32 devices in a mesh: rep: 2 (over y), fs: 4 (over z), tp: 4 (over x, core).
Axes of the slice: x: 2, y: 2, z: 4, core: 2. Of those that a mesh axis runs over, the one named last changes fastest.
Arguments:
- activations: bfloat16 [8, 256, 2048], P(('rep', 'fs'), None, 'tp'), may hold values from -15 to 15
- norm_gain: float32 [2048], replicated, may hold values from 0.1 to 1.9
- w_value: bfloat16 [2048, 2048], P('fs', 'tp'), may hold values from -0.125 to 0.125
- w_gate_conv: bfloat16 [2048, 2048], P('fs', 'tp'), may hold values from -0.125 to 0.125
- conv_weight: float32 [31, 2048], P(None, 'tp'), may hold values from -3 to 3
- chan_gain: float32 [2048], P('tp'), may hold values from 0.1 to 1.9
- w_conv_out: bfloat16 [2048, 2048], P('tp', 'fs'), may hold values from -0.125 to 0.125
- mix_gain: float32 [2048], replicated, may hold values from 0.1 to 1.9
- w_gate: bfloat16 [2048, 3072], P('fs', 'tp'), may hold values from -0.125 to 0.125
- w_up: bfloat16 [2048, 3072], P('fs', 'tp'), may hold values from -0.125 to 0.125
- w_down: bfloat16 [3072, 2048], P('tp', 'fs'), may hold values from -0.109375 to 0.109375
- final_gain: float32 [2048], P('tp'), may hold values from 0.1 to 1.9
Outputs:
- result: bfloat16 [8, 256, 2048], P(('rep', 'fs'), None, 'tp')
The draws below stay inside these ranges and needn't reach their ends.
All inputs are finite; a program needn't handle non-finite values.
Results may differ from the reference program's by a relative error of at most 0.013.
Values may be sent and summed in bfloat16 or wider, within the bound.
A program may use at most 64 MiB of HBM per device.

```python
import jax
import jax.numpy as jnp
from jax import lax

D = 2048
C = 2048
FF = 3072
K = 31
SEQ = 256
BATCH = 8
N_TP = 4


def draw_activations(key, part):
    column = jnp.arange(D, dtype=jnp.float32)
    scale = 0.3 * 10.0 ** (column / (D - 1))
    values = jax.random.normal(key, (BATCH, SEQ, D), jnp.float32) * scale
    return jnp.clip(values, -15.0, 15.0).astype(jnp.bfloat16)


def draw_conv_weight(key, part):
    channel = jnp.arange(C, dtype=jnp.float32)
    scale = 0.35 * 8.0 ** (channel / (C - 1)) / jnp.sqrt(jnp.float32(K))
    values = jnp.clip(jax.random.normal(key, (K, C), jnp.float32), -4.0, 4.0) * scale
    return jnp.clip(values, -3.0, 3.0).astype(jnp.float32)


def levels(key, extent, cuts, least, largest):
    level, own = 1.0, jax.random.fold_in(key, 6)
    for dim, blocks in cuts:
        heights = jnp.exp(jax.random.uniform(jax.random.fold_in(own, dim), (blocks,), jnp.float32, least / len(cuts), largest / len(cuts)))
        level = level * jnp.repeat(heights, extent[dim] // blocks).reshape([-1 if axis == dim else 1 for axis in range(len(extent))])
    return level


def centred(key, shape, scale, limit, pieces=(), kind=jnp.bfloat16):
    array = scale * jax.random.normal(key, shape, jnp.float32)
    if pieces:
        array = array * levels(key, shape, pieces, -0.22, 0.18)
    return jnp.clip(array, -limit, limit).astype(kind)


def setup_inputs(seed: int = 0) -> dict:
    keys = jax.random.split(jax.random.key(seed), 13)
    activations = draw_activations(jax.random.fold_in(keys[12], 71), 0)
    norm_gain = jnp.clip(1.0 + 0.18 * jax.random.normal(keys[1], (D,), jnp.float32), 0.1, 1.9)
    w_value = centred(keys[2], (D, C), D ** -0.5, 0.125, ((0, 4), (1, 4)))
    w_gate_conv = centred(keys[3], (D, C), D ** -0.5, 0.125, ((0, 4), (1, 4)))
    conv_weight = draw_conv_weight(jax.random.fold_in(keys[12], 71), 0)
    chan_gain = jnp.clip(1.0 + 0.18 * jax.random.normal(keys[5], (C,), jnp.float32), 0.1, 1.9)
    w_conv_out = centred(keys[6], (C, D), C ** -0.5, 0.125, ((0, 4), (1, 4)))
    mix_gain = jnp.clip(1.0 + 0.18 * jax.random.normal(keys[7], (D,), jnp.float32), 0.1, 1.9)
    w_gate = centred(keys[8], (D, FF), D ** -0.5, 0.125, ((0, 4), (1, 4)))
    w_up = centred(keys[9], (D, FF), D ** -0.5, 0.125, ((0, 4), (1, 4)))
    w_down = centred(keys[10], (FF, D), FF ** -0.5, 0.109375, ((0, 4), (1, 4)))
    final_gain = jnp.clip(1.0 + 0.18 * jax.random.normal(keys[11], (D,), jnp.float32), 0.1, 1.9)
    return {"activations": activations, "norm_gain": norm_gain, "w_value": w_value, "w_gate_conv": w_gate_conv, "conv_weight": conv_weight, "chan_gain": chan_gain, "w_conv_out": w_conv_out, "mix_gain": mix_gain, "w_gate": w_gate, "w_up": w_up, "w_down": w_down, "final_gain": final_gain}


EPS = 1e-06

def rms_scale(values, gain):
    return values * lax.rsqrt(lax.optimization_barrier(jnp.mean(values * values, axis=-1, keepdims=True)) + EPS) * gain

def blocked_product(left, weight):
    span = weight.shape[0] // N_TP
    total = jnp.zeros((left.shape[0], weight.shape[1]), jnp.float32)
    for block in range(N_TP):
        part = jnp.dot(left[:, block * span:(block + 1) * span], weight[block * span:(block + 1) * span], preferred_element_type=jnp.float32).astype(jnp.bfloat16)
        part = lax.optimization_barrier(part)
        total = total + part.astype(jnp.float32)
    return total

def reference(activations, norm_gain, w_value, w_gate_conv, conv_weight, chan_gain, w_conv_out, mix_gain, w_gate, w_up, w_down, final_gain):

    def one_sequence(sequence):
        residual = sequence.astype(jnp.float32)
        normed_in = rms_scale(residual, norm_gain).astype(jnp.bfloat16)
        value = jnp.dot(normed_in, w_value, preferred_element_type=jnp.float32)
        gate_conv = jnp.dot(normed_in, w_gate_conv, preferred_element_type=jnp.float32)
        glu = value * jax.nn.sigmoid(gate_conv)
        padded = jnp.pad(glu, ((K - 1, 0), (0, 0)))
        conv = jnp.zeros_like(glu)
        for tap in range(K):
            conv = conv + conv_weight[tap][None, :] * padded[tap:tap + SEQ]
        mean = lax.optimization_barrier(jnp.mean(conv, axis=-1, keepdims=True))
        centered = conv - mean
        spread = lax.optimization_barrier(jnp.mean(centered * centered, axis=-1, keepdims=True))
        act = jax.nn.silu(centered * lax.rsqrt(spread + EPS) * chan_gain).astype(jnp.bfloat16)
        first = (residual + blocked_product(act, w_conv_out)).astype(jnp.bfloat16)
        first_f = first.astype(jnp.float32)
        normed_mid = rms_scale(first_f, mix_gain).astype(jnp.bfloat16)
        gate = jnp.dot(normed_mid, w_gate, preferred_element_type=jnp.float32)
        up = jnp.dot(normed_mid, w_up, preferred_element_type=jnp.float32)
        hidden = (jax.nn.silu(gate) * up).astype(jnp.bfloat16)
        second = first_f + blocked_product(hidden, w_down)
        return rms_scale(second, final_gain).astype(jnp.bfloat16)
    return lax.map(one_sequence, activations)
```

```python
import functools

import jax
import jax.numpy as jnp
from jax import lax
from jax.experimental import pallas as pl
from jax.experimental.pallas import tpu as pltpu
from jax.sharding import PartitionSpec as P

EPS = 1e-06
MESH = pl.DeviceIdType.MESH
F32 = jnp.float32
BF16 = jnp.bfloat16


def remote(src, dst, send, recv, target):
    return pltpu.make_async_remote_copy(
        src_ref=src, dst_ref=dst, send_sem=send, recv_sem=recv, device_id=target, device_id_type=MESH
    )


def chunk_of(extent, want):
    return want if extent % want == 0 else extent


def ring_kernel(
    R, F, T, split, length,
    x_ref, ng_ref, cw_ref, cg_ref, mg_ref, fg_ref,
    wv_ref, wg_ref, wo_ref, wga_ref, wup_ref, wd_ref,
    out_ref,
    bv, bg, bo, bga, bup, bd,
    xg, rows, glu, conv, act, part1, part2, got1, got2, firsts, hid, st1, st2, sg1, sg2,
    own_sem, zs, zr, ys, yr, ts, tr,
):
    f = lax.axis_index("fs")
    me = lax.axis_index("tp")
    rep = lax.axis_index("rep")
    count, dt = x_ref.shape
    width = dt * T
    local = [wv_ref, wg_ref, wo_ref, wga_ref, wup_ref, wd_ref]
    bufs = [bv, bg, bo, bga, bup, bd]

    barrier = pltpu.get_barrier_semaphore()
    greeted = 0
    for target in (lax.rem(f + 1, F), lax.rem(f + F - 1, F)):
        pl.semaphore_signal(barrier, inc=1, device_id={"fs": target}, device_id_type=MESH)
        greeted += 1
    if split == 2:
        pl.semaphore_signal(barrier, inc=1, device_id={"rep": 1 - rep}, device_id_type=MESH)
        greeted += 1
    for d in range(1, T):
        pl.semaphore_signal(barrier, inc=1, device_id={"tp": lax.rem(me + d, T)}, device_id_type=MESH)
        greeted += 1
    own = [
        pltpu.make_async_copy(local[w], bufs[w].at[f], own_sem.at[w]) for w in range(6)
    ]
    for copy in own:
        copy.start()
    pl.semaphore_wait(barrier, greeted)

    def half(w):
        n = local[w].shape[0] // split
        return pl.ds(pl.multiple_of((rep if split == 2 else 0) * n, n), n)

    def other(w):
        n = local[w].shape[0] // split
        return pl.ds(pl.multiple_of((1 - rep) * n, n), n)

    def hop(w, side, s):
        shard = f - s if side == 0 else f + s
        target = f + 1 if side == 0 else f - 1
        src = local[w].at[half(w)] if s == 0 else bufs[w].at[shard, half(w)]
        return remote(src, bufs[w].at[shard, half(w)], zs.at[side, w, s], zr.at[side, w, s + 1], {"fs": target})

    def arrival(w, side, s):
        shard = f - s if side == 0 else f + s
        ref = bufs[w].at[shard, half(w)]
        return remote(ref, ref, zs.at[side, w, s], zr.at[side, w, s], {"fs": f})

    def across(w, side, s):
        shard = f - s if side == 0 else f + s
        ref = bufs[w].at[shard, half(w)]
        return remote(ref, ref, ys.at[side, w, s], yr.at[side, w, s], {"rep": 1 - rep})

    def across_in(w, side, s):
        shard = f - s if side == 0 else f + s
        ref = bufs[w].at[shard, other(w)]
        return remote(ref, ref, ys.at[side, w, s], yr.at[side, w, s], {"rep": 1 - rep})

    def has(side, s):
        return f >= s if side == 0 else f + s <= F - 1

    def sends(side, s):
        ahead = f < F - 1 if side == 0 else f > 0
        return jnp.logical_and(has(side, s), ahead)

    def launch(w):
        for side in (0, 1):
            @pl.when(sends(side, 0))
            def _():
                hop(w, side, 0).start()

    def relay(group, stages=range(1, F)):
        for s in stages:
            for w in group:
                for side in (0, 1):
                    @pl.when(has(side, s))
                    def _():
                        arrival(w, side, s).wait_recv()
                        if s < F - 1:
                            @pl.when(sends(side, s))
                            def _():
                                hop(w, side, s).start()
                        if split == 2:
                            across(w, side, s).start()

    def settle(group):
        for w in group:
            own[w].wait()
        if split == 2:
            for s in range(1, F):
                for w in group:
                    for side in (0, 1):
                        @pl.when(has(side, s))
                        def _():
                            across_in(w, side, s).wait_recv()

    def tp_send(k, src, dst_at, d):
        return remote(src, dst_at, ts.at[k, d], tr.at[k, d], {"tp": lax.rem(me + d, T)})

    for w in (0, 1):
        launch(w)
    for d in range(1, T):
        tp_send(0, x_ref, xg.at[me], d).start()
    launch(2)
    xg[me] = x_ref[...]
    for d in range(1, T):
        peer = lax.rem(me + T - d, T)
        tp_send(0, x_ref, xg.at[peer], d).wait_recv()

    block = chunk_of(count, 16)

    def norm_rows(src, gain):
        def step(i, _):
            r = pl.ds(pl.multiple_of(i * block, block), block)
            vals = [src[t, r, :].astype(F32) for t in range(T)]
            ss = sum(jnp.sum(v * v, axis=1, keepdims=True) for v in vals)
            scale = lax.rsqrt(ss / width + EPS)
            for t in range(T):
                rows[r, t * dt:(t + 1) * dt] = (
                    vals[t] * scale * gain[t:t + 1, :]
                ).astype(BF16)
            return 0
        lax.fori_loop(0, count // block, step, 0)

    norm_rows(xg, ng_ref)
    relay((0, 1, 2))
    for w in (3, 4, 5):
        launch(w)
    settle((0, 1))

    chan = bv.shape[2]
    batch = count // length
    taps = cw_ref.shape[0]
    pad = 8 * ((taps - 1 + 7) // 8)
    lead = pad - (taps - 1)

    def columns(buf, c, n):
        block_w = buf[:, :, pl.ds(pl.multiple_of(c * n, n), n)]
        return block_w.reshape(block_w.shape[0] * block_w.shape[1], n)

    nc = chunk_of(chan, 256)

    def glu_step(c, _):
        value = jnp.dot(rows[...], columns(bv, c, nc), preferred_element_type=F32)
        gate = jnp.dot(rows[...], columns(bg, c, nc), preferred_element_type=F32)
        res = value * jax.nn.sigmoid(gate)
        for b in range(batch):
            glu[b, pl.ds(pad, length), pl.ds(pl.multiple_of(c * nc, nc), nc)] = (
                res[b * length:(b + 1) * length]
            )
        return 0

    for b in range(batch):
        glu[b, 0:pad, :] = jnp.zeros((pad, chan), F32)
        glu[b, pad + length:, :] = jnp.zeros((8, chan), F32)
    lax.fori_loop(0, chan // nc, glu_step, 0)
    relay((3,), (1,))

    lanes = chunk_of(chan, 128)
    span = chunk_of(length, 64)
    strips = chan // lanes

    def conv_step(i, _):
        q = lax.rem(i, strips)
        p = i // strips
        cols = pl.ds(pl.multiple_of(q * lanes, lanes), lanes)
        weights = cw_ref[:, cols]
        for b in range(batch):
            total = jnp.zeros((span, lanes), F32)
            for shift in range(8):
                acc = None
                for tap in range(taps):
                    if (lead + tap) % 8 != shift:
                        continue
                    base = lead + tap - shift
                    term = weights[tap:tap + 1, :] * glu[
                        b, pl.ds(pl.multiple_of(p * span + base, 8), span + 8), cols
                    ]
                    acc = term if acc is None else acc + term
                if acc is not None:
                    total = total + acc[shift:shift + span]
            conv[pl.ds(pl.multiple_of(b * length + p * span, span), span), cols] = total
        return 0

    lax.fori_loop(0, strips * (length // span), conv_step, 0)

    lane = lax.broadcasted_iota(jnp.int32, (count, 128), 1)

    def across_lanes(a, b):
        table = jnp.where(lane == 0, a, jnp.where(lane == 1, b, 0.0))
        return jnp.transpose(table)[0:8, :]

    def down_rows(top):
        full = jnp.concatenate([top, jnp.zeros((120, count), F32)], axis=0)
        return jnp.transpose(full)

    values = conv[...]
    local_sum = jnp.sum(values, axis=1, keepdims=True)
    dev = values - local_sum / chan
    st1[...] = across_lanes(local_sum, jnp.sum(dev * dev, axis=1, keepdims=True))
    sg1[me] = st1[...]
    for d in range(1, T):
        tp_send(1, st1, sg1.at[me], d).start()
    relay((4,), (1,))
    for d in range(1, T):
        peer = lax.rem(me + T - d, T)
        tp_send(1, st1, sg1.at[peer], d).wait_recv()
    sums = [sg1[t] for t in range(T)]
    mean = sum(s[0:1, :] for s in sums) / (chan * T)
    spread = sum(
        s[1:2, :] + chan * (s[0:1, :] / chan - mean) * (s[0:1, :] / chan - mean) for s in sums
    ) / (chan * T)
    inv = lax.rsqrt(spread + EPS)
    line = lax.broadcasted_iota(jnp.int32, (8, count), 0)
    table = down_rows(jnp.where(line == 0, mean, jnp.where(line == 1, inv, 0.0)))
    normed = (conv[...] - table[:, 0:1]) * table[:, 1:2] * cg_ref[...]
    act[...] = (normed * jax.nn.sigmoid(normed)).astype(BF16)

    settle((2,))

    def project(src, buf, part):
        dsh = buf.shape[2]
        for j in range(F):
            t, off = (j * dsh) // dt, (j * dsh) % dt
            prod = jnp.dot(src[...], buf[j], preferred_element_type=F32)
            part[t, :, off:off + dsh] = prod.astype(BF16)

    def scatter(k, part, got):
        for d in range(1, T):
            tp_send(k, part.at[lax.rem(me + d, T)], got.at[d - 1], d).start()

    def gathered(k, part, got):
        total = part[me].astype(F32)
        for d in range(1, T):
            tp_send(k, part.at[me], got.at[d - 1], d).wait_recv()
            total = total + got[d - 1].astype(F32)
        return total

    def piece(t):
        return remote(part2.at[t], got2.at[me], ts.at[4, t], tr.at[4, me], {"tp": t})

    def piece_in(t):
        return remote(part2.at[t], got2.at[t], ts.at[4, t], tr.at[4, t], {"tp": t})

    project(act, bo, part1)
    scatter(2, part1, got1)
    relay((5,), (1,))
    first = (x_ref[...].astype(F32) + gathered(2, part1, got1)).astype(BF16)
    firsts[me] = first
    for d in range(1, T):
        tp_send(3, firsts.at[me], firsts.at[me], d).start()
    relay((3,), (2,))
    for d in range(1, T):
        peer = lax.rem(me + T - d, T)
        tp_send(3, firsts.at[peer], firsts.at[peer], d).wait_recv()
    relay((4,), (2,))
    norm_rows(firsts, mg_ref)
    relay((5,), (2,))
    relay((3, 4), range(3, F))
    settle((3, 4))

    ff = bga.shape[2]
    nf = chunk_of(ff, 256)

    def ff_step(c, _):
        gate = jnp.dot(rows[...], columns(bga, c, nf), preferred_element_type=F32)
        up = jnp.dot(rows[...], columns(bup, c, nf), preferred_element_type=F32)
        hid[:, pl.ds(pl.multiple_of(c * nf, nf), nf)] = (
            gate * jax.nn.sigmoid(gate) * up
        ).astype(BF16)
        return 0

    lax.fori_loop(0, ff // nf, ff_step, 0)
    if F == T and bd.shape[2] == dt:
        def down(shard):
            prod = jnp.dot(hid[...], bd[shard], preferred_element_type=F32)
            part2[shard] = prod.astype(BF16)

            @pl.when(shard != me)
            def _():
                piece(shard).start()

        own[5].wait()
        down(f)
        for s in range(1, F):
            if s >= 3:
                relay((5,), (s,))
            for side in (0, 1):
                @pl.when(has(side, s))
                def _():
                    if split == 2:
                        across_in(5, side, s).wait_recv()
                    down(f - s if side == 0 else f + s)
    else:
        relay((5,), range(3, F))
        settle((5,))
        project(hid, bd, part2)
        for d in range(1, T):
            piece(lax.rem(me + d, T)).start()
    second = firsts[me].astype(F32) + part2[me].astype(F32)
    for d in range(1, T):
        peer = lax.rem(me + d, T)
        piece_in(peer).wait_recv()
        second = second + got2[peer].astype(F32)
    total = jnp.sum(second * second, axis=1, keepdims=True)
    conv[:, 0:dt] = second
    st2[...] = across_lanes(total, total)
    sg2[me] = st2[...]
    for d in range(1, T):
        tp_send(5, st2, sg2.at[me], d).start()
    for d in range(1, T):
        peer = lax.rem(me + T - d, T)
        tp_send(5, st2, sg2.at[peer], d).wait_recv()
    full = sum(sg2[t] for t in range(T))
    table = down_rows(full)
    scale = lax.rsqrt(table[:, 0:1] / width + EPS)
    out_ref[...] = (conv[:, 0:dt] * scale * fg_ref[...]).astype(BF16)

    for w in range(6):
        for side in (0, 1):
            for s in range(F):
                if s < F - 1:
                    @pl.when(sends(side, s))
                    def _():
                        hop(w, side, s).wait_send()
                if s >= 1 and split == 2:
                    @pl.when(has(side, s))
                    def _():
                        across(w, side, s).wait_send()
    for d in range(1, T):
        peer = lax.rem(me + d, T)
        tp_send(0, x_ref, xg.at[me], d).wait_send()
        tp_send(1, st1, sg1.at[me], d).wait_send()
        tp_send(2, part1.at[peer], got1.at[d - 1], d).wait_send()
        tp_send(3, firsts.at[me], firsts.at[me], d).wait_send()
        piece(peer).wait_send()
        tp_send(5, st2, sg2.at[me], d).wait_send()


CH = 2


def fast_kernel(
    length,
    x_ref, ng_ref, cw_ref, cg_ref, mg_ref, fg_ref,
    wv_ref, wg_ref, wo_ref, wga_ref, wup_ref, wd_ref,
    out_ref,
    bv, bg, bo, bga, bup, bd,
    xg, rows, accv, accg, glu, conv, act, part, got, q1, q1in, firsts, hid,
    part2, got2, q2, q2in, sec, secb, secin, st1, sg1, st2, sg2, fin, finin,
    own_sem, zs, zr, ms, mr, ys, yr, xos, xor_, ags, agr, sts, str_, rss, rsr, ds_, dr, qs, qr, os_, orr,
):
    f = lax.axis_index("fs")
    me = lax.axis_index("tp")
    rep = lax.axis_index("rep")
    count, dt = x_ref.shape
    T = 4
    width = dt * T
    rows_all = 2 * count
    batch = count // length
    chan, ff = bv.shape[2], bga.shape[2]
    local = [wv_ref, wg_ref, wo_ref, wga_ref, wup_ref, wd_ref]
    bufs = [bv, bg, bo, bga, bup, bd]
    VAL, GATE, CVO, GA, UP, DOWN = range(6)
    outer = jnp.logical_or(f == 0, f == 3)
    near = 1 + f // 3
    po, pi, fo = 3 * (f - 1), 3 - f, 3 * (2 - f)
    sib = me + 1 - 2 * lax.rem(me, 2)
    mir = lax.rem(me + 2, T)
    dia = lax.rem(sib + 2, T)

    def view(ref, w, h, c):
        if w == DOWN:
            n = ref.shape[1] // 2
            k = n // CH
            return ref.at[:, pl.ds(pl.multiple_of(h * n + c * k, k), k)]
        n = ref.shape[0] // 2
        k = n // CH
        return ref.at[pl.ds(pl.multiple_of(h * n + c * k, k), k), :]

    barrier = pltpu.get_barrier_semaphore()

    def greet(**target):
        pl.semaphore_signal(barrier, inc=1, device_id=target, device_id_type=MESH)

    def zsend(w, hs, c):
        h = rep if hs == 0 else 1 - rep
        return remote(
            view(local[w], w, h, c), view(bufs[w].at[f], w, h, c), zs.at[w, hs, c], zr.at[w, hs, c], {"fs": near}
        )

    def xsend():
        return remote(x_ref, xg.at[me, 0], xos, xor_, {"fs": near})

    def result_sends():
        return (
            remote(secb, secin, os_.at[0], orr.at[0], {"fs": po}),
            remote(fin, finin, os_.at[1], orr.at[1], {"fs": po}),
        )

    lane = lax.broadcasted_iota(jnp.int32, (count, 128), 1)
    line = lax.broadcasted_iota(jnp.int32, (8, count), 0)

    def across_lanes(a, b):
        table = jnp.where(lane == 0, a, jnp.where(lane == 1, b, 0.0))
        return jnp.transpose(table)[0:8, :]

    def down_rows(top):
        full = jnp.concatenate([top, jnp.zeros((120, count), F32)], axis=0)
        return jnp.transpose(full)

    @pl.when(outer)
    def _():
        greet(fs=near)
        pl.semaphore_wait(barrier, 1)
        order = [(VAL, 0), (GATE, 0), None, (CVO, 0), (VAL, 1), (GATE, 1), (CVO, 1), (GA, 0), (UP, 0), (GA, 1)]
        for item in order:
            if item is None:
                xsend().start()
            else:
                for c in range(CH):
                    zsend(item[0], item[1], c).start()
        zsend(DOWN, 0, 0).start()
        for c in range(CH):
            zsend(UP, 1, c).start()
        for c in range(1, CH):
            zsend(DOWN, 0, c).start()
        for c in range(CH):
            zsend(DOWN, 1, c).start()
        xsend().wait_send()
        for w in range(6):
            for hs in range(2):
                for c in range(CH):
                    zsend(w, hs, c).wait_send()
        for r in (remote(secb, secin, os_.at[0], orr.at[0], {"fs": near}),
                  remote(fin, finin, os_.at[1], orr.at[1], {"fs": near})):
            r.wait_recv()
        scale = lax.rsqrt(down_rows(finin[...])[:, 0:1] / width + EPS)
        out_ref[...] = (secin[...].astype(F32) * scale * fg_ref[...]).astype(BF16)

    @pl.when(jnp.logical_not(outer))
    def _():
        greet(fs=po)
        greet(fs=pi)
        greet(rep=1 - rep)
        for t in (sib, mir, dia):
            greet(tp=t)
        own = [pltpu.make_async_copy(local[w], bufs[w].at[f], own_sem.at[w]) for w in range(6)]
        for copy in own:
            copy.start()
        pl.semaphore_wait(barrier, 6)

        def arrived(ref, send, recv):
            remote(ref, ref, send, recv, {"fs": f}).wait_recv()

        def mid_own(w, c):
            return remote(
                view(local[w], w, rep, c), view(bufs[w].at[f], w, rep, c), ms.at[w, 0, c], mr.at[w, 0, c], {"fs": pi}
            )

        def mid_fwd(w, c):
            ref = view(bufs[w].at[po], w, rep, c)
            return remote(ref, ref, ms.at[w, 1, c], mr.at[w, 1, c], {"fs": pi})

        def y_fwd(w, k, c):
            ref = view(bufs[w].at[fo if k else pi], w, rep, c)
            return remote(ref, ref, ys.at[w, k, c], yr.at[w, k, c], {"rep": 1 - rep})

        def send_own(w):
            for c in range(CH):
                mid_own(w, c).start()

        def relay_mid(w, c):
            arrived(view(bufs[w].at[po], w, rep, c), zs.at[w, 0, c], zr.at[w, 0, c])
            mid_fwd(w, c).start()

        def relay_y(w, k, c):
            arrived(view(bufs[w].at[fo if k else pi], w, rep, c), ms.at[w, k, c], mr.at[w, k, c])
            y_fwd(w, k, c).start()

        def wait_z(w):
            for c in range(CH):
                arrived(view(bufs[w].at[po], w, 1 - rep, c), zs.at[w, 1, c], zr.at[w, 1, c])

        def wait_y(w, k):
            for c in range(CH):
                arrived(view(bufs[w].at[fo if k else pi], w, 1 - rep, c), ys.at[w, k, c], yr.at[w, k, c])

        def ag(p, buf, slot, kind):
            ref = buf.at[mir if kind == 2 else me, slot]
            return remote(ref, ref, ags.at[p, slot, kind], agr.at[p, slot, kind], {"tp": mir if kind == 1 else sib})

        def ag_in(p, buf, slot, kind):
            ref = buf.at[(sib, mir, dia)[kind], slot]
            return remote(ref, ref, ags.at[p, slot, kind], agr.at[p, slot, kind], {"tp": me})

        def ag_start(p, buf, slot):
            ag(p, buf, slot, 1).start()
            ag(p, buf, slot, 0).start()

        def ag_forward(p, buf, slot):
            ag_in(p, buf, slot, 1).wait_recv()
            ag(p, buf, slot, 2).start()

        def ag_finish(p, buf, slot):
            ag_in(p, buf, slot, 0).wait_recv()
            ag_in(p, buf, slot, 2).wait_recv()

        block = chunk_of(count, 16)

        def norm_rows(src, slot, gain):
            def step(i, _):
                r = pl.ds(pl.multiple_of(i * block, block), block)
                o = pl.ds(pl.multiple_of(slot * count + i * block, block), block)
                vals = [src[t, slot, r, :].astype(F32) for t in range(T)]
                ss = sum(jnp.sum(v * v, axis=1, keepdims=True) for v in vals)
                scale = lax.rsqrt(ss / width + EPS)
                for t in range(T):
                    rows[t, o, :] = (vals[t] * scale * gain[:, t * dt:(t + 1) * dt]).astype(BF16)
                return 0
            lax.fori_loop(0, count // block, step, 0)

        def stat(k, slot, src, dst, d):
            return remote(src, dst, sts.at[k, slot, d], str_.at[k, slot, d], {"tp": lax.rem(me + d, T)})

        def stat_send(k, slot, src, dst):
            for d in range(1, T):
                stat(k, slot, src.at[slot], dst.at[slot, me], d).start()

        def stat_wait(k, slot, src, dst):
            for d in range(1, T):
                stat(k, slot, src.at[slot], dst.at[slot, lax.rem(me + T - d, T)], d).wait_recv()

        xg[me, 1] = x_ref[...]
        send_own(VAL)
        send_own(GATE)
        remote(x_ref, xg.at[me, 1], ags.at[0, 1, 1], agr.at[0, 1, 1], {"tp": mir}).start()
        remote(x_ref, xg.at[me, 1], ags.at[0, 1, 0], agr.at[0, 1, 0], {"tp": sib}).start()
        for c in range(CH):
            relay_mid(VAL, c)
            relay_y(VAL, 0, c)
        ag_forward(0, xg, 1)
        for c in range(CH):
            relay_mid(GATE, c)
            relay_y(GATE, 0, c)
        send_own(CVO)
        ag_finish(0, xg, 1)
        norm_rows(xg, 1, ng_ref)
        relay_y(VAL, 1, 0)
        arrived(xg.at[me, 0], xos, xor_)
        ag_start(0, xg, 0)
        for c in range(1, CH):
            relay_y(VAL, 1, c)
        for c in range(CH):
            relay_mid(CVO, c)
            relay_y(GATE, 1, c)
        send_own(GA)
        send_own(UP)
        ag_forward(0, xg, 0)
        relay_y(CVO, 0, 0)
        ag_finish(0, xg, 0)
        norm_rows(xg, 0, ng_ref)

        pad = glu.shape[1] - length - 8
        taps = cw_ref.shape[0]
        lead = pad - (taps - 1)
        nc = chunk_of(chan, 256)
        for b in range(2 * batch):
            glu[b, 0:pad, :] = jnp.zeros((pad, chan), F32)
            glu[b, pad + length:, :] = jnp.zeros((8, chan), F32)

        def s1(shard, first, last):
            def step(c, _):
                cols = pl.ds(pl.multiple_of(c * nc, nc), nc)
                value = jnp.dot(rows[shard], bv[shard, :, cols], preferred_element_type=F32)
                gate = jnp.dot(rows[shard], bg[shard, :, cols], preferred_element_type=F32)
                if not first:
                    value = value + accv[:, cols]
                    gate = gate + accg[:, cols]
                if last:
                    res = value * jax.nn.sigmoid(gate)
                    for b in range(2 * batch):
                        glu[b, pl.ds(pad, length), cols] = res[b * length:(b + 1) * length]
                else:
                    accv[:, cols] = value
                    accg[:, cols] = gate
                return 0
            lax.fori_loop(0, chan // nc, step, 0)

        own[VAL].wait()
        own[GATE].wait()
        s1(f, True, False)
        wait_y(VAL, 0)
        wait_y(GATE, 0)
        s1(pi, False, False)
        for c in range(1, CH):
            relay_y(CVO, 0, c)
        wait_y(VAL, 1)
        wait_y(GATE, 1)
        s1(fo, False, False)
        relay_y(CVO, 1, 0)
        wait_z(VAL)
        wait_z(GATE)
        s1(po, False, True)
        for c in range(1, CH):
            relay_y(CVO, 1, c)

        lanes = chunk_of(chan, 128)
        span = chunk_of(length, 64)
        strips = chan // lanes

        def convolve(slot):
            def step(i, _):
                s = lax.rem(i, strips)
                p = i // strips
                cols = pl.ds(pl.multiple_of(s * lanes, lanes), lanes)
                weights = cw_ref[:, cols]
                for b in range(batch):
                    total = jnp.zeros((span, lanes), F32)
                    for shift in range(8):
                        acc = None
                        for tap in range(taps):
                            if (lead + tap) % 8 != shift:
                                continue
                            base = lead + tap - shift
                            term = weights[tap:tap + 1, :] * glu[
                                slot * batch + b, pl.ds(pl.multiple_of(p * span + base, 8), span + 8), cols
                            ]
                            acc = term if acc is None else acc + term
                        if acc is not None:
                            total = total + acc[shift:shift + span]
                    at = pl.multiple_of(slot * count + b * length + p * span, span)
                    conv[pl.ds(at, span), cols] = total
                return 0
            lax.fori_loop(0, strips * (length // span), step, 0)

        def span_of(slot):
            return slice(slot * count, (slot + 1) * count)

        def conv_stats(slot):
            values = conv[span_of(slot), :]
            local_sum = jnp.sum(values, axis=1, keepdims=True)
            dev = values - local_sum / chan
            st1[slot] = across_lanes(local_sum, jnp.sum(dev * dev, axis=1, keepdims=True))
            sg1[slot, me] = st1[slot]
            stat_send(0, slot, st1, sg1)

        def activate(slot):
            stat_wait(0, slot, st1, sg1)
            sums = [sg1[slot, t] for t in range(T)]
            mean = sum(s[0:1, :] for s in sums) / (chan * T)
            spread = sum(
                s[1:2, :] + chan * (s[0:1, :] / chan - mean) * (s[0:1, :] / chan - mean) for s in sums
            ) / (chan * T)
            inv = lax.rsqrt(spread + EPS)
            table = down_rows(jnp.where(line == 0, mean, jnp.where(line == 1, inv, 0.0)))
            normed = (conv[span_of(slot), :] - table[:, 0:1]) * table[:, 1:2] * cg_ref[...]
            act[span_of(slot), :] = (normed * jax.nn.sigmoid(normed)).astype(BF16)

        def rs(slot, kind):
            if kind == 2:
                return remote(q1.at[slot], q1in.at[slot], rss.at[slot, 2], rsr.at[slot, 2], {"tp": mir})
            return remote(
                part.at[slot, dia if kind else sib], got.at[slot, kind],
                rss.at[slot, kind], rsr.at[slot, kind], {"tp": sib},
            )

        def project(slot):
            def step(j, _):
                prod = jnp.dot(act[span_of(slot), :], bo[j], preferred_element_type=F32)
                part[slot, j] = prod.astype(BF16)
                return 0
            lax.fori_loop(0, T, step, 0)
            rs(slot, 1).start()
            rs(slot, 0).start()

        def pair_sum(slot):
            rs(slot, 1).wait_recv()
            q1[slot] = (part[slot, mir].astype(F32) + got[slot, 1].astype(F32)).astype(BF16)
            rs(slot, 2).start()

        def finish_first(slot):
            rs(slot, 0).wait_recv()
            total = xg[me, slot].astype(F32) + (part[slot, me].astype(F32) + got[slot, 0].astype(F32))
            rs(slot, 2).wait_recv()
            firsts[me, slot] = (total + q1in[slot].astype(F32)).astype(BF16)
            ag_start(1, firsts, slot)

        convolve(0)
        conv_stats(0)
        relay_y(GA, 0, 0)
        convolve(1)
        conv_stats(1)
        own[CVO].wait()
        wait_y(CVO, 0)
        wait_y(CVO, 1)
        wait_z(CVO)
        activate(0)
        project(0)
        for c in range(1, CH):
            relay_y(GA, 0, c)
        activate(1)
        project(1)
        pair_sum(0)
        relay_mid(GA, 0)
        pair_sum(1)
        relay_y(UP, 0, 0)
        for c in range(1, CH):
            relay_mid(GA, c)
        finish_first(0)
        relay_y(UP, 0, 1)
        relay_mid(UP, 0)
        relay_y(GA, 1, 0)
        finish_first(1)
        ag_forward(1, firsts, 0)
        for c in range(1, CH):
            relay_mid(UP, c)
        send_own(DOWN)
        for c in range(1, CH):
            relay_y(GA, 1, c)
        ag_finish(1, firsts, 0)
        norm_rows(firsts, 0, mg_ref)
        ag_forward(1, firsts, 1)
        relay_y(UP, 1, 0)
        ag_finish(1, firsts, 1)
        norm_rows(firsts, 1, mg_ref)
        for c in range(1, CH):
            relay_y(UP, 1, c)
        relay_mid(DOWN, 0)
        relay_y(DOWN, 0, 0)

        own[GA].wait()
        own[UP].wait()
        for w in (GA, UP):
            wait_y(w, 0)
            wait_y(w, 1)
            wait_z(w)
        nf = chunk_of(ff, 256)

        def ff_step(c, _):
            cols = pl.ds(pl.multiple_of(c * nf, nf), nf)
            gate = sum(jnp.dot(rows[t], bga[t, :, cols], preferred_element_type=F32) for t in range(T))
            up = sum(jnp.dot(rows[t], bup[t, :, cols], preferred_element_type=F32) for t in range(T))
            hid[:, cols] = (gate * jax.nn.sigmoid(gate) * up).astype(BF16)
            return 0

        lax.fori_loop(0, ff // nf, ff_step, 0)

        hn = dt // 2

        def hcols(h):
            return pl.ds(pl.multiple_of(h * hn, hn), hn)

        def pair_send(b, h, n):
            return remote(part2.at[b, :, hcols(h)], got2.at[b, :, hcols(h)], ds_.at[b, n], dr.at[b, n], {"tp": sib})

        def cross(h, n):
            return remote(q2.at[:, hcols(h)], q2in.at[:, hcols(h)], qs.at[n], qr.at[n], {"tp": mir})

        def down(b, n):
            h = rep if n == 0 else 1 - rep
            prod = jnp.dot(hid[...], bd[b, :, hcols(h)], preferred_element_type=F32)
            part2[b, :, hcols(h)] = prod.astype(BF16)

            @pl.when(jnp.logical_or(b == sib, b == dia))
            def _():
                pair_send(b, h, n).start()

        def combine(b, n):
            h = rep if n == 0 else 1 - rep

            @pl.when(b == mir)
            def _():
                pair_send(b, h, n).wait_recv()
                q2[:, hcols(h)] = (part2[b, :, hcols(h)].astype(F32) + got2[b, :, hcols(h)].astype(F32)).astype(BF16)
                cross(h, n).start()

        own[DOWN].wait()
        down(f, 0)
        down(f, 1)
        combine(f, 0)
        for c in range(1, CH):
            relay_mid(DOWN, c)
        down(po, 0)
        combine(f, 1)
        for c in range(1, CH):
            relay_y(DOWN, 0, c)
        down(pi, 0)
        combine(po, 0)
        relay_y(DOWN, 1, 0)
        wait_y(DOWN, 0)
        down(pi, 1)
        combine(pi, 0)
        for c in range(1, CH):
            relay_y(DOWN, 1, c)
        down(fo, 0)
        combine(pi, 1)
        wait_z(DOWN)
        down(po, 1)
        combine(fo, 0)
        wait_y(DOWN, 1)
        down(fo, 1)
        combine(po, 1)
        combine(fo, 1)

        for n in range(2):
            h = rep if n == 0 else 1 - rep
            pair_send(me, h, n).wait_recv()
        for n in range(2):
            h = rep if n == 0 else 1 - rep
            cross(h, n).wait_recv()

        def finish(slot):
            r = span_of(slot)
            second = firsts[me, slot].astype(F32) + part2[me, r, :].astype(F32) + got2[me, r, :].astype(F32)
            second = second + q2in[r, :].astype(F32)
            total = jnp.sum(second * second, axis=1, keepdims=True)
            if slot == 0:
                secb[...] = second.astype(BF16)
                result_sends()[0].start()
            else:
                sec[...] = second
            st2[slot] = across_lanes(total, total)
            sg2[slot, me] = st2[slot]
            stat_send(1, slot, st2, sg2)

        finish(0)
        finish(1)
        stat_wait(1, 0, st2, sg2)
        fin[...] = sum(sg2[0, t] for t in range(T))
        result_sends()[1].start()
        stat_wait(1, 1, st2, sg2)
        table = down_rows(sum(sg2[1, t] for t in range(T)))
        scale = lax.rsqrt(table[:, 0:1] / width + EPS)
        out_ref[...] = (sec[...] * scale * fg_ref[...]).astype(BF16)

        for w in range(6):
            for c in range(CH):
                mid_own(w, c).wait_send()
                mid_fwd(w, c).wait_send()
                for k in range(2):
                    y_fwd(w, k, c).wait_send()
        for slot in range(2):
            for kind in range(3):
                ag(0, xg, slot, kind).wait_send()
                ag(1, firsts, slot, kind).wait_send()
                rs(slot, kind).wait_send()
            for d in range(1, T):
                stat(0, slot, st1.at[slot], sg1.at[slot, me], d).wait_send()
                stat(1, slot, st2.at[slot], sg2.at[slot, me], d).wait_send()
        for n in range(2):
            h = rep if n == 0 else 1 - rep
            pair_send(sib, h, n).wait_send()
            pair_send(dia, h, n).wait_send()
            cross(h, n).wait_send()
        for r in result_sends():
            r.wait_send()


def fast_body(
    activations, norm_gain, w_value, w_gate_conv, conv_weight, chan_gain,
    w_conv_out, mix_gain, w_gate, w_up, w_down, final_gain,
):
    batch, length, dt = activations.shape
    count = batch * length
    weights = (w_value, w_gate_conv, w_conv_out, w_gate, w_up, w_down)
    chan, ff = w_value.shape[1], w_gate.shape[1]
    T = 4
    pad = 8 * ((conv_weight.shape[0] - 1 + 7) // 8)
    rows_all = 2 * count
    vmem, hbm = pl.BlockSpec(memory_space=pltpu.VMEM), pl.BlockSpec(memory_space=pl.ANY)
    dma = pltpu.SemaphoreType.DMA
    V = pltpu.VMEM
    out = pl.pallas_call(
        functools.partial(fast_kernel, length),
        out_shape=jax.ShapeDtypeStruct((count, dt), BF16),
        in_specs=[vmem] * 6 + [hbm] * 6,
        out_specs=vmem,
        scratch_shapes=[V((4,) + w.shape, BF16) for w in weights] + [
            V((T, 2, count, dt), BF16),
            V((T, rows_all, dt), BF16),
            V((rows_all, chan), F32),
            V((rows_all, chan), F32),
            V((2 * batch, pad + length + 8, chan), F32),
            V((rows_all, chan), F32),
            V((rows_all, chan), BF16),
            V((2, T, count, dt), BF16),
            V((2, 2, count, dt), BF16),
            V((2, count, dt), BF16),
            V((2, count, dt), BF16),
            V((T, 2, count, dt), BF16),
            V((rows_all, ff), BF16),
            V((T, rows_all, dt), BF16),
            V((T, rows_all, dt), BF16),
            V((rows_all, dt), BF16),
            V((rows_all, dt), BF16),
            V((count, dt), F32),
            V((count, dt), BF16),
            V((count, dt), BF16),
            V((2, 8, count), F32),
            V((2, T, 8, count), F32),
            V((2, 8, count), F32),
            V((2, T, 8, count), F32),
            V((8, count), F32),
            V((8, count), F32),
            dma((6,)),
            dma((6, 2, CH)),
            dma((6, 2, CH)),
            dma((6, 2, CH)),
            dma((6, 2, CH)),
            dma((6, 2, CH)),
            dma((6, 2, CH)),
            dma(()),
            dma(()),
            dma((2, 2, 3)),
            dma((2, 2, 3)),
            dma((2, 2, T)),
            dma((2, 2, T)),
            dma((2, 3)),
            dma((2, 3)),
            dma((T, 2)),
            dma((T, 2)),
            dma((2,)),
            dma((2,)),
            dma((2,)),
            dma((2,)),
        ],
        compiler_params=pltpu.CompilerParams(
            collective_id=0, has_side_effects=True, vmem_limit_bytes=60 * 1024 * 1024
        ),
        name="block",
    )(
        activations.reshape(count, dt),
        norm_gain.reshape(1, dt * T),
        conv_weight,
        chan_gain.reshape(1, chan),
        mix_gain.reshape(1, dt * T),
        final_gain.reshape(1, dt),
        *weights,
    )
    return out.reshape(batch, length, dt)


def ring_body(
    activations, norm_gain, w_value, w_gate_conv, conv_weight, chan_gain,
    w_conv_out, mix_gain, w_gate, w_up, w_down, final_gain,
):
    batch, length, dt = activations.shape
    count = batch * length
    R, F, T = lax.axis_size("rep"), lax.axis_size("fs"), lax.axis_size("tp")
    weights = (w_value, w_gate_conv, w_conv_out, w_gate, w_up, w_down)
    split = 2 if R == 2 and all(w.shape[0] % 32 == 0 for w in weights) else 1
    width = dt * T
    chan, ff = w_value.shape[1], w_gate.shape[1]
    taps = conv_weight.shape[0]
    pad = 8 * ((taps - 1 + 7) // 8)
    vmem, hbm = pl.BlockSpec(memory_space=pltpu.VMEM), pl.BlockSpec(memory_space=pl.ANY)
    ysh = (2, 6, F) if split == 2 else (1,)
    dma = pltpu.SemaphoreType.DMA
    out = pl.pallas_call(
        functools.partial(ring_kernel, R, F, T, split, length),
        out_shape=jax.ShapeDtypeStruct((count, dt), BF16),
        in_specs=[vmem] * 6 + [hbm] * 6,
        out_specs=vmem,
        scratch_shapes=[pltpu.VMEM((F,) + w.shape, BF16) for w in weights] + [
            pltpu.VMEM((T, count, dt), BF16),
            pltpu.VMEM((count, width), BF16),
            pltpu.VMEM((batch, pad + length + 8, chan), F32),
            pltpu.VMEM((count, max(chan, dt)), F32),
            pltpu.VMEM((count, chan), BF16),
            pltpu.VMEM((T, count, dt), BF16),
            pltpu.VMEM((T, count, dt), BF16),
            pltpu.VMEM((T - 1, count, dt), BF16),
            pltpu.VMEM((T, count, dt), BF16),
            pltpu.VMEM((T, count, dt), BF16),
            pltpu.VMEM((count, ff), BF16),
            pltpu.VMEM((8, count), F32),
            pltpu.VMEM((8, count), F32),
            pltpu.VMEM((T, 8, count), F32),
            pltpu.VMEM((T, 8, count), F32),
            dma((6,)),
            dma((2, 6, F)),
            dma((2, 6, F)),
            dma(ysh),
            dma(ysh),
            dma((6, T)),
            dma((6, T)),
        ],
        compiler_params=pltpu.CompilerParams(
            collective_id=0, has_side_effects=True, vmem_limit_bytes=60 * 1024 * 1024
        ),
        name="block",
    )(
        activations.reshape(count, dt),
        norm_gain.reshape(T, dt),
        conv_weight,
        chan_gain.reshape(1, chan),
        mix_gain.reshape(T, dt),
        final_gain.reshape(1, dt),
        *weights,
    )
    return out.reshape(batch, length, dt)


def solution(mesh):
    in_specs = (
        P(("rep", "fs"), None, "tp"),
        P(),
        P("fs", "tp"),
        P("fs", "tp"),
        P(None, "tp"),
        P("tp"),
        P("tp", "fs"),
        P(),
        P("fs", "tp"),
        P("fs", "tp"),
        P("tp", "fs"),
        P("tp"),
    )
    out_specs = P(("rep", "fs"), None, "tp")
    fast = tuple(mesh.shape[a] for a in ("rep", "fs", "tp")) == (2, 4, 4)
    body = fast_body if fast else ring_body
    return jax.shard_map(body, mesh=mesh, in_specs=in_specs, out_specs=out_specs, check_vma=False)
```

```python
import functools

import jax
import jax.numpy as jnp
from jax import lax
from jax.experimental import pallas as pl
from jax.experimental.pallas import tpu as pltpu
from jax.sharding import PartitionSpec as P

EPS = 1e-06
MESH = pl.DeviceIdType.MESH
F32 = jnp.float32
BF16 = jnp.bfloat16


def remote(src, dst, send, recv, target):
    return pltpu.make_async_remote_copy(
        src_ref=src, dst_ref=dst, send_sem=send, recv_sem=recv, device_id=target, device_id_type=MESH
    )


def chunk_of(extent, want):
    return want if extent % want == 0 else extent


def ring_kernel(
    R, F, T, split, length,
    x_ref, ng_ref, cw_ref, cg_ref, mg_ref, fg_ref,
    wv_ref, wg_ref, wo_ref, wga_ref, wup_ref, wd_ref,
    out_ref,
    bv, bg, bo, bga, bup, bd,
    xg, rows, glu, conv, act, part1, part2, got1, got2, firsts, hid, st1, st2, sg1, sg2,
    own_sem, zs, zr, ys, yr, ts, tr,
):
    f = lax.axis_index("fs")
    me = lax.axis_index("tp")
    rep = lax.axis_index("rep")
    count, dt = x_ref.shape
    width = dt * T
    local = [wv_ref, wg_ref, wo_ref, wga_ref, wup_ref, wd_ref]
    bufs = [bv, bg, bo, bga, bup, bd]

    barrier = pltpu.get_barrier_semaphore()
    greeted = 0
    for target in (lax.rem(f + 1, F), lax.rem(f + F - 1, F)):
        pl.semaphore_signal(barrier, inc=1, device_id={"fs": target}, device_id_type=MESH)
        greeted += 1
    if split == 2:
        pl.semaphore_signal(barrier, inc=1, device_id={"rep": 1 - rep}, device_id_type=MESH)
        greeted += 1
    for d in range(1, T):
        pl.semaphore_signal(barrier, inc=1, device_id={"tp": lax.rem(me + d, T)}, device_id_type=MESH)
        greeted += 1
    own = [
        pltpu.make_async_copy(local[w], bufs[w].at[f], own_sem.at[w]) for w in range(6)
    ]
    for copy in own:
        copy.start()
    pl.semaphore_wait(barrier, greeted)

    def half(w):
        n = local[w].shape[0] // split
        return pl.ds(pl.multiple_of((rep if split == 2 else 0) * n, n), n)

    def other(w):
        n = local[w].shape[0] // split
        return pl.ds(pl.multiple_of((1 - rep) * n, n), n)

    def hop(w, side, s):
        shard = f - s if side == 0 else f + s
        target = f + 1 if side == 0 else f - 1
        src = local[w].at[half(w)] if s == 0 else bufs[w].at[shard, half(w)]
        return remote(src, bufs[w].at[shard, half(w)], zs.at[side, w, s], zr.at[side, w, s + 1], {"fs": target})

    def arrival(w, side, s):
        shard = f - s if side == 0 else f + s
        ref = bufs[w].at[shard, half(w)]
        return remote(ref, ref, zs.at[side, w, s], zr.at[side, w, s], {"fs": f})

    def across(w, side, s):
        shard = f - s if side == 0 else f + s
        ref = bufs[w].at[shard, half(w)]
        return remote(ref, ref, ys.at[side, w, s], yr.at[side, w, s], {"rep": 1 - rep})

    def across_in(w, side, s):
        shard = f - s if side == 0 else f + s
        ref = bufs[w].at[shard, other(w)]
        return remote(ref, ref, ys.at[side, w, s], yr.at[side, w, s], {"rep": 1 - rep})

    def has(side, s):
        return f >= s if side == 0 else f + s <= F - 1

    def sends(side, s):
        ahead = f < F - 1 if side == 0 else f > 0
        return jnp.logical_and(has(side, s), ahead)

    def launch(w):
        for side in (0, 1):
            @pl.when(sends(side, 0))
            def _():
                hop(w, side, 0).start()

    def relay(group, stages=range(1, F)):
        for s in stages:
            for w in group:
                for side in (0, 1):
                    @pl.when(has(side, s))
                    def _():
                        arrival(w, side, s).wait_recv()
                        if s < F - 1:
                            @pl.when(sends(side, s))
                            def _():
                                hop(w, side, s).start()
                        if split == 2:
                            across(w, side, s).start()

    def settle(group):
        for w in group:
            own[w].wait()
        if split == 2:
            for s in range(1, F):
                for w in group:
                    for side in (0, 1):
                        @pl.when(has(side, s))
                        def _():
                            across_in(w, side, s).wait_recv()

    def tp_send(k, src, dst_at, d):
        return remote(src, dst_at, ts.at[k, d], tr.at[k, d], {"tp": lax.rem(me + d, T)})

    for w in (0, 1):
        launch(w)
    for d in range(1, T):
        tp_send(0, x_ref, xg.at[me], d).start()
    launch(2)
    xg[me] = x_ref[...]
    for d in range(1, T):
        peer = lax.rem(me + T - d, T)
        tp_send(0, x_ref, xg.at[peer], d).wait_recv()

    block = chunk_of(count, 16)

    def norm_rows(src, gain):
        def step(i, _):
            r = pl.ds(pl.multiple_of(i * block, block), block)
            vals = [src[t, r, :].astype(F32) for t in range(T)]
            ss = sum(jnp.sum(v * v, axis=1, keepdims=True) for v in vals)
            scale = lax.rsqrt(ss / width + EPS)
            for t in range(T):
                rows[r, t * dt:(t + 1) * dt] = (
                    vals[t] * scale * gain[t:t + 1, :]
                ).astype(BF16)
            return 0
        lax.fori_loop(0, count // block, step, 0)

    norm_rows(xg, ng_ref)
    relay((0, 1, 2))
    for w in (3, 4, 5):
        launch(w)
    settle((0, 1))

    chan = bv.shape[2]
    batch = count // length
    taps = cw_ref.shape[0]
    pad = 8 * ((taps - 1 + 7) // 8)
    lead = pad - (taps - 1)

    def columns(buf, c, n):
        block_w = buf[:, :, pl.ds(pl.multiple_of(c * n, n), n)]
        return block_w.reshape(block_w.shape[0] * block_w.shape[1], n)

    nc = chunk_of(chan, 256)

    def glu_step(c, _):
        value = jnp.dot(rows[...], columns(bv, c, nc), preferred_element_type=F32)
        gate = jnp.dot(rows[...], columns(bg, c, nc), preferred_element_type=F32)
        res = value * jax.nn.sigmoid(gate)
        for b in range(batch):
            glu[b, pl.ds(pad, length), pl.ds(pl.multiple_of(c * nc, nc), nc)] = (
                res[b * length:(b + 1) * length]
            )
        return 0

    for b in range(batch):
        glu[b, 0:pad, :] = jnp.zeros((pad, chan), F32)
        glu[b, pad + length:, :] = jnp.zeros((8, chan), F32)
    lax.fori_loop(0, chan // nc, glu_step, 0)
    relay((3,), (1,))

    lanes = chunk_of(chan, 128)
    span = chunk_of(length, 64)
    strips = chan // lanes

    def conv_step(i, _):
        q = lax.rem(i, strips)
        p = i // strips
        cols = pl.ds(pl.multiple_of(q * lanes, lanes), lanes)
        weights = cw_ref[:, cols]
        for b in range(batch):
            total = jnp.zeros((span, lanes), F32)
            for shift in range(8):
                acc = None
                for tap in range(taps):
                    if (lead + tap) % 8 != shift:
                        continue
                    base = lead + tap - shift
                    term = weights[tap:tap + 1, :] * glu[
                        b, pl.ds(pl.multiple_of(p * span + base, 8), span + 8), cols
                    ]
                    acc = term if acc is None else acc + term
                if acc is not None:
                    total = total + acc[shift:shift + span]
            conv[pl.ds(pl.multiple_of(b * length + p * span, span), span), cols] = total
        return 0

    lax.fori_loop(0, strips * (length // span), conv_step, 0)

    lane = lax.broadcasted_iota(jnp.int32, (count, 128), 1)

    def across_lanes(a, b):
        table = jnp.where(lane == 0, a, jnp.where(lane == 1, b, 0.0))
        return jnp.transpose(table)[0:8, :]

    def down_rows(top):
        full = jnp.concatenate([top, jnp.zeros((120, count), F32)], axis=0)
        return jnp.transpose(full)

    values = conv[...]
    local_sum = jnp.sum(values, axis=1, keepdims=True)
    dev = values - local_sum / chan
    st1[...] = across_lanes(local_sum, jnp.sum(dev * dev, axis=1, keepdims=True))
    sg1[me] = st1[...]
    for d in range(1, T):
        tp_send(1, st1, sg1.at[me], d).start()
    relay((4,), (1,))
    for d in range(1, T):
        peer = lax.rem(me + T - d, T)
        tp_send(1, st1, sg1.at[peer], d).wait_recv()
    sums = [sg1[t] for t in range(T)]
    mean = sum(s[0:1, :] for s in sums) / (chan * T)
    spread = sum(
        s[1:2, :] + chan * (s[0:1, :] / chan - mean) * (s[0:1, :] / chan - mean) for s in sums
    ) / (chan * T)
    inv = lax.rsqrt(spread + EPS)
    line = lax.broadcasted_iota(jnp.int32, (8, count), 0)
    table = down_rows(jnp.where(line == 0, mean, jnp.where(line == 1, inv, 0.0)))
    normed = (conv[...] - table[:, 0:1]) * table[:, 1:2] * cg_ref[...]
    act[...] = (normed * jax.nn.sigmoid(normed)).astype(BF16)

    settle((2,))

    def project(src, buf, part):
        dsh = buf.shape[2]
        for j in range(F):
            t, off = (j * dsh) // dt, (j * dsh) % dt
            prod = jnp.dot(src[...], buf[j], preferred_element_type=F32)
            part[t, :, off:off + dsh] = prod.astype(BF16)

    def scatter(k, part, got):
        for d in range(1, T):
            tp_send(k, part.at[lax.rem(me + d, T)], got.at[d - 1], d).start()

    def gathered(k, part, got):
        total = part[me].astype(F32)
        for d in range(1, T):
            tp_send(k, part.at[me], got.at[d - 1], d).wait_recv()
            total = total + got[d - 1].astype(F32)
        return total

    def piece(t):
        return remote(part2.at[t], got2.at[me], ts.at[4, t], tr.at[4, me], {"tp": t})

    def piece_in(t):
        return remote(part2.at[t], got2.at[t], ts.at[4, t], tr.at[4, t], {"tp": t})

    project(act, bo, part1)
    scatter(2, part1, got1)
    relay((5,), (1,))
    first = (x_ref[...].astype(F32) + gathered(2, part1, got1)).astype(BF16)
    firsts[me] = first
    for d in range(1, T):
        tp_send(3, firsts.at[me], firsts.at[me], d).start()
    relay((3,), (2,))
    for d in range(1, T):
        peer = lax.rem(me + T - d, T)
        tp_send(3, firsts.at[peer], firsts.at[peer], d).wait_recv()
    relay((4,), (2,))
    norm_rows(firsts, mg_ref)
    relay((5,), (2,))
    relay((3, 4), range(3, F))
    settle((3, 4))

    ff = bga.shape[2]
    nf = chunk_of(ff, 256)

    def ff_step(c, _):
        gate = jnp.dot(rows[...], columns(bga, c, nf), preferred_element_type=F32)
        up = jnp.dot(rows[...], columns(bup, c, nf), preferred_element_type=F32)
        hid[:, pl.ds(pl.multiple_of(c * nf, nf), nf)] = (
            gate * jax.nn.sigmoid(gate) * up
        ).astype(BF16)
        return 0

    lax.fori_loop(0, ff // nf, ff_step, 0)
    if F == T and bd.shape[2] == dt:
        def down(shard):
            prod = jnp.dot(hid[...], bd[shard], preferred_element_type=F32)
            part2[shard] = prod.astype(BF16)

            @pl.when(shard != me)
            def _():
                piece(shard).start()

        own[5].wait()
        down(f)
        for s in range(1, F):
            if s >= 3:
                relay((5,), (s,))
            for side in (0, 1):
                @pl.when(has(side, s))
                def _():
                    if split == 2:
                        across_in(5, side, s).wait_recv()
                    down(f - s if side == 0 else f + s)
    else:
        relay((5,), range(3, F))
        settle((5,))
        project(hid, bd, part2)
        for d in range(1, T):
            piece(lax.rem(me + d, T)).start()
    second = firsts[me].astype(F32) + part2[me].astype(F32)
    for d in range(1, T):
        peer = lax.rem(me + d, T)
        piece_in(peer).wait_recv()
        second = second + got2[peer].astype(F32)
    total = jnp.sum(second * second, axis=1, keepdims=True)
    conv[:, 0:dt] = second
    st2[...] = across_lanes(total, total)
    sg2[me] = st2[...]
    for d in range(1, T):
        tp_send(5, st2, sg2.at[me], d).start()
    for d in range(1, T):
        peer = lax.rem(me + T - d, T)
        tp_send(5, st2, sg2.at[peer], d).wait_recv()
    full = sum(sg2[t] for t in range(T))
    table = down_rows(full)
    scale = lax.rsqrt(table[:, 0:1] / width + EPS)
    out_ref[...] = (conv[:, 0:dt] * scale * fg_ref[...]).astype(BF16)

    for w in range(6):
        for side in (0, 1):
            for s in range(F):
                if s < F - 1:
                    @pl.when(sends(side, s))
                    def _():
                        hop(w, side, s).wait_send()
                if s >= 1 and split == 2:
                    @pl.when(has(side, s))
                    def _():
                        across(w, side, s).wait_send()
    for d in range(1, T):
        peer = lax.rem(me + d, T)
        tp_send(0, x_ref, xg.at[me], d).wait_send()
        tp_send(1, st1, sg1.at[me], d).wait_send()
        tp_send(2, part1.at[peer], got1.at[d - 1], d).wait_send()
        tp_send(3, firsts.at[me], firsts.at[me], d).wait_send()
        piece(peer).wait_send()
        tp_send(5, st2, sg2.at[me], d).wait_send()


PIECES = (2, 2, 2, 2, 2, 4)
MOST = max(PIECES)


def fast_kernel(
    length,
    x_ref, ng_hbm, cw_hbm, cg_hbm, mg_hbm, fg_hbm,
    wv_ref, wg_ref, wo_ref, wga_ref, wup_ref, wd_ref,
    out_ref,
    ng_ref, cw_ref, cg_ref, mg_ref, fg_ref, bv, bg, bo, bga, bup, bd,
    xg, rows, accv, accg, glu, conv, act, part, got, q1, q1in, firsts, hid,
    accs, part2, got2, q2, q2in, sec, ssq, secb, secin, st1, sg1, st2, sg2, finin,
    small, own_sem, zs, zr, ms, mr, ys, yr, xos, xor_, ags, agr, sts, str_, rss, rsr, ds_, dr, qs, qr, os_, orr, fs_, fr,
):
    f = lax.axis_index("fs")
    me = lax.axis_index("tp")
    rep = lax.axis_index("rep")
    count, dt = x_ref.shape
    T = 4
    width = dt * T
    rows_all = 2 * count
    batch = count // length
    chan, ff = bv.shape[2], bga.shape[2]
    local = [wv_ref, wg_ref, wo_ref, wga_ref, wup_ref, wd_ref]
    bufs = [bv, bg, bo, bga, bup, bd]
    VAL, GATE, CVO, GA, UP, DOWN = range(6)
    outer = jnp.logical_or(f == 0, f == 3)
    near = 1 + f // 3
    po, pi, fo = 3 * (f - 1), 3 - f, 3 * (2 - f)
    sib = me + 1 - 2 * lax.rem(me, 2)
    mir = lax.rem(me + 2, T)
    dia = lax.rem(sib + 2, T)

    def view(ref, w, h, c):
        if w == DOWN:
            n, m = ref.shape[1] // 2, ref.shape[0] // 2
            k = n // 2
            return ref.at[pl.ds((c % 2) * m, m), pl.ds(pl.multiple_of(h * n + (c // 2) * k, k), k)]
        n = ref.shape[0] // 2
        k = n // PIECES[w]
        return ref.at[pl.ds(pl.multiple_of(h * n + c * k, k), k), :]

    barrier = pltpu.get_barrier_semaphore()

    def greet(**target):
        pl.semaphore_signal(barrier, inc=1, device_id=target, device_id_type=MESH)

    def zsend(w, hs, c):
        h = rep if hs == 0 else 1 - rep
        return remote(
            view(local[w], w, h, c), view(bufs[w].at[f], w, h, c), zs.at[w, hs, c], zr.at[w, hs, c], {"fs": near}
        )

    def xsend():
        return remote(x_ref, xg.at[me, 0], xos, xor_, {"fs": near})

    hn = dt // 2

    def half_of(n):
        return rep if n == 0 else 1 - rep

    def hcols(h):
        return pl.ds(pl.multiple_of(h * hn, hn), hn)

    def result(n, target):
        return remote(
            secb.at[:, hcols(half_of(n))], secin.at[:, hcols(half_of(n))], os_.at[n], orr.at[n], {"fs": target}
        )

    smalls = [
        pltpu.make_async_copy(src, dst, small.at[k])
        for k, (src, dst) in enumerate(
            ((ng_hbm, ng_ref), (cw_hbm, cw_ref), (cg_hbm, cg_ref), (mg_hbm, mg_ref), (fg_hbm, fg_ref))
        )
    ]

    lane = lax.broadcasted_iota(jnp.int32, (count, 128), 1)
    line = lax.broadcasted_iota(jnp.int32, (8, count), 0)

    def across_lanes(a, b):
        table = jnp.where(lane == 0, a, jnp.where(lane == 1, b, 0.0))
        return jnp.transpose(table)[0:8, :]

    def down_rows(top):
        full = jnp.concatenate([top, jnp.zeros((120, count), F32)], axis=0)
        return jnp.transpose(full)

    @pl.when(outer)
    def _():
        for t in range(T):
            greet(fs=near, tp=t)
        smalls[4].start()
        pl.semaphore_wait(barrier, T)
        order = [
            (VAL, 0), (GATE, 0), None, (CVO, 0), (VAL, 1), (GATE, 1), (CVO, 1),
            (GA, 0), (UP, 0), (GA, 1), (DOWN, 0), (UP, 1), (DOWN, 1),
        ]
        for item in order:
            if item is None:
                xsend().start()
            else:
                for c in range(PIECES[item[0]]):
                    zsend(item[0], item[1], c).start()
        xsend().wait_send()
        for w in range(6):
            for hs in range(2):
                for c in range(PIECES[w]):
                    zsend(w, hs, c).wait_send()
        smalls[4].wait()
        for n in range(2):
            result(n, near).wait_recv()
        for t in range(T):
            remote(st2.at[0], finin.at[t], fs_.at[t], fr.at[t], {"fs": near}).wait_recv()
        full = sum(finin[t] for t in range(T))
        scale = lax.rsqrt(down_rows(full)[:, 0:1] / width + EPS)
        out_ref[...] = (secin[...].astype(F32) * scale * fg_ref[...]).astype(BF16)

    @pl.when(jnp.logical_not(outer))
    def _():
        for t in range(T):
            greet(fs=po, tp=t)
        greet(fs=pi)
        greet(rep=1 - rep)
        for t in (sib, mir, dia):
            greet(tp=t)
        own = [pltpu.make_async_copy(local[w], bufs[w].at[f], own_sem.at[w]) for w in range(6)]
        load_x = pltpu.make_async_copy(x_ref, xg.at[me, 1], small.at[5])
        load_x.start()
        for copy in smalls:
            copy.start()
        for copy in own:
            copy.start()
        pl.semaphore_wait(barrier, T + 5)

        def arrived(ref, send, recv):
            remote(ref, ref, send, recv, {"fs": f}).wait_recv()

        def mid_own(w, c):
            return remote(
                view(local[w], w, rep, c), view(bufs[w].at[f], w, rep, c), ms.at[w, 0, c], mr.at[w, 0, c], {"fs": pi}
            )

        def mid_fwd(w, c):
            ref = view(bufs[w].at[po], w, rep, c)
            return remote(ref, ref, ms.at[w, 1, c], mr.at[w, 1, c], {"fs": pi})

        def y_fwd(w, k, c):
            ref = view(bufs[w].at[fo if k else pi], w, rep, c)
            return remote(ref, ref, ys.at[w, k, c], yr.at[w, k, c], {"rep": 1 - rep})

        def send_own(w):
            for c in range(PIECES[w]):
                mid_own(w, c).start()

        def relay_mid(w, c):
            arrived(view(bufs[w].at[po], w, rep, c), zs.at[w, 0, c], zr.at[w, 0, c])
            mid_fwd(w, c).start()

        def relay_y(w, k, c):
            arrived(view(bufs[w].at[fo if k else pi], w, rep, c), ms.at[w, k, c], mr.at[w, k, c])
            y_fwd(w, k, c).start()

        def wait_z(w):
            for c in range(PIECES[w]):
                arrived(view(bufs[w].at[po], w, 1 - rep, c), zs.at[w, 1, c], zr.at[w, 1, c])

        def wait_y(w, k):
            for c in range(PIECES[w]):
                arrived(view(bufs[w].at[fo if k else pi], w, 1 - rep, c), ys.at[w, k, c], yr.at[w, k, c])

        def ag(p, buf, slot, kind):
            ref = buf.at[mir if kind == 2 else me, slot]
            return remote(ref, ref, ags.at[p, slot, kind], agr.at[p, slot, kind], {"tp": mir if kind == 1 else sib})

        def ag_in(p, buf, slot, kind):
            ref = buf.at[(sib, mir, dia)[kind], slot]
            return remote(ref, ref, ags.at[p, slot, kind], agr.at[p, slot, kind], {"tp": me})

        def ag_start(p, buf, slot):
            ag(p, buf, slot, 1).start()
            ag(p, buf, slot, 0).start()

        def ag_forward(p, buf, slot):
            ag_in(p, buf, slot, 1).wait_recv()
            ag(p, buf, slot, 2).start()

        def ag_finish(p, buf, slot):
            ag_in(p, buf, slot, 0).wait_recv()
            ag_in(p, buf, slot, 2).wait_recv()

        block = chunk_of(count, 16)

        def norm_rows(src, slot, gain):
            def step(i, _):
                r = pl.ds(pl.multiple_of(i * block, block), block)
                o = pl.ds(pl.multiple_of(slot * count + i * block, block), block)
                vals = [src[t, slot, r, :].astype(F32) for t in range(T)]
                ss = sum(jnp.sum(v * v, axis=1, keepdims=True) for v in vals)
                scale = lax.rsqrt(ss / width + EPS)
                for t in range(T):
                    rows[t, o, :] = (vals[t] * scale * gain[:, t * dt:(t + 1) * dt]).astype(BF16)
                return 0
            lax.fori_loop(0, count // block, step, 0)

        def stat(k, slot, src, dst, d):
            return remote(src, dst, sts.at[k, slot, d], str_.at[k, slot, d], {"tp": lax.rem(me + d, T)})

        def stat_send(k, slot, src, dst):
            for d in range(1, T):
                stat(k, slot, src.at[slot], dst.at[slot, me], d).start()

        def stat_wait(k, slot, src, dst):
            for d in range(1, T):
                stat(k, slot, src.at[slot], dst.at[slot, lax.rem(me + T - d, T)], d).wait_recv()

        send_own(VAL)
        send_own(GATE)
        load_x.wait()
        ag_start(0, xg, 1)
        for c in range(2):
            relay_mid(VAL, c)
            relay_y(VAL, 0, c)
        relay_mid(GATE, 0)
        ag_forward(0, xg, 1)
        relay_y(GATE, 0, 0)
        relay_mid(GATE, 1)
        relay_y(GATE, 0, 1)
        send_own(CVO)
        ag_finish(0, xg, 1)
        for copy in smalls:
            copy.wait()
        norm_rows(xg, 1, ng_ref)
        relay_y(VAL, 1, 0)
        arrived(xg.at[me, 0], xos, xor_)
        ag_start(0, xg, 0)
        relay_y(VAL, 1, 1)
        relay_mid(CVO, 0)
        relay_y(GATE, 1, 0)
        relay_mid(CVO, 1)
        send_own(GA)
        send_own(UP)
        relay_y(GATE, 1, 1)
        ag_forward(0, xg, 0)
        ag_finish(0, xg, 0)
        norm_rows(xg, 0, ng_ref)
        relay_y(CVO, 0, 0)

        pad = glu.shape[1] - length - 8
        taps = cw_ref.shape[0]
        lead = pad - (taps - 1)
        nc = chunk_of(chan, 256)
        for b in range(2 * batch):
            glu[b, 0:pad, :] = jnp.zeros((pad, chan), F32)
            glu[b, pad + length:, :] = jnp.zeros((8, chan), F32)

        def s1(shard, first, last):
            def step(c, _):
                cols = pl.ds(pl.multiple_of(c * nc, nc), nc)
                value = jnp.dot(rows[shard], bv[shard, :, cols], preferred_element_type=F32)
                gate = jnp.dot(rows[shard], bg[shard, :, cols], preferred_element_type=F32)
                if not first:
                    value = value + accv[:, cols]
                    gate = gate + accg[:, cols]
                if last:
                    res = value * jax.nn.sigmoid(gate)
                    for b in range(2 * batch):
                        glu[b, pl.ds(pad, length), cols] = res[b * length:(b + 1) * length]
                else:
                    accv[:, cols] = value
                    accg[:, cols] = gate
                return 0
            lax.fori_loop(0, chan // nc, step, 0)

        own[VAL].wait()
        own[GATE].wait()
        s1(f, True, False)
        wait_y(VAL, 0)
        wait_y(GATE, 0)
        s1(pi, False, False)
        relay_y(CVO, 0, 1)
        wait_y(VAL, 1)
        wait_y(GATE, 1)
        s1(fo, False, False)
        relay_y(CVO, 1, 0)
        wait_z(VAL)
        wait_z(GATE)
        s1(po, False, True)
        relay_y(CVO, 1, 1)

        lanes = chunk_of(chan, 128)
        span = chunk_of(length, 64)
        strips = chan // lanes

        def convolve(slot):
            def step(i, _):
                s = lax.rem(i, strips)
                p = i // strips
                cols = pl.ds(pl.multiple_of(s * lanes, lanes), lanes)
                weights = cw_ref[:, cols]
                for b in range(batch):
                    total = jnp.zeros((span, lanes), F32)
                    for shift in range(8):
                        acc = None
                        for tap in range(taps):
                            if (lead + tap) % 8 != shift:
                                continue
                            base = lead + tap - shift
                            term = weights[tap:tap + 1, :] * glu[
                                slot * batch + b, pl.ds(pl.multiple_of(p * span + base, 8), span + 8), cols
                            ]
                            acc = term if acc is None else acc + term
                        if acc is not None:
                            total = total + acc[shift:shift + span]
                    at = pl.multiple_of(slot * count + b * length + p * span, span)
                    conv[pl.ds(at, span), cols] = total
                return 0
            lax.fori_loop(0, strips * (length // span), step, 0)

        def span_of(slot):
            return slice(slot * count, (slot + 1) * count)

        def conv_stats(slot):
            values = conv[span_of(slot), :]
            local_sum = jnp.sum(values, axis=1, keepdims=True)
            dev = values - local_sum / chan
            st1[slot] = across_lanes(local_sum, jnp.sum(dev * dev, axis=1, keepdims=True))
            sg1[slot, me] = st1[slot]
            stat_send(0, slot, st1, sg1)

        def activate(slot):
            stat_wait(0, slot, st1, sg1)
            sums = [sg1[slot, t] for t in range(T)]
            mean = sum(s[0:1, :] for s in sums) / (chan * T)
            spread = sum(
                s[1:2, :] + chan * (s[0:1, :] / chan - mean) * (s[0:1, :] / chan - mean) for s in sums
            ) / (chan * T)
            inv = lax.rsqrt(spread + EPS)
            table = down_rows(jnp.where(line == 0, mean, jnp.where(line == 1, inv, 0.0)))
            normed = (conv[span_of(slot), :] - table[:, 0:1]) * table[:, 1:2] * cg_ref[...]
            act[span_of(slot), :] = (normed * jax.nn.sigmoid(normed)).astype(BF16)

        def rs(slot, kind):
            if kind == 2:
                return remote(q1.at[slot], q1in.at[slot], rss.at[slot, 2], rsr.at[slot, 2], {"tp": mir})
            return remote(
                part.at[slot, dia if kind else sib], got.at[slot, kind],
                rss.at[slot, kind], rsr.at[slot, kind], {"tp": sib},
            )

        def project(slot):
            def step(j, _):
                prod = jnp.dot(act[span_of(slot), :], bo[j], preferred_element_type=F32)
                part[slot, j] = prod.astype(BF16)
                return 0
            lax.fori_loop(0, T, step, 0)
            rs(slot, 1).start()
            rs(slot, 0).start()

        def pair_sum(slot):
            rs(slot, 1).wait_recv()
            q1[slot] = (part[slot, mir].astype(F32) + got[slot, 1].astype(F32)).astype(BF16)
            rs(slot, 2).start()

        def finish_first(slot):
            rs(slot, 0).wait_recv()
            total = xg[me, slot].astype(F32) + (part[slot, me].astype(F32) + got[slot, 0].astype(F32))
            rs(slot, 2).wait_recv()
            firsts[me, slot] = (total + q1in[slot].astype(F32)).astype(BF16)
            ag_start(1, firsts, slot)

        convolve(0)
        conv_stats(0)
        convolve(1)
        conv_stats(1)
        relay_y(GA, 0, 0)
        own[CVO].wait()
        wait_y(CVO, 0)
        wait_y(CVO, 1)
        wait_z(CVO)
        activate(0)
        project(0)
        activate(1)
        relay_mid(GA, 0)
        project(1)
        pair_sum(0)
        relay_y(GA, 0, 1)
        pair_sum(1)
        relay_mid(GA, 1)
        relay_y(UP, 0, 0)
        finish_first(0)
        relay_mid(UP, 0)
        relay_y(UP, 0, 1)
        relay_mid(UP, 1)
        send_own(DOWN)
        relay_y(GA, 1, 0)
        finish_first(1)
        relay_y(GA, 1, 1)
        ag_forward(1, firsts, 0)
        ag_finish(1, firsts, 0)
        norm_rows(firsts, 0, mg_ref)
        relay_y(UP, 1, 0)
        ag_forward(1, firsts, 1)
        relay_y(UP, 1, 1)
        ag_finish(1, firsts, 1)
        norm_rows(firsts, 1, mg_ref)
        relay_mid(DOWN, 0)
        relay_y(DOWN, 0, 0)

        nf = chunk_of(ff, 256)

        def s5(w, shard, first, last=False):
            def step(c, _):
                cols = pl.ds(pl.multiple_of(c * nf, nf), nf)
                value = jnp.dot(rows[shard], bufs[w][shard, :, cols], preferred_element_type=F32)
                if not first:
                    value = value + accs[w - GA, :, cols]
                if last:
                    gate = accs[0, :, cols]
                    hid[:, cols] = (gate * jax.nn.sigmoid(gate) * value).astype(BF16)
                else:
                    accs[w - GA, :, cols] = value
                return 0
            lax.fori_loop(0, ff // nf, step, 0)

        own[GA].wait()
        own[UP].wait()
        wait_y(GA, 0)
        wait_y(GA, 1)
        wait_z(GA)
        wait_y(UP, 0)
        s5(GA, f, True)
        relay_mid(DOWN, 1)
        s5(GA, pi, False)
        relay_mid(DOWN, 2)
        relay_y(DOWN, 0, 1)
        s5(GA, po, False)
        s5(GA, fo, False)
        relay_mid(DOWN, 3)
        s5(UP, f, True)
        s5(UP, pi, False)
        relay_y(DOWN, 0, 2)
        wait_y(UP, 1)
        s5(UP, fo, False)
        relay_y(DOWN, 0, 3)
        relay_y(DOWN, 1, 0)
        wait_z(UP)
        s5(UP, po, False, True)
        relay_y(DOWN, 1, 1)

        def pair_send(b, h, n):
            return remote(part2.at[b, :, hcols(h)], got2.at[b, :, hcols(h)], ds_.at[b, n], dr.at[b, n], {"tp": sib})

        def cross(h, n):
            return remote(q2.at[:, hcols(h)], q2in.at[:, hcols(h)], qs.at[n], qr.at[n], {"tp": mir})

        def down(b, n):
            h = half_of(n)
            prod = jnp.dot(hid[...], bd[b, :, hcols(h)], preferred_element_type=F32)
            part2[b, :, hcols(h)] = prod.astype(BF16)

            @pl.when(jnp.logical_or(b == sib, b == dia))
            def _():
                pair_send(b, h, n).start()

        def combine(b, n):
            h = half_of(n)

            @pl.when(b == mir)
            def _():
                pair_send(b, h, n).wait_recv()
                q2[:, hcols(h)] = (part2[b, :, hcols(h)].astype(F32) + got2[b, :, hcols(h)].astype(F32)).astype(BF16)
                cross(h, n).start()

        def outer_stat(d):
            return remote(
                st2.at[0], finin.at[me], fs_.at[d], fr.at[me], {"fs": po, "tp": lax.rem(me + d, T)}
            )

        def finish(n):
            h = half_of(n)
            pair_send(me, h, n).wait_recv()
            cross(h, n).wait_recv()
            cols = hcols(h)
            for slot in range(2):
                r = span_of(slot)
                second = firsts[me, slot, :, cols].astype(F32) + part2[me, r, cols].astype(F32)
                second = second + got2[me, r, cols].astype(F32) + q2in[r, cols].astype(F32)
                if slot == 0:
                    secb[:, cols] = second.astype(BF16)
                    result(n, po).start()
                else:
                    sec[:, cols] = second
                total = jnp.sum(second * second, axis=1, keepdims=True)
                if n == 0:
                    ssq[r, :] = total
                    continue
                total = total + ssq[r, :]
                st2[slot] = across_lanes(total, total)
                if slot == 0:
                    for d in range(T):
                        outer_stat(d).start()
                else:
                    sg2[me] = st2[1]
                    for d in range(1, T):
                        stat(1, 1, st2.at[1], sg2.at[me], d).start()

        own[DOWN].wait()
        down(f, 0)
        down(f, 1)
        relay_y(DOWN, 1, 2)
        combine(f, 0)
        down(po, 0)
        combine(f, 1)
        down(pi, 0)
        combine(po, 0)
        wait_y(DOWN, 0)
        down(pi, 1)
        combine(pi, 0)
        relay_y(DOWN, 1, 3)
        down(fo, 0)
        combine(pi, 1)
        combine(fo, 0)
        wait_z(DOWN)
        down(po, 1)
        combine(po, 1)
        wait_y(DOWN, 1)
        down(fo, 1)
        finish(0)
        combine(fo, 1)
        finish(1)
        for d in range(1, T):
            stat(1, 1, st2.at[1], sg2.at[lax.rem(me + T - d, T)], d).wait_recv()
        table = down_rows(sum(sg2[t] for t in range(T)))
        scale = lax.rsqrt(table[:, 0:1] / width + EPS)
        out_ref[...] = (sec[...] * scale * fg_ref[...]).astype(BF16)

        for w in range(6):
            for c in range(PIECES[w]):
                mid_own(w, c).wait_send()
                mid_fwd(w, c).wait_send()
                for k in range(2):
                    y_fwd(w, k, c).wait_send()
        for slot in range(2):
            for kind in range(3):
                ag(0, xg, slot, kind).wait_send()
                ag(1, firsts, slot, kind).wait_send()
                rs(slot, kind).wait_send()
            for d in range(1, T):
                stat(0, slot, st1.at[slot], sg1.at[slot, me], d).wait_send()
        for n in range(2):
            h = half_of(n)
            pair_send(sib, h, n).wait_send()
            pair_send(dia, h, n).wait_send()
            cross(h, n).wait_send()
            result(n, po).wait_send()
        for d in range(T):
            outer_stat(d).wait_send()
        for d in range(1, T):
            stat(1, 1, st2.at[1], sg2.at[me], d).wait_send()


def fast_body(
    activations, norm_gain, w_value, w_gate_conv, conv_weight, chan_gain,
    w_conv_out, mix_gain, w_gate, w_up, w_down, final_gain,
):
    batch, length, dt = activations.shape
    count = batch * length
    weights = (w_value, w_gate_conv, w_conv_out, w_gate, w_up, w_down)
    chan, ff = w_value.shape[1], w_gate.shape[1]
    T = 4
    pad = 8 * ((conv_weight.shape[0] - 1 + 7) // 8)
    rows_all = 2 * count
    vmem, hbm = pl.BlockSpec(memory_space=pltpu.VMEM), pl.BlockSpec(memory_space=pl.ANY)
    dma = pltpu.SemaphoreType.DMA
    V = pltpu.VMEM
    out = pl.pallas_call(
        functools.partial(fast_kernel, length),
        out_shape=jax.ShapeDtypeStruct((count, dt), BF16),
        in_specs=[hbm] * 12,
        out_specs=vmem,
        scratch_shapes=[
            V((1, dt * T), F32),
            V(conv_weight.shape, F32),
            V((1, chan), F32),
            V((1, dt * T), F32),
            V((1, dt), F32),
        ] + [V((4,) + w.shape, BF16) for w in weights] + [
            V((T, 2, count, dt), BF16),
            V((T, rows_all, dt), BF16),
            V((rows_all, chan), F32),
            V((rows_all, chan), F32),
            V((2 * batch, pad + length + 8, chan), F32),
            V((rows_all, chan), F32),
            V((rows_all, chan), BF16),
            V((2, T, count, dt), BF16),
            V((2, 2, count, dt), BF16),
            V((2, count, dt), BF16),
            V((2, count, dt), BF16),
            V((T, 2, count, dt), BF16),
            V((rows_all, ff), BF16),
            V((2, rows_all, ff), F32),
            V((T, rows_all, dt), BF16),
            V((T, rows_all, dt), BF16),
            V((rows_all, dt), BF16),
            V((rows_all, dt), BF16),
            V((count, dt), F32),
            V((rows_all, 1), F32),
            V((count, dt), BF16),
            V((count, dt), BF16),
            V((2, 8, count), F32),
            V((2, T, 8, count), F32),
            V((2, 8, count), F32),
            V((T, 8, count), F32),
            V((T, 8, count), F32),
            dma((6,)),
            dma((6,)),
            dma((6, 2, MOST)),
            dma((6, 2, MOST)),
            dma((6, 2, MOST)),
            dma((6, 2, MOST)),
            dma((6, 2, MOST)),
            dma((6, 2, MOST)),
            dma(()),
            dma(()),
            dma((2, 2, 3)),
            dma((2, 2, 3)),
            dma((2, 2, T)),
            dma((2, 2, T)),
            dma((2, 3)),
            dma((2, 3)),
            dma((T, 2)),
            dma((T, 2)),
            dma((2,)),
            dma((2,)),
            dma((2,)),
            dma((2,)),
            dma((T,)),
            dma((T,)),
        ],
        compiler_params=pltpu.CompilerParams(
            collective_id=0, has_side_effects=True, vmem_limit_bytes=60 * 1024 * 1024
        ),
        name="block",
    )(
        activations.reshape(count, dt),
        norm_gain.reshape(1, dt * T),
        conv_weight,
        chan_gain.reshape(1, chan),
        mix_gain.reshape(1, dt * T),
        final_gain.reshape(1, dt),
        *weights,
    )
    return out.reshape(batch, length, dt)


def ring_body(
    activations, norm_gain, w_value, w_gate_conv, conv_weight, chan_gain,
    w_conv_out, mix_gain, w_gate, w_up, w_down, final_gain,
):
    batch, length, dt = activations.shape
    count = batch * length
    R, F, T = lax.axis_size("rep"), lax.axis_size("fs"), lax.axis_size("tp")
    weights = (w_value, w_gate_conv, w_conv_out, w_gate, w_up, w_down)
    split = 2 if R == 2 and all(w.shape[0] % 32 == 0 for w in weights) else 1
    width = dt * T
    chan, ff = w_value.shape[1], w_gate.shape[1]
    taps = conv_weight.shape[0]
    pad = 8 * ((taps - 1 + 7) // 8)
    vmem, hbm = pl.BlockSpec(memory_space=pltpu.VMEM), pl.BlockSpec(memory_space=pl.ANY)
    ysh = (2, 6, F) if split == 2 else (1,)
    dma = pltpu.SemaphoreType.DMA
    out = pl.pallas_call(
        functools.partial(ring_kernel, R, F, T, split, length),
        out_shape=jax.ShapeDtypeStruct((count, dt), BF16),
        in_specs=[vmem] * 6 + [hbm] * 6,
        out_specs=vmem,
        scratch_shapes=[pltpu.VMEM((F,) + w.shape, BF16) for w in weights] + [
            pltpu.VMEM((T, count, dt), BF16),
            pltpu.VMEM((count, width), BF16),
            pltpu.VMEM((batch, pad + length + 8, chan), F32),
            pltpu.VMEM((count, max(chan, dt)), F32),
            pltpu.VMEM((count, chan), BF16),
            pltpu.VMEM((T, count, dt), BF16),
            pltpu.VMEM((T, count, dt), BF16),
            pltpu.VMEM((T - 1, count, dt), BF16),
            pltpu.VMEM((T, count, dt), BF16),
            pltpu.VMEM((T, count, dt), BF16),
            pltpu.VMEM((count, ff), BF16),
            pltpu.VMEM((8, count), F32),
            pltpu.VMEM((8, count), F32),
            pltpu.VMEM((T, 8, count), F32),
            pltpu.VMEM((T, 8, count), F32),
            dma((6,)),
            dma((2, 6, F)),
            dma((2, 6, F)),
            dma(ysh),
            dma(ysh),
            dma((6, T)),
            dma((6, T)),
        ],
        compiler_params=pltpu.CompilerParams(
            collective_id=0, has_side_effects=True, vmem_limit_bytes=60 * 1024 * 1024
        ),
        name="block",
    )(
        activations.reshape(count, dt),
        norm_gain.reshape(T, dt),
        conv_weight,
        chan_gain.reshape(1, chan),
        mix_gain.reshape(T, dt),
        final_gain.reshape(1, dt),
        *weights,
    )
    return out.reshape(batch, length, dt)


def solution(mesh):
    in_specs = (
        P(("rep", "fs"), None, "tp"),
        P(),
        P("fs", "tp"),
        P("fs", "tp"),
        P(None, "tp"),
        P("tp"),
        P("tp", "fs"),
        P(),
        P("fs", "tp"),
        P("fs", "tp"),
        P("tp", "fs"),
        P("tp"),
    )
    out_specs = P(("rep", "fs"), None, "tp")
    fast = tuple(mesh.shape[a] for a in ("rep", "fs", "tp")) == (2, 4, 4)
    body = fast_body if fast else ring_body
    return jax.shard_map(body, mesh=mesh, in_specs=in_specs, out_specs=out_specs, check_vma=False)
```

```python
import functools

import jax
import jax.numpy as jnp
from jax import lax
from jax.experimental import pallas as pl
from jax.experimental.pallas import tpu as pltpu
from jax.sharding import PartitionSpec as P

EPS = 1e-06
MESH = pl.DeviceIdType.MESH
F32 = jnp.float32
BF16 = jnp.bfloat16


def remote(src, dst, send, recv, target):
    return pltpu.make_async_remote_copy(
        src_ref=src, dst_ref=dst, send_sem=send, recv_sem=recv, device_id=target, device_id_type=MESH
    )


def chunk_of(extent, want):
    return want if extent % want == 0 else extent


def ring_kernel(
    R, F, T, split, length,
    x_ref, ng_ref, cw_ref, cg_ref, mg_ref, fg_ref,
    wv_ref, wg_ref, wo_ref, wga_ref, wup_ref, wd_ref,
    out_ref,
    bv, bg, bo, bga, bup, bd,
    xg, rows, glu, conv, act, part1, part2, got1, got2, firsts, hid, st1, st2, sg1, sg2,
    own_sem, zs, zr, ys, yr, ts, tr,
):
    f = lax.axis_index("fs")
    me = lax.axis_index("tp")
    rep = lax.axis_index("rep")
    count, dt = x_ref.shape
    width = dt * T
    local = [wv_ref, wg_ref, wo_ref, wga_ref, wup_ref, wd_ref]
    bufs = [bv, bg, bo, bga, bup, bd]

    barrier = pltpu.get_barrier_semaphore()
    greeted = 0
    for target in (lax.rem(f + 1, F), lax.rem(f + F - 1, F)):
        pl.semaphore_signal(barrier, inc=1, device_id={"fs": target}, device_id_type=MESH)
        greeted += 1
    if split == 2:
        pl.semaphore_signal(barrier, inc=1, device_id={"rep": 1 - rep}, device_id_type=MESH)
        greeted += 1
    for d in range(1, T):
        pl.semaphore_signal(barrier, inc=1, device_id={"tp": lax.rem(me + d, T)}, device_id_type=MESH)
        greeted += 1
    own = [
        pltpu.make_async_copy(local[w], bufs[w].at[f], own_sem.at[w]) for w in range(6)
    ]
    for copy in own:
        copy.start()
    pl.semaphore_wait(barrier, greeted)

    def half(w):
        n = local[w].shape[0] // split
        return pl.ds(pl.multiple_of((rep if split == 2 else 0) * n, n), n)

    def other(w):
        n = local[w].shape[0] // split
        return pl.ds(pl.multiple_of((1 - rep) * n, n), n)

    def hop(w, side, s):
        shard = f - s if side == 0 else f + s
        target = f + 1 if side == 0 else f - 1
        src = local[w].at[half(w)] if s == 0 else bufs[w].at[shard, half(w)]
        return remote(src, bufs[w].at[shard, half(w)], zs.at[side, w, s], zr.at[side, w, s + 1], {"fs": target})

    def arrival(w, side, s):
        shard = f - s if side == 0 else f + s
        ref = bufs[w].at[shard, half(w)]
        return remote(ref, ref, zs.at[side, w, s], zr.at[side, w, s], {"fs": f})

    def across(w, side, s):
        shard = f - s if side == 0 else f + s
        ref = bufs[w].at[shard, half(w)]
        return remote(ref, ref, ys.at[side, w, s], yr.at[side, w, s], {"rep": 1 - rep})

    def across_in(w, side, s):
        shard = f - s if side == 0 else f + s
        ref = bufs[w].at[shard, other(w)]
        return remote(ref, ref, ys.at[side, w, s], yr.at[side, w, s], {"rep": 1 - rep})

    def has(side, s):
        return f >= s if side == 0 else f + s <= F - 1

    def sends(side, s):
        ahead = f < F - 1 if side == 0 else f > 0
        return jnp.logical_and(has(side, s), ahead)

    def launch(w):
        for side in (0, 1):
            @pl.when(sends(side, 0))
            def _():
                hop(w, side, 0).start()

    def relay(group, stages=range(1, F)):
        for s in stages:
            for w in group:
                for side in (0, 1):
                    @pl.when(has(side, s))
                    def _():
                        arrival(w, side, s).wait_recv()
                        if s < F - 1:
                            @pl.when(sends(side, s))
                            def _():
                                hop(w, side, s).start()
                        if split == 2:
                            across(w, side, s).start()

    def settle(group):
        for w in group:
            own[w].wait()
        if split == 2:
            for s in range(1, F):
                for w in group:
                    for side in (0, 1):
                        @pl.when(has(side, s))
                        def _():
                            across_in(w, side, s).wait_recv()

    def tp_send(k, src, dst_at, d):
        return remote(src, dst_at, ts.at[k, d], tr.at[k, d], {"tp": lax.rem(me + d, T)})

    for w in (0, 1):
        launch(w)
    for d in range(1, T):
        tp_send(0, x_ref, xg.at[me], d).start()
    launch(2)
    xg[me] = x_ref[...]
    for d in range(1, T):
        peer = lax.rem(me + T - d, T)
        tp_send(0, x_ref, xg.at[peer], d).wait_recv()

    block = chunk_of(count, 16)

    def norm_rows(src, gain):
        def step(i, _):
            r = pl.ds(pl.multiple_of(i * block, block), block)
            vals = [src[t, r, :].astype(F32) for t in range(T)]
            ss = sum(jnp.sum(v * v, axis=1, keepdims=True) for v in vals)
            scale = lax.rsqrt(ss / width + EPS)
            for t in range(T):
                rows[r, t * dt:(t + 1) * dt] = (
                    vals[t] * scale * gain[t:t + 1, :]
                ).astype(BF16)
            return 0
        lax.fori_loop(0, count // block, step, 0)

    norm_rows(xg, ng_ref)
    relay((0, 1, 2))
    for w in (3, 4, 5):
        launch(w)
    settle((0, 1))

    chan = bv.shape[2]
    batch = count // length
    taps = cw_ref.shape[0]
    pad = 8 * ((taps - 1 + 7) // 8)
    lead = pad - (taps - 1)

    def columns(buf, c, n):
        block_w = buf[:, :, pl.ds(pl.multiple_of(c * n, n), n)]
        return block_w.reshape(block_w.shape[0] * block_w.shape[1], n)

    nc = chunk_of(chan, 256)

    def glu_step(c, _):
        value = jnp.dot(rows[...], columns(bv, c, nc), preferred_element_type=F32)
        gate = jnp.dot(rows[...], columns(bg, c, nc), preferred_element_type=F32)
        res = value * jax.nn.sigmoid(gate)
        for b in range(batch):
            glu[b, pl.ds(pad, length), pl.ds(pl.multiple_of(c * nc, nc), nc)] = (
                res[b * length:(b + 1) * length]
            )
        return 0

    for b in range(batch):
        glu[b, 0:pad, :] = jnp.zeros((pad, chan), F32)
        glu[b, pad + length:, :] = jnp.zeros((8, chan), F32)
    lax.fori_loop(0, chan // nc, glu_step, 0)
    relay((3,), (1,))

    lanes = chunk_of(chan, 128)
    span = chunk_of(length, 64)
    strips = chan // lanes

    def conv_step(i, _):
        q = lax.rem(i, strips)
        p = i // strips
        cols = pl.ds(pl.multiple_of(q * lanes, lanes), lanes)
        weights = cw_ref[:, cols]
        for b in range(batch):
            total = jnp.zeros((span, lanes), F32)
            for shift in range(8):
                acc = None
                for tap in range(taps):
                    if (lead + tap) % 8 != shift:
                        continue
                    base = lead + tap - shift
                    term = weights[tap:tap + 1, :] * glu[
                        b, pl.ds(pl.multiple_of(p * span + base, 8), span + 8), cols
                    ]
                    acc = term if acc is None else acc + term
                if acc is not None:
                    total = total + acc[shift:shift + span]
            conv[pl.ds(pl.multiple_of(b * length + p * span, span), span), cols] = total
        return 0

    lax.fori_loop(0, strips * (length // span), conv_step, 0)

    lane = lax.broadcasted_iota(jnp.int32, (count, 128), 1)

    def across_lanes(a, b):
        table = jnp.where(lane == 0, a, jnp.where(lane == 1, b, 0.0))
        return jnp.transpose(table)[0:8, :]

    def down_rows(top):
        full = jnp.concatenate([top, jnp.zeros((120, count), F32)], axis=0)
        return jnp.transpose(full)

    values = conv[...]
    local_sum = jnp.sum(values, axis=1, keepdims=True)
    dev = values - local_sum / chan
    st1[...] = across_lanes(local_sum, jnp.sum(dev * dev, axis=1, keepdims=True))
    sg1[me] = st1[...]
    for d in range(1, T):
        tp_send(1, st1, sg1.at[me], d).start()
    relay((4,), (1,))
    for d in range(1, T):
        peer = lax.rem(me + T - d, T)
        tp_send(1, st1, sg1.at[peer], d).wait_recv()
    sums = [sg1[t] for t in range(T)]
    mean = sum(s[0:1, :] for s in sums) / (chan * T)
    spread = sum(
        s[1:2, :] + chan * (s[0:1, :] / chan - mean) * (s[0:1, :] / chan - mean) for s in sums
    ) / (chan * T)
    inv = lax.rsqrt(spread + EPS)
    line = lax.broadcasted_iota(jnp.int32, (8, count), 0)
    table = down_rows(jnp.where(line == 0, mean, jnp.where(line == 1, inv, 0.0)))
    normed = (conv[...] - table[:, 0:1]) * table[:, 1:2] * cg_ref[...]
    act[...] = (normed * jax.nn.sigmoid(normed)).astype(BF16)

    settle((2,))

    def project(src, buf, part):
        dsh = buf.shape[2]
        for j in range(F):
            t, off = (j * dsh) // dt, (j * dsh) % dt
            prod = jnp.dot(src[...], buf[j], preferred_element_type=F32)
            part[t, :, off:off + dsh] = prod.astype(BF16)

    def scatter(k, part, got):
        for d in range(1, T):
            tp_send(k, part.at[lax.rem(me + d, T)], got.at[d - 1], d).start()

    def gathered(k, part, got):
        total = part[me].astype(F32)
        for d in range(1, T):
            tp_send(k, part.at[me], got.at[d - 1], d).wait_recv()
            total = total + got[d - 1].astype(F32)
        return total

    def piece(t):
        return remote(part2.at[t], got2.at[me], ts.at[4, t], tr.at[4, me], {"tp": t})

    def piece_in(t):
        return remote(part2.at[t], got2.at[t], ts.at[4, t], tr.at[4, t], {"tp": t})

    project(act, bo, part1)
    scatter(2, part1, got1)
    relay((5,), (1,))
    first = (x_ref[...].astype(F32) + gathered(2, part1, got1)).astype(BF16)
    firsts[me] = first
    for d in range(1, T):
        tp_send(3, firsts.at[me], firsts.at[me], d).start()
    relay((3,), (2,))
    for d in range(1, T):
        peer = lax.rem(me + T - d, T)
        tp_send(3, firsts.at[peer], firsts.at[peer], d).wait_recv()
    relay((4,), (2,))
    norm_rows(firsts, mg_ref)
    relay((5,), (2,))
    relay((3, 4), range(3, F))
    settle((3, 4))

    ff = bga.shape[2]
    nf = chunk_of(ff, 256)

    def ff_step(c, _):
        gate = jnp.dot(rows[...], columns(bga, c, nf), preferred_element_type=F32)
        up = jnp.dot(rows[...], columns(bup, c, nf), preferred_element_type=F32)
        hid[:, pl.ds(pl.multiple_of(c * nf, nf), nf)] = (
            gate * jax.nn.sigmoid(gate) * up
        ).astype(BF16)
        return 0

    lax.fori_loop(0, ff // nf, ff_step, 0)
    if F == T and bd.shape[2] == dt:
        def down(shard):
            prod = jnp.dot(hid[...], bd[shard], preferred_element_type=F32)
            part2[shard] = prod.astype(BF16)

            @pl.when(shard != me)
            def _():
                piece(shard).start()

        own[5].wait()
        down(f)
        for s in range(1, F):
            if s >= 3:
                relay((5,), (s,))
            for side in (0, 1):
                @pl.when(has(side, s))
                def _():
                    if split == 2:
                        across_in(5, side, s).wait_recv()
                    down(f - s if side == 0 else f + s)
    else:
        relay((5,), range(3, F))
        settle((5,))
        project(hid, bd, part2)
        for d in range(1, T):
            piece(lax.rem(me + d, T)).start()
    second = firsts[me].astype(F32) + part2[me].astype(F32)
    for d in range(1, T):
        peer = lax.rem(me + d, T)
        piece_in(peer).wait_recv()
        second = second + got2[peer].astype(F32)
    total = jnp.sum(second * second, axis=1, keepdims=True)
    conv[:, 0:dt] = second
    st2[...] = across_lanes(total, total)
    sg2[me] = st2[...]
    for d in range(1, T):
        tp_send(5, st2, sg2.at[me], d).start()
    for d in range(1, T):
        peer = lax.rem(me + T - d, T)
        tp_send(5, st2, sg2.at[peer], d).wait_recv()
    full = sum(sg2[t] for t in range(T))
    table = down_rows(full)
    scale = lax.rsqrt(table[:, 0:1] / width + EPS)
    out_ref[...] = (conv[:, 0:dt] * scale * fg_ref[...]).astype(BF16)

    for w in range(6):
        for side in (0, 1):
            for s in range(F):
                if s < F - 1:
                    @pl.when(sends(side, s))
                    def _():
                        hop(w, side, s).wait_send()
                if s >= 1 and split == 2:
                    @pl.when(has(side, s))
                    def _():
                        across(w, side, s).wait_send()
    for d in range(1, T):
        peer = lax.rem(me + d, T)
        tp_send(0, x_ref, xg.at[me], d).wait_send()
        tp_send(1, st1, sg1.at[me], d).wait_send()
        tp_send(2, part1.at[peer], got1.at[d - 1], d).wait_send()
        tp_send(3, firsts.at[me], firsts.at[me], d).wait_send()
        piece(peer).wait_send()
        tp_send(5, st2, sg2.at[me], d).wait_send()


PIECES = (2, 2, 2, 2, 2, 4)
FIRST = tuple(sum(PIECES[:w]) for w in range(6))
GROUP = (0, 0, 0, 1, 1, 2)


def fast_kernel(
    length,
    x_ref, ng_hbm, cw_hbm, cg_hbm, mg_hbm, fg_hbm,
    wv_ref, wg_ref, wo_ref, wga_ref, wup_ref, wd_ref,
    out_ref,
    ng_ref, cw_ref, cg_ref, mg_ref, fg_ref, bv, bg, bo, bga, bup, bd,
    xg, rows, accv, accg, glu, conv, act, part, got, q1, q1in, firsts, hid,
    accs, part2, got2, q2, q2in, sec, ssq, secb, secin, st1, sg1, st2, sg2, finin,
    small, own_sem, zs, zr, zr2, ms, mr, md, ys, yr, xos, xor_, ags, agr, sts, str_, rss, rsr, ds_, dr, qs, qr, os_, orr, fs_, fr,
):
    f = lax.axis_index("fs")
    me = lax.axis_index("tp")
    rep = lax.axis_index("rep")
    count, dt = x_ref.shape
    T = 4
    width = dt * T
    rows_all = 2 * count
    batch = count // length
    chan, ff = bv.shape[2], bga.shape[2]
    local = [wv_ref, wg_ref, wo_ref, wga_ref, wup_ref, wd_ref]
    bufs = [bv, bg, bo, bga, bup, bd]
    VAL, GATE, CVO, GA, UP, DOWN = range(6)
    outer = jnp.logical_or(f == 0, f == 3)
    near = 1 + f // 3
    po, pi, fo = 3 * (f - 1), 3 - f, 3 * (2 - f)
    sib = me + 1 - 2 * lax.rem(me, 2)
    mir = lax.rem(me + 2, T)
    dia = lax.rem(sib + 2, T)

    def view(ref, w, h, c):
        if w == DOWN:
            n, m = ref.shape[1] // 2, ref.shape[0] // 2
            k = n // 2
            return ref.at[pl.ds((c % 2) * m, m), pl.ds(pl.multiple_of(h * n + (c // 2) * k, k), k)]
        n = ref.shape[0] // 2
        k = n // PIECES[w]
        return ref.at[pl.ds(pl.multiple_of(h * n + c * k, k), k), :]

    barrier = pltpu.get_barrier_semaphore()

    def greet(**target):
        pl.semaphore_signal(barrier, inc=1, device_id=target, device_id_type=MESH)

    def zsend(w, hs, c):
        h = rep if hs == 0 else 1 - rep
        sem = zr2.at[w] if hs else zr.at[FIRST[w] + c]
        return remote(view(local[w], w, h, c), view(bufs[w].at[f], w, h, c), zs.at[GROUP[w]], sem, {"fs": near})

    def all_sent(sems, extra=1):
        for g, ref in enumerate((bufs[VAL].at[0:3], bufs[GA].at[0:2], bufs[DOWN].at[0, :, 0:bd.shape[2] * extra // 4])):
            remote(ref, ref, sems.at[g], sems.at[g], {"fs": f}).wait_send()

    def xsend():
        return remote(x_ref, xg.at[me, 0], xos, xor_, {"fs": near})

    hn = dt // 2

    def ucols(j):
        if j == 0:
            return pl.ds(pl.multiple_of(rep * hn, hn), hn)
        return pl.ds(pl.multiple_of((1 - rep) * hn + (j - 1) * (hn // 2), hn // 2), hn // 2)

    def result(cols, target):
        return remote(secb.at[:, cols], secin.at[:, cols], os_, orr, {"fs": target})

    smalls = [
        pltpu.make_async_copy(src, dst, small.at[k])
        for k, (src, dst) in enumerate(
            ((ng_hbm, ng_ref), (cw_hbm, cw_ref), (cg_hbm, cg_ref), (mg_hbm, mg_ref), (fg_hbm, fg_ref))
        )
    ]

    lane = lax.broadcasted_iota(jnp.int32, (count, 128), 1)
    line = lax.broadcasted_iota(jnp.int32, (8, count), 0)

    def across_lanes(a, b):
        table = jnp.where(lane == 0, a, jnp.where(lane == 1, b, 0.0))
        return jnp.transpose(table)[0:8, :]

    def down_rows(top):
        full = jnp.concatenate([top, jnp.zeros((120, count), F32)], axis=0)
        return jnp.transpose(full)

    @pl.when(outer)
    def _():
        for t in range(T):
            greet(fs=near, tp=t)
        smalls[4].start()
        pl.semaphore_wait(barrier, T)
        order = [
            (VAL, 0), (GATE, 0), None, (CVO, 0), (VAL, 1), (GATE, 1), (CVO, 1),
            (GA, 0), (UP, 0), (GA, 1), (UP, 1), (DOWN, 0), (DOWN, 1),
        ]
        for item in order:
            if item is None:
                xsend().start()
            else:
                for c in range(PIECES[item[0]]):
                    zsend(item[0], item[1], c).start()
        xsend().wait_send()
        all_sent(zs, 4)
        smalls[4].wait()
        remote(secb, secin, os_, orr, {"fs": near}).wait_recv()
        remote(finin, finin, fs_, fr, {"fs": near}).wait_recv()
        full = sum(finin[t] for t in range(T))
        scale = lax.rsqrt(down_rows(full)[:, 0:1] / width + EPS)
        out_ref[...] = (secin[...].astype(F32) * scale * fg_ref[...]).astype(BF16)

    @pl.when(jnp.logical_not(outer))
    def _():
        for t in range(T):
            greet(fs=po, tp=t)
        greet(fs=pi)
        greet(rep=1 - rep)
        for t in (sib, mir, dia):
            greet(tp=t)
        own = [pltpu.make_async_copy(local[w], bufs[w].at[f], own_sem.at[w]) for w in range(6)]
        load_x = pltpu.make_async_copy(x_ref, xg.at[me, 1], small.at[5])
        load_x.start()
        for copy in smalls:
            copy.start()
        for copy in own:
            copy.start()
        pl.semaphore_wait(barrier, T + 5)

        def arrived(ref, send, recv):
            remote(ref, ref, send, recv, {"fs": f}).wait_recv()

        def mid_own(w, c):
            return remote(
                view(local[w], w, rep, c), view(bufs[w].at[f], w, rep, c), ms.at[GROUP[w]], mr.at[0, FIRST[w] + c], {"fs": pi}
            )

        def mid_fwd(w, c):
            ref = view(bufs[w].at[po], w, rep, c)
            return remote(ref, ref, ms.at[GROUP[w]], mr.at[1, FIRST[w] + c], {"fs": pi})

        def mid_direct(c):
            return remote(
                view(local[DOWN], DOWN, 1 - rep, c), view(bufs[DOWN].at[f], DOWN, 1 - rep, c), md.at[0], md.at[1], {"fs": pi}
            )

        def y_fwd(w, k, c):
            ref = view(bufs[w].at[fo if k else pi], w, rep, c)
            sem = yr.at[k, w + c // 2 if w == DOWN else w]
            return remote(ref, ref, ys.at[GROUP[w]], sem, {"rep": 1 - rep})

        def send_own(w):
            for c in range(PIECES[w]):
                mid_own(w, c).start()

        def relay_mid(w, c):
            arrived(view(bufs[w].at[po], w, rep, c), zs.at[GROUP[w]], zr.at[FIRST[w] + c])
            mid_fwd(w, c).start()

        def wait_mid(w, k, c):
            arrived(view(bufs[w].at[fo if k else pi], w, rep, c), ms.at[GROUP[w]], mr.at[k, FIRST[w] + c])

        def relay_y(w, k, c):
            wait_mid(w, k, c)
            y_fwd(w, k, c).start()

        def other(w, shard):
            if w == DOWN:
                return bufs[w].at[shard, :, pl.ds(pl.multiple_of((1 - rep) * hn, hn), hn)]
            n = bufs[w].shape[1] // 2
            return bufs[w].at[shard, pl.ds(pl.multiple_of((1 - rep) * n, n), n), :]

        def wait_z(w):
            arrived(other(w, po), zs.at[GROUP[w]], zr2.at[w])

        def wait_y(w, k):
            arrived(other(w, fo if k else pi), ys.at[GROUP[w]], yr.at[k, w])

        def wait_y_down(k, j):
            ref = bufs[DOWN].at[fo if k else pi, :, ucols(j)]
            arrived(ref, ys.at[2], yr.at[k, DOWN + j - 1])

        def wait_direct():
            arrived(bufs[DOWN].at[pi, :, ucols(2)], md.at[0], md.at[1])

        def ag(p, buf, slot, kind):
            ref = buf.at[mir if kind == 2 else me, slot]
            return remote(
                ref, ref, ags.at[p, slot], agr.at[p, slot, 1 if kind == 1 else 0], {"tp": mir if kind == 1 else sib}
            )

        def ag_start(p, buf, slot):
            ag(p, buf, slot, 1).start()
            ag(p, buf, slot, 0).start()

        def ag_forward(p, buf, slot):
            arrived(buf.at[mir, slot], ags.at[p, slot], agr.at[p, slot, 1])
            ag(p, buf, slot, 2).start()

        def ag_finish(p, buf, slot):
            arrived(buf.at[0:2, slot], ags.at[p, slot], agr.at[p, slot, 0])

        block = chunk_of(count, 16)

        def norm_rows(src, slot, gain):
            def step(i, _):
                r = pl.ds(pl.multiple_of(i * block, block), block)
                o = pl.ds(pl.multiple_of(slot * count + i * block, block), block)
                vals = [src[t, slot, r, :].astype(F32) for t in range(T)]
                ss = sum(jnp.sum(v * v, axis=1, keepdims=True) for v in vals)
                scale = lax.rsqrt(ss / width + EPS)
                for t in range(T):
                    rows[t, o, :] = (vals[t] * scale * gain[:, t * dt:(t + 1) * dt]).astype(BF16)
                return 0
            lax.fori_loop(0, count // block, step, 0)

        def stat(k, src, dst, d):
            return remote(src, dst, sts.at[k], str_.at[k], {"tp": lax.rem(me + d, T)})

        send_own(VAL)
        send_own(GATE)
        load_x.wait()
        ag_start(0, xg, 1)
        for c in range(2):
            relay_mid(VAL, c)
            relay_y(VAL, 0, c)
        relay_mid(GATE, 0)
        ag_forward(0, xg, 1)
        relay_y(GATE, 0, 0)
        relay_mid(GATE, 1)
        relay_y(GATE, 0, 1)
        send_own(CVO)
        ag_finish(0, xg, 1)
        for copy in smalls:
            copy.wait()
        norm_rows(xg, 1, ng_ref)
        relay_y(VAL, 1, 0)
        arrived(xg.at[me, 0], xos, xor_)
        ag_start(0, xg, 0)
        relay_y(VAL, 1, 1)
        relay_mid(CVO, 0)
        relay_y(GATE, 1, 0)
        relay_mid(CVO, 1)
        send_own(GA)
        send_own(UP)
        relay_y(GATE, 1, 1)
        ag_forward(0, xg, 0)
        ag_finish(0, xg, 0)
        norm_rows(xg, 0, ng_ref)
        relay_y(CVO, 0, 0)

        pad = glu.shape[1] - length - 8
        taps = cw_ref.shape[0]
        lead = pad - (taps - 1)
        nc = chunk_of(chan, 256)
        for b in range(2 * batch):
            glu[b, 0:pad, :] = jnp.zeros((pad, chan), F32)
            glu[b, pad + length:, :] = jnp.zeros((8, chan), F32)

        def s1(shard, first, last):
            def step(c, _):
                cols = pl.ds(pl.multiple_of(c * nc, nc), nc)
                value = jnp.dot(rows[shard], bv[shard, :, cols], preferred_element_type=F32)
                gate = jnp.dot(rows[shard], bg[shard, :, cols], preferred_element_type=F32)
                if not first:
                    value = value + accv[:, cols]
                    gate = gate + accg[:, cols]
                if last:
                    res = value * jax.nn.sigmoid(gate)
                    for b in range(2 * batch):
                        glu[b, pl.ds(pad, length), cols] = res[b * length:(b + 1) * length]
                else:
                    accv[:, cols] = value
                    accg[:, cols] = gate
                return 0
            lax.fori_loop(0, chan // nc, step, 0)

        own[VAL].wait()
        own[GATE].wait()
        s1(f, True, False)
        wait_y(VAL, 0)
        wait_y(GATE, 0)
        s1(pi, False, False)
        relay_y(CVO, 0, 1)
        wait_y(VAL, 1)
        wait_y(GATE, 1)
        s1(fo, False, False)
        relay_y(CVO, 1, 0)
        wait_z(VAL)
        wait_z(GATE)
        s1(po, False, True)
        relay_y(CVO, 1, 1)

        lanes = chunk_of(chan, 128)
        span = chunk_of(length, 64)
        strips = chan // lanes

        def convolve(slot):
            def step(i, _):
                s = lax.rem(i, strips)
                p = i // strips
                cols = pl.ds(pl.multiple_of(s * lanes, lanes), lanes)
                weights = cw_ref[:, cols]
                for b in range(batch):
                    total = jnp.zeros((span, lanes), F32)
                    for shift in range(8):
                        acc = None
                        for tap in range(taps):
                            if (lead + tap) % 8 != shift:
                                continue
                            base = lead + tap - shift
                            term = weights[tap:tap + 1, :] * glu[
                                slot * batch + b, pl.ds(pl.multiple_of(p * span + base, 8), span + 8), cols
                            ]
                            acc = term if acc is None else acc + term
                        if acc is not None:
                            total = total + acc[shift:shift + span]
                    at = pl.multiple_of(slot * count + b * length + p * span, span)
                    conv[pl.ds(at, span), cols] = total
                return 0
            lax.fori_loop(0, strips * (length // span), step, 0)

        def span_of(slot):
            return slice(slot * count, (slot + 1) * count)

        def conv_stats(slot):
            values = conv[span_of(slot), :]
            local_sum = jnp.sum(values, axis=1, keepdims=True)
            dev = values - local_sum / chan
            st1[slot] = across_lanes(local_sum, jnp.sum(dev * dev, axis=1, keepdims=True))
            sg1[slot, me] = st1[slot]
            for d in range(1, T):
                stat(slot, st1.at[slot], sg1.at[slot, me], d).start()

        def activate(slot):
            arrived(sg1.at[slot, 0:3], sts.at[slot], str_.at[slot])
            sums = [sg1[slot, t] for t in range(T)]
            mean = sum(s[0:1, :] for s in sums) / (chan * T)
            spread = sum(
                s[1:2, :] + chan * (s[0:1, :] / chan - mean) * (s[0:1, :] / chan - mean) for s in sums
            ) / (chan * T)
            inv = lax.rsqrt(spread + EPS)
            table = down_rows(jnp.where(line == 0, mean, jnp.where(line == 1, inv, 0.0)))
            normed = (conv[span_of(slot), :] - table[:, 0:1]) * table[:, 1:2] * cg_ref[...]
            act[span_of(slot), :] = (normed * jax.nn.sigmoid(normed)).astype(BF16)

        def rs(slot, kind):
            if kind == 2:
                return remote(q1.at[slot], q1in.at[slot], rss.at[slot], rsr.at[slot, 0], {"tp": mir})
            return remote(
                part.at[slot, dia if kind else sib], got.at[slot, kind], rss.at[slot], rsr.at[slot, kind], {"tp": sib}
            )

        def project(slot):
            def step(j, _):
                prod = jnp.dot(act[span_of(slot), :], bo[j], preferred_element_type=F32)
                part[slot, j] = prod.astype(BF16)
                return 0
            lax.fori_loop(0, T, step, 0)
            rs(slot, 1).start()
            rs(slot, 0).start()

        def pair_sum(slot):
            rs(slot, 1).wait_recv()
            q1[slot] = (part[slot, mir].astype(F32) + got[slot, 1].astype(F32)).astype(BF16)
            rs(slot, 2).start()

        def finish_first(slot):
            arrived(part.at[slot, 0:2], rss.at[slot], rsr.at[slot, 0])
            total = xg[me, slot].astype(F32) + (part[slot, me].astype(F32) + got[slot, 0].astype(F32))
            firsts[me, slot] = (total + q1in[slot].astype(F32)).astype(BF16)
            ag_start(1, firsts, slot)

        convolve(0)
        conv_stats(0)
        convolve(1)
        conv_stats(1)
        relay_y(GA, 0, 0)
        own[CVO].wait()
        wait_y(CVO, 0)
        wait_y(CVO, 1)
        wait_z(CVO)
        activate(0)
        project(0)
        activate(1)
        relay_mid(GA, 0)
        project(1)
        pair_sum(0)
        relay_y(GA, 0, 1)
        pair_sum(1)
        relay_mid(GA, 1)
        relay_y(UP, 0, 0)
        finish_first(0)
        relay_mid(UP, 0)
        relay_y(UP, 0, 1)
        relay_mid(UP, 1)
        send_own(DOWN)
        relay_y(GA, 1, 0)
        finish_first(1)
        relay_y(GA, 1, 1)
        ag_forward(1, firsts, 0)
        relay_y(UP, 1, 0)
        ag_finish(1, firsts, 0)
        norm_rows(firsts, 0, mg_ref)
        ag_forward(1, firsts, 1)
        relay_y(UP, 1, 1)
        ag_finish(1, firsts, 1)
        relay_y(DOWN, 0, 0)
        norm_rows(firsts, 1, mg_ref)
        relay_y(DOWN, 0, 1)

        nf = chunk_of(ff, 256)

        def s5(w, keep):
            def step(c, _):
                cols = pl.ds(pl.multiple_of(c * nf, nf), nf)
                value = sum(jnp.dot(rows[t], bufs[w][t, :, cols], preferred_element_type=F32) for t in range(T))
                if keep:
                    accs[:, cols] = value
                else:
                    gate = accs[:, cols]
                    hid[:, cols] = (gate * jax.nn.sigmoid(gate) * value).astype(BF16)
                return 0
            lax.fori_loop(0, ff // nf, step, 0)

        own[GA].wait()
        own[UP].wait()
        wait_y(GA, 0)
        wait_y(GA, 1)
        wait_z(GA)
        s5(GA, True)
        relay_mid(DOWN, 0)
        wait_y(UP, 0)
        wait_z(UP)
        wait_y(UP, 1)
        s5(UP, False)
        relay_mid(DOWN, 1)

        def pair_send(b, j):
            ref = part2.at[b, :, ucols(j)]
            return remote(ref, got2.at[b, :, ucols(j)], ds_, dr.at[lax.rem(b // 2 + me // 2, 2), j], {"tp": sib})

        def cross(j):
            return remote(q2.at[:, ucols(j)], q2in.at[:, ucols(j)], qs, qr.at[j], {"tp": mir})

        def down(b, j):
            cols = ucols(j)
            prod = jnp.dot(hid[...], bd[b, :, cols], preferred_element_type=F32)
            part2[b, :, cols] = prod.astype(BF16)

            @pl.when(jnp.logical_or(b == sib, b == dia))
            def _():
                pair_send(b, j).start()

        def combine(b, j):
            cols = ucols(j)

            @pl.when(b == mir)
            def _():
                pair_send(b, j).wait_recv()
                q2[:, cols] = (part2[b, :, cols].astype(F32) + got2[b, :, cols].astype(F32)).astype(BF16)
                cross(j).start()

        def outer_stat(d):
            return remote(st2.at[0], finin.at[me], fs_, fr, {"fs": po, "tp": lax.rem(me + d, T)})

        def finish(j):
            pair_send(me, j).wait_recv()
            cross(j).wait_recv()
            cols = ucols(j)
            for slot in range(2):
                r = span_of(slot)
                second = firsts[me, slot, :, cols].astype(F32) + part2[me, r, cols].astype(F32)
                second = second + got2[me, r, cols].astype(F32) + q2in[r, cols].astype(F32)
                if slot == 0:
                    secb[:, cols] = second.astype(BF16)
                    result(cols, po).start()
                else:
                    sec[:, cols] = second
                total = jnp.sum(second * second, axis=1, keepdims=True)
                if j > 0:
                    total = total + ssq[r, :]
                if j < 2:
                    ssq[r, :] = total
                    continue
                st2[slot] = across_lanes(total, total)
                if slot == 0:
                    for d in range(T):
                        outer_stat(d).start()
                else:
                    sg2[me] = st2[1]
                    for d in range(1, T):
                        stat(2, st2.at[1], sg2.at[me], d).start()

        own[DOWN].wait()
        wait_mid(DOWN, 0, 2)
        wait_mid(DOWN, 0, 3)
        down(pi, 0)
        down(f, 0)
        relay_mid(DOWN, 2)
        combine(pi, 0)
        relay_y(DOWN, 1, 0)
        combine(f, 0)
        wait_y_down(0, 1)
        down(pi, 1)
        down(f, 1)
        relay_mid(DOWN, 3)
        mid_direct(2).start()
        mid_direct(3).start()
        combine(pi, 1)
        relay_y(DOWN, 1, 1)
        combine(f, 1)
        down(po, 0)
        down(f, 2)
        relay_y(DOWN, 1, 2)
        combine(po, 0)
        combine(f, 2)
        wait_y_down(1, 1)
        down(fo, 1)
        relay_y(DOWN, 1, 3)
        down(fo, 0)
        combine(fo, 1)
        combine(fo, 0)
        wait_z(DOWN)
        down(po, 1)
        down(po, 2)
        combine(po, 1)
        wait_direct()
        down(pi, 2)
        wait_y_down(1, 2)
        down(fo, 2)
        combine(po, 2)
        combine(pi, 2)
        combine(fo, 2)
        finish(0)
        finish(1)
        finish(2)
        arrived(sg2.at[0:3], sts.at[2], str_.at[2])
        table = down_rows(sum(sg2[t] for t in range(T)))
        scale = lax.rsqrt(table[:, 0:1] / width + EPS)
        out_ref[...] = (sec[...] * scale * fg_ref[...]).astype(BF16)

        def sent(ref, sem):
            remote(ref, ref, sem, sem, {"fs": f}).wait_send()

        all_sent(ms, 4)
        all_sent(ys, 3)
        sent(bufs[DOWN].at[f, :, ucols(2)], md.at[0])
        for slot in range(2):
            sent(xg.at[0:3, slot], ags.at[0, slot])
            sent(firsts.at[0:3, slot], ags.at[1, slot])
            sent(part.at[slot, 0:3], rss.at[slot])
            sent(sg1.at[slot, 0:3], sts.at[slot])
        sent(sg2.at[0:3], sts.at[2])
        sent(part2.at[0:2], ds_)
        sent(q2, qs)
        sent(secb, os_)
        sent(finin, fs_)


def fast_body(
    activations, norm_gain, w_value, w_gate_conv, conv_weight, chan_gain,
    w_conv_out, mix_gain, w_gate, w_up, w_down, final_gain,
):
    batch, length, dt = activations.shape
    count = batch * length
    weights = (w_value, w_gate_conv, w_conv_out, w_gate, w_up, w_down)
    chan, ff = w_value.shape[1], w_gate.shape[1]
    T = 4
    pad = 8 * ((conv_weight.shape[0] - 1 + 7) // 8)
    rows_all = 2 * count
    vmem, hbm = pl.BlockSpec(memory_space=pltpu.VMEM), pl.BlockSpec(memory_space=pl.ANY)
    dma = pltpu.SemaphoreType.DMA
    V = pltpu.VMEM
    out = pl.pallas_call(
        functools.partial(fast_kernel, length),
        out_shape=jax.ShapeDtypeStruct((count, dt), BF16),
        in_specs=[hbm] * 12,
        out_specs=vmem,
        scratch_shapes=[
            V((1, dt * T), F32),
            V(conv_weight.shape, F32),
            V((1, chan), F32),
            V((1, dt * T), F32),
            V((1, dt), F32),
        ] + [V((4,) + w.shape, BF16) for w in weights] + [
            V((T, 2, count, dt), BF16),
            V((T, rows_all, dt), BF16),
            V((rows_all, chan), F32),
            V((rows_all, chan), F32),
            V((2 * batch, pad + length + 8, chan), F32),
            V((rows_all, chan), F32),
            V((rows_all, chan), BF16),
            V((2, T, count, dt), BF16),
            V((2, 2, count, dt), BF16),
            V((2, count, dt), BF16),
            V((2, count, dt), BF16),
            V((T, 2, count, dt), BF16),
            V((rows_all, ff), BF16),
            V((rows_all, ff), F32),
            V((T, rows_all, dt), BF16),
            V((T, rows_all, dt), BF16),
            V((rows_all, dt), BF16),
            V((rows_all, dt), BF16),
            V((count, dt), F32),
            V((rows_all, 1), F32),
            V((count, dt), BF16),
            V((count, dt), BF16),
            V((2, 8, count), F32),
            V((2, T, 8, count), F32),
            V((2, 8, count), F32),
            V((T, 8, count), F32),
            V((T, 8, count), F32),
            dma((6,)),
            dma((6,)),
            dma((3,)),
            dma((sum(PIECES),)),
            dma((6,)),
            dma((3,)),
            dma((2, sum(PIECES))),
            dma((2,)),
            dma((3,)),
            dma((2, 7)),
            dma(()),
            dma(()),
            dma((2, 2)),
            dma((2, 2, 2)),
            dma((3,)),
            dma((3,)),
            dma((2,)),
            dma((2, 2)),
            dma(()),
            dma((2, 3)),
            dma(()),
            dma((3,)),
            dma(()),
            dma(()),
            dma(()),
            dma(()),
        ],
        compiler_params=pltpu.CompilerParams(
            collective_id=0, has_side_effects=True, vmem_limit_bytes=60 * 1024 * 1024
        ),
        name="block",
    )(
        activations.reshape(count, dt),
        norm_gain.reshape(1, dt * T),
        conv_weight,
        chan_gain.reshape(1, chan),
        mix_gain.reshape(1, dt * T),
        final_gain.reshape(1, dt),
        *weights,
    )
    return out.reshape(batch, length, dt)


def ring_body(
    activations, norm_gain, w_value, w_gate_conv, conv_weight, chan_gain,
    w_conv_out, mix_gain, w_gate, w_up, w_down, final_gain,
):
    batch, length, dt = activations.shape
    count = batch * length
    R, F, T = lax.axis_size("rep"), lax.axis_size("fs"), lax.axis_size("tp")
    weights = (w_value, w_gate_conv, w_conv_out, w_gate, w_up, w_down)
    split = 2 if R == 2 and all(w.shape[0] % 32 == 0 for w in weights) else 1
    width = dt * T
    chan, ff = w_value.shape[1], w_gate.shape[1]
    taps = conv_weight.shape[0]
    pad = 8 * ((taps - 1 + 7) // 8)
    vmem, hbm = pl.BlockSpec(memory_space=pltpu.VMEM), pl.BlockSpec(memory_space=pl.ANY)
    ysh = (2, 6, F) if split == 2 else (1,)
    dma = pltpu.SemaphoreType.DMA
    out = pl.pallas_call(
        functools.partial(ring_kernel, R, F, T, split, length),
        out_shape=jax.ShapeDtypeStruct((count, dt), BF16),
        in_specs=[vmem] * 6 + [hbm] * 6,
        out_specs=vmem,
        scratch_shapes=[pltpu.VMEM((F,) + w.shape, BF16) for w in weights] + [
            pltpu.VMEM((T, count, dt), BF16),
            pltpu.VMEM((count, width), BF16),
            pltpu.VMEM((batch, pad + length + 8, chan), F32),
            pltpu.VMEM((count, max(chan, dt)), F32),
            pltpu.VMEM((count, chan), BF16),
            pltpu.VMEM((T, count, dt), BF16),
            pltpu.VMEM((T, count, dt), BF16),
            pltpu.VMEM((T - 1, count, dt), BF16),
            pltpu.VMEM((T, count, dt), BF16),
            pltpu.VMEM((T, count, dt), BF16),
            pltpu.VMEM((count, ff), BF16),
            pltpu.VMEM((8, count), F32),
            pltpu.VMEM((8, count), F32),
            pltpu.VMEM((T, 8, count), F32),
            pltpu.VMEM((T, 8, count), F32),
            dma((6,)),
            dma((2, 6, F)),
            dma((2, 6, F)),
            dma(ysh),
            dma(ysh),
            dma((6, T)),
            dma((6, T)),
        ],
        compiler_params=pltpu.CompilerParams(
            collective_id=0, has_side_effects=True, vmem_limit_bytes=60 * 1024 * 1024
        ),
        name="block",
    )(
        activations.reshape(count, dt),
        norm_gain.reshape(T, dt),
        conv_weight,
        chan_gain.reshape(1, chan),
        mix_gain.reshape(T, dt),
        final_gain.reshape(1, dt),
        *weights,
    )
    return out.reshape(batch, length, dt)


def solution(mesh):
    in_specs = (
        P(("rep", "fs"), None, "tp"),
        P(),
        P("fs", "tp"),
        P("fs", "tp"),
        P(None, "tp"),
        P("tp"),
        P("tp", "fs"),
        P(),
        P("fs", "tp"),
        P("fs", "tp"),
        P("tp", "fs"),
        P("tp"),
    )
    out_specs = P(("rep", "fs"), None, "tp")
    fast = tuple(mesh.shape[a] for a in ("rep", "fs", "tp")) == (2, 4, 4)
    body = fast_body if fast else ring_body
    return jax.shard_map(body, mesh=mesh, in_specs=in_specs, out_specs=out_specs, check_vma=False)
```

```python
import functools

import jax
import jax.numpy as jnp
from jax import lax
from jax.experimental import pallas as pl
from jax.experimental.pallas import tpu as pltpu
from jax.sharding import PartitionSpec as P

EPS = 1e-06
MESH = pl.DeviceIdType.MESH
F32 = jnp.float32
BF16 = jnp.bfloat16


def remote(src, dst, send, recv, target):
    return pltpu.make_async_remote_copy(
        src_ref=src, dst_ref=dst, send_sem=send, recv_sem=recv, device_id=target, device_id_type=MESH
    )


def chunk_of(extent, want):
    return want if extent % want == 0 else extent


def ring_kernel(
    R, F, T, split, length,
    x_ref, ng_ref, cw_ref, cg_ref, mg_ref, fg_ref,
    wv_ref, wg_ref, wo_ref, wga_ref, wup_ref, wd_ref,
    out_ref,
    bv, bg, bo, bga, bup, bd,
    xg, rows, glu, conv, act, part1, part2, got1, got2, firsts, hid, st1, st2, sg1, sg2,
    own_sem, zs, zr, ys, yr, ts, tr,
):
    f = lax.axis_index("fs")
    me = lax.axis_index("tp")
    rep = lax.axis_index("rep")
    count, dt = x_ref.shape
    width = dt * T
    local = [wv_ref, wg_ref, wo_ref, wga_ref, wup_ref, wd_ref]
    bufs = [bv, bg, bo, bga, bup, bd]

    barrier = pltpu.get_barrier_semaphore()
    greeted = 0
    for target in (lax.rem(f + 1, F), lax.rem(f + F - 1, F)):
        pl.semaphore_signal(barrier, inc=1, device_id={"fs": target}, device_id_type=MESH)
        greeted += 1
    if split == 2:
        pl.semaphore_signal(barrier, inc=1, device_id={"rep": 1 - rep}, device_id_type=MESH)
        greeted += 1
    for d in range(1, T):
        pl.semaphore_signal(barrier, inc=1, device_id={"tp": lax.rem(me + d, T)}, device_id_type=MESH)
        greeted += 1
    own = [
        pltpu.make_async_copy(local[w], bufs[w].at[f], own_sem.at[w]) for w in range(6)
    ]
    for copy in own:
        copy.start()
    pl.semaphore_wait(barrier, greeted)

    def half(w):
        n = local[w].shape[0] // split
        return pl.ds(pl.multiple_of((rep if split == 2 else 0) * n, n), n)

    def other(w):
        n = local[w].shape[0] // split
        return pl.ds(pl.multiple_of((1 - rep) * n, n), n)

    def hop(w, side, s):
        shard = f - s if side == 0 else f + s
        target = f + 1 if side == 0 else f - 1
        src = local[w].at[half(w)] if s == 0 else bufs[w].at[shard, half(w)]
        return remote(src, bufs[w].at[shard, half(w)], zs.at[side, w, s], zr.at[side, w, s + 1], {"fs": target})

    def arrival(w, side, s):
        shard = f - s if side == 0 else f + s
        ref = bufs[w].at[shard, half(w)]
        return remote(ref, ref, zs.at[side, w, s], zr.at[side, w, s], {"fs": f})

    def across(w, side, s):
        shard = f - s if side == 0 else f + s
        ref = bufs[w].at[shard, half(w)]
        return remote(ref, ref, ys.at[side, w, s], yr.at[side, w, s], {"rep": 1 - rep})

    def across_in(w, side, s):
        shard = f - s if side == 0 else f + s
        ref = bufs[w].at[shard, other(w)]
        return remote(ref, ref, ys.at[side, w, s], yr.at[side, w, s], {"rep": 1 - rep})

    def has(side, s):
        return f >= s if side == 0 else f + s <= F - 1

    def sends(side, s):
        ahead = f < F - 1 if side == 0 else f > 0
        return jnp.logical_and(has(side, s), ahead)

    def launch(w):
        for side in (0, 1):
            @pl.when(sends(side, 0))
            def _():
                hop(w, side, 0).start()

    def relay(group, stages=range(1, F)):
        for s in stages:
            for w in group:
                for side in (0, 1):
                    @pl.when(has(side, s))
                    def _():
                        arrival(w, side, s).wait_recv()
                        if s < F - 1:
                            @pl.when(sends(side, s))
                            def _():
                                hop(w, side, s).start()
                        if split == 2:
                            across(w, side, s).start()

    def settle(group):
        for w in group:
            own[w].wait()
        if split == 2:
            for s in range(1, F):
                for w in group:
                    for side in (0, 1):
                        @pl.when(has(side, s))
                        def _():
                            across_in(w, side, s).wait_recv()

    def tp_send(k, src, dst_at, d):
        return remote(src, dst_at, ts.at[k, d], tr.at[k, d], {"tp": lax.rem(me + d, T)})

    for w in (0, 1):
        launch(w)
    for d in range(1, T):
        tp_send(0, x_ref, xg.at[me], d).start()
    launch(2)
    xg[me] = x_ref[...]
    for d in range(1, T):
        peer = lax.rem(me + T - d, T)
        tp_send(0, x_ref, xg.at[peer], d).wait_recv()

    block = chunk_of(count, 16)

    def norm_rows(src, gain):
        def step(i, _):
            r = pl.ds(pl.multiple_of(i * block, block), block)
            vals = [src[t, r, :].astype(F32) for t in range(T)]
            ss = sum(jnp.sum(v * v, axis=1, keepdims=True) for v in vals)
            scale = lax.rsqrt(ss / width + EPS)
            for t in range(T):
                rows[r, t * dt:(t + 1) * dt] = (
                    vals[t] * scale * gain[t:t + 1, :]
                ).astype(BF16)
            return 0
        lax.fori_loop(0, count // block, step, 0)

    norm_rows(xg, ng_ref)
    relay((0, 1, 2))
    for w in (3, 4, 5):
        launch(w)
    settle((0, 1))

    chan = bv.shape[2]
    batch = count // length
    taps = cw_ref.shape[0]
    pad = 8 * ((taps - 1 + 7) // 8)
    lead = pad - (taps - 1)

    def columns(buf, c, n):
        block_w = buf[:, :, pl.ds(pl.multiple_of(c * n, n), n)]
        return block_w.reshape(block_w.shape[0] * block_w.shape[1], n)

    nc = chunk_of(chan, 256)

    def glu_step(c, _):
        value = jnp.dot(rows[...], columns(bv, c, nc), preferred_element_type=F32)
        gate = jnp.dot(rows[...], columns(bg, c, nc), preferred_element_type=F32)
        res = value * jax.nn.sigmoid(gate)
        for b in range(batch):
            glu[b, pl.ds(pad, length), pl.ds(pl.multiple_of(c * nc, nc), nc)] = (
                res[b * length:(b + 1) * length]
            )
        return 0

    for b in range(batch):
        glu[b, 0:pad, :] = jnp.zeros((pad, chan), F32)
        glu[b, pad + length:, :] = jnp.zeros((8, chan), F32)
    lax.fori_loop(0, chan // nc, glu_step, 0)
    relay((3,), (1,))

    lanes = chunk_of(chan, 128)
    span = chunk_of(length, 64)
    strips = chan // lanes

    def conv_step(i, _):
        q = lax.rem(i, strips)
        p = i // strips
        cols = pl.ds(pl.multiple_of(q * lanes, lanes), lanes)
        weights = cw_ref[:, cols]
        for b in range(batch):
            total = jnp.zeros((span, lanes), F32)
            for shift in range(8):
                acc = None
                for tap in range(taps):
                    if (lead + tap) % 8 != shift:
                        continue
                    base = lead + tap - shift
                    term = weights[tap:tap + 1, :] * glu[
                        b, pl.ds(pl.multiple_of(p * span + base, 8), span + 8), cols
                    ]
                    acc = term if acc is None else acc + term
                if acc is not None:
                    total = total + acc[shift:shift + span]
            conv[pl.ds(pl.multiple_of(b * length + p * span, span), span), cols] = total
        return 0

    lax.fori_loop(0, strips * (length // span), conv_step, 0)

    lane = lax.broadcasted_iota(jnp.int32, (count, 128), 1)

    def across_lanes(a, b):
        table = jnp.where(lane == 0, a, jnp.where(lane == 1, b, 0.0))
        return jnp.transpose(table)[0:8, :]

    def down_rows(top):
        full = jnp.concatenate([top, jnp.zeros((120, count), F32)], axis=0)
        return jnp.transpose(full)

    values = conv[...]
    local_sum = jnp.sum(values, axis=1, keepdims=True)
    dev = values - local_sum / chan
    st1[...] = across_lanes(local_sum, jnp.sum(dev * dev, axis=1, keepdims=True))
    sg1[me] = st1[...]
    for d in range(1, T):
        tp_send(1, st1, sg1.at[me], d).start()
    relay((4,), (1,))
    for d in range(1, T):
        peer = lax.rem(me + T - d, T)
        tp_send(1, st1, sg1.at[peer], d).wait_recv()
    sums = [sg1[t] for t in range(T)]
    mean = sum(s[0:1, :] for s in sums) / (chan * T)
    spread = sum(
        s[1:2, :] + chan * (s[0:1, :] / chan - mean) * (s[0:1, :] / chan - mean) for s in sums
    ) / (chan * T)
    inv = lax.rsqrt(spread + EPS)
    line = lax.broadcasted_iota(jnp.int32, (8, count), 0)
    table = down_rows(jnp.where(line == 0, mean, jnp.where(line == 1, inv, 0.0)))
    normed = (conv[...] - table[:, 0:1]) * table[:, 1:2] * cg_ref[...]
    act[...] = (normed * jax.nn.sigmoid(normed)).astype(BF16)

    settle((2,))

    def project(src, buf, part):
        dsh = buf.shape[2]
        for j in range(F):
            t, off = (j * dsh) // dt, (j * dsh) % dt
            prod = jnp.dot(src[...], buf[j], preferred_element_type=F32)
            part[t, :, off:off + dsh] = prod.astype(BF16)

    def scatter(k, part, got):
        for d in range(1, T):
            tp_send(k, part.at[lax.rem(me + d, T)], got.at[d - 1], d).start()

    def gathered(k, part, got):
        total = part[me].astype(F32)
        for d in range(1, T):
            tp_send(k, part.at[me], got.at[d - 1], d).wait_recv()
            total = total + got[d - 1].astype(F32)
        return total

    def piece(t):
        return remote(part2.at[t], got2.at[me], ts.at[4, t], tr.at[4, me], {"tp": t})

    def piece_in(t):
        return remote(part2.at[t], got2.at[t], ts.at[4, t], tr.at[4, t], {"tp": t})

    project(act, bo, part1)
    scatter(2, part1, got1)
    relay((5,), (1,))
    first = (x_ref[...].astype(F32) + gathered(2, part1, got1)).astype(BF16)
    firsts[me] = first
    for d in range(1, T):
        tp_send(3, firsts.at[me], firsts.at[me], d).start()
    relay((3,), (2,))
    for d in range(1, T):
        peer = lax.rem(me + T - d, T)
        tp_send(3, firsts.at[peer], firsts.at[peer], d).wait_recv()
    relay((4,), (2,))
    norm_rows(firsts, mg_ref)
    relay((5,), (2,))
    relay((3, 4), range(3, F))
    settle((3, 4))

    ff = bga.shape[2]
    nf = chunk_of(ff, 256)

    def ff_step(c, _):
        gate = jnp.dot(rows[...], columns(bga, c, nf), preferred_element_type=F32)
        up = jnp.dot(rows[...], columns(bup, c, nf), preferred_element_type=F32)
        hid[:, pl.ds(pl.multiple_of(c * nf, nf), nf)] = (
            gate * jax.nn.sigmoid(gate) * up
        ).astype(BF16)
        return 0

    lax.fori_loop(0, ff // nf, ff_step, 0)
    if F == T and bd.shape[2] == dt:
        def down(shard):
            prod = jnp.dot(hid[...], bd[shard], preferred_element_type=F32)
            part2[shard] = prod.astype(BF16)

            @pl.when(shard != me)
            def _():
                piece(shard).start()

        own[5].wait()
        down(f)
        for s in range(1, F):
            if s >= 3:
                relay((5,), (s,))
            for side in (0, 1):
                @pl.when(has(side, s))
                def _():
                    if split == 2:
                        across_in(5, side, s).wait_recv()
                    down(f - s if side == 0 else f + s)
    else:
        relay((5,), range(3, F))
        settle((5,))
        project(hid, bd, part2)
        for d in range(1, T):
            piece(lax.rem(me + d, T)).start()
    second = firsts[me].astype(F32) + part2[me].astype(F32)
    for d in range(1, T):
        peer = lax.rem(me + d, T)
        piece_in(peer).wait_recv()
        second = second + got2[peer].astype(F32)
    total = jnp.sum(second * second, axis=1, keepdims=True)
    conv[:, 0:dt] = second
    st2[...] = across_lanes(total, total)
    sg2[me] = st2[...]
    for d in range(1, T):
        tp_send(5, st2, sg2.at[me], d).start()
    for d in range(1, T):
        peer = lax.rem(me + T - d, T)
        tp_send(5, st2, sg2.at[peer], d).wait_recv()
    full = sum(sg2[t] for t in range(T))
    table = down_rows(full)
    scale = lax.rsqrt(table[:, 0:1] / width + EPS)
    out_ref[...] = (conv[:, 0:dt] * scale * fg_ref[...]).astype(BF16)

    for w in range(6):
        for side in (0, 1):
            for s in range(F):
                if s < F - 1:
                    @pl.when(sends(side, s))
                    def _():
                        hop(w, side, s).wait_send()
                if s >= 1 and split == 2:
                    @pl.when(has(side, s))
                    def _():
                        across(w, side, s).wait_send()
    for d in range(1, T):
        peer = lax.rem(me + d, T)
        tp_send(0, x_ref, xg.at[me], d).wait_send()
        tp_send(1, st1, sg1.at[me], d).wait_send()
        tp_send(2, part1.at[peer], got1.at[d - 1], d).wait_send()
        tp_send(3, firsts.at[me], firsts.at[me], d).wait_send()
        piece(peer).wait_send()
        tp_send(5, st2, sg2.at[me], d).wait_send()


PIECES = (2, 2, 2, 2, 2, 4)
FIRST = tuple(sum(PIECES[:w]) for w in range(6))
GROUP = (0, 0, 0, 1, 1, 2)


def fast_kernel(
    length,
    x_ref, ng_hbm, cw_hbm, cg_hbm, mg_hbm, fg_hbm,
    wv_ref, wg_ref, wo_ref, wga_ref, wup_ref, wd_ref,
    out_ref,
    ng_ref, cw_ref, cg_ref, mg_ref, fg_ref, bv, bg, bo, bga, bup, bd,
    xg, rows, accv, accg, glu, conv, act, part, got, q1, q1in, firsts, hid,
    accs, part2, got2, q2, q2in, sec, ssq, secb, secin, st1, sg1, st2, sg2, finin,
    small, own_sem, zs, zr, zr2, ms, mr, md, ys, yr, xos, xor_, ags, agr, sts, str_, rss, rsr, ds_, dr, qs, qr, os_, orr, fs_, fr,
):
    f = lax.axis_index("fs")
    me = lax.axis_index("tp")
    rep = lax.axis_index("rep")
    count, dt = x_ref.shape
    T = 4
    width = dt * T
    rows_all = 2 * count
    batch = count // length
    chan, ff = bv.shape[2], bga.shape[2]
    local = [wv_ref, wg_ref, wo_ref, wga_ref, wup_ref, wd_ref]
    bufs = [bv, bg, bo, bga, bup, bd]
    VAL, GATE, CVO, GA, UP, DOWN = range(6)
    outer = jnp.logical_or(f == 0, f == 3)
    near = 1 + f // 3
    po, pi, fo = 3 * (f - 1), 3 - f, 3 * (2 - f)
    sib = me + 1 - 2 * lax.rem(me, 2)
    mir = lax.rem(me + 2, T)
    dia = lax.rem(sib + 2, T)

    def view(ref, w, h, c):
        if w == DOWN:
            n, m = ref.shape[1] // 2, ref.shape[0] // 2
            k = n // 2
            return ref.at[pl.ds((c % 2) * m, m), pl.ds(pl.multiple_of(h * n + (c // 2) * k, k), k)]
        n = ref.shape[0] // 2
        k = n // PIECES[w]
        return ref.at[pl.ds(pl.multiple_of(h * n + c * k, k), k), :]

    barrier = pltpu.get_barrier_semaphore()

    def greet(**target):
        pl.semaphore_signal(barrier, inc=1, device_id=target, device_id_type=MESH)

    def zsend(w, hs, c):
        h = rep if hs == 0 else 1 - rep
        sem = zr2.at[w + c // 2 if w == DOWN else w] if hs else zr.at[FIRST[w] + c]
        return remote(view(local[w], w, h, c), view(bufs[w].at[f], w, h, c), zs.at[GROUP[w]], sem, {"fs": near})

    def all_sent(sems, eighths):
        n = bd.shape[1] * eighths // 8
        for g, ref in enumerate((bufs[VAL].at[0:3], bufs[GA].at[0:2], bufs[DOWN].at[0, 0:n, :])):
            remote(ref, ref, sems.at[g], sems.at[g], {"fs": f}).wait_send()

    def xsend():
        return remote(x_ref, xg.at[me, 0], xos, xor_, {"fs": near})

    hn = dt // 2

    def ucols(j):
        if j == 0:
            return pl.ds(pl.multiple_of(rep * hn, hn), hn)
        return pl.ds(pl.multiple_of((1 - rep) * hn + min(j - 1, 1) * (hn // 2), hn // 2), hn // 2)

    def urows(j):
        return slice(0, rows_all) if j < 2 else slice((j - 2) * count, (j - 1) * count)

    def result(cols, target):
        return remote(secb.at[:, cols], secin.at[:, cols], os_, orr, {"fs": target})

    smalls = [
        pltpu.make_async_copy(src, dst, small.at[k])
        for k, (src, dst) in enumerate(
            ((ng_hbm, ng_ref), (cw_hbm, cw_ref), (cg_hbm, cg_ref), (mg_hbm, mg_ref), (fg_hbm, fg_ref))
        )
    ]

    lane = lax.broadcasted_iota(jnp.int32, (count, 128), 1)
    line = lax.broadcasted_iota(jnp.int32, (8, count), 0)

    def across_lanes(a, b):
        table = jnp.where(lane == 0, a, jnp.where(lane == 1, b, 0.0))
        return jnp.transpose(table)[0:8, :]

    def down_rows(top):
        full = jnp.concatenate([top, jnp.zeros((120, count), F32)], axis=0)
        return jnp.transpose(full)

    @pl.when(outer)
    def _():
        for t in range(T):
            greet(fs=near, tp=t)
        smalls[4].start()
        pl.semaphore_wait(barrier, T)
        order = [
            (VAL, 0), (GATE, 0), None, (CVO, 0), (VAL, 1), (GATE, 1), (CVO, 1),
            (GA, 0), (UP, 0), (GA, 1), (UP, 1), (DOWN, 0), (DOWN, 1),
        ]
        for item in order:
            if item is None:
                xsend().start()
            else:
                for c in range(1 if item == (DOWN, 1) else 0, PIECES[item[0]]):
                    zsend(item[0], item[1], c).start()
        xsend().wait_send()
        all_sent(zs, 7)
        smalls[4].wait()
        remote(secb, secin, os_, orr, {"fs": near}).wait_recv()
        remote(finin, finin, fs_, fr, {"fs": near}).wait_recv()
        full = sum(finin[t] for t in range(T))
        scale = lax.rsqrt(down_rows(full)[:, 0:1] / width + EPS)
        out_ref[...] = (secin[...].astype(F32) * scale * fg_ref[...]).astype(BF16)

    @pl.when(jnp.logical_not(outer))
    def _():
        for t in range(T):
            greet(fs=po, tp=t)
        greet(fs=pi)
        greet(rep=1 - rep)
        for t in (sib, mir, dia):
            greet(tp=t)
        own = [pltpu.make_async_copy(local[w], bufs[w].at[f], own_sem.at[w]) for w in range(6)]
        load_x = pltpu.make_async_copy(x_ref, xg.at[me, 1], small.at[5])
        load_x.start()
        for copy in smalls:
            copy.start()
        for copy in own:
            copy.start()
        pl.semaphore_wait(barrier, T + 5)

        def arrived(ref, send, recv):
            remote(ref, ref, send, recv, {"fs": f}).wait_recv()

        def mid_own(w, c):
            return remote(
                view(local[w], w, rep, c), view(bufs[w].at[f], w, rep, c), ms.at[GROUP[w]], mr.at[0, FIRST[w] + c], {"fs": pi}
            )

        def mid_fwd(w, c):
            ref = view(bufs[w].at[po], w, rep, c)
            return remote(ref, ref, ms.at[GROUP[w]], mr.at[1, FIRST[w] + c], {"fs": pi})

        def mid_direct(c):
            return remote(
                view(local[DOWN], DOWN, 1 - rep, c), view(bufs[DOWN].at[f], DOWN, 1 - rep, c), md.at[0], md.at[1], {"fs": pi}
            )

        def y_fwd(w, k, c):
            ref = view(bufs[w].at[fo if k else pi], w, rep, c)
            sem = yr.at[k, w + c // 2 if w == DOWN else w]
            return remote(ref, ref, ys.at[GROUP[w]], sem, {"rep": 1 - rep})

        def y_outer():
            ref = view(bufs[DOWN].at[po], DOWN, rep, 0)
            return remote(ref, ref, ys.at[2], yr.at[0, 6], {"rep": 1 - rep})

        def wait_z_down(j):
            if j == 1:
                arrived(view(bufs[DOWN].at[po], DOWN, 1 - rep, 0), ys.at[2], yr.at[0, 6])
                arrived(view(bufs[DOWN].at[po], DOWN, 1 - rep, 1), zs.at[2], zr2.at[DOWN])
            else:
                arrived(bufs[DOWN].at[po, :, ucols(2)], zs.at[2], zr2.at[DOWN + 1])

        def send_own(w):
            for c in range(PIECES[w]):
                mid_own(w, c).start()

        def relay_mid(w, c):
            arrived(view(bufs[w].at[po], w, rep, c), zs.at[GROUP[w]], zr.at[FIRST[w] + c])
            mid_fwd(w, c).start()

        def wait_mid(w, k, c):
            arrived(view(bufs[w].at[fo if k else pi], w, rep, c), ms.at[GROUP[w]], mr.at[k, FIRST[w] + c])

        def relay_y(w, k, c):
            wait_mid(w, k, c)
            y_fwd(w, k, c).start()

        def other(w, shard):
            n = bufs[w].shape[1] // 2
            return bufs[w].at[shard, pl.ds(pl.multiple_of((1 - rep) * n, n), n), :]

        def wait_z(w):
            arrived(other(w, po), zs.at[GROUP[w]], zr2.at[w])

        def wait_y(w, k):
            arrived(other(w, fo if k else pi), ys.at[GROUP[w]], yr.at[k, w])

        def wait_y_down(k, j):
            ref = bufs[DOWN].at[fo if k else pi, :, ucols(j)]
            arrived(ref, ys.at[2], yr.at[k, DOWN + j - 1])

        def wait_direct():
            arrived(bufs[DOWN].at[pi, :, ucols(2)], md.at[0], md.at[1])

        def ag(p, buf, slot, kind):
            ref = buf.at[mir if kind == 2 else me, slot]
            return remote(
                ref, ref, ags.at[p, slot], agr.at[p, slot, 1 if kind == 1 else 0], {"tp": mir if kind == 1 else sib}
            )

        def ag_start(p, buf, slot):
            ag(p, buf, slot, 1).start()
            ag(p, buf, slot, 0).start()

        def ag_forward(p, buf, slot):
            arrived(buf.at[mir, slot], ags.at[p, slot], agr.at[p, slot, 1])
            ag(p, buf, slot, 2).start()

        def ag_finish(p, buf, slot):
            arrived(buf.at[0:2, slot], ags.at[p, slot], agr.at[p, slot, 0])

        block = chunk_of(count, 16)

        def norm_rows(src, slot, gain):
            def step(i, _):
                r = pl.ds(pl.multiple_of(i * block, block), block)
                o = pl.ds(pl.multiple_of(slot * count + i * block, block), block)
                vals = [src[t, slot, r, :].astype(F32) for t in range(T)]
                ss = sum(jnp.sum(v * v, axis=1, keepdims=True) for v in vals)
                scale = lax.rsqrt(ss / width + EPS)
                for t in range(T):
                    rows[t, o, :] = (vals[t] * scale * gain[:, t * dt:(t + 1) * dt]).astype(BF16)
                return 0
            lax.fori_loop(0, count // block, step, 0)

        def stat(k, src, dst, d):
            return remote(src, dst, sts.at[k], str_.at[k], {"tp": lax.rem(me + d, T)})

        send_own(VAL)
        send_own(GATE)
        load_x.wait()
        ag_start(0, xg, 1)
        for c in range(2):
            relay_mid(VAL, c)
            relay_y(VAL, 0, c)
        relay_mid(GATE, 0)
        ag_forward(0, xg, 1)
        relay_y(GATE, 0, 0)
        relay_mid(GATE, 1)
        relay_y(GATE, 0, 1)
        send_own(CVO)
        ag_finish(0, xg, 1)
        for copy in smalls:
            copy.wait()
        norm_rows(xg, 1, ng_ref)
        relay_y(VAL, 1, 0)
        arrived(xg.at[me, 0], xos, xor_)
        ag_start(0, xg, 0)
        relay_y(VAL, 1, 1)
        relay_mid(CVO, 0)
        relay_y(GATE, 1, 0)
        relay_mid(CVO, 1)
        send_own(GA)
        send_own(UP)
        relay_y(GATE, 1, 1)
        ag_forward(0, xg, 0)
        ag_finish(0, xg, 0)
        norm_rows(xg, 0, ng_ref)
        relay_y(CVO, 0, 0)

        pad = glu.shape[1] - length - 8
        taps = cw_ref.shape[0]
        lead = pad - (taps - 1)
        nc = chunk_of(chan, 256)
        for b in range(2 * batch):
            glu[b, 0:pad, :] = jnp.zeros((pad, chan), F32)
            glu[b, pad + length:, :] = jnp.zeros((8, chan), F32)

        def s1(shard, first, last):
            def step(c, _):
                cols = pl.ds(pl.multiple_of(c * nc, nc), nc)
                value = jnp.dot(rows[shard], bv[shard, :, cols], preferred_element_type=F32)
                gate = jnp.dot(rows[shard], bg[shard, :, cols], preferred_element_type=F32)
                if not first:
                    value = value + accv[:, cols]
                    gate = gate + accg[:, cols]
                if last:
                    res = value * jax.nn.sigmoid(gate)
                    for b in range(2 * batch):
                        glu[b, pl.ds(pad, length), cols] = res[b * length:(b + 1) * length]
                else:
                    accv[:, cols] = value
                    accg[:, cols] = gate
                return 0
            lax.fori_loop(0, chan // nc, step, 0)

        own[VAL].wait()
        own[GATE].wait()
        s1(f, True, False)
        wait_y(VAL, 0)
        wait_y(GATE, 0)
        s1(pi, False, False)
        relay_y(CVO, 0, 1)
        wait_y(VAL, 1)
        wait_y(GATE, 1)
        s1(fo, False, False)
        relay_y(CVO, 1, 0)
        wait_z(VAL)
        wait_z(GATE)
        s1(po, False, True)
        relay_y(CVO, 1, 1)

        lanes = chunk_of(chan, 128)
        span = chunk_of(length, 64)
        strips = chan // lanes

        def convolve(slot):
            def step(i, _):
                s = lax.rem(i, strips)
                p = i // strips
                cols = pl.ds(pl.multiple_of(s * lanes, lanes), lanes)
                weights = cw_ref[:, cols]
                for b in range(batch):
                    total = jnp.zeros((span, lanes), F32)
                    for shift in range(8):
                        acc = None
                        for tap in range(taps):
                            if (lead + tap) % 8 != shift:
                                continue
                            base = lead + tap - shift
                            term = weights[tap:tap + 1, :] * glu[
                                slot * batch + b, pl.ds(pl.multiple_of(p * span + base, 8), span + 8), cols
                            ]
                            acc = term if acc is None else acc + term
                        if acc is not None:
                            total = total + acc[shift:shift + span]
                    at = pl.multiple_of(slot * count + b * length + p * span, span)
                    conv[pl.ds(at, span), cols] = total
                return 0
            lax.fori_loop(0, strips * (length // span), step, 0)

        def span_of(slot):
            return slice(slot * count, (slot + 1) * count)

        def conv_stats(slot):
            values = conv[span_of(slot), :]
            local_sum = jnp.sum(values, axis=1, keepdims=True)
            dev = values - local_sum / chan
            st1[slot] = across_lanes(local_sum, jnp.sum(dev * dev, axis=1, keepdims=True))
            sg1[slot, me] = st1[slot]
            for d in range(1, T):
                stat(slot, st1.at[slot], sg1.at[slot, me], d).start()

        def activate(slot):
            arrived(sg1.at[slot, 0:3], sts.at[slot], str_.at[slot])
            sums = [sg1[slot, t] for t in range(T)]
            mean = sum(s[0:1, :] for s in sums) / (chan * T)
            spread = sum(
                s[1:2, :] + chan * (s[0:1, :] / chan - mean) * (s[0:1, :] / chan - mean) for s in sums
            ) / (chan * T)
            inv = lax.rsqrt(spread + EPS)
            table = down_rows(jnp.where(line == 0, mean, jnp.where(line == 1, inv, 0.0)))
            normed = (conv[span_of(slot), :] - table[:, 0:1]) * table[:, 1:2] * cg_ref[...]
            act[span_of(slot), :] = (normed * jax.nn.sigmoid(normed)).astype(BF16)

        def rs(slot, kind):
            if kind == 2:
                return remote(q1.at[slot], q1in.at[slot], rss.at[slot], rsr.at[slot, 0], {"tp": mir})
            return remote(
                part.at[slot, dia if kind else sib], got.at[slot, kind], rss.at[slot], rsr.at[slot, kind], {"tp": sib}
            )

        def project(slot):
            def step(j, _):
                prod = jnp.dot(act[span_of(slot), :], bo[j], preferred_element_type=F32)
                part[slot, j] = prod.astype(BF16)
                return 0
            lax.fori_loop(0, T, step, 0)
            rs(slot, 1).start()
            rs(slot, 0).start()

        def pair_sum(slot):
            rs(slot, 1).wait_recv()
            q1[slot] = (part[slot, mir].astype(F32) + got[slot, 1].astype(F32)).astype(BF16)
            rs(slot, 2).start()

        def finish_first(slot):
            arrived(part.at[slot, 0:2], rss.at[slot], rsr.at[slot, 0])
            total = xg[me, slot].astype(F32) + (part[slot, me].astype(F32) + got[slot, 0].astype(F32))
            firsts[me, slot] = (total + q1in[slot].astype(F32)).astype(BF16)
            ag_start(1, firsts, slot)

        convolve(0)
        conv_stats(0)
        convolve(1)
        conv_stats(1)
        relay_y(GA, 0, 0)
        own[CVO].wait()
        wait_y(CVO, 0)
        wait_y(CVO, 1)
        wait_z(CVO)
        activate(0)
        project(0)
        activate(1)
        relay_mid(GA, 0)
        project(1)
        pair_sum(0)
        relay_y(GA, 0, 1)
        pair_sum(1)
        relay_mid(GA, 1)
        relay_y(UP, 0, 0)
        finish_first(0)
        relay_mid(UP, 0)
        relay_y(UP, 0, 1)
        relay_mid(UP, 1)
        send_own(DOWN)
        relay_y(GA, 1, 0)
        finish_first(1)
        relay_y(GA, 1, 1)
        ag_forward(1, firsts, 0)
        relay_y(UP, 1, 0)
        ag_finish(1, firsts, 0)
        norm_rows(firsts, 0, mg_ref)
        ag_forward(1, firsts, 1)
        relay_y(UP, 1, 1)
        ag_finish(1, firsts, 1)
        relay_y(DOWN, 0, 0)
        norm_rows(firsts, 1, mg_ref)
        relay_y(DOWN, 0, 1)

        nf = chunk_of(ff, 256)

        def s5(w, keep):
            def step(c, _):
                cols = pl.ds(pl.multiple_of(c * nf, nf), nf)
                value = sum(jnp.dot(rows[t], bufs[w][t, :, cols], preferred_element_type=F32) for t in range(T))
                if keep:
                    accs[:, cols] = value
                else:
                    gate = accs[:, cols]
                    hid[:, cols] = (gate * jax.nn.sigmoid(gate) * value).astype(BF16)
                return 0
            lax.fori_loop(0, ff // nf, step, 0)

        own[GA].wait()
        own[UP].wait()
        wait_y(GA, 0)
        wait_y(GA, 1)
        wait_z(GA)
        s5(GA, True)
        relay_mid(DOWN, 0)
        y_outer().start()
        wait_y(UP, 0)
        wait_z(UP)
        wait_y(UP, 1)
        s5(UP, False)

        def pair_send(b, j):
            at = (b, urows(j), ucols(j))
            return remote(part2.at[at], got2.at[at], ds_, dr.at[lax.rem(b // 2 + me // 2, 2), j], {"tp": sib})

        def cross(j):
            at = (urows(j), ucols(j))
            return remote(q2.at[at], q2in.at[at], qs, qr.at[j], {"tp": mir})

        def down(b, j):
            r, cols = urows(j), ucols(j)
            prod = jnp.dot(hid[r, :], bd[b, :, cols], preferred_element_type=F32)
            part2[b, r, cols] = prod.astype(BF16)

            @pl.when(jnp.logical_or(b == sib, b == dia))
            def _():
                pair_send(b, j).start()

        def combine(b, j):
            r, cols = urows(j), ucols(j)

            @pl.when(b == mir)
            def _():
                pair_send(b, j).wait_recv()
                q2[r, cols] = (part2[b, r, cols].astype(F32) + got2[b, r, cols].astype(F32)).astype(BF16)
                cross(j).start()

        def outer_stat(d):
            return remote(st2.at[0], finin.at[me], fs_, fr, {"fs": po, "tp": lax.rem(me + d, T)})

        def finish(b, j):
            @pl.when(b == me)
            def _():
                pair_send(me, j).wait_recv()
                cross(j).wait_recv()
                cols = ucols(j)
                for slot in (0, 1) if j < 2 else (j - 2,):
                    r = span_of(slot)
                    second = firsts[me, slot, :, cols].astype(F32) + part2[me, r, cols].astype(F32)
                    second = second + got2[me, r, cols].astype(F32) + q2in[r, cols].astype(F32)
                    total = jnp.sum(second * second, axis=1, keepdims=True)
                    if j > 0:
                        total = total + ssq[r, :]
                    if slot == 0:
                        secb[:, cols] = second.astype(BF16)
                        result(cols, po).start()
                    else:
                        sec[:, cols] = second
                    if j < 2:
                        ssq[r, :] = total
                        continue
                    st2[slot] = across_lanes(total, total)
                    if slot == 0:
                        for d in range(T):
                            outer_stat(d).start()
                    else:
                        sg2[me] = st2[1]
                        for d in range(1, T):
                            stat(2, st2.at[1], sg2.at[me], d).start()

        own[DOWN].wait()
        relay_mid(DOWN, 1)
        wait_mid(DOWN, 0, 2)
        wait_mid(DOWN, 0, 3)
        down(pi, 0)
        down(f, 0)
        relay_y(DOWN, 1, 0)
        relay_mid(DOWN, 2)
        combine(pi, 0)
        down(f, 1)
        combine(f, 0)
        wait_y_down(0, 1)
        down(pi, 1)
        relay_mid(DOWN, 3)
        mid_direct(2).start()
        mid_direct(3).start()
        relay_y(DOWN, 1, 1)
        combine(f, 1)
        combine(pi, 1)
        down(po, 0)
        down(f, 2)
        down(f, 3)
        relay_y(DOWN, 1, 2)
        combine(po, 0)
        combine(f, 2)
        combine(f, 3)
        relay_y(DOWN, 1, 3)
        wait_y_down(1, 1)
        down(fo, 1)
        down(fo, 0)
        for j in range(4):
            finish(f, j)
        combine(fo, 1)
        combine(fo, 0)
        wait_z_down(1)
        down(po, 1)
        finish(pi, 0)
        finish(po, 0)
        combine(po, 1)
        finish(pi, 1)
        wait_z_down(2)
        down(po, 2)
        down(po, 3)
        wait_direct()
        down(pi, 2)
        wait_y_down(1, 2)
        down(fo, 2)
        combine(po, 2)
        combine(pi, 2)
        down(pi, 3)
        down(fo, 3)
        combine(fo, 2)
        combine(po, 3)
        combine(pi, 3)
        combine(fo, 3)
        finish(po, 1)
        finish(fo, 0)
        finish(fo, 1)
        for j in (2, 3):
            for b in (po, pi, fo):
                finish(b, j)
        arrived(sg2.at[0:3], sts.at[2], str_.at[2])
        table = down_rows(sum(sg2[t] for t in range(T)))
        scale = lax.rsqrt(table[:, 0:1] / width + EPS)
        out_ref[...] = (sec[...] * scale * fg_ref[...]).astype(BF16)

        def sent(ref, sem):
            remote(ref, ref, sem, sem, {"fs": f}).wait_send()

        all_sent(ms, 8)
        all_sent(ys, 7)
        sent(bufs[DOWN].at[f, :, ucols(2)], md.at[0])
        for slot in range(2):
            sent(xg.at[0:3, slot], ags.at[0, slot])
            sent(firsts.at[0:3, slot], ags.at[1, slot])
            sent(part.at[slot, 0:3], rss.at[slot])
            sent(sg1.at[slot, 0:3], sts.at[slot])
        sent(sg2.at[0:3], sts.at[2])
        sent(part2.at[0:2], ds_)
        sent(q2, qs)
        sent(secb, os_)
        sent(finin, fs_)


def fast_body(
    activations, norm_gain, w_value, w_gate_conv, conv_weight, chan_gain,
    w_conv_out, mix_gain, w_gate, w_up, w_down, final_gain,
):
    batch, length, dt = activations.shape
    count = batch * length
    weights = (w_value, w_gate_conv, w_conv_out, w_gate, w_up, w_down)
    chan, ff = w_value.shape[1], w_gate.shape[1]
    T = 4
    pad = 8 * ((conv_weight.shape[0] - 1 + 7) // 8)
    rows_all = 2 * count
    vmem, hbm = pl.BlockSpec(memory_space=pltpu.VMEM), pl.BlockSpec(memory_space=pl.ANY)
    dma = pltpu.SemaphoreType.DMA
    V = pltpu.VMEM
    out = pl.pallas_call(
        functools.partial(fast_kernel, length),
        out_shape=pltpu.VMEM((count, dt), BF16),
        in_specs=[hbm] * 12,
        out_specs=vmem,
        scratch_shapes=[
            V((1, dt * T), F32),
            V(conv_weight.shape, F32),
            V((1, chan), F32),
            V((1, dt * T), F32),
            V((1, dt), F32),
        ] + [V((4,) + w.shape, BF16) for w in weights] + [
            V((T, 2, count, dt), BF16),
            V((T, rows_all, dt), BF16),
            V((rows_all, chan), F32),
            V((rows_all, chan), F32),
            V((2 * batch, pad + length + 8, chan), F32),
            V((rows_all, chan), F32),
            V((rows_all, chan), BF16),
            V((2, T, count, dt), BF16),
            V((2, 2, count, dt), BF16),
            V((2, count, dt), BF16),
            V((2, count, dt), BF16),
            V((T, 2, count, dt), BF16),
            V((rows_all, ff), BF16),
            V((rows_all, ff), F32),
            V((T, rows_all, dt), BF16),
            V((T, rows_all, dt), BF16),
            V((rows_all, dt), BF16),
            V((rows_all, dt), BF16),
            V((count, dt), F32),
            V((rows_all, 1), F32),
            V((count, dt), BF16),
            V((count, dt), BF16),
            V((2, 8, count), F32),
            V((2, T, 8, count), F32),
            V((2, 8, count), F32),
            V((T, 8, count), F32),
            V((T, 8, count), F32),
            dma((6,)),
            dma((6,)),
            dma((3,)),
            dma((sum(PIECES),)),
            dma((7,)),
            dma((3,)),
            dma((2, sum(PIECES))),
            dma((2,)),
            dma((3,)),
            dma((2, 7)),
            dma(()),
            dma(()),
            dma((2, 2)),
            dma((2, 2, 2)),
            dma((3,)),
            dma((3,)),
            dma((2,)),
            dma((2, 2)),
            dma(()),
            dma((2, 4)),
            dma(()),
            dma((4,)),
            dma(()),
            dma(()),
            dma(()),
            dma(()),
        ],
        compiler_params=pltpu.CompilerParams(
            collective_id=0, has_side_effects=True, vmem_limit_bytes=60 * 1024 * 1024
        ),
        name="block",
    )(
        activations.reshape(count, dt),
        norm_gain.reshape(1, dt * T),
        conv_weight,
        chan_gain.reshape(1, chan),
        mix_gain.reshape(1, dt * T),
        final_gain.reshape(1, dt),
        *weights,
    )
    return out.reshape(batch, length, dt)


def ring_body(
    activations, norm_gain, w_value, w_gate_conv, conv_weight, chan_gain,
    w_conv_out, mix_gain, w_gate, w_up, w_down, final_gain,
):
    batch, length, dt = activations.shape
    count = batch * length
    R, F, T = lax.axis_size("rep"), lax.axis_size("fs"), lax.axis_size("tp")
    weights = (w_value, w_gate_conv, w_conv_out, w_gate, w_up, w_down)
    split = 2 if R == 2 and all(w.shape[0] % 32 == 0 for w in weights) else 1
    width = dt * T
    chan, ff = w_value.shape[1], w_gate.shape[1]
    taps = conv_weight.shape[0]
    pad = 8 * ((taps - 1 + 7) // 8)
    vmem, hbm = pl.BlockSpec(memory_space=pltpu.VMEM), pl.BlockSpec(memory_space=pl.ANY)
    ysh = (2, 6, F) if split == 2 else (1,)
    dma = pltpu.SemaphoreType.DMA
    out = pl.pallas_call(
        functools.partial(ring_kernel, R, F, T, split, length),
        out_shape=jax.ShapeDtypeStruct((count, dt), BF16),
        in_specs=[vmem] * 6 + [hbm] * 6,
        out_specs=vmem,
        scratch_shapes=[pltpu.VMEM((F,) + w.shape, BF16) for w in weights] + [
            pltpu.VMEM((T, count, dt), BF16),
            pltpu.VMEM((count, width), BF16),
            pltpu.VMEM((batch, pad + length + 8, chan), F32),
            pltpu.VMEM((count, max(chan, dt)), F32),
            pltpu.VMEM((count, chan), BF16),
            pltpu.VMEM((T, count, dt), BF16),
            pltpu.VMEM((T, count, dt), BF16),
            pltpu.VMEM((T - 1, count, dt), BF16),
            pltpu.VMEM((T, count, dt), BF16),
            pltpu.VMEM((T, count, dt), BF16),
            pltpu.VMEM((count, ff), BF16),
            pltpu.VMEM((8, count), F32),
            pltpu.VMEM((8, count), F32),
            pltpu.VMEM((T, 8, count), F32),
            pltpu.VMEM((T, 8, count), F32),
            dma((6,)),
            dma((2, 6, F)),
            dma((2, 6, F)),
            dma(ysh),
            dma(ysh),
            dma((6, T)),
            dma((6, T)),
        ],
        compiler_params=pltpu.CompilerParams(
            collective_id=0, has_side_effects=True, vmem_limit_bytes=60 * 1024 * 1024
        ),
        name="block",
    )(
        activations.reshape(count, dt),
        norm_gain.reshape(T, dt),
        conv_weight,
        chan_gain.reshape(1, chan),
        mix_gain.reshape(T, dt),
        final_gain.reshape(1, dt),
        *weights,
    )
    return out.reshape(batch, length, dt)


def solution(mesh):
    in_specs = (
        P(("rep", "fs"), None, "tp"),
        P(),
        P("fs", "tp"),
        P("fs", "tp"),
        P(None, "tp"),
        P("tp"),
        P("tp", "fs"),
        P(),
        P("fs", "tp"),
        P("fs", "tp"),
        P("tp", "fs"),
        P("tp"),
    )
    out_specs = P(("rep", "fs"), None, "tp")
    fast = tuple(mesh.shape[a] for a in ("rep", "fs", "tp")) == (2, 4, 4)
    body = fast_body if fast else ring_body
    return jax.shard_map(body, mesh=mesh, in_specs=in_specs, out_specs=out_specs, check_vma=False)
```

```python
import functools

import jax
import jax.numpy as jnp
from jax import lax
from jax.experimental import pallas as pl
from jax.experimental.pallas import tpu as pltpu
from jax.sharding import PartitionSpec as P

EPS = 1e-06
MESH = pl.DeviceIdType.MESH
F32 = jnp.float32
BF16 = jnp.bfloat16


def remote(src, dst, send, recv, target):
    return pltpu.make_async_remote_copy(
        src_ref=src, dst_ref=dst, send_sem=send, recv_sem=recv, device_id=target, device_id_type=MESH
    )


def chunk_of(extent, want):
    return want if extent % want == 0 else extent


def ring_kernel(
    R, F, T, split, length,
    x_ref, ng_ref, cw_ref, cg_ref, mg_ref, fg_ref,
    wv_ref, wg_ref, wo_ref, wga_ref, wup_ref, wd_ref,
    out_ref,
    bv, bg, bo, bga, bup, bd,
    xg, rows, glu, conv, act, part1, part2, got1, got2, firsts, hid, st1, st2, sg1, sg2,
    own_sem, zs, zr, ys, yr, ts, tr,
):
    f = lax.axis_index("fs")
    me = lax.axis_index("tp")
    rep = lax.axis_index("rep")
    count, dt = x_ref.shape
    width = dt * T
    local = [wv_ref, wg_ref, wo_ref, wga_ref, wup_ref, wd_ref]
    bufs = [bv, bg, bo, bga, bup, bd]

    barrier = pltpu.get_barrier_semaphore()
    greeted = 0
    for target in (lax.rem(f + 1, F), lax.rem(f + F - 1, F)):
        pl.semaphore_signal(barrier, inc=1, device_id={"fs": target}, device_id_type=MESH)
        greeted += 1
    if split == 2:
        pl.semaphore_signal(barrier, inc=1, device_id={"rep": 1 - rep}, device_id_type=MESH)
        greeted += 1
    for d in range(1, T):
        pl.semaphore_signal(barrier, inc=1, device_id={"tp": lax.rem(me + d, T)}, device_id_type=MESH)
        greeted += 1
    own = [
        pltpu.make_async_copy(local[w], bufs[w].at[f], own_sem.at[w]) for w in range(6)
    ]
    for copy in own:
        copy.start()
    pl.semaphore_wait(barrier, greeted)

    def half(w):
        n = local[w].shape[0] // split
        return pl.ds(pl.multiple_of((rep if split == 2 else 0) * n, n), n)

    def other(w):
        n = local[w].shape[0] // split
        return pl.ds(pl.multiple_of((1 - rep) * n, n), n)

    def hop(w, side, s):
        shard = f - s if side == 0 else f + s
        target = f + 1 if side == 0 else f - 1
        src = local[w].at[half(w)] if s == 0 else bufs[w].at[shard, half(w)]
        return remote(src, bufs[w].at[shard, half(w)], zs.at[side, w, s], zr.at[side, w, s + 1], {"fs": target})

    def arrival(w, side, s):
        shard = f - s if side == 0 else f + s
        ref = bufs[w].at[shard, half(w)]
        return remote(ref, ref, zs.at[side, w, s], zr.at[side, w, s], {"fs": f})

    def across(w, side, s):
        shard = f - s if side == 0 else f + s
        ref = bufs[w].at[shard, half(w)]
        return remote(ref, ref, ys.at[side, w, s], yr.at[side, w, s], {"rep": 1 - rep})

    def across_in(w, side, s):
        shard = f - s if side == 0 else f + s
        ref = bufs[w].at[shard, other(w)]
        return remote(ref, ref, ys.at[side, w, s], yr.at[side, w, s], {"rep": 1 - rep})

    def has(side, s):
        return f >= s if side == 0 else f + s <= F - 1

    def sends(side, s):
        ahead = f < F - 1 if side == 0 else f > 0
        return jnp.logical_and(has(side, s), ahead)

    def launch(w):
        for side in (0, 1):
            @pl.when(sends(side, 0))
            def _():
                hop(w, side, 0).start()

    def relay(group, stages=range(1, F)):
        for s in stages:
            for w in group:
                for side in (0, 1):
                    @pl.when(has(side, s))
                    def _():
                        arrival(w, side, s).wait_recv()
                        if s < F - 1:
                            @pl.when(sends(side, s))
                            def _():
                                hop(w, side, s).start()
                        if split == 2:
                            across(w, side, s).start()

    def settle(group):
        for w in group:
            own[w].wait()
        if split == 2:
            for s in range(1, F):
                for w in group:
                    for side in (0, 1):
                        @pl.when(has(side, s))
                        def _():
                            across_in(w, side, s).wait_recv()

    def tp_send(k, src, dst_at, d):
        return remote(src, dst_at, ts.at[k, d], tr.at[k, d], {"tp": lax.rem(me + d, T)})

    for w in (0, 1):
        launch(w)
    for d in range(1, T):
        tp_send(0, x_ref, xg.at[me], d).start()
    launch(2)
    xg[me] = x_ref[...]
    for d in range(1, T):
        peer = lax.rem(me + T - d, T)
        tp_send(0, x_ref, xg.at[peer], d).wait_recv()

    block = chunk_of(count, 16)

    def norm_rows(src, gain):
        def step(i, _):
            r = pl.ds(pl.multiple_of(i * block, block), block)
            vals = [src[t, r, :].astype(F32) for t in range(T)]
            ss = sum(jnp.sum(v * v, axis=1, keepdims=True) for v in vals)
            scale = lax.rsqrt(ss / width + EPS)
            for t in range(T):
                rows[r, t * dt:(t + 1) * dt] = (
                    vals[t] * scale * gain[t:t + 1, :]
                ).astype(BF16)
            return 0
        lax.fori_loop(0, count // block, step, 0)

    norm_rows(xg, ng_ref)
    relay((0, 1, 2))
    for w in (3, 4, 5):
        launch(w)
    settle((0, 1))

    chan = bv.shape[2]
    batch = count // length
    taps = cw_ref.shape[0]
    pad = 8 * ((taps - 1 + 7) // 8)
    lead = pad - (taps - 1)

    def columns(buf, c, n):
        block_w = buf[:, :, pl.ds(pl.multiple_of(c * n, n), n)]
        return block_w.reshape(block_w.shape[0] * block_w.shape[1], n)

    nc = chunk_of(chan, 256)

    def glu_step(c, _):
        value = jnp.dot(rows[...], columns(bv, c, nc), preferred_element_type=F32)
        gate = jnp.dot(rows[...], columns(bg, c, nc), preferred_element_type=F32)
        res = value * jax.nn.sigmoid(gate)
        for b in range(batch):
            glu[b, pl.ds(pad, length), pl.ds(pl.multiple_of(c * nc, nc), nc)] = (
                res[b * length:(b + 1) * length]
            )
        return 0

    for b in range(batch):
        glu[b, 0:pad, :] = jnp.zeros((pad, chan), F32)
        glu[b, pad + length:, :] = jnp.zeros((8, chan), F32)
    lax.fori_loop(0, chan // nc, glu_step, 0)
    relay((3,), (1,))

    lanes = chunk_of(chan, 128)
    span = chunk_of(length, 64)
    strips = chan // lanes

    def conv_step(i, _):
        q = lax.rem(i, strips)
        p = i // strips
        cols = pl.ds(pl.multiple_of(q * lanes, lanes), lanes)
        weights = cw_ref[:, cols]
        for b in range(batch):
            total = jnp.zeros((span, lanes), F32)
            for shift in range(8):
                acc = None
                for tap in range(taps):
                    if (lead + tap) % 8 != shift:
                        continue
                    base = lead + tap - shift
                    term = weights[tap:tap + 1, :] * glu[
                        b, pl.ds(pl.multiple_of(p * span + base, 8), span + 8), cols
                    ]
                    acc = term if acc is None else acc + term
                if acc is not None:
                    total = total + acc[shift:shift + span]
            conv[pl.ds(pl.multiple_of(b * length + p * span, span), span), cols] = total
        return 0

    lax.fori_loop(0, strips * (length // span), conv_step, 0)

    lane = lax.broadcasted_iota(jnp.int32, (count, 128), 1)

    def across_lanes(a, b):
        table = jnp.where(lane == 0, a, jnp.where(lane == 1, b, 0.0))
        return jnp.transpose(table)[0:8, :]

    def down_rows(top):
        full = jnp.concatenate([top, jnp.zeros((120, count), F32)], axis=0)
        return jnp.transpose(full)

    values = conv[...]
    local_sum = jnp.sum(values, axis=1, keepdims=True)
    dev = values - local_sum / chan
    st1[...] = across_lanes(local_sum, jnp.sum(dev * dev, axis=1, keepdims=True))
    sg1[me] = st1[...]
    for d in range(1, T):
        tp_send(1, st1, sg1.at[me], d).start()
    relay((4,), (1,))
    for d in range(1, T):
        peer = lax.rem(me + T - d, T)
        tp_send(1, st1, sg1.at[peer], d).wait_recv()
    sums = [sg1[t] for t in range(T)]
    mean = sum(s[0:1, :] for s in sums) / (chan * T)
    spread = sum(
        s[1:2, :] + chan * (s[0:1, :] / chan - mean) * (s[0:1, :] / chan - mean) for s in sums
    ) / (chan * T)
    inv = lax.rsqrt(spread + EPS)
    line = lax.broadcasted_iota(jnp.int32, (8, count), 0)
    table = down_rows(jnp.where(line == 0, mean, jnp.where(line == 1, inv, 0.0)))
    normed = (conv[...] - table[:, 0:1]) * table[:, 1:2] * cg_ref[...]
    act[...] = (normed * jax.nn.sigmoid(normed)).astype(BF16)

    settle((2,))

    def project(src, buf, part):
        dsh = buf.shape[2]
        for j in range(F):
            t, off = (j * dsh) // dt, (j * dsh) % dt
            prod = jnp.dot(src[...], buf[j], preferred_element_type=F32)
            part[t, :, off:off + dsh] = prod.astype(BF16)

    def scatter(k, part, got):
        for d in range(1, T):
            tp_send(k, part.at[lax.rem(me + d, T)], got.at[d - 1], d).start()

    def gathered(k, part, got):
        total = part[me].astype(F32)
        for d in range(1, T):
            tp_send(k, part.at[me], got.at[d - 1], d).wait_recv()
            total = total + got[d - 1].astype(F32)
        return total

    def piece(t):
        return remote(part2.at[t], got2.at[me], ts.at[4, t], tr.at[4, me], {"tp": t})

    def piece_in(t):
        return remote(part2.at[t], got2.at[t], ts.at[4, t], tr.at[4, t], {"tp": t})

    project(act, bo, part1)
    scatter(2, part1, got1)
    relay((5,), (1,))
    first = (x_ref[...].astype(F32) + gathered(2, part1, got1)).astype(BF16)
    firsts[me] = first
    for d in range(1, T):
        tp_send(3, firsts.at[me], firsts.at[me], d).start()
    relay((3,), (2,))
    for d in range(1, T):
        peer = lax.rem(me + T - d, T)
        tp_send(3, firsts.at[peer], firsts.at[peer], d).wait_recv()
    relay((4,), (2,))
    norm_rows(firsts, mg_ref)
    relay((5,), (2,))
    relay((3, 4), range(3, F))
    settle((3, 4))

    ff = bga.shape[2]
    nf = chunk_of(ff, 256)

    def ff_step(c, _):
        gate = jnp.dot(rows[...], columns(bga, c, nf), preferred_element_type=F32)
        up = jnp.dot(rows[...], columns(bup, c, nf), preferred_element_type=F32)
        hid[:, pl.ds(pl.multiple_of(c * nf, nf), nf)] = (
            gate * jax.nn.sigmoid(gate) * up
        ).astype(BF16)
        return 0

    lax.fori_loop(0, ff // nf, ff_step, 0)
    if F == T and bd.shape[2] == dt:
        def down(shard):
            prod = jnp.dot(hid[...], bd[shard], preferred_element_type=F32)
            part2[shard] = prod.astype(BF16)

            @pl.when(shard != me)
            def _():
                piece(shard).start()

        own[5].wait()
        down(f)
        for s in range(1, F):
            if s >= 3:
                relay((5,), (s,))
            for side in (0, 1):
                @pl.when(has(side, s))
                def _():
                    if split == 2:
                        across_in(5, side, s).wait_recv()
                    down(f - s if side == 0 else f + s)
    else:
        relay((5,), range(3, F))
        settle((5,))
        project(hid, bd, part2)
        for d in range(1, T):
            piece(lax.rem(me + d, T)).start()
    second = firsts[me].astype(F32) + part2[me].astype(F32)
    for d in range(1, T):
        peer = lax.rem(me + d, T)
        piece_in(peer).wait_recv()
        second = second + got2[peer].astype(F32)
    total = jnp.sum(second * second, axis=1, keepdims=True)
    conv[:, 0:dt] = second
    st2[...] = across_lanes(total, total)
    sg2[me] = st2[...]
    for d in range(1, T):
        tp_send(5, st2, sg2.at[me], d).start()
    for d in range(1, T):
        peer = lax.rem(me + T - d, T)
        tp_send(5, st2, sg2.at[peer], d).wait_recv()
    full = sum(sg2[t] for t in range(T))
    table = down_rows(full)
    scale = lax.rsqrt(table[:, 0:1] / width + EPS)
    out_ref[...] = (conv[:, 0:dt] * scale * fg_ref[...]).astype(BF16)

    for w in range(6):
        for side in (0, 1):
            for s in range(F):
                if s < F - 1:
                    @pl.when(sends(side, s))
                    def _():
                        hop(w, side, s).wait_send()
                if s >= 1 and split == 2:
                    @pl.when(has(side, s))
                    def _():
                        across(w, side, s).wait_send()
    for d in range(1, T):
        peer = lax.rem(me + d, T)
        tp_send(0, x_ref, xg.at[me], d).wait_send()
        tp_send(1, st1, sg1.at[me], d).wait_send()
        tp_send(2, part1.at[peer], got1.at[d - 1], d).wait_send()
        tp_send(3, firsts.at[me], firsts.at[me], d).wait_send()
        piece(peer).wait_send()
        tp_send(5, st2, sg2.at[me], d).wait_send()


PIECES = (2, 2, 2, 2, 2, 4)
FIRST = tuple(sum(PIECES[:w]) for w in range(6))
GROUP = (0, 0, 0, 1, 1, 2)


def fast_kernel(
    length,
    x_ref, ng_hbm, cw_hbm, cg_hbm, mg_hbm, fg_hbm,
    wv_ref, wg_ref, wo_ref, wga_ref, wup_ref, wd_ref,
    out_ref,
    ng_ref, cw_ref, cg_ref, mg_ref, fg_ref, bv, bg, bo, bga, bup, bd,
    xg, rows, accv, accg, glu, conv, act, part, got, q1, q1in, firsts, hid,
    accs, part2, got2, q2, q2in, sec, ssq, secb, secin, st1, sg1, st2, sg2, finin,
    small, own_sem, zs, zr, zr2, ms, mr, md, ys, yr, xos, xor_, ags, agr, sts, str_, rss, rsr, ds_, dr, qs, qr, os_, orr, fs_, fr,
):
    f = lax.axis_index("fs")
    me = lax.axis_index("tp")
    rep = lax.axis_index("rep")
    count, dt = x_ref.shape
    T = 4
    width = dt * T
    rows_all = 2 * count
    batch = count // length
    chan, ff = bv.shape[2], bga.shape[2]
    local = [wv_ref, wg_ref, wo_ref, wga_ref, wup_ref, wd_ref]
    bufs = [bv, bg, bo, bga, bup, bd]
    VAL, GATE, CVO, GA, UP, DOWN = range(6)
    outer = jnp.logical_or(f == 0, f == 3)
    near = 1 + f // 3
    po, pi, fo = 3 * (f - 1), 3 - f, 3 * (2 - f)
    sib = me + 1 - 2 * lax.rem(me, 2)
    mir = lax.rem(me + 2, T)
    dia = lax.rem(sib + 2, T)

    def view(ref, w, h, c):
        if w == DOWN:
            n, m = ref.shape[1] // 2, ref.shape[0] // 2
            k = n // 2
            return ref.at[pl.ds((c % 2) * m, m), pl.ds(pl.multiple_of(h * n + (c // 2) * k, k), k)]
        n = ref.shape[0] // 2
        k = n // PIECES[w]
        return ref.at[pl.ds(pl.multiple_of(h * n + c * k, k), k), :]

    barrier = pltpu.get_barrier_semaphore()

    def greet(**target):
        pl.semaphore_signal(barrier, inc=1, device_id=target, device_id_type=MESH)

    def zsend(w, hs, c):
        h = rep if hs == 0 else 1 - rep
        sem = zr2.at[w + c // 2 if w == DOWN else w] if hs else zr.at[FIRST[w] + c]
        return remote(view(local[w], w, h, c), view(bufs[w].at[f], w, h, c), zs.at[GROUP[w]], sem, {"fs": near})

    def all_sent(sems, eighths):
        n = bd.shape[1] * eighths // 8
        for g, ref in enumerate((bufs[VAL].at[0:3], bufs[GA].at[0:2], bufs[DOWN].at[0, 0:n, :])):
            remote(ref, ref, sems.at[g], sems.at[g], {"fs": f}).wait_send()

    def xsend():
        return remote(x_ref, xg.at[me, 0], xos, xor_, {"fs": near})

    hn = dt // 2

    def ucols(j):
        if j == 0:
            return pl.ds(pl.multiple_of(rep * hn, hn), hn)
        if j > 3:
            return pl.ds(pl.multiple_of(rep * hn + (j - 4) * (hn // 2), hn // 2), hn // 2)
        return pl.ds(pl.multiple_of((1 - rep) * hn + min(j - 1, 1) * (hn // 2), hn // 2), hn // 2)

    def urows(j):
        return slice((j - 2) * count, (j - 1) * count) if j in (2, 3) else slice(0, rows_all)

    def result(cols, target):
        return remote(secb.at[:, cols], secin.at[:, cols], os_, orr, {"fs": target})

    smalls = [
        pltpu.make_async_copy(src, dst, small.at[k])
        for k, (src, dst) in enumerate(
            ((ng_hbm, ng_ref), (cw_hbm, cw_ref), (cg_hbm, cg_ref), (mg_hbm, mg_ref), (fg_hbm, fg_ref))
        )
    ]

    lane = lax.broadcasted_iota(jnp.int32, (count, 128), 1)
    line = lax.broadcasted_iota(jnp.int32, (8, count), 0)

    def across_lanes(a, b):
        table = jnp.where(lane == 0, a, jnp.where(lane == 1, b, 0.0))
        return jnp.transpose(table)[0:8, :]

    def down_rows(top):
        full = jnp.concatenate([top, jnp.zeros((120, count), F32)], axis=0)
        return jnp.transpose(full)

    @pl.when(outer)
    def _():
        for t in range(T):
            greet(fs=near, tp=t)
        smalls[4].start()
        pl.semaphore_wait(barrier, T)
        order = [
            (VAL, 0), (GATE, 0), None, (CVO, 0), (VAL, 1), (GATE, 1), (CVO, 1),
            (GA, 0), (UP, 0), (GA, 1), (UP, 1), (DOWN, 0), (DOWN, 1),
        ]
        for item in order:
            if item is None:
                xsend().start()
            else:
                for c in range(1 if item == (DOWN, 1) else 0, PIECES[item[0]]):
                    zsend(item[0], item[1], c).start()
        xsend().wait_send()
        all_sent(zs, 7)
        smalls[4].wait()
        remote(secb, secin, os_, orr, {"fs": near}).wait_recv()
        remote(finin, finin, fs_, fr, {"fs": near}).wait_recv()
        full = sum(finin[t] for t in range(T))
        scale = lax.rsqrt(down_rows(full)[:, 0:1] / width + EPS)
        out_ref[...] = (secin[...].astype(F32) * scale * fg_ref[...]).astype(BF16)

    @pl.when(jnp.logical_not(outer))
    def _():
        for t in range(T):
            greet(fs=po, tp=t)
        greet(fs=pi)
        greet(rep=1 - rep)
        for t in (sib, mir, dia):
            greet(tp=t)
        own = [pltpu.make_async_copy(local[w], bufs[w].at[f], own_sem.at[w]) for w in range(6)]
        load_x = pltpu.make_async_copy(x_ref, xg.at[me, 1], small.at[5])
        load_x.start()
        for copy in smalls:
            copy.start()
        for copy in own:
            copy.start()
        pl.semaphore_wait(barrier, T + 5)

        def arrived(ref, send, recv):
            remote(ref, ref, send, recv, {"fs": f}).wait_recv()

        def mid_own(w, c):
            return remote(
                view(local[w], w, rep, c), view(bufs[w].at[f], w, rep, c), ms.at[GROUP[w]], mr.at[0, FIRST[w] + c], {"fs": pi}
            )

        def mid_fwd(w, c):
            ref = view(bufs[w].at[po], w, rep, c)
            return remote(ref, ref, ms.at[GROUP[w]], mr.at[1, FIRST[w] + c], {"fs": pi})

        def mid_direct(c):
            return remote(
                view(local[DOWN], DOWN, 1 - rep, c), view(bufs[DOWN].at[f], DOWN, 1 - rep, c), md.at[0], md.at[1], {"fs": pi}
            )

        def y_fwd(w, k, c):
            ref = view(bufs[w].at[fo if k else pi], w, rep, c)
            sem = yr.at[k, w + c // 2 if w == DOWN else w]
            return remote(ref, ref, ys.at[GROUP[w]], sem, {"rep": 1 - rep})

        def y_outer():
            ref = view(bufs[DOWN].at[po], DOWN, rep, 0)
            return remote(ref, ref, ys.at[2], yr.at[0, 6], {"rep": 1 - rep})

        def wait_z_down(j):
            if j == 1:
                arrived(view(bufs[DOWN].at[po], DOWN, 1 - rep, 0), ys.at[2], yr.at[0, 6])
                arrived(view(bufs[DOWN].at[po], DOWN, 1 - rep, 1), zs.at[2], zr2.at[DOWN])
            else:
                arrived(bufs[DOWN].at[po, :, ucols(2)], zs.at[2], zr2.at[DOWN + 1])

        def send_own(w):
            for c in range(PIECES[w]):
                mid_own(w, c).start()

        def relay_mid(w, c):
            arrived(view(bufs[w].at[po], w, rep, c), zs.at[GROUP[w]], zr.at[FIRST[w] + c])
            mid_fwd(w, c).start()

        def wait_mid(w, k, c):
            arrived(view(bufs[w].at[fo if k else pi], w, rep, c), ms.at[GROUP[w]], mr.at[k, FIRST[w] + c])

        def relay_y(w, k, c):
            wait_mid(w, k, c)
            y_fwd(w, k, c).start()

        def other(w, shard):
            n = bufs[w].shape[1] // 2
            return bufs[w].at[shard, pl.ds(pl.multiple_of((1 - rep) * n, n), n), :]

        def wait_z(w):
            arrived(other(w, po), zs.at[GROUP[w]], zr2.at[w])

        def wait_y(w, k):
            arrived(other(w, fo if k else pi), ys.at[GROUP[w]], yr.at[k, w])

        def wait_y_down(k, j):
            ref = bufs[DOWN].at[fo if k else pi, :, ucols(j)]
            arrived(ref, ys.at[2], yr.at[k, DOWN + j - 1])

        def wait_direct():
            arrived(bufs[DOWN].at[pi, :, ucols(2)], md.at[0], md.at[1])

        def ag(p, buf, slot, kind):
            ref = buf.at[mir if kind == 2 else me, slot]
            return remote(
                ref, ref, ags.at[p, slot], agr.at[p, slot, 1 if kind == 1 else 0], {"tp": mir if kind == 1 else sib}
            )

        def ag_start(p, buf, slot):
            ag(p, buf, slot, 1).start()
            ag(p, buf, slot, 0).start()

        def ag_forward(p, buf, slot):
            arrived(buf.at[mir, slot], ags.at[p, slot], agr.at[p, slot, 1])
            ag(p, buf, slot, 2).start()

        def ag_finish(p, buf, slot):
            arrived(buf.at[0:2, slot], ags.at[p, slot], agr.at[p, slot, 0])

        block = chunk_of(count, 16)

        def norm_rows(src, slot, gain):
            def step(i, _):
                r = pl.ds(pl.multiple_of(i * block, block), block)
                o = pl.ds(pl.multiple_of(slot * count + i * block, block), block)
                vals = [src[t, slot, r, :].astype(F32) for t in range(T)]
                ss = sum(jnp.sum(v * v, axis=1, keepdims=True) for v in vals)
                scale = lax.rsqrt(ss / width + EPS)
                for t in range(T):
                    rows[t, o, :] = (vals[t] * scale * gain[:, t * dt:(t + 1) * dt]).astype(BF16)
                return 0
            lax.fori_loop(0, count // block, step, 0)

        def stat(k, src, dst, d):
            return remote(src, dst, sts.at[k], str_.at[k], {"tp": lax.rem(me + d, T)})

        send_own(VAL)
        send_own(GATE)
        load_x.wait()
        ag_start(0, xg, 1)
        for c in range(2):
            relay_mid(VAL, c)
            relay_y(VAL, 0, c)
        relay_mid(GATE, 0)
        ag_forward(0, xg, 1)
        relay_y(GATE, 0, 0)
        relay_mid(GATE, 1)
        relay_y(GATE, 0, 1)
        send_own(CVO)
        ag_finish(0, xg, 1)
        for copy in smalls:
            copy.wait()
        norm_rows(xg, 1, ng_ref)
        relay_y(VAL, 1, 0)
        arrived(xg.at[me, 0], xos, xor_)
        ag_start(0, xg, 0)
        relay_y(VAL, 1, 1)
        relay_mid(CVO, 0)
        relay_y(GATE, 1, 0)
        relay_mid(CVO, 1)
        send_own(GA)
        send_own(UP)
        relay_y(GATE, 1, 1)
        ag_forward(0, xg, 0)
        ag_finish(0, xg, 0)
        norm_rows(xg, 0, ng_ref)
        relay_y(CVO, 0, 0)

        pad = glu.shape[1] - length - 8
        taps = cw_ref.shape[0]
        lead = pad - (taps - 1)
        nc = chunk_of(chan, 256)
        for b in range(2 * batch):
            glu[b, 0:pad, :] = jnp.zeros((pad, chan), F32)
            glu[b, pad + length:, :] = jnp.zeros((8, chan), F32)

        def s1(shard, first, last):
            def step(c, _):
                cols = pl.ds(pl.multiple_of(c * nc, nc), nc)
                value = jnp.dot(rows[shard], bv[shard, :, cols], preferred_element_type=F32)
                gate = jnp.dot(rows[shard], bg[shard, :, cols], preferred_element_type=F32)
                if not first:
                    value = value + accv[:, cols]
                    gate = gate + accg[:, cols]
                if last:
                    res = value * jax.nn.sigmoid(gate)
                    for b in range(2 * batch):
                        glu[b, pl.ds(pad, length), cols] = res[b * length:(b + 1) * length]
                else:
                    accv[:, cols] = value
                    accg[:, cols] = gate
                return 0
            lax.fori_loop(0, chan // nc, step, 0)

        own[VAL].wait()
        own[GATE].wait()
        s1(f, True, False)
        wait_y(VAL, 0)
        wait_y(GATE, 0)
        s1(pi, False, False)
        relay_y(CVO, 0, 1)
        wait_y(VAL, 1)
        wait_y(GATE, 1)
        s1(fo, False, False)
        relay_y(CVO, 1, 0)
        wait_z(VAL)
        wait_z(GATE)
        s1(po, False, True)
        relay_y(CVO, 1, 1)

        lanes = chunk_of(chan, 128)
        span = chunk_of(length, 64)
        strips = chan // lanes

        def convolve(slot):
            def step(i, _):
                s = lax.rem(i, strips)
                p = i // strips
                cols = pl.ds(pl.multiple_of(s * lanes, lanes), lanes)
                weights = cw_ref[:, cols]
                for b in range(batch):
                    total = jnp.zeros((span, lanes), F32)
                    for shift in range(8):
                        acc = None
                        for tap in range(taps):
                            if (lead + tap) % 8 != shift:
                                continue
                            base = lead + tap - shift
                            term = weights[tap:tap + 1, :] * glu[
                                slot * batch + b, pl.ds(pl.multiple_of(p * span + base, 8), span + 8), cols
                            ]
                            acc = term if acc is None else acc + term
                        if acc is not None:
                            total = total + acc[shift:shift + span]
                    at = pl.multiple_of(slot * count + b * length + p * span, span)
                    conv[pl.ds(at, span), cols] = total
                return 0
            lax.fori_loop(0, strips * (length // span), step, 0)

        def span_of(slot):
            return slice(slot * count, (slot + 1) * count)

        def conv_stats(slot):
            values = conv[span_of(slot), :]
            local_sum = jnp.sum(values, axis=1, keepdims=True)
            dev = values - local_sum / chan
            st1[slot] = across_lanes(local_sum, jnp.sum(dev * dev, axis=1, keepdims=True))
            sg1[slot, me] = st1[slot]
            for d in range(1, T):
                stat(slot, st1.at[slot], sg1.at[slot, me], d).start()

        def activate(slot):
            arrived(sg1.at[slot, 0:3], sts.at[slot], str_.at[slot])
            sums = [sg1[slot, t] for t in range(T)]
            mean = sum(s[0:1, :] for s in sums) / (chan * T)
            spread = sum(
                s[1:2, :] + chan * (s[0:1, :] / chan - mean) * (s[0:1, :] / chan - mean) for s in sums
            ) / (chan * T)
            inv = lax.rsqrt(spread + EPS)
            table = down_rows(jnp.where(line == 0, mean, jnp.where(line == 1, inv, 0.0)))
            normed = (conv[span_of(slot), :] - table[:, 0:1]) * table[:, 1:2] * cg_ref[...]
            act[span_of(slot), :] = (normed * jax.nn.sigmoid(normed)).astype(BF16)

        def rs(slot, kind):
            if kind == 2:
                return remote(q1.at[slot], q1in.at[slot], rss.at[slot], rsr.at[slot, 0], {"tp": mir})
            return remote(
                part.at[slot, dia if kind else sib], got.at[slot, kind], rss.at[slot], rsr.at[slot, kind], {"tp": sib}
            )

        def project(slot):
            def step(j, _):
                prod = jnp.dot(act[span_of(slot), :], bo[j], preferred_element_type=F32)
                part[slot, j] = prod.astype(BF16)
                return 0
            lax.fori_loop(0, T, step, 0)
            rs(slot, 1).start()
            rs(slot, 0).start()

        def pair_sum(slot):
            rs(slot, 1).wait_recv()
            q1[slot] = (part[slot, mir].astype(F32) + got[slot, 1].astype(F32)).astype(BF16)
            rs(slot, 2).start()

        def finish_first(slot):
            arrived(part.at[slot, 0:2], rss.at[slot], rsr.at[slot, 0])
            total = xg[me, slot].astype(F32) + (part[slot, me].astype(F32) + got[slot, 0].astype(F32))
            firsts[me, slot] = (total + q1in[slot].astype(F32)).astype(BF16)
            ag_start(1, firsts, slot)

        convolve(0)
        conv_stats(0)
        convolve(1)
        conv_stats(1)
        relay_y(GA, 0, 0)
        own[CVO].wait()
        wait_y(CVO, 0)
        wait_y(CVO, 1)
        wait_z(CVO)
        activate(0)
        project(0)
        activate(1)
        relay_mid(GA, 0)
        project(1)
        pair_sum(0)
        relay_y(GA, 0, 1)
        pair_sum(1)
        relay_mid(GA, 1)
        relay_y(UP, 0, 0)
        finish_first(0)
        relay_mid(UP, 0)
        relay_y(UP, 0, 1)
        relay_mid(UP, 1)
        send_own(DOWN)
        relay_y(GA, 1, 0)
        finish_first(1)
        relay_y(GA, 1, 1)
        ag_forward(1, firsts, 0)
        relay_y(UP, 1, 0)
        ag_finish(1, firsts, 0)
        norm_rows(firsts, 0, mg_ref)
        ag_forward(1, firsts, 1)
        relay_y(UP, 1, 1)
        ag_finish(1, firsts, 1)
        relay_y(DOWN, 0, 0)
        norm_rows(firsts, 1, mg_ref)
        relay_y(DOWN, 0, 1)

        nf = chunk_of(ff, 256)

        def s5(w, keep):
            def step(c, _):
                cols = pl.ds(pl.multiple_of(c * nf, nf), nf)
                value = sum(jnp.dot(rows[t], bufs[w][t, :, cols], preferred_element_type=F32) for t in range(T))
                if keep:
                    accs[:, cols] = value
                else:
                    gate = accs[:, cols]
                    hid[:, cols] = (gate * jax.nn.sigmoid(gate) * value).astype(BF16)
                return 0
            lax.fori_loop(0, ff // nf, step, 0)

        own[GA].wait()
        own[UP].wait()
        wait_y(GA, 0)
        wait_y(GA, 1)
        wait_z(GA)
        s5(GA, True)
        relay_mid(DOWN, 0)
        y_outer().start()
        wait_y(UP, 0)
        wait_z(UP)
        wait_y(UP, 1)
        s5(UP, False)

        def pair_send(b, j):
            at = (b, urows(j), ucols(j))
            return remote(part2.at[at], got2.at[at], ds_, dr.at[lax.rem(b // 2 + me // 2, 2), j], {"tp": sib})

        def cross(j):
            at = (urows(j), ucols(j))
            return remote(q2.at[at], q2in.at[at], qs, qr.at[j], {"tp": mir})

        def down(b, j):
            r, cols = urows(j), ucols(j)
            prod = jnp.dot(hid[r, :], bd[b, :, cols], preferred_element_type=F32)
            part2[b, r, cols] = prod.astype(BF16)

            @pl.when(jnp.logical_or(b == sib, b == dia))
            def _():
                pair_send(b, j).start()

        def combine(b, j):
            r, cols = urows(j), ucols(j)

            @pl.when(b == mir)
            def _():
                pair_send(b, j).wait_recv()
                q2[r, cols] = (part2[b, r, cols].astype(F32) + got2[b, r, cols].astype(F32)).astype(BF16)
                cross(j).start()

        def outer_stat(d):
            return remote(st2.at[0], finin.at[me], fs_, fr, {"fs": po, "tp": lax.rem(me + d, T)})

        def finish(b, j):
            @pl.when(b == me)
            def _():
                pair_send(me, j).wait_recv()
                cross(j).wait_recv()
                cols = ucols(j)
                for slot in (j - 2,) if j in (2, 3) else (0, 1):
                    r = span_of(slot)
                    second = firsts[me, slot, :, cols].astype(F32) + part2[me, r, cols].astype(F32)
                    second = second + got2[me, r, cols].astype(F32) + q2in[r, cols].astype(F32)
                    total = jnp.sum(second * second, axis=1, keepdims=True)
                    if j not in (0, 4):
                        total = total + ssq[r, :]
                    if slot == 0:
                        secb[:, cols] = second.astype(BF16)
                        result(cols, po).start()
                    else:
                        sec[:, cols] = second
                    if j not in (2, 3):
                        ssq[r, :] = total
                        continue
                    st2[slot] = across_lanes(total, total)
                    if slot == 0:
                        for d in range(T):
                            outer_stat(d).start()
                    else:
                        sg2[me] = st2[1]
                        for d in range(1, T):
                            stat(2, st2.at[1], sg2.at[me], d).start()

        own[DOWN].wait()
        relay_mid(DOWN, 1)
        wait_mid(DOWN, 0, 2)
        wait_mid(DOWN, 0, 3)
        down(pi, 0)
        down(f, 0)
        relay_y(DOWN, 1, 0)
        relay_mid(DOWN, 2)
        combine(pi, 0)
        down(f, 1)
        combine(f, 0)
        wait_y_down(0, 1)
        down(pi, 1)
        relay_mid(DOWN, 3)
        mid_direct(2).start()
        mid_direct(3).start()
        relay_y(DOWN, 1, 1)
        combine(f, 1)
        combine(pi, 1)
        down(po, 0)
        down(fo, 4)
        relay_y(DOWN, 1, 2)
        down(f, 2)
        down(f, 3)
        combine(po, 0)
        combine(fo, 4)
        relay_y(DOWN, 1, 3)
        combine(f, 2)
        combine(f, 3)
        down(fo, 5)
        wait_y_down(1, 1)
        down(fo, 1)
        finish(f, 0)
        finish(pi, 0)
        combine(fo, 5)
        wait_z_down(1)
        down(po, 1)
        combine(fo, 1)
        finish(f, 1)
        finish(pi, 1)
        combine(po, 1)
        wait_z_down(2)
        down(po, 2)
        down(po, 3)
        wait_direct()
        down(pi, 2)
        wait_y_down(1, 2)
        down(fo, 2)
        combine(po, 2)
        combine(pi, 2)
        down(pi, 3)
        down(fo, 3)
        combine(fo, 2)
        combine(po, 3)
        combine(pi, 3)
        combine(fo, 3)
        finish(po, 0)
        finish(fo, 4)
        finish(po, 1)
        finish(fo, 5)
        finish(fo, 1)
        for j in (2, 3):
            for b in (f, po, pi, fo):
                finish(b, j)
        arrived(sg2.at[0:3], sts.at[2], str_.at[2])
        table = down_rows(sum(sg2[t] for t in range(T)))
        scale = lax.rsqrt(table[:, 0:1] / width + EPS)
        out_ref[...] = (sec[...] * scale * fg_ref[...]).astype(BF16)

        def sent(ref, sem):
            remote(ref, ref, sem, sem, {"fs": f}).wait_send()

        all_sent(ms, 8)
        all_sent(ys, 7)
        sent(bufs[DOWN].at[f, :, ucols(2)], md.at[0])
        for slot in range(2):
            sent(xg.at[0:3, slot], ags.at[0, slot])
            sent(firsts.at[0:3, slot], ags.at[1, slot])
            sent(part.at[slot, 0:3], rss.at[slot])
            sent(sg1.at[slot, 0:3], sts.at[slot])
        sent(sg2.at[0:3], sts.at[2])
        sent(part2.at[0:2], ds_)
        sent(q2, qs)
        sent(secb, os_)
        sent(finin, fs_)


def fast_body(
    activations, norm_gain, w_value, w_gate_conv, conv_weight, chan_gain,
    w_conv_out, mix_gain, w_gate, w_up, w_down, final_gain,
):
    batch, length, dt = activations.shape
    count = batch * length
    weights = (w_value, w_gate_conv, w_conv_out, w_gate, w_up, w_down)
    chan, ff = w_value.shape[1], w_gate.shape[1]
    T = 4
    pad = 8 * ((conv_weight.shape[0] - 1 + 7) // 8)
    rows_all = 2 * count
    vmem, hbm = pl.BlockSpec(memory_space=pltpu.VMEM), pl.BlockSpec(memory_space=pl.ANY)
    dma = pltpu.SemaphoreType.DMA
    V = pltpu.VMEM
    out = pl.pallas_call(
        functools.partial(fast_kernel, length),
        out_shape=pltpu.VMEM((count, dt), BF16),
        in_specs=[hbm] * 12,
        out_specs=vmem,
        scratch_shapes=[
            V((1, dt * T), F32),
            V(conv_weight.shape, F32),
            V((1, chan), F32),
            V((1, dt * T), F32),
            V((1, dt), F32),
        ] + [V((4,) + w.shape, BF16) for w in weights] + [
            V((T, 2, count, dt), BF16),
            V((T, rows_all, dt), BF16),
            V((rows_all, chan), F32),
            V((rows_all, chan), F32),
            V((2 * batch, pad + length + 8, chan), F32),
            V((rows_all, chan), F32),
            V((rows_all, chan), BF16),
            V((2, T, count, dt), BF16),
            V((2, 2, count, dt), BF16),
            V((2, count, dt), BF16),
            V((2, count, dt), BF16),
            V((T, 2, count, dt), BF16),
            V((rows_all, ff), BF16),
            V((rows_all, ff), F32),
            V((T, rows_all, dt), BF16),
            V((T, rows_all, dt), BF16),
            V((rows_all, dt), BF16),
            V((rows_all, dt), BF16),
            V((count, dt), F32),
            V((rows_all, 1), F32),
            V((count, dt), BF16),
            V((count, dt), BF16),
            V((2, 8, count), F32),
            V((2, T, 8, count), F32),
            V((2, 8, count), F32),
            V((T, 8, count), F32),
            V((T, 8, count), F32),
            dma((6,)),
            dma((6,)),
            dma((3,)),
            dma((sum(PIECES),)),
            dma((7,)),
            dma((3,)),
            dma((2, sum(PIECES))),
            dma((2,)),
            dma((3,)),
            dma((2, 7)),
            dma(()),
            dma(()),
            dma((2, 2)),
            dma((2, 2, 2)),
            dma((3,)),
            dma((3,)),
            dma((2,)),
            dma((2, 2)),
            dma(()),
            dma((2, 6)),
            dma(()),
            dma((6,)),
            dma(()),
            dma(()),
            dma(()),
            dma(()),
        ],
        compiler_params=pltpu.CompilerParams(
            collective_id=0, has_side_effects=True, vmem_limit_bytes=60 * 1024 * 1024
        ),
        name="block",
    )(
        activations.reshape(count, dt),
        norm_gain.reshape(1, dt * T),
        conv_weight,
        chan_gain.reshape(1, chan),
        mix_gain.reshape(1, dt * T),
        final_gain.reshape(1, dt),
        *weights,
    )
    return out.reshape(batch, length, dt)


def ring_body(
    activations, norm_gain, w_value, w_gate_conv, conv_weight, chan_gain,
    w_conv_out, mix_gain, w_gate, w_up, w_down, final_gain,
):
    batch, length, dt = activations.shape
    count = batch * length
    R, F, T = lax.axis_size("rep"), lax.axis_size("fs"), lax.axis_size("tp")
    weights = (w_value, w_gate_conv, w_conv_out, w_gate, w_up, w_down)
    split = 2 if R == 2 and all(w.shape[0] % 32 == 0 for w in weights) else 1
    width = dt * T
    chan, ff = w_value.shape[1], w_gate.shape[1]
    taps = conv_weight.shape[0]
    pad = 8 * ((taps - 1 + 7) // 8)
    vmem, hbm = pl.BlockSpec(memory_space=pltpu.VMEM), pl.BlockSpec(memory_space=pl.ANY)
    ysh = (2, 6, F) if split == 2 else (1,)
    dma = pltpu.SemaphoreType.DMA
    out = pl.pallas_call(
        functools.partial(ring_kernel, R, F, T, split, length),
        out_shape=jax.ShapeDtypeStruct((count, dt), BF16),
        in_specs=[vmem] * 6 + [hbm] * 6,
        out_specs=vmem,
        scratch_shapes=[pltpu.VMEM((F,) + w.shape, BF16) for w in weights] + [
            pltpu.VMEM((T, count, dt), BF16),
            pltpu.VMEM((count, width), BF16),
            pltpu.VMEM((batch, pad + length + 8, chan), F32),
            pltpu.VMEM((count, max(chan, dt)), F32),
            pltpu.VMEM((count, chan), BF16),
            pltpu.VMEM((T, count, dt), BF16),
            pltpu.VMEM((T, count, dt), BF16),
            pltpu.VMEM((T - 1, count, dt), BF16),
            pltpu.VMEM((T, count, dt), BF16),
            pltpu.VMEM((T, count, dt), BF16),
            pltpu.VMEM((count, ff), BF16),
            pltpu.VMEM((8, count), F32),
            pltpu.VMEM((8, count), F32),
            pltpu.VMEM((T, 8, count), F32),
            pltpu.VMEM((T, 8, count), F32),
            dma((6,)),
            dma((2, 6, F)),
            dma((2, 6, F)),
            dma(ysh),
            dma(ysh),
            dma((6, T)),
            dma((6, T)),
        ],
        compiler_params=pltpu.CompilerParams(
            collective_id=0, has_side_effects=True, vmem_limit_bytes=60 * 1024 * 1024
        ),
        name="block",
    )(
        activations.reshape(count, dt),
        norm_gain.reshape(T, dt),
        conv_weight,
        chan_gain.reshape(1, chan),
        mix_gain.reshape(T, dt),
        final_gain.reshape(1, dt),
        *weights,
    )
    return out.reshape(batch, length, dt)


def solution(mesh):
    in_specs = (
        P(("rep", "fs"), None, "tp"),
        P(),
        P("fs", "tp"),
        P("fs", "tp"),
        P(None, "tp"),
        P("tp"),
        P("tp", "fs"),
        P(),
        P("fs", "tp"),
        P("fs", "tp"),
        P("tp", "fs"),
        P("tp"),
    )
    out_specs = P(("rep", "fs"), None, "tp")
    fast = tuple(mesh.shape[a] for a in ("rep", "fs", "tp")) == (2, 4, 4)
    body = fast_body if fast else ring_body
    return jax.shard_map(body, mesh=mesh, in_specs=in_specs, out_specs=out_specs, check_vma=False)
```

```python
import functools

import jax
import jax.numpy as jnp
from jax import lax
from jax.experimental import pallas as pl
from jax.experimental.pallas import tpu as pltpu
from jax.sharding import PartitionSpec as P

EPS = 1e-06
MESH = pl.DeviceIdType.MESH
F32 = jnp.float32
BF16 = jnp.bfloat16


def remote(src, dst, send, recv, target):
    return pltpu.make_async_remote_copy(
        src_ref=src, dst_ref=dst, send_sem=send, recv_sem=recv, device_id=target, device_id_type=MESH
    )


def chunk_of(extent, want):
    return want if extent % want == 0 else extent


def ring_kernel(
    R, F, T, split, length,
    x_ref, ng_ref, cw_ref, cg_ref, mg_ref, fg_ref,
    wv_ref, wg_ref, wo_ref, wga_ref, wup_ref, wd_ref,
    out_ref,
    bv, bg, bo, bga, bup, bd,
    xg, rows, glu, conv, act, part1, part2, got1, got2, firsts, hid, st1, st2, sg1, sg2,
    own_sem, zs, zr, ys, yr, ts, tr,
):
    f = lax.axis_index("fs")
    me = lax.axis_index("tp")
    rep = lax.axis_index("rep")
    count, dt = x_ref.shape
    width = dt * T
    local = [wv_ref, wg_ref, wo_ref, wga_ref, wup_ref, wd_ref]
    bufs = [bv, bg, bo, bga, bup, bd]

    barrier = pltpu.get_barrier_semaphore()
    greeted = 0
    for target in (lax.rem(f + 1, F), lax.rem(f + F - 1, F)):
        pl.semaphore_signal(barrier, inc=1, device_id={"fs": target}, device_id_type=MESH)
        greeted += 1
    if split == 2:
        pl.semaphore_signal(barrier, inc=1, device_id={"rep": 1 - rep}, device_id_type=MESH)
        greeted += 1
    for d in range(1, T):
        pl.semaphore_signal(barrier, inc=1, device_id={"tp": lax.rem(me + d, T)}, device_id_type=MESH)
        greeted += 1
    own = [
        pltpu.make_async_copy(local[w], bufs[w].at[f], own_sem.at[w]) for w in range(6)
    ]
    for copy in own:
        copy.start()
    pl.semaphore_wait(barrier, greeted)

    def half(w):
        n = local[w].shape[0] // split
        return pl.ds(pl.multiple_of((rep if split == 2 else 0) * n, n), n)

    def other(w):
        n = local[w].shape[0] // split
        return pl.ds(pl.multiple_of((1 - rep) * n, n), n)

    def hop(w, side, s):
        shard = f - s if side == 0 else f + s
        target = f + 1 if side == 0 else f - 1
        src = local[w].at[half(w)] if s == 0 else bufs[w].at[shard, half(w)]
        return remote(src, bufs[w].at[shard, half(w)], zs.at[side, w, s], zr.at[side, w, s + 1], {"fs": target})

    def arrival(w, side, s):
        shard = f - s if side == 0 else f + s
        ref = bufs[w].at[shard, half(w)]
        return remote(ref, ref, zs.at[side, w, s], zr.at[side, w, s], {"fs": f})

    def across(w, side, s):
        shard = f - s if side == 0 else f + s
        ref = bufs[w].at[shard, half(w)]
        return remote(ref, ref, ys.at[side, w, s], yr.at[side, w, s], {"rep": 1 - rep})

    def across_in(w, side, s):
        shard = f - s if side == 0 else f + s
        ref = bufs[w].at[shard, other(w)]
        return remote(ref, ref, ys.at[side, w, s], yr.at[side, w, s], {"rep": 1 - rep})

    def has(side, s):
        return f >= s if side == 0 else f + s <= F - 1

    def sends(side, s):
        ahead = f < F - 1 if side == 0 else f > 0
        return jnp.logical_and(has(side, s), ahead)

    def launch(w):
        for side in (0, 1):
            @pl.when(sends(side, 0))
            def _():
                hop(w, side, 0).start()

    def relay(group, stages=range(1, F)):
        for s in stages:
            for w in group:
                for side in (0, 1):
                    @pl.when(has(side, s))
                    def _():
                        arrival(w, side, s).wait_recv()
                        if s < F - 1:
                            @pl.when(sends(side, s))
                            def _():
                                hop(w, side, s).start()
                        if split == 2:
                            across(w, side, s).start()

    def settle(group):
        for w in group:
            own[w].wait()
        if split == 2:
            for s in range(1, F):
                for w in group:
                    for side in (0, 1):
                        @pl.when(has(side, s))
                        def _():
                            across_in(w, side, s).wait_recv()

    def tp_send(k, src, dst_at, d):
        return remote(src, dst_at, ts.at[k, d], tr.at[k, d], {"tp": lax.rem(me + d, T)})

    for w in (0, 1):
        launch(w)
    for d in range(1, T):
        tp_send(0, x_ref, xg.at[me], d).start()
    launch(2)
    xg[me] = x_ref[...]
    for d in range(1, T):
        peer = lax.rem(me + T - d, T)
        tp_send(0, x_ref, xg.at[peer], d).wait_recv()

    block = chunk_of(count, 16)

    def norm_rows(src, gain):
        def step(i, _):
            r = pl.ds(pl.multiple_of(i * block, block), block)
            vals = [src[t, r, :].astype(F32) for t in range(T)]
            ss = sum(jnp.sum(v * v, axis=1, keepdims=True) for v in vals)
            scale = lax.rsqrt(ss / width + EPS)
            for t in range(T):
                rows[r, t * dt:(t + 1) * dt] = (
                    vals[t] * scale * gain[t:t + 1, :]
                ).astype(BF16)
            return 0
        lax.fori_loop(0, count // block, step, 0)

    norm_rows(xg, ng_ref)
    relay((0, 1, 2))
    for w in (3, 4, 5):
        launch(w)
    settle((0, 1))

    chan = bv.shape[2]
    batch = count // length
    taps = cw_ref.shape[0]
    pad = 8 * ((taps - 1 + 7) // 8)
    lead = pad - (taps - 1)

    def columns(buf, c, n):
        block_w = buf[:, :, pl.ds(pl.multiple_of(c * n, n), n)]
        return block_w.reshape(block_w.shape[0] * block_w.shape[1], n)

    nc = chunk_of(chan, 256)

    def glu_step(c, _):
        value = jnp.dot(rows[...], columns(bv, c, nc), preferred_element_type=F32)
        gate = jnp.dot(rows[...], columns(bg, c, nc), preferred_element_type=F32)
        res = value * jax.nn.sigmoid(gate)
        for b in range(batch):
            glu[b, pl.ds(pad, length), pl.ds(pl.multiple_of(c * nc, nc), nc)] = (
                res[b * length:(b + 1) * length]
            )
        return 0

    for b in range(batch):
        glu[b, 0:pad, :] = jnp.zeros((pad, chan), F32)
        glu[b, pad + length:, :] = jnp.zeros((8, chan), F32)
    lax.fori_loop(0, chan // nc, glu_step, 0)
    relay((3,), (1,))

    lanes = chunk_of(chan, 128)
    span = chunk_of(length, 64)
    strips = chan // lanes

    def conv_step(i, _):
        q = lax.rem(i, strips)
        p = i // strips
        cols = pl.ds(pl.multiple_of(q * lanes, lanes), lanes)
        weights = cw_ref[:, cols]
        for b in range(batch):
            total = jnp.zeros((span, lanes), F32)
            for shift in range(8):
                acc = None
                for tap in range(taps):
                    if (lead + tap) % 8 != shift:
                        continue
                    base = lead + tap - shift
                    term = weights[tap:tap + 1, :] * glu[
                        b, pl.ds(pl.multiple_of(p * span + base, 8), span + 8), cols
                    ]
                    acc = term if acc is None else acc + term
                if acc is not None:
                    total = total + acc[shift:shift + span]
            conv[pl.ds(pl.multiple_of(b * length + p * span, span), span), cols] = total
        return 0

    lax.fori_loop(0, strips * (length // span), conv_step, 0)

    lane = lax.broadcasted_iota(jnp.int32, (count, 128), 1)

    def across_lanes(a, b):
        table = jnp.where(lane == 0, a, jnp.where(lane == 1, b, 0.0))
        return jnp.transpose(table)[0:8, :]

    def down_rows(top):
        full = jnp.concatenate([top, jnp.zeros((120, count), F32)], axis=0)
        return jnp.transpose(full)

    values = conv[...]
    local_sum = jnp.sum(values, axis=1, keepdims=True)
    dev = values - local_sum / chan
    st1[...] = across_lanes(local_sum, jnp.sum(dev * dev, axis=1, keepdims=True))
    sg1[me] = st1[...]
    for d in range(1, T):
        tp_send(1, st1, sg1.at[me], d).start()
    relay((4,), (1,))
    for d in range(1, T):
        peer = lax.rem(me + T - d, T)
        tp_send(1, st1, sg1.at[peer], d).wait_recv()
    sums = [sg1[t] for t in range(T)]
    mean = sum(s[0:1, :] for s in sums) / (chan * T)
    spread = sum(
        s[1:2, :] + chan * (s[0:1, :] / chan - mean) * (s[0:1, :] / chan - mean) for s in sums
    ) / (chan * T)
    inv = lax.rsqrt(spread + EPS)
    line = lax.broadcasted_iota(jnp.int32, (8, count), 0)
    table = down_rows(jnp.where(line == 0, mean, jnp.where(line == 1, inv, 0.0)))
    normed = (conv[...] - table[:, 0:1]) * table[:, 1:2] * cg_ref[...]
    act[...] = (normed * jax.nn.sigmoid(normed)).astype(BF16)

    settle((2,))

    def project(src, buf, part):
        dsh = buf.shape[2]
        for j in range(F):
            t, off = (j * dsh) // dt, (j * dsh) % dt
            prod = jnp.dot(src[...], buf[j], preferred_element_type=F32)
            part[t, :, off:off + dsh] = prod.astype(BF16)

    def scatter(k, part, got):
        for d in range(1, T):
            tp_send(k, part.at[lax.rem(me + d, T)], got.at[d - 1], d).start()

    def gathered(k, part, got):
        total = part[me].astype(F32)
        for d in range(1, T):
            tp_send(k, part.at[me], got.at[d - 1], d).wait_recv()
            total = total + got[d - 1].astype(F32)
        return total

    def piece(t):
        return remote(part2.at[t], got2.at[me], ts.at[4, t], tr.at[4, me], {"tp": t})

    def piece_in(t):
        return remote(part2.at[t], got2.at[t], ts.at[4, t], tr.at[4, t], {"tp": t})

    project(act, bo, part1)
    scatter(2, part1, got1)
    relay((5,), (1,))
    first = (x_ref[...].astype(F32) + gathered(2, part1, got1)).astype(BF16)
    firsts[me] = first
    for d in range(1, T):
        tp_send(3, firsts.at[me], firsts.at[me], d).start()
    relay((3,), (2,))
    for d in range(1, T):
        peer = lax.rem(me + T - d, T)
        tp_send(3, firsts.at[peer], firsts.at[peer], d).wait_recv()
    relay((4,), (2,))
    norm_rows(firsts, mg_ref)
    relay((5,), (2,))
    relay((3, 4), range(3, F))
    settle((3, 4))

    ff = bga.shape[2]
    nf = chunk_of(ff, 256)

    def ff_step(c, _):
        gate = jnp.dot(rows[...], columns(bga, c, nf), preferred_element_type=F32)
        up = jnp.dot(rows[...], columns(bup, c, nf), preferred_element_type=F32)
        hid[:, pl.ds(pl.multiple_of(c * nf, nf), nf)] = (
            gate * jax.nn.sigmoid(gate) * up
        ).astype(BF16)
        return 0

    lax.fori_loop(0, ff // nf, ff_step, 0)
    if F == T and bd.shape[2] == dt:
        def down(shard):
            prod = jnp.dot(hid[...], bd[shard], preferred_element_type=F32)
            part2[shard] = prod.astype(BF16)

            @pl.when(shard != me)
            def _():
                piece(shard).start()

        own[5].wait()
        down(f)
        for s in range(1, F):
            if s >= 3:
                relay((5,), (s,))
            for side in (0, 1):
                @pl.when(has(side, s))
                def _():
                    if split == 2:
                        across_in(5, side, s).wait_recv()
                    down(f - s if side == 0 else f + s)
    else:
        relay((5,), range(3, F))
        settle((5,))
        project(hid, bd, part2)
        for d in range(1, T):
            piece(lax.rem(me + d, T)).start()
    second = firsts[me].astype(F32) + part2[me].astype(F32)
    for d in range(1, T):
        peer = lax.rem(me + d, T)
        piece_in(peer).wait_recv()
        second = second + got2[peer].astype(F32)
    total = jnp.sum(second * second, axis=1, keepdims=True)
    conv[:, 0:dt] = second
    st2[...] = across_lanes(total, total)
    sg2[me] = st2[...]
    for d in range(1, T):
        tp_send(5, st2, sg2.at[me], d).start()
    for d in range(1, T):
        peer = lax.rem(me + T - d, T)
        tp_send(5, st2, sg2.at[peer], d).wait_recv()
    full = sum(sg2[t] for t in range(T))
    table = down_rows(full)
    scale = lax.rsqrt(table[:, 0:1] / width + EPS)
    out_ref[...] = (conv[:, 0:dt] * scale * fg_ref[...]).astype(BF16)

    for w in range(6):
        for side in (0, 1):
            for s in range(F):
                if s < F - 1:
                    @pl.when(sends(side, s))
                    def _():
                        hop(w, side, s).wait_send()
                if s >= 1 and split == 2:
                    @pl.when(has(side, s))
                    def _():
                        across(w, side, s).wait_send()
    for d in range(1, T):
        peer = lax.rem(me + d, T)
        tp_send(0, x_ref, xg.at[me], d).wait_send()
        tp_send(1, st1, sg1.at[me], d).wait_send()
        tp_send(2, part1.at[peer], got1.at[d - 1], d).wait_send()
        tp_send(3, firsts.at[me], firsts.at[me], d).wait_send()
        piece(peer).wait_send()
        tp_send(5, st2, sg2.at[me], d).wait_send()


PIECES = (2, 2, 2, 2, 2, 8)
FIRST = tuple(sum(PIECES[:w]) for w in range(6))
GROUP = (0, 0, 0, 1, 1, 2)


def fast_kernel(
    length,
    x_ref, ng_hbm, cw_hbm, cg_hbm, mg_hbm, fg_hbm,
    wv_ref, wg_ref, wo_ref, wga_ref, wup_ref, wd_ref,
    out_ref,
    ng_ref, cw_ref, cg_ref, mg_ref, fg_ref, bv, bg, bo, bga, bup, bd,
    xg, rows, accv, accg, glu, conv, act, part, got, q1, q1in, firsts, hid,
    accs, part2, got2, q2, q2in, sec, ssq, secb, secin, st1, sg1, st2, sg2, finin,
    small, own_sem, zs, zr, zr2, ms, mr, md, ys, yr, xos, xor_, ags, agr, sts, str_, rss, rsr, ds_, dr, qs, qr, os_, orr, fs_, fr,
):
    f = lax.axis_index("fs")
    me = lax.axis_index("tp")
    rep = lax.axis_index("rep")
    count, dt = x_ref.shape
    T = 4
    width = dt * T
    rows_all = 2 * count
    batch = count // length
    chan, ff = bv.shape[2], bga.shape[2]
    local = [wv_ref, wg_ref, wo_ref, wga_ref, wup_ref, wd_ref]
    bufs = [bv, bg, bo, bga, bup, bd]
    VAL, GATE, CVO, GA, UP, DOWN = range(6)
    outer = jnp.logical_or(f == 0, f == 3)
    near = 1 + f // 3
    po, pi, fo = 3 * (f - 1), 3 - f, 3 * (2 - f)
    sib = me + 1 - 2 * lax.rem(me, 2)
    mir = lax.rem(me + 2, T)
    dia = lax.rem(sib + 2, T)

    def view(ref, w, h, c):
        if w == DOWN:
            n, m = ref.shape[1] // 2, ref.shape[0] // 4
            k = n // 2
            return ref.at[pl.ds((c % 4) * m, m), pl.ds(pl.multiple_of(h * n + (c // 4) * k, k), k)]
        n = ref.shape[0] // 2
        k = n // PIECES[w]
        return ref.at[pl.ds(pl.multiple_of(h * n + c * k, k), k), :]

    barrier = pltpu.get_barrier_semaphore()

    def greet(**target):
        pl.semaphore_signal(barrier, inc=1, device_id=target, device_id_type=MESH)

    def zsend(w, hs, c):
        h = rep if hs == 0 else 1 - rep
        sem = zr2.at[w + c // 4 if w == DOWN else w] if hs else zr.at[FIRST[w] + c]
        return remote(view(local[w], w, h, c), view(bufs[w].at[f], w, h, c), zs.at[GROUP[w]], sem, {"fs": near})

    def all_sent(sems, eighths):
        n = bd.shape[1] * eighths // 8
        for g, ref in enumerate((bufs[VAL].at[0:3], bufs[GA].at[0:2], bufs[DOWN].at[0, 0:n, :])):
            remote(ref, ref, sems.at[g], sems.at[g], {"fs": f}).wait_send()

    def xsend():
        return remote(x_ref, xg.at[me, 0], xos, xor_, {"fs": near})

    hn = dt // 2

    def ucols(j):
        if j == 0:
            return pl.ds(pl.multiple_of(rep * hn, hn), hn)
        if j > 3:
            return pl.ds(pl.multiple_of(rep * hn + (j - 4) * (hn // 2), hn // 2), hn // 2)
        return pl.ds(pl.multiple_of((1 - rep) * hn + min(j - 1, 1) * (hn // 2), hn // 2), hn // 2)

    def urows(j):
        return slice((j - 2) * count, (j - 1) * count) if j in (2, 3) else slice(0, rows_all)

    def result(cols, target):
        return remote(secb.at[:, cols], secin.at[:, cols], os_, orr, {"fs": target})

    smalls = [
        pltpu.make_async_copy(src, dst, small.at[k])
        for k, (src, dst) in enumerate(
            ((ng_hbm, ng_ref), (cw_hbm, cw_ref), (cg_hbm, cg_ref), (mg_hbm, mg_ref), (fg_hbm, fg_ref))
        )
    ]

    lane = lax.broadcasted_iota(jnp.int32, (count, 128), 1)
    line = lax.broadcasted_iota(jnp.int32, (8, count), 0)

    def across_lanes(a, b):
        table = jnp.where(lane == 0, a, jnp.where(lane == 1, b, 0.0))
        return jnp.transpose(table)[0:8, :]

    def down_rows(top):
        full = jnp.concatenate([top, jnp.zeros((120, count), F32)], axis=0)
        return jnp.transpose(full)

    @pl.when(outer)
    def _():
        for t in range(T):
            greet(fs=near, tp=t)
        smalls[4].start()
        pl.semaphore_wait(barrier, T)
        order = [
            (VAL, 0), (GATE, 0), None, (CVO, 0), (VAL, 1), (GATE, 1), (CVO, 1),
            (GA, 0), (UP, 0), (GA, 1), (UP, 1), (DOWN, 0), (DOWN, 1),
        ]
        for item in order:
            if item is None:
                xsend().start()
            else:
                for c in range(PIECES[item[0]]):
                    zsend(item[0], item[1], c).start()
        xsend().wait_send()
        all_sent(zs, 8)
        smalls[4].wait()
        remote(secb, secin, os_, orr, {"fs": near}).wait_recv()
        remote(finin, finin, fs_, fr, {"fs": near}).wait_recv()
        full = sum(finin[t] for t in range(T))
        scale = lax.rsqrt(down_rows(full)[:, 0:1] / width + EPS)
        out_ref[...] = (secin[...].astype(F32) * scale * fg_ref[...]).astype(BF16)

    @pl.when(jnp.logical_not(outer))
    def _():
        for t in range(T):
            greet(fs=po, tp=t)
        greet(fs=pi)
        greet(rep=1 - rep)
        for t in (sib, mir, dia):
            greet(tp=t)
        own = [pltpu.make_async_copy(local[w], bufs[w].at[f], own_sem.at[w]) for w in range(6)]
        load_x = pltpu.make_async_copy(x_ref, xg.at[me, 1], small.at[5])
        load_x.start()
        for copy in smalls:
            copy.start()
        for copy in own:
            copy.start()
        pl.semaphore_wait(barrier, T + 5)

        def arrived(ref, send, recv):
            remote(ref, ref, send, recv, {"fs": f}).wait_recv()

        def mid_own(w, c):
            return remote(
                view(local[w], w, rep, c), view(bufs[w].at[f], w, rep, c), ms.at[GROUP[w]], mr.at[0, FIRST[w] + c], {"fs": pi}
            )

        def mid_fwd(w, c):
            ref = view(bufs[w].at[po], w, rep, c)
            return remote(ref, ref, ms.at[GROUP[w]], mr.at[1, FIRST[w] + c], {"fs": pi})

        def mid_direct(c):
            return remote(
                view(local[DOWN], DOWN, 1 - rep, c), view(bufs[DOWN].at[f], DOWN, 1 - rep, c), md.at[0], md.at[1], {"fs": pi}
            )

        def y_fwd(w, k, c):
            ref = view(bufs[w].at[fo if k else pi], w, rep, c)
            sem = yr.at[k, w + c // 4 if w == DOWN else w]
            return remote(ref, ref, ys.at[GROUP[w]], sem, {"rep": 1 - rep})

        def wait_z_down(j):
            arrived(bufs[DOWN].at[po, :, ucols(j)], zs.at[2], zr2.at[DOWN + j - 1])

        def send_own(w):
            for c in range(PIECES[w]):
                mid_own(w, c).start()

        def relay_mid(w, c):
            arrived(view(bufs[w].at[po], w, rep, c), zs.at[GROUP[w]], zr.at[FIRST[w] + c])
            mid_fwd(w, c).start()

        def wait_mid(w, k, c):
            arrived(view(bufs[w].at[fo if k else pi], w, rep, c), ms.at[GROUP[w]], mr.at[k, FIRST[w] + c])

        def relay_y(w, k, c):
            wait_mid(w, k, c)
            y_fwd(w, k, c).start()

        def other(w, shard):
            n = bufs[w].shape[1] // 2
            return bufs[w].at[shard, pl.ds(pl.multiple_of((1 - rep) * n, n), n), :]

        def wait_z(w):
            arrived(other(w, po), zs.at[GROUP[w]], zr2.at[w])

        def wait_y(w, k):
            arrived(other(w, fo if k else pi), ys.at[GROUP[w]], yr.at[k, w])

        def wait_y_down(k, j):
            ref = bufs[DOWN].at[fo if k else pi, :, ucols(j)]
            arrived(ref, ys.at[2], yr.at[k, DOWN + j - 1])

        def wait_last():
            m = bd.shape[1] // 2
            arrived(bufs[DOWN].at[pi, 0:m, ucols(2)], ys.at[2], yr.at[0, 6])
            arrived(bufs[DOWN].at[pi, m:2 * m, ucols(2)], md.at[0], md.at[1])

        def ag(p, buf, slot, kind):
            ref = buf.at[mir if kind == 2 else me, slot]
            return remote(
                ref, ref, ags.at[p, slot], agr.at[p, slot, 1 if kind == 1 else 0], {"tp": mir if kind == 1 else sib}
            )

        def ag_start(p, buf, slot):
            ag(p, buf, slot, 1).start()
            ag(p, buf, slot, 0).start()

        def ag_forward(p, buf, slot):
            arrived(buf.at[mir, slot], ags.at[p, slot], agr.at[p, slot, 1])
            ag(p, buf, slot, 2).start()

        def ag_finish(p, buf, slot):
            arrived(buf.at[0:2, slot], ags.at[p, slot], agr.at[p, slot, 0])

        block = chunk_of(count, 32)

        def norm_rows(src, slot, gain):
            def step(i, _):
                r = pl.ds(pl.multiple_of(i * block, block), block)
                o = pl.ds(pl.multiple_of(slot * count + i * block, block), block)
                vals = [src[t, slot, r, :].astype(F32) for t in range(T)]
                ss = sum(jnp.sum(v * v, axis=1, keepdims=True) for v in vals)
                scale = lax.rsqrt(ss / width + EPS)
                for t in range(T):
                    rows[t, o, :] = (vals[t] * scale * gain[:, t * dt:(t + 1) * dt]).astype(BF16)
                return 0
            lax.fori_loop(0, count // block, step, 0)

        def stat(k, src, dst, d):
            return remote(src, dst, sts.at[k], str_.at[k], {"tp": lax.rem(me + d, T)})

        send_own(VAL)
        send_own(GATE)
        load_x.wait()
        ag_start(0, xg, 1)
        for c in range(2):
            relay_mid(VAL, c)
            relay_y(VAL, 0, c)
        relay_mid(GATE, 0)
        ag_forward(0, xg, 1)
        relay_y(GATE, 0, 0)
        relay_mid(GATE, 1)
        relay_y(GATE, 0, 1)
        send_own(CVO)
        ag_finish(0, xg, 1)
        for copy in smalls:
            copy.wait()
        norm_rows(xg, 1, ng_ref)
        relay_y(VAL, 1, 0)
        arrived(xg.at[me, 0], xos, xor_)
        ag_start(0, xg, 0)
        relay_y(VAL, 1, 1)
        relay_mid(CVO, 0)
        relay_y(GATE, 1, 0)
        relay_mid(CVO, 1)
        send_own(GA)
        send_own(UP)
        relay_y(GATE, 1, 1)
        ag_forward(0, xg, 0)
        ag_finish(0, xg, 0)
        norm_rows(xg, 0, ng_ref)
        relay_y(CVO, 0, 0)

        pad = glu.shape[1] - length - 8
        taps = cw_ref.shape[0]
        lead = pad - (taps - 1)
        nc = chunk_of(chan, 256)
        for b in range(2 * batch):
            glu[b, 0:pad, :] = jnp.zeros((pad, chan), F32)
            glu[b, pad + length:, :] = jnp.zeros((8, chan), F32)

        def s1(shard, first, last):
            def step(c, _):
                cols = pl.ds(pl.multiple_of(c * nc, nc), nc)
                value = jnp.dot(rows[shard], bv[shard, :, cols], preferred_element_type=F32)
                gate = jnp.dot(rows[shard], bg[shard, :, cols], preferred_element_type=F32)
                if not first:
                    value = value + accv[:, cols]
                    gate = gate + accg[:, cols]
                if last:
                    res = value * jax.nn.sigmoid(gate)
                    for b in range(2 * batch):
                        glu[b, pl.ds(pad, length), cols] = res[b * length:(b + 1) * length]
                else:
                    accv[:, cols] = value
                    accg[:, cols] = gate
                return 0
            lax.fori_loop(0, chan // nc, step, 0)

        own[VAL].wait()
        own[GATE].wait()
        s1(f, True, False)
        wait_y(VAL, 0)
        wait_y(GATE, 0)
        s1(pi, False, False)
        relay_y(CVO, 0, 1)
        wait_y(VAL, 1)
        wait_y(GATE, 1)
        s1(fo, False, False)
        relay_y(CVO, 1, 0)
        wait_z(VAL)
        wait_z(GATE)
        s1(po, False, True)
        relay_y(CVO, 1, 1)

        lanes = chunk_of(chan, 128)
        span = chunk_of(length, 64)
        strips = chan // lanes

        def convolve(slot):
            def step(i, _):
                s = lax.rem(i, strips)
                p = i // strips
                cols = pl.ds(pl.multiple_of(s * lanes, lanes), lanes)
                weights = cw_ref[:, cols]
                for b in range(batch):
                    total = jnp.zeros((span, lanes), F32)
                    for shift in range(8):
                        acc = None
                        for tap in range(taps):
                            if (lead + tap) % 8 != shift:
                                continue
                            base = lead + tap - shift
                            term = weights[tap:tap + 1, :] * glu[
                                slot * batch + b, pl.ds(pl.multiple_of(p * span + base, 8), span + 8), cols
                            ]
                            acc = term if acc is None else acc + term
                        if acc is not None:
                            total = total + acc[shift:shift + span]
                    at = pl.multiple_of(slot * count + b * length + p * span, span)
                    conv[pl.ds(at, span), cols] = total
                return 0
            lax.fori_loop(0, strips * (length // span), step, 0)

        def span_of(slot):
            return slice(slot * count, (slot + 1) * count)

        def conv_stats(slot):
            values = conv[span_of(slot), :]
            local_sum = jnp.sum(values, axis=1, keepdims=True)
            dev = values - local_sum / chan
            st1[slot] = across_lanes(local_sum, jnp.sum(dev * dev, axis=1, keepdims=True))
            sg1[slot, me] = st1[slot]
            for d in range(1, T):
                stat(slot, st1.at[slot], sg1.at[slot, me], d).start()

        def activate(slot):
            arrived(sg1.at[slot, 0:3], sts.at[slot], str_.at[slot])
            sums = [sg1[slot, t] for t in range(T)]
            mean = sum(s[0:1, :] for s in sums) / (chan * T)
            spread = sum(
                s[1:2, :] + chan * (s[0:1, :] / chan - mean) * (s[0:1, :] / chan - mean) for s in sums
            ) / (chan * T)
            inv = lax.rsqrt(spread + EPS)
            table = down_rows(jnp.where(line == 0, mean, jnp.where(line == 1, inv, 0.0)))
            normed = (conv[span_of(slot), :] - table[:, 0:1]) * table[:, 1:2] * cg_ref[...]
            act[span_of(slot), :] = (normed * jax.nn.sigmoid(normed)).astype(BF16)

        def rs(slot, kind):
            if kind == 2:
                return remote(q1.at[slot], q1in.at[slot], rss.at[slot], rsr.at[slot, 0], {"tp": mir})
            return remote(
                part.at[slot, dia if kind else sib], got.at[slot, kind], rss.at[slot], rsr.at[slot, kind], {"tp": sib}
            )

        def project(slot):
            def step(j, _):
                prod = jnp.dot(act[span_of(slot), :], bo[j], preferred_element_type=F32)
                part[slot, j] = prod.astype(BF16)
                return 0
            lax.fori_loop(0, T, step, 0)
            rs(slot, 1).start()
            rs(slot, 0).start()

        def pair_sum(slot):
            rs(slot, 1).wait_recv()
            q1[slot] = (part[slot, mir].astype(F32) + got[slot, 1].astype(F32)).astype(BF16)
            rs(slot, 2).start()

        def finish_first(slot):
            arrived(part.at[slot, 0:2], rss.at[slot], rsr.at[slot, 0])
            total = xg[me, slot].astype(F32) + (part[slot, me].astype(F32) + got[slot, 0].astype(F32))
            firsts[me, slot] = (total + q1in[slot].astype(F32)).astype(BF16)
            ag_start(1, firsts, slot)

        convolve(0)
        conv_stats(0)
        convolve(1)
        conv_stats(1)
        relay_y(GA, 0, 0)
        own[CVO].wait()
        wait_y(CVO, 0)
        wait_y(CVO, 1)
        wait_z(CVO)
        activate(0)
        project(0)
        activate(1)
        project(1)
        pair_sum(0)
        relay_y(GA, 0, 1)
        relay_mid(GA, 0)
        pair_sum(1)
        relay_y(UP, 0, 0)
        relay_mid(GA, 1)
        relay_y(UP, 0, 1)
        finish_first(0)
        relay_mid(UP, 0)
        relay_y(GA, 1, 0)
        finish_first(1)
        relay_mid(UP, 1)
        send_own(DOWN)
        mid_direct(6).start()
        relay_y(GA, 1, 1)
        relay_y(UP, 1, 0)
        ag_forward(1, firsts, 0)
        ag_finish(1, firsts, 0)
        norm_rows(firsts, 0, mg_ref)
        relay_y(UP, 1, 1)
        ag_forward(1, firsts, 1)
        ag_finish(1, firsts, 1)
        relay_y(DOWN, 0, 0)
        relay_y(DOWN, 0, 1)
        norm_rows(firsts, 1, mg_ref)
        relay_y(DOWN, 0, 2)
        relay_y(DOWN, 0, 3)

        nf = chunk_of(ff, 256)

        def s5(w, shards, keep):
            def step(c, _):
                cols = pl.ds(pl.multiple_of(c * nf, nf), nf)
                value = sum(jnp.dot(rows[t], bufs[w][t, :, cols], preferred_element_type=F32) for t in shards)
                if keep:
                    accs[w - GA, :, cols] = value
                else:
                    gate = accs[0, :, cols]
                    hid[:, cols] = (gate * jax.nn.sigmoid(gate) * (value + accs[1, :, cols])).astype(BF16)
                return 0
            lax.fori_loop(0, ff // nf, step, 0)

        own[GA].wait()
        own[UP].wait()
        wait_y(GA, 0)
        wait_y(GA, 1)
        wait_z(GA)
        s5(GA, (f, pi, po, fo), True)
        relay_mid(DOWN, 0)
        wait_y(UP, 0)
        wait_z(UP)
        s5(UP, (f, pi, po), True)
        relay_mid(DOWN, 1)
        relay_y(DOWN, 0, 4)
        relay_y(DOWN, 0, 5)
        wait_y(UP, 1)
        s5(UP, (fo,), False)

        def pair_send(b, j):
            at = (b, urows(j), ucols(j))
            return remote(part2.at[at], got2.at[at], ds_, dr.at[lax.rem(b // 2 + me // 2, 2), j], {"tp": sib})

        def cross(j):
            at = (urows(j), ucols(j))
            return remote(q2.at[at], q2in.at[at], qs, qr.at[j], {"tp": mir})

        def down(b, j):
            r, cols = urows(j), ucols(j)
            prod = jnp.dot(hid[r, :], bd[b, :, cols], preferred_element_type=F32)
            part2[b, r, cols] = prod.astype(BF16)

            @pl.when(jnp.logical_or(b == sib, b == dia))
            def _():
                pair_send(b, j).start()

        def combine(b, j):
            r, cols = urows(j), ucols(j)

            @pl.when(b == mir)
            def _():
                pair_send(b, j).wait_recv()
                q2[r, cols] = (part2[b, r, cols].astype(F32) + got2[b, r, cols].astype(F32)).astype(BF16)
                cross(j).start()

        def outer_stat(t):
            return remote(st2.at[0], finin.at[me], fs_, fr, {"fs": po, "tp": t})

        def finish(b, j):
            @pl.when(b == me)
            def _():
                pair_send(me, j).wait_recv()
                cross(j).wait_recv()
                cols = ucols(j)
                for slot in (j - 2,) if j in (2, 3) else (0, 1):
                    r = span_of(slot)
                    second = firsts[me, slot, :, cols].astype(F32) + part2[me, r, cols].astype(F32)
                    second = second + got2[me, r, cols].astype(F32) + q2in[r, cols].astype(F32)
                    total = jnp.sum(second * second, axis=1, keepdims=True)
                    if j not in (0, 4):
                        total = total + ssq[r, :]
                    if slot == 0:
                        secb[:, cols] = second.astype(BF16)
                    else:
                        sec[:, cols] = second
                    if j not in (2, 3):
                        ssq[r, :] = total
                    else:
                        st2[slot] = across_lanes(total, total)
                    if j == 2:
                        for t in (mir, dia, me, sib):
                            outer_stat(t).start()
                    if j == 3:
                        sg2[me] = st2[1]
                        for d in (2, 1, 3):
                            stat(2, st2.at[1], sg2.at[me], d).start()
                    if slot == 0:
                        result(cols, po).start()

        own[DOWN].wait()
        for c in range(6, 8):
            wait_mid(DOWN, 0, c)
        down(pi, 0)
        down(f, 0)
        relay_mid(DOWN, 2)
        relay_mid(DOWN, 3)
        combine(pi, 0)
        down(f, 1)
        combine(f, 0)
        wait_y_down(0, 1)
        down(pi, 1)
        relay_mid(DOWN, 4)
        relay_mid(DOWN, 5)
        relay_y(DOWN, 1, 0)
        relay_y(DOWN, 1, 1)
        combine(f, 1)
        combine(pi, 1)
        down(f, 2)
        down(f, 3)
        relay_mid(DOWN, 6)
        relay_mid(DOWN, 7)
        mid_direct(7).start()
        relay_y(DOWN, 1, 2)
        relay_y(DOWN, 1, 3)
        down(po, 0)
        down(fo, 4)
        relay_y(DOWN, 1, 4)
        relay_y(DOWN, 1, 5)
        combine(f, 2)
        combine(f, 3)
        combine(po, 0)
        combine(fo, 4)
        relay_y(DOWN, 1, 6)
        relay_y(DOWN, 1, 7)
        down(fo, 5)
        wait_y_down(1, 1)
        down(fo, 1)
        finish(f, 0)
        finish(pi, 0)
        combine(fo, 5)
        wait_z_down(1)
        down(po, 1)
        combine(fo, 1)
        finish(f, 1)
        finish(pi, 1)
        combine(po, 1)
        wait_z_down(2)
        down(po, 2)
        down(po, 3)
        finish(po, 0)
        wait_last()
        down(pi, 2)
        wait_y_down(1, 2)
        down(fo, 2)
        combine(po, 2)
        combine(pi, 2)
        down(pi, 3)
        down(fo, 3)
        combine(fo, 2)
        combine(po, 3)
        combine(pi, 3)
        combine(fo, 3)
        finish(fo, 4)
        finish(po, 1)
        finish(fo, 5)
        finish(fo, 1)
        for j in (2, 3):
            for b in (f, po, pi, fo):
                finish(b, j)
        arrived(sg2.at[0:3], sts.at[2], str_.at[2])
        table = down_rows(sum(sg2[t] for t in range(T)))
        scale = lax.rsqrt(table[:, 0:1] / width + EPS)
        out_ref[...] = (sec[...] * scale * fg_ref[...]).astype(BF16)

        def sent(ref, sem):
            remote(ref, ref, sem, sem, {"fs": f}).wait_send()

        all_sent(ms, 8)
        all_sent(ys, 7)
        sent(bufs[DOWN].at[f, 0:bd.shape[1] // 2, ucols(2)], md.at[0])
        for slot in range(2):
            sent(xg.at[0:3, slot], ags.at[0, slot])
            sent(firsts.at[0:3, slot], ags.at[1, slot])
            sent(part.at[slot, 0:3], rss.at[slot])
            sent(sg1.at[slot, 0:3], sts.at[slot])
        sent(sg2.at[0:3], sts.at[2])
        sent(part2.at[0:2], ds_)
        sent(q2, qs)
        sent(secb, os_)
        sent(finin, fs_)


def fast_body(
    activations, norm_gain, w_value, w_gate_conv, conv_weight, chan_gain,
    w_conv_out, mix_gain, w_gate, w_up, w_down, final_gain,
):
    batch, length, dt = activations.shape
    count = batch * length
    weights = (w_value, w_gate_conv, w_conv_out, w_gate, w_up, w_down)
    chan, ff = w_value.shape[1], w_gate.shape[1]
    T = 4
    pad = 8 * ((conv_weight.shape[0] - 1 + 7) // 8)
    rows_all = 2 * count
    vmem, hbm = pl.BlockSpec(memory_space=pltpu.VMEM), pl.BlockSpec(memory_space=pl.ANY)
    dma = pltpu.SemaphoreType.DMA
    V = pltpu.VMEM
    out = pl.pallas_call(
        functools.partial(fast_kernel, length),
        out_shape=pltpu.VMEM((count, dt), BF16),
        in_specs=[hbm] * 12,
        out_specs=vmem,
        scratch_shapes=[
            V((1, dt * T), F32),
            V(conv_weight.shape, F32),
            V((1, chan), F32),
            V((1, dt * T), F32),
            V((1, dt), F32),
        ] + [V((4,) + w.shape, BF16) for w in weights] + [
            V((T, 2, count, dt), BF16),
            V((T, rows_all, dt), BF16),
            V((rows_all, chan), F32),
            V((rows_all, chan), F32),
            V((2 * batch, pad + length + 8, chan), F32),
            V((rows_all, chan), F32),
            V((rows_all, chan), BF16),
            V((2, T, count, dt), BF16),
            V((2, 2, count, dt), BF16),
            V((2, count, dt), BF16),
            V((2, count, dt), BF16),
            V((T, 2, count, dt), BF16),
            V((rows_all, ff), BF16),
            V((2, rows_all, ff), F32),
            V((T, rows_all, dt), BF16),
            V((T, rows_all, dt), BF16),
            V((rows_all, dt), BF16),
            V((rows_all, dt), BF16),
            V((count, dt), F32),
            V((rows_all, 1), F32),
            V((count, dt), BF16),
            V((count, dt), BF16),
            V((2, 8, count), F32),
            V((2, T, 8, count), F32),
            V((2, 8, count), F32),
            V((T, 8, count), F32),
            V((T, 8, count), F32),
            dma((6,)),
            dma((6,)),
            dma((3,)),
            dma((sum(PIECES),)),
            dma((7,)),
            dma((3,)),
            dma((2, sum(PIECES))),
            dma((2,)),
            dma((3,)),
            dma((2, 7)),
            dma(()),
            dma(()),
            dma((2, 2)),
            dma((2, 2, 2)),
            dma((3,)),
            dma((3,)),
            dma((2,)),
            dma((2, 2)),
            dma(()),
            dma((2, 6)),
            dma(()),
            dma((6,)),
            dma(()),
            dma(()),
            dma(()),
            dma(()),
        ],
        compiler_params=pltpu.CompilerParams(
            collective_id=0, has_side_effects=True, vmem_limit_bytes=60 * 1024 * 1024
        ),
        name="block",
    )(
        activations.reshape(count, dt),
        norm_gain.reshape(1, dt * T),
        conv_weight,
        chan_gain.reshape(1, chan),
        mix_gain.reshape(1, dt * T),
        final_gain.reshape(1, dt),
        *weights,
    )
    return out.reshape(batch, length, dt)


def ring_body(
    activations, norm_gain, w_value, w_gate_conv, conv_weight, chan_gain,
    w_conv_out, mix_gain, w_gate, w_up, w_down, final_gain,
):
    batch, length, dt = activations.shape
    count = batch * length
    R, F, T = lax.axis_size("rep"), lax.axis_size("fs"), lax.axis_size("tp")
    weights = (w_value, w_gate_conv, w_conv_out, w_gate, w_up, w_down)
    split = 2 if R == 2 and all(w.shape[0] % 32 == 0 for w in weights) else 1
    width = dt * T
    chan, ff = w_value.shape[1], w_gate.shape[1]
    taps = conv_weight.shape[0]
    pad = 8 * ((taps - 1 + 7) // 8)
    vmem, hbm = pl.BlockSpec(memory_space=pltpu.VMEM), pl.BlockSpec(memory_space=pl.ANY)
    ysh = (2, 6, F) if split == 2 else (1,)
    dma = pltpu.SemaphoreType.DMA
    out = pl.pallas_call(
        functools.partial(ring_kernel, R, F, T, split, length),
        out_shape=jax.ShapeDtypeStruct((count, dt), BF16),
        in_specs=[vmem] * 6 + [hbm] * 6,
        out_specs=vmem,
        scratch_shapes=[pltpu.VMEM((F,) + w.shape, BF16) for w in weights] + [
            pltpu.VMEM((T, count, dt), BF16),
            pltpu.VMEM((count, width), BF16),
            pltpu.VMEM((batch, pad + length + 8, chan), F32),
            pltpu.VMEM((count, max(chan, dt)), F32),
            pltpu.VMEM((count, chan), BF16),
            pltpu.VMEM((T, count, dt), BF16),
            pltpu.VMEM((T, count, dt), BF16),
            pltpu.VMEM((T - 1, count, dt), BF16),
            pltpu.VMEM((T, count, dt), BF16),
            pltpu.VMEM((T, count, dt), BF16),
            pltpu.VMEM((count, ff), BF16),
            pltpu.VMEM((8, count), F32),
            pltpu.VMEM((8, count), F32),
            pltpu.VMEM((T, 8, count), F32),
            pltpu.VMEM((T, 8, count), F32),
            dma((6,)),
            dma((2, 6, F)),
            dma((2, 6, F)),
            dma(ysh),
            dma(ysh),
            dma((6, T)),
            dma((6, T)),
        ],
        compiler_params=pltpu.CompilerParams(
            collective_id=0, has_side_effects=True, vmem_limit_bytes=60 * 1024 * 1024
        ),
        name="block",
    )(
        activations.reshape(count, dt),
        norm_gain.reshape(T, dt),
        conv_weight,
        chan_gain.reshape(1, chan),
        mix_gain.reshape(T, dt),
        final_gain.reshape(1, dt),
        *weights,
    )
    return out.reshape(batch, length, dt)


def solution(mesh):
    in_specs = (
        P(("rep", "fs"), None, "tp"),
        P(),
        P("fs", "tp"),
        P("fs", "tp"),
        P(None, "tp"),
        P("tp"),
        P("tp", "fs"),
        P(),
        P("fs", "tp"),
        P("fs", "tp"),
        P("tp", "fs"),
        P("tp"),
    )
    out_specs = P(("rep", "fs"), None, "tp")
    fast = tuple(mesh.shape[a] for a in ("rep", "fs", "tp")) == (2, 4, 4)
    body = fast_body if fast else ring_body
    return jax.shard_map(body, mesh=mesh, in_specs=in_specs, out_specs=out_specs, check_vma=False)
```

```python
import functools

import jax
import jax.numpy as jnp
from jax import lax
from jax.experimental import pallas as pl
from jax.experimental.pallas import tpu as pltpu
from jax.sharding import PartitionSpec as P

EPS = 1e-06
MESH = pl.DeviceIdType.MESH
F32 = jnp.float32
BF16 = jnp.bfloat16


def remote(src, dst, send, recv, target):
    return pltpu.make_async_remote_copy(
        src_ref=src, dst_ref=dst, send_sem=send, recv_sem=recv, device_id=target, device_id_type=MESH
    )


def chunk_of(extent, want):
    return want if extent % want == 0 else extent


def ring_kernel(
    R, F, T, split, length,
    x_ref, ng_ref, cw_ref, cg_ref, mg_ref, fg_ref,
    wv_ref, wg_ref, wo_ref, wga_ref, wup_ref, wd_ref,
    out_ref,
    bv, bg, bo, bga, bup, bd,
    xg, rows, glu, conv, act, part1, part2, got1, got2, firsts, hid, st1, st2, sg1, sg2,
    own_sem, zs, zr, ys, yr, ts, tr,
):
    f = lax.axis_index("fs")
    me = lax.axis_index("tp")
    rep = lax.axis_index("rep")
    count, dt = x_ref.shape
    width = dt * T
    local = [wv_ref, wg_ref, wo_ref, wga_ref, wup_ref, wd_ref]
    bufs = [bv, bg, bo, bga, bup, bd]

    barrier = pltpu.get_barrier_semaphore()
    greeted = 0
    for target in (lax.rem(f + 1, F), lax.rem(f + F - 1, F)):
        pl.semaphore_signal(barrier, inc=1, device_id={"fs": target}, device_id_type=MESH)
        greeted += 1
    if split == 2:
        pl.semaphore_signal(barrier, inc=1, device_id={"rep": 1 - rep}, device_id_type=MESH)
        greeted += 1
    for d in range(1, T):
        pl.semaphore_signal(barrier, inc=1, device_id={"tp": lax.rem(me + d, T)}, device_id_type=MESH)
        greeted += 1
    own = [
        pltpu.make_async_copy(local[w], bufs[w].at[f], own_sem.at[w]) for w in range(6)
    ]
    for copy in own:
        copy.start()
    pl.semaphore_wait(barrier, greeted)

    def half(w):
        n = local[w].shape[0] // split
        return pl.ds(pl.multiple_of((rep if split == 2 else 0) * n, n), n)

    def other(w):
        n = local[w].shape[0] // split
        return pl.ds(pl.multiple_of((1 - rep) * n, n), n)

    def hop(w, side, s):
        shard = f - s if side == 0 else f + s
        target = f + 1 if side == 0 else f - 1
        src = local[w].at[half(w)] if s == 0 else bufs[w].at[shard, half(w)]
        return remote(src, bufs[w].at[shard, half(w)], zs.at[side, w, s], zr.at[side, w, s + 1], {"fs": target})

    def arrival(w, side, s):
        shard = f - s if side == 0 else f + s
        ref = bufs[w].at[shard, half(w)]
        return remote(ref, ref, zs.at[side, w, s], zr.at[side, w, s], {"fs": f})

    def across(w, side, s):
        shard = f - s if side == 0 else f + s
        ref = bufs[w].at[shard, half(w)]
        return remote(ref, ref, ys.at[side, w, s], yr.at[side, w, s], {"rep": 1 - rep})

    def across_in(w, side, s):
        shard = f - s if side == 0 else f + s
        ref = bufs[w].at[shard, other(w)]
        return remote(ref, ref, ys.at[side, w, s], yr.at[side, w, s], {"rep": 1 - rep})

    def has(side, s):
        return f >= s if side == 0 else f + s <= F - 1

    def sends(side, s):
        ahead = f < F - 1 if side == 0 else f > 0
        return jnp.logical_and(has(side, s), ahead)

    def launch(w):
        for side in (0, 1):
            @pl.when(sends(side, 0))
            def _():
                hop(w, side, 0).start()

    def relay(group, stages=range(1, F)):
        for s in stages:
            for w in group:
                for side in (0, 1):
                    @pl.when(has(side, s))
                    def _():
                        arrival(w, side, s).wait_recv()
                        if s < F - 1:
                            @pl.when(sends(side, s))
                            def _():
                                hop(w, side, s).start()
                        if split == 2:
                            across(w, side, s).start()

    def settle(group):
        for w in group:
            own[w].wait()
        if split == 2:
            for s in range(1, F):
                for w in group:
                    for side in (0, 1):
                        @pl.when(has(side, s))
                        def _():
                            across_in(w, side, s).wait_recv()

    def tp_send(k, src, dst_at, d):
        return remote(src, dst_at, ts.at[k, d], tr.at[k, d], {"tp": lax.rem(me + d, T)})

    for w in (0, 1):
        launch(w)
    for d in range(1, T):
        tp_send(0, x_ref, xg.at[me], d).start()
    launch(2)
    xg[me] = x_ref[...]
    for d in range(1, T):
        peer = lax.rem(me + T - d, T)
        tp_send(0, x_ref, xg.at[peer], d).wait_recv()

    block = chunk_of(count, 16)

    def norm_rows(src, gain):
        def step(i, _):
            r = pl.ds(pl.multiple_of(i * block, block), block)
            vals = [src[t, r, :].astype(F32) for t in range(T)]
            ss = sum(jnp.sum(v * v, axis=1, keepdims=True) for v in vals)
            scale = lax.rsqrt(ss / width + EPS)
            for t in range(T):
                rows[r, t * dt:(t + 1) * dt] = (
                    vals[t] * scale * gain[t:t + 1, :]
                ).astype(BF16)
            return 0
        lax.fori_loop(0, count // block, step, 0)

    norm_rows(xg, ng_ref)
    relay((0, 1, 2))
    for w in (3, 4, 5):
        launch(w)
    settle((0, 1))

    chan = bv.shape[2]
    batch = count // length
    taps = cw_ref.shape[0]
    pad = 8 * ((taps - 1 + 7) // 8)
    lead = pad - (taps - 1)

    def columns(buf, c, n):
        block_w = buf[:, :, pl.ds(pl.multiple_of(c * n, n), n)]
        return block_w.reshape(block_w.shape[0] * block_w.shape[1], n)

    nc = chunk_of(chan, 256)

    def glu_step(c, _):
        value = jnp.dot(rows[...], columns(bv, c, nc), preferred_element_type=F32)
        gate = jnp.dot(rows[...], columns(bg, c, nc), preferred_element_type=F32)
        res = value * jax.nn.sigmoid(gate)
        for b in range(batch):
            glu[b, pl.ds(pad, length), pl.ds(pl.multiple_of(c * nc, nc), nc)] = (
                res[b * length:(b + 1) * length]
            )
        return 0

    for b in range(batch):
        glu[b, 0:pad, :] = jnp.zeros((pad, chan), F32)
        glu[b, pad + length:, :] = jnp.zeros((8, chan), F32)
    lax.fori_loop(0, chan // nc, glu_step, 0)
    relay((3,), (1,))

    lanes = chunk_of(chan, 128)
    span = chunk_of(length, 64)
    strips = chan // lanes

    def conv_step(i, _):
        q = lax.rem(i, strips)
        p = i // strips
        cols = pl.ds(pl.multiple_of(q * lanes, lanes), lanes)
        weights = cw_ref[:, cols]
        for b in range(batch):
            total = jnp.zeros((span, lanes), F32)
            for shift in range(8):
                acc = None
                for tap in range(taps):
                    if (lead + tap) % 8 != shift:
                        continue
                    base = lead + tap - shift
                    term = weights[tap:tap + 1, :] * glu[
                        b, pl.ds(pl.multiple_of(p * span + base, 8), span + 8), cols
                    ]
                    acc = term if acc is None else acc + term
                if acc is not None:
                    total = total + acc[shift:shift + span]
            conv[pl.ds(pl.multiple_of(b * length + p * span, span), span), cols] = total
        return 0

    lax.fori_loop(0, strips * (length // span), conv_step, 0)

    lane = lax.broadcasted_iota(jnp.int32, (count, 128), 1)

    def across_lanes(a, b):
        table = jnp.where(lane == 0, a, jnp.where(lane == 1, b, 0.0))
        return jnp.transpose(table)[0:8, :]

    def down_rows(top):
        full = jnp.concatenate([top, jnp.zeros((120, count), F32)], axis=0)
        return jnp.transpose(full)

    values = conv[...]
    local_sum = jnp.sum(values, axis=1, keepdims=True)
    dev = values - local_sum / chan
    st1[...] = across_lanes(local_sum, jnp.sum(dev * dev, axis=1, keepdims=True))
    sg1[me] = st1[...]
    for d in range(1, T):
        tp_send(1, st1, sg1.at[me], d).start()
    relay((4,), (1,))
    for d in range(1, T):
        peer = lax.rem(me + T - d, T)
        tp_send(1, st1, sg1.at[peer], d).wait_recv()
    sums = [sg1[t] for t in range(T)]
    mean = sum(s[0:1, :] for s in sums) / (chan * T)
    spread = sum(
        s[1:2, :] + chan * (s[0:1, :] / chan - mean) * (s[0:1, :] / chan - mean) for s in sums
    ) / (chan * T)
    inv = lax.rsqrt(spread + EPS)
    line = lax.broadcasted_iota(jnp.int32, (8, count), 0)
    table = down_rows(jnp.where(line == 0, mean, jnp.where(line == 1, inv, 0.0)))
    normed = (conv[...] - table[:, 0:1]) * table[:, 1:2] * cg_ref[...]
    act[...] = (normed * jax.nn.sigmoid(normed)).astype(BF16)

    settle((2,))

    def project(src, buf, part):
        dsh = buf.shape[2]
        for j in range(F):
            t, off = (j * dsh) // dt, (j * dsh) % dt
            prod = jnp.dot(src[...], buf[j], preferred_element_type=F32)
            part[t, :, off:off + dsh] = prod.astype(BF16)

    def scatter(k, part, got):
        for d in range(1, T):
            tp_send(k, part.at[lax.rem(me + d, T)], got.at[d - 1], d).start()

    def gathered(k, part, got):
        total = part[me].astype(F32)
        for d in range(1, T):
            tp_send(k, part.at[me], got.at[d - 1], d).wait_recv()
            total = total + got[d - 1].astype(F32)
        return total

    def piece(t):
        return remote(part2.at[t], got2.at[me], ts.at[4, t], tr.at[4, me], {"tp": t})

    def piece_in(t):
        return remote(part2.at[t], got2.at[t], ts.at[4, t], tr.at[4, t], {"tp": t})

    project(act, bo, part1)
    scatter(2, part1, got1)
    relay((5,), (1,))
    first = (x_ref[...].astype(F32) + gathered(2, part1, got1)).astype(BF16)
    firsts[me] = first
    for d in range(1, T):
        tp_send(3, firsts.at[me], firsts.at[me], d).start()
    relay((3,), (2,))
    for d in range(1, T):
        peer = lax.rem(me + T - d, T)
        tp_send(3, firsts.at[peer], firsts.at[peer], d).wait_recv()
    relay((4,), (2,))
    norm_rows(firsts, mg_ref)
    relay((5,), (2,))
    relay((3, 4), range(3, F))
    settle((3, 4))

    ff = bga.shape[2]
    nf = chunk_of(ff, 256)

    def ff_step(c, _):
        gate = jnp.dot(rows[...], columns(bga, c, nf), preferred_element_type=F32)
        up = jnp.dot(rows[...], columns(bup, c, nf), preferred_element_type=F32)
        hid[:, pl.ds(pl.multiple_of(c * nf, nf), nf)] = (
            gate * jax.nn.sigmoid(gate) * up
        ).astype(BF16)
        return 0

    lax.fori_loop(0, ff // nf, ff_step, 0)
    if F == T and bd.shape[2] == dt:
        def down(shard):
            prod = jnp.dot(hid[...], bd[shard], preferred_element_type=F32)
            part2[shard] = prod.astype(BF16)

            @pl.when(shard != me)
            def _():
                piece(shard).start()

        own[5].wait()
        down(f)
        for s in range(1, F):
            if s >= 3:
                relay((5,), (s,))
            for side in (0, 1):
                @pl.when(has(side, s))
                def _():
                    if split == 2:
                        across_in(5, side, s).wait_recv()
                    down(f - s if side == 0 else f + s)
    else:
        relay((5,), range(3, F))
        settle((5,))
        project(hid, bd, part2)
        for d in range(1, T):
            piece(lax.rem(me + d, T)).start()
    second = firsts[me].astype(F32) + part2[me].astype(F32)
    for d in range(1, T):
        peer = lax.rem(me + d, T)
        piece_in(peer).wait_recv()
        second = second + got2[peer].astype(F32)
    total = jnp.sum(second * second, axis=1, keepdims=True)
    conv[:, 0:dt] = second
    st2[...] = across_lanes(total, total)
    sg2[me] = st2[...]
    for d in range(1, T):
        tp_send(5, st2, sg2.at[me], d).start()
    for d in range(1, T):
        peer = lax.rem(me + T - d, T)
        tp_send(5, st2, sg2.at[peer], d).wait_recv()
    full = sum(sg2[t] for t in range(T))
    table = down_rows(full)
    scale = lax.rsqrt(table[:, 0:1] / width + EPS)
    out_ref[...] = (conv[:, 0:dt] * scale * fg_ref[...]).astype(BF16)

    for w in range(6):
        for side in (0, 1):
            for s in range(F):
                if s < F - 1:
                    @pl.when(sends(side, s))
                    def _():
                        hop(w, side, s).wait_send()
                if s >= 1 and split == 2:
                    @pl.when(has(side, s))
                    def _():
                        across(w, side, s).wait_send()
    for d in range(1, T):
        peer = lax.rem(me + d, T)
        tp_send(0, x_ref, xg.at[me], d).wait_send()
        tp_send(1, st1, sg1.at[me], d).wait_send()
        tp_send(2, part1.at[peer], got1.at[d - 1], d).wait_send()
        tp_send(3, firsts.at[me], firsts.at[me], d).wait_send()
        piece(peer).wait_send()
        tp_send(5, st2, sg2.at[me], d).wait_send()


PIECES = (2, 2, 2, 2, 2, 8)
FIRST = tuple(sum(PIECES[:w]) for w in range(6))
GROUP = (0, 0, 0, 1, 1, 2)


def fast_kernel(
    length,
    x_ref, ng_hbm, cw_hbm, cg_hbm, mg_hbm, fg_hbm,
    wv_ref, wg_ref, wo_ref, wga_ref, wup_ref, wd_ref,
    out_ref,
    ng_ref, cw_ref, cg_ref, mg_ref, fg_ref, bv, bg, bo, bga, bup, bd,
    xg, rows, accv, accg, glu, conv, act, part, got, q1, q1in, firsts, hid,
    accs, part2, got2, q2, q2in, sec, ssq, secb, secin, st1, sg1, st2, sg2, finin,
    small, own_sem, zs, zr, zr2, ms, mr, md, ys, yr, xos, xor_, ags, agr, sts, str_, rss, rsr, ds_, dr, qs, qr, os_, orr, fs_, fr,
):
    f = lax.axis_index("fs")
    me = lax.axis_index("tp")
    rep = lax.axis_index("rep")
    count, dt = x_ref.shape
    T = 4
    width = dt * T
    rows_all = 2 * count
    batch = count // length
    chan, ff = bv.shape[2], bga.shape[2]
    local = [wv_ref, wg_ref, wo_ref, wga_ref, wup_ref, wd_ref]
    bufs = [bv, bg, bo, bga, bup, bd]
    VAL, GATE, CVO, GA, UP, DOWN = range(6)
    outer = jnp.logical_or(f == 0, f == 3)
    near = 1 + f // 3
    po, pi, fo = 3 * (f - 1), 3 - f, 3 * (2 - f)
    sib = me + 1 - 2 * lax.rem(me, 2)
    mir = lax.rem(me + 2, T)
    dia = lax.rem(sib + 2, T)

    def view(ref, w, h, c):
        if w == DOWN:
            n, m = ref.shape[1] // 2, ref.shape[0] // 4
            k = n // 2
            return ref.at[pl.ds((c % 4) * m, m), pl.ds(pl.multiple_of(h * n + (c // 4) * k, k), k)]
        n = ref.shape[0] // 2
        k = n // PIECES[w]
        return ref.at[pl.ds(pl.multiple_of(h * n + c * k, k), k), :]

    barrier = pltpu.get_barrier_semaphore()

    def greet(**target):
        pl.semaphore_signal(barrier, inc=1, device_id=target, device_id_type=MESH)

    def zsend(w, hs, c):
        h = rep if hs == 0 else 1 - rep
        sem = zr2.at[w + c // 4 if w == DOWN else w] if hs else zr.at[FIRST[w] + c]
        return remote(view(local[w], w, h, c), view(bufs[w].at[f], w, h, c), zs.at[GROUP[w]], sem, {"fs": near})

    def all_sent(sems, eighths):
        n = bd.shape[1] * eighths // 8
        for g, ref in enumerate((bufs[VAL].at[0:3], bufs[GA].at[0:2], bufs[DOWN].at[0, 0:n, :])):
            remote(ref, ref, sems.at[g], sems.at[g], {"fs": f}).wait_send()

    def xsend():
        return remote(x_ref, xg.at[me, 0], xos, xor_, {"fs": near})

    hn = dt // 2

    def ucols(j):
        if j == 0:
            return pl.ds(pl.multiple_of(rep * hn, hn), hn)
        if j > 3:
            return pl.ds(pl.multiple_of(rep * hn + (j - 4) * (hn // 2), hn // 2), hn // 2)
        return pl.ds(pl.multiple_of((1 - rep) * hn + min(j - 1, 1) * (hn // 2), hn // 2), hn // 2)

    def urows(j):
        return slice((j - 2) * count, (j - 1) * count) if j in (2, 3) else slice(0, rows_all)

    def result(cols, target):
        return remote(secb.at[:, cols], secin.at[:, cols], os_, orr, {"fs": target})

    smalls = [
        pltpu.make_async_copy(src, dst, small.at[k])
        for k, (src, dst) in enumerate(
            ((ng_hbm, ng_ref), (cw_hbm, cw_ref), (cg_hbm, cg_ref), (mg_hbm, mg_ref), (fg_hbm, fg_ref))
        )
    ]

    lane = lax.broadcasted_iota(jnp.int32, (count, 128), 1)
    line = lax.broadcasted_iota(jnp.int32, (8, count), 0)

    def across_lanes(a, b):
        table = jnp.where(lane == 0, a, jnp.where(lane == 1, b, 0.0))
        return jnp.transpose(table)[0:8, :]

    def down_rows(top):
        full = jnp.concatenate([top, jnp.zeros((120, count), F32)], axis=0)
        return jnp.transpose(full)

    @pl.when(outer)
    def _():
        greet(fs=near)
        smalls[4].start()
        pl.semaphore_wait(barrier, 1)
        order = [
            (VAL, 0), (GATE, 0), None, (CVO, 0), (VAL, 1), (GATE, 1), (CVO, 1),
            (GA, 0), (UP, 0), (GA, 1),
        ]
        for item in order:
            if item is None:
                xsend().start()
            else:
                for c in range(PIECES[item[0]]):
                    zsend(item[0], item[1], c).start()
        zsend(UP, 1, 0).start()
        zsend(DOWN, 0, 0).start()
        zsend(DOWN, 0, 1).start()
        zsend(UP, 1, 1).start()
        for c in range(2, PIECES[DOWN]):
            zsend(DOWN, 0, c).start()
        for c in range(PIECES[DOWN]):
            zsend(DOWN, 1, c).start()
        xsend().wait_send()
        all_sent(zs, 8)
        smalls[4].wait()
        remote(secb, secin, os_, orr, {"fs": near}).wait_recv()
        remote(finin, finin, fs_, fr, {"fs": near}).wait_recv()
        full = sum(finin[t] for t in range(T))
        scale = lax.rsqrt(down_rows(full)[:, 0:1] / width + EPS)
        out_ref[...] = (secin[...].astype(F32) * scale * fg_ref[...]).astype(BF16)

    @pl.when(jnp.logical_not(outer))
    def _():
        greet(fs=po)
        greet(fs=pi)
        greet(rep=1 - rep)
        for t in (sib, mir):
            greet(tp=t)
        own = [pltpu.make_async_copy(local[w], bufs[w].at[f], own_sem.at[w]) for w in range(6)]
        load_x = pltpu.make_async_copy(x_ref, xg.at[me, 1], small.at[5])
        load_x.start()
        for copy in smalls:
            copy.start()
        for copy in own:
            copy.start()
        pl.semaphore_wait(barrier, 5)

        def arrived(ref, send, recv):
            remote(ref, ref, send, recv, {"fs": f}).wait_recv()

        def mid_own(w, c):
            return remote(
                view(local[w], w, rep, c), view(bufs[w].at[f], w, rep, c), ms.at[GROUP[w]], mr.at[0, FIRST[w] + c], {"fs": pi}
            )

        def mid_fwd(w, c):
            ref = view(bufs[w].at[po], w, rep, c)
            return remote(ref, ref, ms.at[GROUP[w]], mr.at[1, FIRST[w] + c], {"fs": pi})

        def mid_direct(c):
            return remote(
                view(local[DOWN], DOWN, 1 - rep, c), view(bufs[DOWN].at[f], DOWN, 1 - rep, c), md.at[0], md.at[1], {"fs": pi}
            )

        def y_fwd(w, k, c):
            ref = view(bufs[w].at[fo if k else pi], w, rep, c)
            sem = yr.at[k, w + c // 4 if w == DOWN else w]
            return remote(ref, ref, ys.at[GROUP[w]], sem, {"rep": 1 - rep})

        def wait_z_down(j):
            arrived(bufs[DOWN].at[po, :, ucols(j)], zs.at[2], zr2.at[DOWN + j - 1])

        def send_own(w):
            for c in range(PIECES[w]):
                mid_own(w, c).start()

        def relay_mid(w, c):
            arrived(view(bufs[w].at[po], w, rep, c), zs.at[GROUP[w]], zr.at[FIRST[w] + c])
            mid_fwd(w, c).start()

        def wait_mid(w, k, c):
            arrived(view(bufs[w].at[fo if k else pi], w, rep, c), ms.at[GROUP[w]], mr.at[k, FIRST[w] + c])

        def relay_y(w, k, c):
            wait_mid(w, k, c)
            y_fwd(w, k, c).start()

        def other(w, shard):
            n = bufs[w].shape[1] // 2
            return bufs[w].at[shard, pl.ds(pl.multiple_of((1 - rep) * n, n), n), :]

        def wait_z(w):
            arrived(other(w, po), zs.at[GROUP[w]], zr2.at[w])

        def wait_y(w, k):
            arrived(other(w, fo if k else pi), ys.at[GROUP[w]], yr.at[k, w])

        def wait_y_down(k, j):
            ref = bufs[DOWN].at[fo if k else pi, :, ucols(j)]
            arrived(ref, ys.at[2], yr.at[k, DOWN + j - 1])

        def wait_last():
            m = bd.shape[1] // 2
            arrived(bufs[DOWN].at[pi, 0:m, ucols(2)], ys.at[2], yr.at[0, 6])
            arrived(bufs[DOWN].at[pi, m:2 * m, ucols(2)], md.at[0], md.at[1])

        def ag(p, buf, slot, kind):
            ref = buf.at[mir if kind == 2 else me, slot]
            return remote(
                ref, ref, ags.at[p, slot], agr.at[p, slot, 1 if kind == 1 else 0], {"tp": mir if kind == 1 else sib}
            )

        def ag_start(p, buf, slot):
            ag(p, buf, slot, 1).start()
            ag(p, buf, slot, 0).start()

        def ag_forward(p, buf, slot):
            arrived(buf.at[mir, slot], ags.at[p, slot], agr.at[p, slot, 1])
            ag(p, buf, slot, 2).start()

        def ag_finish(p, buf, slot):
            arrived(buf.at[0:2, slot], ags.at[p, slot], agr.at[p, slot, 0])

        block = chunk_of(count, 32)

        def norm_rows(src, slot, gain):
            def step(i, _):
                r = pl.ds(pl.multiple_of(i * block, block), block)
                o = pl.ds(pl.multiple_of(slot * count + i * block, block), block)
                vals = [src[t, slot, r, :].astype(F32) for t in range(T)]
                ss = sum(jnp.sum(v * v, axis=1, keepdims=True) for v in vals)
                scale = lax.rsqrt(ss / width + EPS)
                for t in range(T):
                    rows[t, o, :] = (vals[t] * scale * gain[:, t * dt:(t + 1) * dt]).astype(BF16)
                return 0
            lax.fori_loop(0, count // block, step, 0)

        def stat(k, src, dst, d):
            return remote(src, dst, sts.at[k], str_.at[k], {"tp": lax.rem(me + d, T)})

        send_own(VAL)
        send_own(GATE)
        load_x.wait()
        ag_start(0, xg, 1)
        for c in range(2):
            relay_mid(VAL, c)
            relay_y(VAL, 0, c)
        relay_mid(GATE, 0)
        ag_forward(0, xg, 1)
        relay_y(GATE, 0, 0)
        relay_mid(GATE, 1)
        relay_y(GATE, 0, 1)
        send_own(CVO)
        ag_finish(0, xg, 1)
        for copy in smalls:
            copy.wait()
        norm_rows(xg, 1, ng_ref)
        relay_y(VAL, 1, 0)
        arrived(xg.at[me, 0], xos, xor_)
        ag_start(0, xg, 0)
        relay_y(VAL, 1, 1)
        relay_mid(CVO, 0)
        relay_y(GATE, 1, 0)
        relay_mid(CVO, 1)
        send_own(GA)
        send_own(UP)
        relay_y(GATE, 1, 1)
        ag_forward(0, xg, 0)
        ag_finish(0, xg, 0)
        norm_rows(xg, 0, ng_ref)
        relay_y(CVO, 0, 0)

        pad = glu.shape[1] - length - 8
        taps = cw_ref.shape[0]
        lead = pad - (taps - 1)
        nc = chunk_of(chan, 256)
        for b in range(2 * batch):
            glu[b, 0:pad, :] = jnp.zeros((pad, chan), F32)
            glu[b, pad + length:, :] = jnp.zeros((8, chan), F32)

        def s1(shard, first, last):
            def step(c, _):
                cols = pl.ds(pl.multiple_of(c * nc, nc), nc)
                value = jnp.dot(rows[shard], bv[shard, :, cols], preferred_element_type=F32)
                gate = jnp.dot(rows[shard], bg[shard, :, cols], preferred_element_type=F32)
                if not first:
                    value = value + accv[:, cols]
                    gate = gate + accg[:, cols]
                if last:
                    res = value * jax.nn.sigmoid(gate)
                    for b in range(2 * batch):
                        glu[b, pl.ds(pad, length), cols] = res[b * length:(b + 1) * length]
                else:
                    accv[:, cols] = value
                    accg[:, cols] = gate
                return 0
            lax.fori_loop(0, chan // nc, step, 0)

        own[VAL].wait()
        own[GATE].wait()
        s1(f, True, False)
        wait_y(VAL, 0)
        wait_y(GATE, 0)
        s1(pi, False, False)
        relay_y(CVO, 0, 1)
        wait_y(VAL, 1)
        wait_y(GATE, 1)
        s1(fo, False, False)
        relay_y(CVO, 1, 0)
        wait_z(VAL)
        wait_z(GATE)
        s1(po, False, True)
        relay_y(CVO, 1, 1)

        lanes = chunk_of(chan, 128)
        span = chunk_of(length, 64)
        strips = chan // lanes

        def convolve(slot):
            def step(i, _):
                s = lax.rem(i, strips)
                p = i // strips
                cols = pl.ds(pl.multiple_of(s * lanes, lanes), lanes)
                weights = cw_ref[:, cols]
                for b in range(batch):
                    total = jnp.zeros((span, lanes), F32)
                    for shift in range(8):
                        acc = None
                        for tap in range(taps):
                            if (lead + tap) % 8 != shift:
                                continue
                            base = lead + tap - shift
                            term = weights[tap:tap + 1, :] * glu[
                                slot * batch + b, pl.ds(pl.multiple_of(p * span + base, 8), span + 8), cols
                            ]
                            acc = term if acc is None else acc + term
                        if acc is not None:
                            total = total + acc[shift:shift + span]
                    at = pl.multiple_of(slot * count + b * length + p * span, span)
                    conv[pl.ds(at, span), cols] = total
                return 0
            lax.fori_loop(0, strips * (length // span), step, 0)

        def span_of(slot):
            return slice(slot * count, (slot + 1) * count)

        def conv_stats(slot):
            values = conv[span_of(slot), :]
            local_sum = jnp.sum(values, axis=1, keepdims=True)
            dev = values - local_sum / chan
            st1[slot] = across_lanes(local_sum, jnp.sum(dev * dev, axis=1, keepdims=True))
            sg1[slot, me] = st1[slot]
            for d in range(1, T):
                stat(slot, st1.at[slot], sg1.at[slot, me], d).start()

        def activate(slot):
            arrived(sg1.at[slot, 0:3], sts.at[slot], str_.at[slot])
            sums = [sg1[slot, t] for t in range(T)]
            mean = sum(s[0:1, :] for s in sums) / (chan * T)
            spread = sum(
                s[1:2, :] + chan * (s[0:1, :] / chan - mean) * (s[0:1, :] / chan - mean) for s in sums
            ) / (chan * T)
            inv = lax.rsqrt(spread + EPS)
            table = down_rows(jnp.where(line == 0, mean, jnp.where(line == 1, inv, 0.0)))
            normed = (conv[span_of(slot), :] - table[:, 0:1]) * table[:, 1:2] * cg_ref[...]
            act[span_of(slot), :] = (normed * jax.nn.sigmoid(normed)).astype(BF16)

        def rs(slot, kind):
            if kind == 2:
                return remote(q1.at[slot], q1in.at[slot], rss.at[slot], rsr.at[slot, 0], {"tp": mir})
            return remote(
                part.at[slot, dia if kind else sib], got.at[slot, kind], rss.at[slot], rsr.at[slot, kind], {"tp": sib}
            )

        def project(slot):
            def step(j, _):
                prod = jnp.dot(act[span_of(slot), :], bo[j], preferred_element_type=F32)
                part[slot, j] = prod.astype(BF16)
                return 0
            lax.fori_loop(0, T, step, 0)
            rs(slot, 1).start()
            rs(slot, 0).start()

        def pair_sum(slot):
            rs(slot, 1).wait_recv()
            q1[slot] = (part[slot, mir].astype(F32) + got[slot, 1].astype(F32)).astype(BF16)
            rs(slot, 2).start()

        def finish_first(slot):
            arrived(part.at[slot, 0:2], rss.at[slot], rsr.at[slot, 0])
            total = xg[me, slot].astype(F32) + (part[slot, me].astype(F32) + got[slot, 0].astype(F32))
            firsts[me, slot] = (total + q1in[slot].astype(F32)).astype(BF16)
            ag_start(1, firsts, slot)

        convolve(0)
        conv_stats(0)
        convolve(1)
        conv_stats(1)
        relay_y(GA, 0, 0)
        own[CVO].wait()
        wait_y(CVO, 0)
        wait_y(CVO, 1)
        wait_z(CVO)
        activate(0)
        project(0)
        activate(1)
        project(1)
        pair_sum(0)
        relay_y(GA, 0, 1)
        relay_mid(GA, 0)
        pair_sum(1)
        relay_y(UP, 0, 0)
        relay_mid(GA, 1)
        relay_y(UP, 0, 1)
        finish_first(0)
        relay_mid(UP, 0)
        relay_y(GA, 1, 0)
        finish_first(1)
        relay_mid(UP, 1)
        send_own(DOWN)
        mid_direct(6).start()
        relay_y(GA, 1, 1)
        relay_y(UP, 1, 0)
        ag_forward(1, firsts, 0)
        ag_finish(1, firsts, 0)
        norm_rows(firsts, 0, mg_ref)
        relay_y(UP, 1, 1)
        ag_forward(1, firsts, 1)
        ag_finish(1, firsts, 1)
        relay_y(DOWN, 0, 0)
        relay_y(DOWN, 0, 1)
        norm_rows(firsts, 1, mg_ref)
        relay_y(DOWN, 0, 2)
        relay_y(DOWN, 0, 3)

        nf = chunk_of(ff, 256)

        def s5(w, shards, keep):
            def step(c, _):
                cols = pl.ds(pl.multiple_of(c * nf, nf), nf)
                value = sum(jnp.dot(rows[t], bufs[w][t, :, cols], preferred_element_type=F32) for t in shards)
                if keep:
                    accs[w - GA, :, cols] = value
                else:
                    gate = accs[0, :, cols]
                    hid[:, cols] = (gate * jax.nn.sigmoid(gate) * (value + accs[1, :, cols])).astype(BF16)
                return 0
            lax.fori_loop(0, ff // nf, step, 0)

        own[GA].wait()
        own[UP].wait()
        wait_y(GA, 0)
        wait_y(GA, 1)
        wait_z(GA)
        relay_mid(DOWN, 0)
        s5(GA, (f, pi, po, fo), True)
        relay_mid(DOWN, 1)
        wait_y(UP, 0)
        s5(UP, (f, pi), True)
        relay_y(DOWN, 0, 4)
        relay_y(DOWN, 0, 5)
        wait_z(UP)
        wait_y(UP, 1)
        s5(UP, (po, fo), False)

        def pair_send(b, j):
            at = (b, urows(j), ucols(j))
            return remote(part2.at[at], got2.at[at], ds_, dr.at[lax.rem(b // 2 + me // 2, 2), j], {"tp": sib})

        def cross(j):
            at = (urows(j), ucols(j))
            return remote(q2.at[at], q2in.at[at], qs, qr.at[j], {"tp": mir})

        def down(b, j):
            r, cols = urows(j), ucols(j)
            prod = jnp.dot(hid[r, :], bd[b, :, cols], preferred_element_type=F32)
            part2[b, r, cols] = prod.astype(BF16)

            @pl.when(jnp.logical_or(b == sib, b == dia))
            def _():
                pair_send(b, j).start()

        def combine(b, j):
            r, cols = urows(j), ucols(j)

            @pl.when(b == mir)
            def _():
                pair_send(b, j).wait_recv()
                q2[r, cols] = (part2[b, r, cols].astype(F32) + got2[b, r, cols].astype(F32)).astype(BF16)
                cross(j).start()

        def outer_stat(t):
            return remote(st2.at[0], finin.at[me], fs_, fr, {"fs": po, "tp": t})

        def finish(b, j):
            @pl.when(b == me)
            def _():
                pair_send(me, j).wait_recv()
                cross(j).wait_recv()
                cols = ucols(j)
                for slot in (j - 2,) if j in (2, 3) else (0, 1):
                    r = span_of(slot)
                    second = firsts[me, slot, :, cols].astype(F32) + part2[me, r, cols].astype(F32)
                    second = second + got2[me, r, cols].astype(F32) + q2in[r, cols].astype(F32)
                    total = jnp.sum(second * second, axis=1, keepdims=True)
                    if j not in (0, 4):
                        total = total + ssq[r, :]
                    if slot == 0:
                        secb[:, cols] = second.astype(BF16)
                    else:
                        sec[:, cols] = second
                    if j not in (2, 3):
                        ssq[r, :] = total
                    else:
                        st2[slot] = across_lanes(total, total)
                    if j == 2:
                        for t in (mir, dia, me, sib):
                            outer_stat(t).start()
                    if j == 3:
                        sg2[me] = st2[1]
                        for d in (2, 1, 3):
                            stat(2, st2.at[1], sg2.at[me], d).start()
                    if slot == 0:
                        result(cols, po).start()

        own[DOWN].wait()
        for c in range(6, 8):
            wait_mid(DOWN, 0, c)
        down(pi, 0)
        down(f, 0)
        relay_mid(DOWN, 2)
        relay_mid(DOWN, 3)
        combine(pi, 0)
        down(f, 1)
        combine(f, 0)
        wait_y_down(0, 1)
        down(pi, 1)
        relay_mid(DOWN, 4)
        relay_mid(DOWN, 5)
        relay_y(DOWN, 1, 0)
        relay_y(DOWN, 1, 1)
        combine(f, 1)
        combine(pi, 1)
        down(f, 2)
        down(f, 3)
        relay_mid(DOWN, 6)
        relay_mid(DOWN, 7)
        mid_direct(7).start()
        relay_y(DOWN, 1, 2)
        relay_y(DOWN, 1, 3)
        down(po, 0)
        down(fo, 4)
        relay_y(DOWN, 1, 4)
        relay_y(DOWN, 1, 5)
        combine(f, 2)
        combine(f, 3)
        combine(po, 0)
        combine(fo, 4)
        relay_y(DOWN, 1, 6)
        relay_y(DOWN, 1, 7)
        down(fo, 5)
        wait_y_down(1, 1)
        down(fo, 1)
        finish(f, 0)
        finish(pi, 0)
        combine(fo, 5)
        wait_z_down(1)
        down(po, 1)
        combine(fo, 1)
        finish(f, 1)
        finish(pi, 1)
        combine(po, 1)
        wait_z_down(2)
        down(po, 2)
        down(po, 3)
        finish(po, 0)
        wait_last()
        down(pi, 2)
        wait_y_down(1, 2)
        down(fo, 2)
        combine(po, 2)
        combine(pi, 2)
        down(pi, 3)
        down(fo, 3)
        combine(fo, 2)
        combine(po, 3)
        combine(pi, 3)
        combine(fo, 3)
        finish(fo, 4)
        finish(po, 1)
        finish(fo, 5)
        finish(fo, 1)
        for j in (2, 3):
            for b in (f, po, pi, fo):
                finish(b, j)
        arrived(sg2.at[0:3], sts.at[2], str_.at[2])
        table = down_rows(sum(sg2[t] for t in range(T)))
        scale = lax.rsqrt(table[:, 0:1] / width + EPS)
        out_ref[...] = (sec[...] * scale * fg_ref[...]).astype(BF16)

        def sent(ref, sem):
            remote(ref, ref, sem, sem, {"fs": f}).wait_send()

        all_sent(ms, 8)
        all_sent(ys, 7)
        sent(bufs[DOWN].at[f, 0:bd.shape[1] // 2, ucols(2)], md.at[0])
        for slot in range(2):
            sent(xg.at[0:3, slot], ags.at[0, slot])
            sent(firsts.at[0:3, slot], ags.at[1, slot])
            sent(part.at[slot, 0:3], rss.at[slot])
            sent(sg1.at[slot, 0:3], sts.at[slot])
        sent(sg2.at[0:3], sts.at[2])
        sent(part2.at[0:2], ds_)
        sent(q2, qs)
        sent(secb, os_)
        sent(finin, fs_)


def fast_body(
    activations, norm_gain, w_value, w_gate_conv, conv_weight, chan_gain,
    w_conv_out, mix_gain, w_gate, w_up, w_down, final_gain,
):
    batch, length, dt = activations.shape
    count = batch * length
    weights = (w_value, w_gate_conv, w_conv_out, w_gate, w_up, w_down)
    chan, ff = w_value.shape[1], w_gate.shape[1]
    T = 4
    pad = 8 * ((conv_weight.shape[0] - 1 + 7) // 8)
    rows_all = 2 * count
    vmem, hbm = pl.BlockSpec(memory_space=pltpu.VMEM), pl.BlockSpec(memory_space=pl.ANY)
    dma = pltpu.SemaphoreType.DMA
    V = pltpu.VMEM
    out = pl.pallas_call(
        functools.partial(fast_kernel, length),
        out_shape=pltpu.VMEM((count, dt), BF16),
        in_specs=[hbm] * 12,
        out_specs=vmem,
        scratch_shapes=[
            V((1, dt * T), F32),
            V(conv_weight.shape, F32),
            V((1, chan), F32),
            V((1, dt * T), F32),
            V((1, dt), F32),
        ] + [V((4,) + w.shape, BF16) for w in weights] + [
            V((T, 2, count, dt), BF16),
            V((T, rows_all, dt), BF16),
            V((rows_all, chan), F32),
            V((rows_all, chan), F32),
            V((2 * batch, pad + length + 8, chan), F32),
            V((rows_all, chan), F32),
            V((rows_all, chan), BF16),
            V((2, T, count, dt), BF16),
            V((2, 2, count, dt), BF16),
            V((2, count, dt), BF16),
            V((2, count, dt), BF16),
            V((T, 2, count, dt), BF16),
            V((rows_all, ff), BF16),
            V((2, rows_all, ff), F32),
            V((T, rows_all, dt), BF16),
            V((T, rows_all, dt), BF16),
            V((rows_all, dt), BF16),
            V((rows_all, dt), BF16),
            V((count, dt), F32),
            V((rows_all, 1), F32),
            V((count, dt), BF16),
            V((count, dt), BF16),
            V((2, 8, count), F32),
            V((2, T, 8, count), F32),
            V((2, 8, count), F32),
            V((T, 8, count), F32),
            V((T, 8, count), F32),
            dma((6,)),
            dma((6,)),
            dma((3,)),
            dma((sum(PIECES),)),
            dma((7,)),
            dma((3,)),
            dma((2, sum(PIECES))),
            dma((2,)),
            dma((3,)),
            dma((2, 7)),
            dma(()),
            dma(()),
            dma((2, 2)),
            dma((2, 2, 2)),
            dma((3,)),
            dma((3,)),
            dma((2,)),
            dma((2, 2)),
            dma(()),
            dma((2, 6)),
            dma(()),
            dma((6,)),
            dma(()),
            dma(()),
            dma(()),
            dma(()),
        ],
        compiler_params=pltpu.CompilerParams(
            collective_id=0, has_side_effects=True, vmem_limit_bytes=60 * 1024 * 1024
        ),
        name="block",
    )(
        activations.reshape(count, dt),
        norm_gain.reshape(1, dt * T),
        conv_weight,
        chan_gain.reshape(1, chan),
        mix_gain.reshape(1, dt * T),
        final_gain.reshape(1, dt),
        *weights,
    )
    return out.reshape(batch, length, dt)


def ring_body(
    activations, norm_gain, w_value, w_gate_conv, conv_weight, chan_gain,
    w_conv_out, mix_gain, w_gate, w_up, w_down, final_gain,
):
    batch, length, dt = activations.shape
    count = batch * length
    R, F, T = lax.axis_size("rep"), lax.axis_size("fs"), lax.axis_size("tp")
    weights = (w_value, w_gate_conv, w_conv_out, w_gate, w_up, w_down)
    split = 2 if R == 2 and all(w.shape[0] % 32 == 0 for w in weights) else 1
    width = dt * T
    chan, ff = w_value.shape[1], w_gate.shape[1]
    taps = conv_weight.shape[0]
    pad = 8 * ((taps - 1 + 7) // 8)
    vmem, hbm = pl.BlockSpec(memory_space=pltpu.VMEM), pl.BlockSpec(memory_space=pl.ANY)
    ysh = (2, 6, F) if split == 2 else (1,)
    dma = pltpu.SemaphoreType.DMA
    out = pl.pallas_call(
        functools.partial(ring_kernel, R, F, T, split, length),
        out_shape=jax.ShapeDtypeStruct((count, dt), BF16),
        in_specs=[vmem] * 6 + [hbm] * 6,
        out_specs=vmem,
        scratch_shapes=[pltpu.VMEM((F,) + w.shape, BF16) for w in weights] + [
            pltpu.VMEM((T, count, dt), BF16),
            pltpu.VMEM((count, width), BF16),
            pltpu.VMEM((batch, pad + length + 8, chan), F32),
            pltpu.VMEM((count, max(chan, dt)), F32),
            pltpu.VMEM((count, chan), BF16),
            pltpu.VMEM((T, count, dt), BF16),
            pltpu.VMEM((T, count, dt), BF16),
            pltpu.VMEM((T - 1, count, dt), BF16),
            pltpu.VMEM((T, count, dt), BF16),
            pltpu.VMEM((T, count, dt), BF16),
            pltpu.VMEM((count, ff), BF16),
            pltpu.VMEM((8, count), F32),
            pltpu.VMEM((8, count), F32),
            pltpu.VMEM((T, 8, count), F32),
            pltpu.VMEM((T, 8, count), F32),
            dma((6,)),
            dma((2, 6, F)),
            dma((2, 6, F)),
            dma(ysh),
            dma(ysh),
            dma((6, T)),
            dma((6, T)),
        ],
        compiler_params=pltpu.CompilerParams(
            collective_id=0, has_side_effects=True, vmem_limit_bytes=60 * 1024 * 1024
        ),
        name="block",
    )(
        activations.reshape(count, dt),
        norm_gain.reshape(T, dt),
        conv_weight,
        chan_gain.reshape(1, chan),
        mix_gain.reshape(T, dt),
        final_gain.reshape(1, dt),
        *weights,
    )
    return out.reshape(batch, length, dt)


def solution(mesh):
    in_specs = (
        P(("rep", "fs"), None, "tp"),
        P(),
        P("fs", "tp"),
        P("fs", "tp"),
        P(None, "tp"),
        P("tp"),
        P("tp", "fs"),
        P(),
        P("fs", "tp"),
        P("fs", "tp"),
        P("tp", "fs"),
        P("tp"),
    )
    out_specs = P(("rep", "fs"), None, "tp")
    fast = tuple(mesh.shape[a] for a in ("rep", "fs", "tp")) == (2, 4, 4)
    body = fast_body if fast else ring_body
    return jax.shard_map(body, mesh=mesh, in_specs=in_specs, out_specs=out_specs, check_vma=False)
```

```python
import functools

import jax
import jax.numpy as jnp
from jax import lax
from jax.experimental import pallas as pl
from jax.experimental.pallas import tpu as pltpu
from jax.sharding import PartitionSpec as P

EPS = 1e-06
MESH = pl.DeviceIdType.MESH
F32 = jnp.float32
BF16 = jnp.bfloat16


def remote(src, dst, send, recv, target):
    return pltpu.make_async_remote_copy(
        src_ref=src, dst_ref=dst, send_sem=send, recv_sem=recv, device_id=target, device_id_type=MESH
    )


def chunk_of(extent, want):
    return want if extent % want == 0 else extent


def ring_kernel(
    R, F, T, split, length,
    x_ref, ng_ref, cw_ref, cg_ref, mg_ref, fg_ref,
    wv_ref, wg_ref, wo_ref, wga_ref, wup_ref, wd_ref,
    out_ref,
    bv, bg, bo, bga, bup, bd,
    xg, rows, glu, conv, act, part1, part2, got1, got2, firsts, hid, st1, st2, sg1, sg2,
    own_sem, zs, zr, ys, yr, ts, tr,
):
    f = lax.axis_index("fs")
    me = lax.axis_index("tp")
    rep = lax.axis_index("rep")
    count, dt = x_ref.shape
    width = dt * T
    local = [wv_ref, wg_ref, wo_ref, wga_ref, wup_ref, wd_ref]
    bufs = [bv, bg, bo, bga, bup, bd]

    barrier = pltpu.get_barrier_semaphore()
    greeted = 0
    for target in (lax.rem(f + 1, F), lax.rem(f + F - 1, F)):
        pl.semaphore_signal(barrier, inc=1, device_id={"fs": target}, device_id_type=MESH)
        greeted += 1
    if split == 2:
        pl.semaphore_signal(barrier, inc=1, device_id={"rep": 1 - rep}, device_id_type=MESH)
        greeted += 1
    for d in range(1, T):
        pl.semaphore_signal(barrier, inc=1, device_id={"tp": lax.rem(me + d, T)}, device_id_type=MESH)
        greeted += 1
    own = [
        pltpu.make_async_copy(local[w], bufs[w].at[f], own_sem.at[w]) for w in range(6)
    ]
    for copy in own:
        copy.start()
    pl.semaphore_wait(barrier, greeted)

    def half(w):
        n = local[w].shape[0] // split
        return pl.ds(pl.multiple_of((rep if split == 2 else 0) * n, n), n)

    def other(w):
        n = local[w].shape[0] // split
        return pl.ds(pl.multiple_of((1 - rep) * n, n), n)

    def hop(w, side, s):
        shard = f - s if side == 0 else f + s
        target = f + 1 if side == 0 else f - 1
        src = local[w].at[half(w)] if s == 0 else bufs[w].at[shard, half(w)]
        return remote(src, bufs[w].at[shard, half(w)], zs.at[side, w, s], zr.at[side, w, s + 1], {"fs": target})

    def arrival(w, side, s):
        shard = f - s if side == 0 else f + s
        ref = bufs[w].at[shard, half(w)]
        return remote(ref, ref, zs.at[side, w, s], zr.at[side, w, s], {"fs": f})

    def across(w, side, s):
        shard = f - s if side == 0 else f + s
        ref = bufs[w].at[shard, half(w)]
        return remote(ref, ref, ys.at[side, w, s], yr.at[side, w, s], {"rep": 1 - rep})

    def across_in(w, side, s):
        shard = f - s if side == 0 else f + s
        ref = bufs[w].at[shard, other(w)]
        return remote(ref, ref, ys.at[side, w, s], yr.at[side, w, s], {"rep": 1 - rep})

    def has(side, s):
        return f >= s if side == 0 else f + s <= F - 1

    def sends(side, s):
        ahead = f < F - 1 if side == 0 else f > 0
        return jnp.logical_and(has(side, s), ahead)

    def launch(w):
        for side in (0, 1):
            @pl.when(sends(side, 0))
            def _():
                hop(w, side, 0).start()

    def relay(group, stages=range(1, F)):
        for s in stages:
            for w in group:
                for side in (0, 1):
                    @pl.when(has(side, s))
                    def _():
                        arrival(w, side, s).wait_recv()
                        if s < F - 1:
                            @pl.when(sends(side, s))
                            def _():
                                hop(w, side, s).start()
                        if split == 2:
                            across(w, side, s).start()

    def settle(group):
        for w in group:
            own[w].wait()
        if split == 2:
            for s in range(1, F):
                for w in group:
                    for side in (0, 1):
                        @pl.when(has(side, s))
                        def _():
                            across_in(w, side, s).wait_recv()

    def tp_send(k, src, dst_at, d):
        return remote(src, dst_at, ts.at[k, d], tr.at[k, d], {"tp": lax.rem(me + d, T)})

    for w in (0, 1):
        launch(w)
    for d in range(1, T):
        tp_send(0, x_ref, xg.at[me], d).start()
    launch(2)
    xg[me] = x_ref[...]
    for d in range(1, T):
        peer = lax.rem(me + T - d, T)
        tp_send(0, x_ref, xg.at[peer], d).wait_recv()

    block = chunk_of(count, 16)

    def norm_rows(src, gain):
        def step(i, _):
            r = pl.ds(pl.multiple_of(i * block, block), block)
            vals = [src[t, r, :].astype(F32) for t in range(T)]
            ss = sum(jnp.sum(v * v, axis=1, keepdims=True) for v in vals)
            scale = lax.rsqrt(ss / width + EPS)
            for t in range(T):
                rows[r, t * dt:(t + 1) * dt] = (
                    vals[t] * scale * gain[t:t + 1, :]
                ).astype(BF16)
            return 0
        lax.fori_loop(0, count // block, step, 0)

    norm_rows(xg, ng_ref)
    relay((0, 1, 2))
    for w in (3, 4, 5):
        launch(w)
    settle((0, 1))

    chan = bv.shape[2]
    batch = count // length
    taps = cw_ref.shape[0]
    pad = 8 * ((taps - 1 + 7) // 8)
    lead = pad - (taps - 1)

    def columns(buf, c, n):
        block_w = buf[:, :, pl.ds(pl.multiple_of(c * n, n), n)]
        return block_w.reshape(block_w.shape[0] * block_w.shape[1], n)

    nc = chunk_of(chan, 256)

    def glu_step(c, _):
        value = jnp.dot(rows[...], columns(bv, c, nc), preferred_element_type=F32)
        gate = jnp.dot(rows[...], columns(bg, c, nc), preferred_element_type=F32)
        res = value * jax.nn.sigmoid(gate)
        for b in range(batch):
            glu[b, pl.ds(pad, length), pl.ds(pl.multiple_of(c * nc, nc), nc)] = (
                res[b * length:(b + 1) * length]
            )
        return 0

    for b in range(batch):
        glu[b, 0:pad, :] = jnp.zeros((pad, chan), F32)
        glu[b, pad + length:, :] = jnp.zeros((8, chan), F32)
    lax.fori_loop(0, chan // nc, glu_step, 0)
    relay((3,), (1,))

    lanes = chunk_of(chan, 128)
    span = chunk_of(length, 64)
    strips = chan // lanes

    def conv_step(i, _):
        q = lax.rem(i, strips)
        p = i // strips
        cols = pl.ds(pl.multiple_of(q * lanes, lanes), lanes)
        weights = cw_ref[:, cols]
        for b in range(batch):
            total = jnp.zeros((span, lanes), F32)
            for shift in range(8):
                acc = None
                for tap in range(taps):
                    if (lead + tap) % 8 != shift:
                        continue
                    base = lead + tap - shift
                    term = weights[tap:tap + 1, :] * glu[
                        b, pl.ds(pl.multiple_of(p * span + base, 8), span + 8), cols
                    ]
                    acc = term if acc is None else acc + term
                if acc is not None:
                    total = total + acc[shift:shift + span]
            conv[pl.ds(pl.multiple_of(b * length + p * span, span), span), cols] = total
        return 0

    lax.fori_loop(0, strips * (length // span), conv_step, 0)

    lane = lax.broadcasted_iota(jnp.int32, (count, 128), 1)

    def across_lanes(a, b):
        table = jnp.where(lane == 0, a, jnp.where(lane == 1, b, 0.0))
        return jnp.transpose(table)[0:8, :]

    def down_rows(top):
        full = jnp.concatenate([top, jnp.zeros((120, count), F32)], axis=0)
        return jnp.transpose(full)

    values = conv[...]
    local_sum = jnp.sum(values, axis=1, keepdims=True)
    dev = values - local_sum / chan
    st1[...] = across_lanes(local_sum, jnp.sum(dev * dev, axis=1, keepdims=True))
    sg1[me] = st1[...]
    for d in range(1, T):
        tp_send(1, st1, sg1.at[me], d).start()
    relay((4,), (1,))
    for d in range(1, T):
        peer = lax.rem(me + T - d, T)
        tp_send(1, st1, sg1.at[peer], d).wait_recv()
    sums = [sg1[t] for t in range(T)]
    mean = sum(s[0:1, :] for s in sums) / (chan * T)
    spread = sum(
        s[1:2, :] + chan * (s[0:1, :] / chan - mean) * (s[0:1, :] / chan - mean) for s in sums
    ) / (chan * T)
    inv = lax.rsqrt(spread + EPS)
    line = lax.broadcasted_iota(jnp.int32, (8, count), 0)
    table = down_rows(jnp.where(line == 0, mean, jnp.where(line == 1, inv, 0.0)))
    normed = (conv[...] - table[:, 0:1]) * table[:, 1:2] * cg_ref[...]
    act[...] = (normed * jax.nn.sigmoid(normed)).astype(BF16)

    settle((2,))

    def project(src, buf, part):
        dsh = buf.shape[2]
        for j in range(F):
            t, off = (j * dsh) // dt, (j * dsh) % dt
            prod = jnp.dot(src[...], buf[j], preferred_element_type=F32)
            part[t, :, off:off + dsh] = prod.astype(BF16)

    def scatter(k, part, got):
        for d in range(1, T):
            tp_send(k, part.at[lax.rem(me + d, T)], got.at[d - 1], d).start()

    def gathered(k, part, got):
        total = part[me].astype(F32)
        for d in range(1, T):
            tp_send(k, part.at[me], got.at[d - 1], d).wait_recv()
            total = total + got[d - 1].astype(F32)
        return total

    def piece(t):
        return remote(part2.at[t], got2.at[me], ts.at[4, t], tr.at[4, me], {"tp": t})

    def piece_in(t):
        return remote(part2.at[t], got2.at[t], ts.at[4, t], tr.at[4, t], {"tp": t})

    project(act, bo, part1)
    scatter(2, part1, got1)
    relay((5,), (1,))
    first = (x_ref[...].astype(F32) + gathered(2, part1, got1)).astype(BF16)
    firsts[me] = first
    for d in range(1, T):
        tp_send(3, firsts.at[me], firsts.at[me], d).start()
    relay((3,), (2,))
    for d in range(1, T):
        peer = lax.rem(me + T - d, T)
        tp_send(3, firsts.at[peer], firsts.at[peer], d).wait_recv()
    relay((4,), (2,))
    norm_rows(firsts, mg_ref)
    relay((5,), (2,))
    relay((3, 4), range(3, F))
    settle((3, 4))

    ff = bga.shape[2]
    nf = chunk_of(ff, 256)

    def ff_step(c, _):
        gate = jnp.dot(rows[...], columns(bga, c, nf), preferred_element_type=F32)
        up = jnp.dot(rows[...], columns(bup, c, nf), preferred_element_type=F32)
        hid[:, pl.ds(pl.multiple_of(c * nf, nf), nf)] = (
            gate * jax.nn.sigmoid(gate) * up
        ).astype(BF16)
        return 0

    lax.fori_loop(0, ff // nf, ff_step, 0)
    if F == T and bd.shape[2] == dt:
        def down(shard):
            prod = jnp.dot(hid[...], bd[shard], preferred_element_type=F32)
            part2[shard] = prod.astype(BF16)

            @pl.when(shard != me)
            def _():
                piece(shard).start()

        own[5].wait()
        down(f)
        for s in range(1, F):
            if s >= 3:
                relay((5,), (s,))
            for side in (0, 1):
                @pl.when(has(side, s))
                def _():
                    if split == 2:
                        across_in(5, side, s).wait_recv()
                    down(f - s if side == 0 else f + s)
    else:
        relay((5,), range(3, F))
        settle((5,))
        project(hid, bd, part2)
        for d in range(1, T):
            piece(lax.rem(me + d, T)).start()
    second = firsts[me].astype(F32) + part2[me].astype(F32)
    for d in range(1, T):
        peer = lax.rem(me + d, T)
        piece_in(peer).wait_recv()
        second = second + got2[peer].astype(F32)
    total = jnp.sum(second * second, axis=1, keepdims=True)
    conv[:, 0:dt] = second
    st2[...] = across_lanes(total, total)
    sg2[me] = st2[...]
    for d in range(1, T):
        tp_send(5, st2, sg2.at[me], d).start()
    for d in range(1, T):
        peer = lax.rem(me + T - d, T)
        tp_send(5, st2, sg2.at[peer], d).wait_recv()
    full = sum(sg2[t] for t in range(T))
    table = down_rows(full)
    scale = lax.rsqrt(table[:, 0:1] / width + EPS)
    out_ref[...] = (conv[:, 0:dt] * scale * fg_ref[...]).astype(BF16)

    for w in range(6):
        for side in (0, 1):
            for s in range(F):
                if s < F - 1:
                    @pl.when(sends(side, s))
                    def _():
                        hop(w, side, s).wait_send()
                if s >= 1 and split == 2:
                    @pl.when(has(side, s))
                    def _():
                        across(w, side, s).wait_send()
    for d in range(1, T):
        peer = lax.rem(me + d, T)
        tp_send(0, x_ref, xg.at[me], d).wait_send()
        tp_send(1, st1, sg1.at[me], d).wait_send()
        tp_send(2, part1.at[peer], got1.at[d - 1], d).wait_send()
        tp_send(3, firsts.at[me], firsts.at[me], d).wait_send()
        piece(peer).wait_send()
        tp_send(5, st2, sg2.at[me], d).wait_send()


PIECES = (2, 2, 2, 2, 2, 8)
FIRST = tuple(sum(PIECES[:w]) for w in range(6))
GROUP = (0, 0, 0, 1, 1, 2)


def fast_kernel(
    length,
    x_ref, ng_hbm, cw_hbm, cg_hbm, mg_hbm, fg_hbm,
    wv_ref, wg_ref, wo_ref, wga_ref, wup_ref, wd_ref,
    out_ref,
    ng_ref, cw_ref, cg_ref, mg_ref, fg_ref, bv, bg, bo, bga, bup, bd,
    xg, rows, accv, accg, glu, conv, act, part, got, q1, q1in, firsts, hid,
    accs, part2, got2, q2, q2in, sec, ssq, secb, secin, st1, sg1, st2, sg2, finin,
    small, own_sem, zs, zr, zr2, ms, mr, md, ys, yr, xos, xor_, ags, agr, sts, str_, rss, rsr, ds_, dr, qs, qr, os_, orr, fs_, fr,
):
    f = lax.axis_index("fs")
    me = lax.axis_index("tp")
    rep = lax.axis_index("rep")
    count, dt = x_ref.shape
    T = 4
    width = dt * T
    rows_all = 2 * count
    batch = count // length
    chan, ff = bv.shape[2], bga.shape[2]
    local = [wv_ref, wg_ref, wo_ref, wga_ref, wup_ref, wd_ref]
    bufs = [bv, bg, bo, bga, bup, bd]
    VAL, GATE, CVO, GA, UP, DOWN = range(6)
    outer = jnp.logical_or(f == 0, f == 3)
    near = 1 + f // 3
    po, pi, fo = 3 * (f - 1), 3 - f, 3 * (2 - f)
    sib = me + 1 - 2 * lax.rem(me, 2)
    mir = lax.rem(me + 2, T)
    dia = lax.rem(sib + 2, T)

    def view(ref, w, h, c):
        if w == DOWN:
            n, m = ref.shape[1] // 2, ref.shape[0] // 4
            k = n // 2
            return ref.at[pl.ds((c % 4) * m, m), pl.ds(pl.multiple_of(h * n + (c // 4) * k, k), k)]
        n = ref.shape[0] // 2
        k = n // PIECES[w]
        return ref.at[pl.ds(pl.multiple_of(h * n + c * k, k), k), :]

    barrier = pltpu.get_barrier_semaphore()

    def greet(**target):
        pl.semaphore_signal(barrier, inc=1, device_id=target, device_id_type=MESH)

    def zsend(w, hs, c):
        h = rep if hs == 0 else 1 - rep
        sem = zr2.at[w + c // 4 if w == DOWN else w] if hs else zr.at[FIRST[w] + c]
        return remote(view(local[w], w, h, c), view(bufs[w].at[f], w, h, c), zs.at[GROUP[w]], sem, {"fs": near})

    def all_sent(sems, eighths):
        n = bd.shape[1] * eighths // 8
        for g, ref in enumerate((bufs[VAL].at[0:3], bufs[GA].at[0:2], bufs[DOWN].at[0, 0:n, :])):
            remote(ref, ref, sems.at[g], sems.at[g], {"fs": f}).wait_send()

    def xsend():
        return remote(x_ref, xg.at[me, 0], xos, xor_, {"fs": near})

    hn = dt // 2

    def ucols(j):
        if j == 0:
            return pl.ds(pl.multiple_of(rep * hn, hn), hn)
        if j > 3:
            return pl.ds(pl.multiple_of(rep * hn + (j - 4) * (hn // 2), hn // 2), hn // 2)
        return pl.ds(pl.multiple_of((1 - rep) * hn + min(j - 1, 1) * (hn // 2), hn // 2), hn // 2)

    def urows(j):
        return slice((j - 2) * count, (j - 1) * count) if j in (2, 3) else slice(0, rows_all)

    def result(cols, target):
        return remote(secb.at[:, cols], secin.at[:, cols], os_, orr, {"fs": target})

    smalls = [
        pltpu.make_async_copy(src, dst, small.at[k])
        for k, (src, dst) in enumerate(
            ((ng_hbm, ng_ref), (cw_hbm, cw_ref), (cg_hbm, cg_ref), (mg_hbm, mg_ref), (fg_hbm, fg_ref))
        )
    ]

    lane = lax.broadcasted_iota(jnp.int32, (count, 128), 1)
    line = lax.broadcasted_iota(jnp.int32, (8, count), 0)

    def across_lanes(a, b):
        table = jnp.where(lane == 0, a, jnp.where(lane == 1, b, 0.0))
        return jnp.transpose(table)[0:8, :]

    def down_rows(top):
        full = jnp.concatenate([top, jnp.zeros((120, count), F32)], axis=0)
        return jnp.transpose(full)

    @pl.when(outer)
    def _():
        greet(fs=near)
        smalls[4].start()
        pl.semaphore_wait(barrier, 1)
        order = [
            (VAL, 0), (GATE, 0), None, (CVO, 0), (VAL, 1), (GATE, 1), (CVO, 1),
            (GA, 0), (UP, 0), (GA, 1),
        ]
        for item in order:
            if item is None:
                xsend().start()
            else:
                for c in range(PIECES[item[0]]):
                    zsend(item[0], item[1], c).start()
        zsend(UP, 1, 0).start()
        zsend(DOWN, 0, 0).start()
        zsend(DOWN, 0, 1).start()
        zsend(UP, 1, 1).start()
        for c in range(2, PIECES[DOWN]):
            zsend(DOWN, 0, c).start()
        for c in range(PIECES[DOWN]):
            zsend(DOWN, 1, c).start()
        xsend().wait_send()
        all_sent(zs, 8)
        smalls[4].wait()
        remote(secb, secin, os_, orr, {"fs": near}).wait_recv()
        remote(finin, finin, fs_, fr, {"fs": near}).wait_recv()
        full = sum(finin[t] for t in range(T))
        scale = lax.rsqrt(down_rows(full)[:, 0:1] / width + EPS)
        out_ref[...] = (secin[...].astype(F32) * scale * fg_ref[...]).astype(BF16)

    @pl.when(jnp.logical_not(outer))
    def _():
        greet(fs=po)
        greet(fs=pi)
        greet(rep=1 - rep)
        for t in (sib, mir):
            greet(tp=t)
        own = [pltpu.make_async_copy(local[w], bufs[w].at[f], own_sem.at[w]) for w in range(6)]
        load_x = pltpu.make_async_copy(x_ref, xg.at[me, 1], small.at[5])
        load_x.start()
        for copy in smalls:
            copy.start()
        for copy in own:
            copy.start()
        pl.semaphore_wait(barrier, 5)

        def arrived(ref, send, recv):
            remote(ref, ref, send, recv, {"fs": f}).wait_recv()

        def mid_own(w, c):
            return remote(
                view(local[w], w, rep, c), view(bufs[w].at[f], w, rep, c), ms.at[GROUP[w]], mr.at[0, FIRST[w] + c], {"fs": pi}
            )

        def mid_fwd(w, c):
            ref = view(bufs[w].at[po], w, rep, c)
            return remote(ref, ref, ms.at[GROUP[w]], mr.at[1, FIRST[w] + c], {"fs": pi})

        def mid_direct(c):
            return remote(
                view(local[DOWN], DOWN, 1 - rep, c), view(bufs[DOWN].at[f], DOWN, 1 - rep, c), md.at[0], md.at[1], {"fs": pi}
            )

        def y_fwd(w, k, c):
            ref = view(bufs[w].at[fo if k else pi], w, rep, c)
            sem = yr.at[k, w + c // 4 if w == DOWN else w]
            return remote(ref, ref, ys.at[GROUP[w]], sem, {"rep": 1 - rep})

        def wait_z_down(j):
            arrived(bufs[DOWN].at[po, :, ucols(j)], zs.at[2], zr2.at[DOWN + j - 1])

        def send_own(w):
            for c in range(PIECES[w]):
                mid_own(w, c).start()

        def relay_mid(w, c):
            arrived(view(bufs[w].at[po], w, rep, c), zs.at[GROUP[w]], zr.at[FIRST[w] + c])
            mid_fwd(w, c).start()

        def wait_mid(w, k, c):
            arrived(view(bufs[w].at[fo if k else pi], w, rep, c), ms.at[GROUP[w]], mr.at[k, FIRST[w] + c])

        def relay_y(w, k, c):
            wait_mid(w, k, c)
            y_fwd(w, k, c).start()

        def other(w, shard):
            n = bufs[w].shape[1] // 2
            return bufs[w].at[shard, pl.ds(pl.multiple_of((1 - rep) * n, n), n), :]

        def wait_z(w):
            arrived(other(w, po), zs.at[GROUP[w]], zr2.at[w])

        def wait_y(w, k):
            arrived(other(w, fo if k else pi), ys.at[GROUP[w]], yr.at[k, w])

        def wait_y_down(k, j):
            ref = bufs[DOWN].at[fo if k else pi, :, ucols(j)]
            arrived(ref, ys.at[2], yr.at[k, DOWN + j - 1])

        def wait_last():
            m = bd.shape[1] // 2
            arrived(bufs[DOWN].at[pi, 0:m, ucols(2)], ys.at[2], yr.at[0, 6])
            arrived(bufs[DOWN].at[pi, m:2 * m, ucols(2)], md.at[0], md.at[1])

        def ag(p, buf, slot, kind):
            ref = buf.at[mir if kind == 2 else me, slot]
            return remote(
                ref, ref, ags.at[p, slot], agr.at[p, slot, 1 if kind == 1 else 0], {"tp": mir if kind == 1 else sib}
            )

        def ag_start(p, buf, slot):
            ag(p, buf, slot, 1).start()
            ag(p, buf, slot, 0).start()

        def ag_forward(p, buf, slot):
            arrived(buf.at[mir, slot], ags.at[p, slot], agr.at[p, slot, 1])
            ag(p, buf, slot, 2).start()

        def ag_finish(p, buf, slot):
            arrived(buf.at[0:2, slot], ags.at[p, slot], agr.at[p, slot, 0])

        block = chunk_of(count, 32)

        def norm_rows(src, slot, gain):
            def step(i, _):
                r = pl.ds(pl.multiple_of(i * block, block), block)
                o = pl.ds(pl.multiple_of(slot * count + i * block, block), block)
                vals = [src[t, slot, r, :].astype(F32) for t in range(T)]
                ss = sum(jnp.sum(v * v, axis=1, keepdims=True) for v in vals)
                scale = lax.rsqrt(ss / width + EPS)
                for t in range(T):
                    rows[t, o, :] = (vals[t] * scale * gain[:, t * dt:(t + 1) * dt]).astype(BF16)
                return 0
            lax.fori_loop(0, count // block, step, 0)

        def stat(k, src, dst, d):
            return remote(src, dst, sts.at[k], str_.at[k], {"tp": lax.rem(me + d, T)})

        send_own(VAL)
        send_own(GATE)
        load_x.wait()
        ag_start(0, xg, 1)
        for c in range(2):
            relay_mid(VAL, c)
            relay_y(VAL, 0, c)
        relay_mid(GATE, 0)
        ag_forward(0, xg, 1)
        relay_y(GATE, 0, 0)
        relay_mid(GATE, 1)
        relay_y(GATE, 0, 1)
        send_own(CVO)
        ag_finish(0, xg, 1)
        for copy in smalls:
            copy.wait()
        norm_rows(xg, 1, ng_ref)
        relay_y(VAL, 1, 0)
        arrived(xg.at[me, 0], xos, xor_)
        ag_start(0, xg, 0)
        relay_y(VAL, 1, 1)
        relay_mid(CVO, 0)
        relay_y(GATE, 1, 0)
        relay_mid(CVO, 1)
        send_own(GA)
        send_own(UP)
        relay_y(GATE, 1, 1)
        ag_forward(0, xg, 0)
        ag_finish(0, xg, 0)
        norm_rows(xg, 0, ng_ref)
        relay_y(CVO, 0, 0)

        pad = glu.shape[1] - length - 8
        taps = cw_ref.shape[0]
        lead = pad - (taps - 1)
        nc = chunk_of(chan, 256)
        for b in range(2 * batch):
            glu[b, 0:pad, :] = jnp.zeros((pad, chan), F32)
            glu[b, pad + length:, :] = jnp.zeros((8, chan), F32)

        def s1(shard, first, last):
            def step(c, _):
                cols = pl.ds(pl.multiple_of(c * nc, nc), nc)
                value = jnp.dot(rows[shard], bv[shard, :, cols], preferred_element_type=F32)
                gate = jnp.dot(rows[shard], bg[shard, :, cols], preferred_element_type=F32)
                if not first:
                    value = value + accv[:, cols]
                    gate = gate + accg[:, cols]
                if last:
                    res = value * jax.nn.sigmoid(gate)
                    for b in range(2 * batch):
                        glu[b, pl.ds(pad, length), cols] = res[b * length:(b + 1) * length]
                else:
                    accv[:, cols] = value
                    accg[:, cols] = gate
                return 0
            lax.fori_loop(0, chan // nc, step, 0)

        own[VAL].wait()
        own[GATE].wait()
        s1(f, True, False)
        wait_y(VAL, 0)
        wait_y(GATE, 0)
        s1(pi, False, False)
        relay_y(CVO, 0, 1)
        wait_y(VAL, 1)
        wait_y(GATE, 1)
        s1(fo, False, False)
        relay_y(CVO, 1, 0)
        wait_z(VAL)
        wait_z(GATE)
        s1(po, False, True)
        relay_y(CVO, 1, 1)

        lanes = chunk_of(chan, 128)
        span = chunk_of(length, 64)
        strips = chan // lanes

        def convolve(slot):
            def step(i, _):
                s = lax.rem(i, strips)
                p = i // strips
                cols = pl.ds(pl.multiple_of(s * lanes, lanes), lanes)
                weights = cw_ref[:, cols]
                for b in range(batch):
                    total = jnp.zeros((span, lanes), F32)
                    for shift in range(8):
                        acc = None
                        for tap in range(taps):
                            if (lead + tap) % 8 != shift:
                                continue
                            base = lead + tap - shift
                            term = weights[tap:tap + 1, :] * glu[
                                slot * batch + b, pl.ds(pl.multiple_of(p * span + base, 8), span + 8), cols
                            ]
                            acc = term if acc is None else acc + term
                        if acc is not None:
                            total = total + acc[shift:shift + span]
                    at = pl.multiple_of(slot * count + b * length + p * span, span)
                    conv[pl.ds(at, span), cols] = total
                return 0
            lax.fori_loop(0, strips * (length // span), step, 0)

        def span_of(slot):
            return slice(slot * count, (slot + 1) * count)

        def conv_stats(slot):
            values = conv[span_of(slot), :]
            local_sum = jnp.sum(values, axis=1, keepdims=True)
            dev = values - local_sum / chan
            st1[slot] = across_lanes(local_sum, jnp.sum(dev * dev, axis=1, keepdims=True))
            sg1[slot, me] = st1[slot]
            for d in range(1, T):
                stat(slot, st1.at[slot], sg1.at[slot, me], d).start()

        def activate(slot):
            arrived(sg1.at[slot, 0:3], sts.at[slot], str_.at[slot])
            sums = [sg1[slot, t] for t in range(T)]
            mean = sum(s[0:1, :] for s in sums) / (chan * T)
            spread = sum(
                s[1:2, :] + chan * (s[0:1, :] / chan - mean) * (s[0:1, :] / chan - mean) for s in sums
            ) / (chan * T)
            inv = lax.rsqrt(spread + EPS)
            table = down_rows(jnp.where(line == 0, mean, jnp.where(line == 1, inv, 0.0)))
            normed = (conv[span_of(slot), :] - table[:, 0:1]) * table[:, 1:2] * cg_ref[...]
            act[span_of(slot), :] = (normed * jax.nn.sigmoid(normed)).astype(BF16)

        def rs(slot, kind):
            if kind == 2:
                return remote(q1.at[slot], q1in.at[slot], rss.at[slot], rsr.at[slot, 0], {"tp": mir})
            return remote(
                part.at[slot, dia if kind else sib], got.at[slot, kind], rss.at[slot], rsr.at[slot, kind], {"tp": sib}
            )

        def project(slot):
            def step(j, _):
                prod = jnp.dot(act[span_of(slot), :], bo[j], preferred_element_type=F32)
                part[slot, j] = prod.astype(BF16)
                return 0
            lax.fori_loop(0, T, step, 0)
            rs(slot, 1).start()
            rs(slot, 0).start()

        def pair_sum(slot):
            rs(slot, 1).wait_recv()
            q1[slot] = (part[slot, mir].astype(F32) + got[slot, 1].astype(F32)).astype(BF16)
            rs(slot, 2).start()

        def finish_first(slot):
            arrived(part.at[slot, 0:2], rss.at[slot], rsr.at[slot, 0])
            total = xg[me, slot].astype(F32) + (part[slot, me].astype(F32) + got[slot, 0].astype(F32))
            firsts[me, slot] = (total + q1in[slot].astype(F32)).astype(BF16)
            ag_start(1, firsts, slot)

        convolve(0)
        conv_stats(0)
        convolve(1)
        conv_stats(1)
        relay_y(GA, 0, 0)
        own[CVO].wait()
        wait_y(CVO, 0)
        wait_y(CVO, 1)
        wait_z(CVO)
        activate(0)
        project(0)
        activate(1)
        project(1)
        pair_sum(0)
        relay_y(GA, 0, 1)
        relay_mid(GA, 0)
        pair_sum(1)
        relay_y(UP, 0, 0)
        relay_mid(GA, 1)
        relay_y(UP, 0, 1)
        finish_first(0)
        relay_mid(UP, 0)
        relay_y(GA, 1, 0)
        finish_first(1)
        relay_mid(UP, 1)
        send_own(DOWN)
        relay_y(GA, 1, 1)
        relay_y(UP, 1, 0)
        ag_forward(1, firsts, 0)
        ag_finish(1, firsts, 0)
        norm_rows(firsts, 0, mg_ref)
        relay_y(UP, 1, 1)
        ag_forward(1, firsts, 1)
        ag_finish(1, firsts, 1)
        relay_y(DOWN, 0, 0)
        relay_y(DOWN, 0, 1)
        norm_rows(firsts, 1, mg_ref)
        relay_y(DOWN, 0, 2)
        relay_y(DOWN, 0, 3)

        nf = chunk_of(ff, 256)

        def s5(w, shards, keep):
            def step(c, _):
                cols = pl.ds(pl.multiple_of(c * nf, nf), nf)
                value = sum(jnp.dot(rows[t], bufs[w][t, :, cols], preferred_element_type=F32) for t in shards)
                if keep:
                    accs[w - GA, :, cols] = value
                else:
                    gate = accs[0, :, cols]
                    hid[:, cols] = (gate * jax.nn.sigmoid(gate) * (value + accs[1, :, cols])).astype(BF16)
                return 0
            lax.fori_loop(0, ff // nf, step, 0)

        own[GA].wait()
        own[UP].wait()
        wait_y(GA, 0)
        wait_y(GA, 1)
        wait_z(GA)
        relay_mid(DOWN, 0)
        s5(GA, (f, pi, po, fo), True)
        relay_mid(DOWN, 1)
        wait_y(UP, 0)
        s5(UP, (f, pi), True)
        relay_y(DOWN, 0, 4)
        relay_y(DOWN, 0, 5)
        wait_z(UP)
        wait_y(UP, 1)
        s5(UP, (po, fo), False)

        def pair_send(b, j):
            at = (b, urows(j), ucols(j))
            return remote(part2.at[at], got2.at[at], ds_, dr.at[lax.rem(b // 2 + me // 2, 2), j], {"tp": sib})

        def cross(j):
            at = (urows(j), ucols(j))
            return remote(q2.at[at], q2in.at[at], qs, qr.at[j], {"tp": mir})

        def down(b, j):
            r, cols = urows(j), ucols(j)
            prod = jnp.dot(hid[r, :], bd[b, :, cols], preferred_element_type=F32)
            part2[b, r, cols] = prod.astype(BF16)

            @pl.when(jnp.logical_or(b == sib, b == dia))
            def _():
                pair_send(b, j).start()

        def combine(b, j):
            r, cols = urows(j), ucols(j)

            @pl.when(b == mir)
            def _():
                pair_send(b, j).wait_recv()
                q2[r, cols] = (part2[b, r, cols].astype(F32) + got2[b, r, cols].astype(F32)).astype(BF16)
                cross(j).start()

        def outer_stat(t):
            return remote(st2.at[0], finin.at[me], fs_, fr, {"fs": po, "tp": t})

        def finish(b, j):
            @pl.when(b == me)
            def _():
                pair_send(me, j).wait_recv()
                cross(j).wait_recv()
                cols = ucols(j)
                for slot in (j - 2,) if j in (2, 3) else (0, 1):
                    r = span_of(slot)
                    second = firsts[me, slot, :, cols].astype(F32) + part2[me, r, cols].astype(F32)
                    second = second + got2[me, r, cols].astype(F32) + q2in[r, cols].astype(F32)
                    total = jnp.sum(second * second, axis=1, keepdims=True)
                    if j not in (0, 4):
                        total = total + ssq[r, :]
                    if slot == 0:
                        secb[:, cols] = second.astype(BF16)
                    else:
                        sec[:, cols] = second
                    if j not in (2, 3):
                        ssq[r, :] = total
                    else:
                        st2[slot] = across_lanes(total, total)
                    if j == 2:
                        for t in (mir, dia, me, sib):
                            outer_stat(t).start()
                    if j == 3:
                        sg2[me] = st2[1]
                        for d in (2, 1, 3):
                            stat(2, st2.at[1], sg2.at[me], d).start()
                    if slot == 0:
                        result(cols, po).start()

        own[DOWN].wait()
        for c in range(6, 8):
            wait_mid(DOWN, 0, c)
        down(pi, 0)
        down(f, 0)
        relay_mid(DOWN, 2)
        relay_mid(DOWN, 3)
        combine(pi, 0)
        down(f, 1)
        combine(f, 0)
        wait_y_down(0, 1)
        down(pi, 1)
        relay_mid(DOWN, 4)
        relay_mid(DOWN, 5)
        relay_y(DOWN, 1, 0)
        relay_y(DOWN, 1, 1)
        combine(f, 1)
        combine(pi, 1)
        down(f, 2)
        down(f, 3)
        relay_mid(DOWN, 6)
        relay_mid(DOWN, 7)
        mid_direct(6).start()
        mid_direct(7).start()
        relay_y(DOWN, 1, 2)
        relay_y(DOWN, 1, 3)
        down(po, 0)
        down(fo, 4)
        relay_y(DOWN, 1, 4)
        relay_y(DOWN, 1, 5)
        combine(f, 2)
        combine(f, 3)
        combine(po, 0)
        combine(fo, 4)
        relay_y(DOWN, 1, 6)
        relay_y(DOWN, 1, 7)
        down(fo, 5)
        wait_y_down(1, 1)
        down(fo, 1)
        finish(f, 0)
        finish(pi, 0)
        combine(fo, 5)
        wait_z_down(1)
        down(po, 1)
        combine(fo, 1)
        wait_last()
        down(pi, 2)
        down(pi, 3)
        finish(f, 1)
        finish(pi, 1)
        combine(po, 1)
        wait_z_down(2)
        down(po, 2)
        down(po, 3)
        combine(pi, 2)
        combine(pi, 3)
        finish(po, 0)
        wait_y_down(1, 2)
        down(fo, 2)
        combine(po, 2)
        down(fo, 3)
        combine(fo, 2)
        combine(po, 3)
        combine(fo, 3)
        finish(fo, 4)
        finish(po, 1)
        finish(fo, 5)
        finish(fo, 1)
        for j in (2, 3):
            for b in (f, po, pi, fo):
                finish(b, j)
        arrived(sg2.at[0:3], sts.at[2], str_.at[2])
        table = down_rows(sum(sg2[t] for t in range(T)))
        scale = lax.rsqrt(table[:, 0:1] / width + EPS)
        out_ref[...] = (sec[...] * scale * fg_ref[...]).astype(BF16)

        def sent(ref, sem):
            remote(ref, ref, sem, sem, {"fs": f}).wait_send()

        all_sent(ms, 8)
        all_sent(ys, 7)
        sent(bufs[DOWN].at[f, 0:bd.shape[1] // 2, ucols(2)], md.at[0])
        for slot in range(2):
            sent(xg.at[0:3, slot], ags.at[0, slot])
            sent(firsts.at[0:3, slot], ags.at[1, slot])
            sent(part.at[slot, 0:3], rss.at[slot])
            sent(sg1.at[slot, 0:3], sts.at[slot])
        sent(sg2.at[0:3], sts.at[2])
        sent(part2.at[0:2], ds_)
        sent(q2, qs)
        sent(secb, os_)
        sent(finin, fs_)


def fast_body(
    activations, norm_gain, w_value, w_gate_conv, conv_weight, chan_gain,
    w_conv_out, mix_gain, w_gate, w_up, w_down, final_gain,
):
    batch, length, dt = activations.shape
    count = batch * length
    weights = (w_value, w_gate_conv, w_conv_out, w_gate, w_up, w_down)
    chan, ff = w_value.shape[1], w_gate.shape[1]
    T = 4
    pad = 8 * ((conv_weight.shape[0] - 1 + 7) // 8)
    rows_all = 2 * count
    vmem, hbm = pl.BlockSpec(memory_space=pltpu.VMEM), pl.BlockSpec(memory_space=pl.ANY)
    dma = pltpu.SemaphoreType.DMA
    V = pltpu.VMEM
    out = pl.pallas_call(
        functools.partial(fast_kernel, length),
        out_shape=pltpu.VMEM((count, dt), BF16),
        in_specs=[hbm] * 12,
        out_specs=vmem,
        scratch_shapes=[
            V((1, dt * T), F32),
            V(conv_weight.shape, F32),
            V((1, chan), F32),
            V((1, dt * T), F32),
            V((1, dt), F32),
        ] + [V((4,) + w.shape, BF16) for w in weights] + [
            V((T, 2, count, dt), BF16),
            V((T, rows_all, dt), BF16),
            V((rows_all, chan), F32),
            V((rows_all, chan), F32),
            V((2 * batch, pad + length + 8, chan), F32),
            V((rows_all, chan), F32),
            V((rows_all, chan), BF16),
            V((2, T, count, dt), BF16),
            V((2, 2, count, dt), BF16),
            V((2, count, dt), BF16),
            V((2, count, dt), BF16),
            V((T, 2, count, dt), BF16),
            V((rows_all, ff), BF16),
            V((2, rows_all, ff), F32),
            V((T, rows_all, dt), BF16),
            V((T, rows_all, dt), BF16),
            V((rows_all, dt), BF16),
            V((rows_all, dt), BF16),
            V((count, dt), F32),
            V((rows_all, 1), F32),
            V((count, dt), BF16),
            V((count, dt), BF16),
            V((2, 8, count), F32),
            V((2, T, 8, count), F32),
            V((2, 8, count), F32),
            V((T, 8, count), F32),
            V((T, 8, count), F32),
            dma((6,)),
            dma((6,)),
            dma((3,)),
            dma((sum(PIECES),)),
            dma((7,)),
            dma((3,)),
            dma((2, sum(PIECES))),
            dma((2,)),
            dma((3,)),
            dma((2, 7)),
            dma(()),
            dma(()),
            dma((2, 2)),
            dma((2, 2, 2)),
            dma((3,)),
            dma((3,)),
            dma((2,)),
            dma((2, 2)),
            dma(()),
            dma((2, 6)),
            dma(()),
            dma((6,)),
            dma(()),
            dma(()),
            dma(()),
            dma(()),
        ],
        compiler_params=pltpu.CompilerParams(
            collective_id=0, has_side_effects=True, vmem_limit_bytes=60 * 1024 * 1024
        ),
        name="block",
    )(
        activations.reshape(count, dt),
        norm_gain.reshape(1, dt * T),
        conv_weight,
        chan_gain.reshape(1, chan),
        mix_gain.reshape(1, dt * T),
        final_gain.reshape(1, dt),
        *weights,
    )
    return out.reshape(batch, length, dt)


def ring_body(
    activations, norm_gain, w_value, w_gate_conv, conv_weight, chan_gain,
    w_conv_out, mix_gain, w_gate, w_up, w_down, final_gain,
):
    batch, length, dt = activations.shape
    count = batch * length
    R, F, T = lax.axis_size("rep"), lax.axis_size("fs"), lax.axis_size("tp")
    weights = (w_value, w_gate_conv, w_conv_out, w_gate, w_up, w_down)
    split = 2 if R == 2 and all(w.shape[0] % 32 == 0 for w in weights) else 1
    width = dt * T
    chan, ff = w_value.shape[1], w_gate.shape[1]
    taps = conv_weight.shape[0]
    pad = 8 * ((taps - 1 + 7) // 8)
    vmem, hbm = pl.BlockSpec(memory_space=pltpu.VMEM), pl.BlockSpec(memory_space=pl.ANY)
    ysh = (2, 6, F) if split == 2 else (1,)
    dma = pltpu.SemaphoreType.DMA
    out = pl.pallas_call(
        functools.partial(ring_kernel, R, F, T, split, length),
        out_shape=jax.ShapeDtypeStruct((count, dt), BF16),
        in_specs=[vmem] * 6 + [hbm] * 6,
        out_specs=vmem,
        scratch_shapes=[pltpu.VMEM((F,) + w.shape, BF16) for w in weights] + [
            pltpu.VMEM((T, count, dt), BF16),
            pltpu.VMEM((count, width), BF16),
            pltpu.VMEM((batch, pad + length + 8, chan), F32),
            pltpu.VMEM((count, max(chan, dt)), F32),
            pltpu.VMEM((count, chan), BF16),
            pltpu.VMEM((T, count, dt), BF16),
            pltpu.VMEM((T, count, dt), BF16),
            pltpu.VMEM((T - 1, count, dt), BF16),
            pltpu.VMEM((T, count, dt), BF16),
            pltpu.VMEM((T, count, dt), BF16),
            pltpu.VMEM((count, ff), BF16),
            pltpu.VMEM((8, count), F32),
            pltpu.VMEM((8, count), F32),
            pltpu.VMEM((T, 8, count), F32),
            pltpu.VMEM((T, 8, count), F32),
            dma((6,)),
            dma((2, 6, F)),
            dma((2, 6, F)),
            dma(ysh),
            dma(ysh),
            dma((6, T)),
            dma((6, T)),
        ],
        compiler_params=pltpu.CompilerParams(
            collective_id=0, has_side_effects=True, vmem_limit_bytes=60 * 1024 * 1024
        ),
        name="block",
    )(
        activations.reshape(count, dt),
        norm_gain.reshape(T, dt),
        conv_weight,
        chan_gain.reshape(1, chan),
        mix_gain.reshape(T, dt),
        final_gain.reshape(1, dt),
        *weights,
    )
    return out.reshape(batch, length, dt)


def solution(mesh):
    in_specs = (
        P(("rep", "fs"), None, "tp"),
        P(),
        P("fs", "tp"),
        P("fs", "tp"),
        P(None, "tp"),
        P("tp"),
        P("tp", "fs"),
        P(),
        P("fs", "tp"),
        P("fs", "tp"),
        P("tp", "fs"),
        P("tp"),
    )
    out_specs = P(("rep", "fs"), None, "tp")
    fast = tuple(mesh.shape[a] for a in ("rep", "fs", "tp")) == (2, 4, 4)
    body = fast_body if fast else ring_body
    return jax.shard_map(body, mesh=mesh, in_specs=in_specs, out_specs=out_specs, check_vma=False)
```

```python
import functools

import jax
import jax.numpy as jnp
from jax import lax
from jax.experimental import pallas as pl
from jax.experimental.pallas import tpu as pltpu
from jax.sharding import PartitionSpec as P

EPS = 1e-06
MESH = pl.DeviceIdType.MESH
F32 = jnp.float32
BF16 = jnp.bfloat16


def remote(src, dst, send, recv, target):
    return pltpu.make_async_remote_copy(
        src_ref=src, dst_ref=dst, send_sem=send, recv_sem=recv, device_id=target, device_id_type=MESH
    )


def chunk_of(extent, want):
    return want if extent % want == 0 else extent


def ring_kernel(
    R, F, T, split, length,
    x_ref, ng_ref, cw_ref, cg_ref, mg_ref, fg_ref,
    wv_ref, wg_ref, wo_ref, wga_ref, wup_ref, wd_ref,
    out_ref,
    bv, bg, bo, bga, bup, bd,
    xg, rows, glu, conv, act, part1, part2, got1, got2, firsts, hid, st1, st2, sg1, sg2,
    own_sem, zs, zr, ys, yr, ts, tr,
):
    f = lax.axis_index("fs")
    me = lax.axis_index("tp")
    rep = lax.axis_index("rep")
    count, dt = x_ref.shape
    width = dt * T
    local = [wv_ref, wg_ref, wo_ref, wga_ref, wup_ref, wd_ref]
    bufs = [bv, bg, bo, bga, bup, bd]

    barrier = pltpu.get_barrier_semaphore()
    greeted = 0
    for target in (lax.rem(f + 1, F), lax.rem(f + F - 1, F)):
        pl.semaphore_signal(barrier, inc=1, device_id={"fs": target}, device_id_type=MESH)
        greeted += 1
    if split == 2:
        pl.semaphore_signal(barrier, inc=1, device_id={"rep": 1 - rep}, device_id_type=MESH)
        greeted += 1
    for d in range(1, T):
        pl.semaphore_signal(barrier, inc=1, device_id={"tp": lax.rem(me + d, T)}, device_id_type=MESH)
        greeted += 1
    own = [
        pltpu.make_async_copy(local[w], bufs[w].at[f], own_sem.at[w]) for w in range(6)
    ]
    for copy in own:
        copy.start()
    pl.semaphore_wait(barrier, greeted)

    def half(w):
        n = local[w].shape[0] // split
        return pl.ds(pl.multiple_of((rep if split == 2 else 0) * n, n), n)

    def other(w):
        n = local[w].shape[0] // split
        return pl.ds(pl.multiple_of((1 - rep) * n, n), n)

    def hop(w, side, s):
        shard = f - s if side == 0 else f + s
        target = f + 1 if side == 0 else f - 1
        src = local[w].at[half(w)] if s == 0 else bufs[w].at[shard, half(w)]
        return remote(src, bufs[w].at[shard, half(w)], zs.at[side, w, s], zr.at[side, w, s + 1], {"fs": target})

    def arrival(w, side, s):
        shard = f - s if side == 0 else f + s
        ref = bufs[w].at[shard, half(w)]
        return remote(ref, ref, zs.at[side, w, s], zr.at[side, w, s], {"fs": f})

    def across(w, side, s):
        shard = f - s if side == 0 else f + s
        ref = bufs[w].at[shard, half(w)]
        return remote(ref, ref, ys.at[side, w, s], yr.at[side, w, s], {"rep": 1 - rep})

    def across_in(w, side, s):
        shard = f - s if side == 0 else f + s
        ref = bufs[w].at[shard, other(w)]
        return remote(ref, ref, ys.at[side, w, s], yr.at[side, w, s], {"rep": 1 - rep})

    def has(side, s):
        return f >= s if side == 0 else f + s <= F - 1

    def sends(side, s):
        ahead = f < F - 1 if side == 0 else f > 0
        return jnp.logical_and(has(side, s), ahead)

    def launch(w):
        for side in (0, 1):
            @pl.when(sends(side, 0))
            def _():
                hop(w, side, 0).start()

    def relay(group, stages=range(1, F)):
        for s in stages:
            for w in group:
                for side in (0, 1):
                    @pl.when(has(side, s))
                    def _():
                        arrival(w, side, s).wait_recv()
                        if s < F - 1:
                            @pl.when(sends(side, s))
                            def _():
                                hop(w, side, s).start()
                        if split == 2:
                            across(w, side, s).start()

    def settle(group):
        for w in group:
            own[w].wait()
        if split == 2:
            for s in range(1, F):
                for w in group:
                    for side in (0, 1):
                        @pl.when(has(side, s))
                        def _():
                            across_in(w, side, s).wait_recv()

    def tp_send(k, src, dst_at, d):
        return remote(src, dst_at, ts.at[k, d], tr.at[k, d], {"tp": lax.rem(me + d, T)})

    for w in (0, 1):
        launch(w)
    for d in range(1, T):
        tp_send(0, x_ref, xg.at[me], d).start()
    launch(2)
    xg[me] = x_ref[...]
    for d in range(1, T):
        peer = lax.rem(me + T - d, T)
        tp_send(0, x_ref, xg.at[peer], d).wait_recv()

    block = chunk_of(count, 16)

    def norm_rows(src, gain):
        def step(i, _):
            r = pl.ds(pl.multiple_of(i * block, block), block)
            vals = [src[t, r, :].astype(F32) for t in range(T)]
            ss = sum(jnp.sum(v * v, axis=1, keepdims=True) for v in vals)
            scale = lax.rsqrt(ss / width + EPS)
            for t in range(T):
                rows[r, t * dt:(t + 1) * dt] = (
                    vals[t] * scale * gain[t:t + 1, :]
                ).astype(BF16)
            return 0
        lax.fori_loop(0, count // block, step, 0)

    norm_rows(xg, ng_ref)
    relay((0, 1, 2))
    for w in (3, 4, 5):
        launch(w)
    settle((0, 1))

    chan = bv.shape[2]
    batch = count // length
    taps = cw_ref.shape[0]
    pad = 8 * ((taps - 1 + 7) // 8)
    lead = pad - (taps - 1)

    def columns(buf, c, n):
        block_w = buf[:, :, pl.ds(pl.multiple_of(c * n, n), n)]
        return block_w.reshape(block_w.shape[0] * block_w.shape[1], n)

    nc = chunk_of(chan, 256)

    def glu_step(c, _):
        value = jnp.dot(rows[...], columns(bv, c, nc), preferred_element_type=F32)
        gate = jnp.dot(rows[...], columns(bg, c, nc), preferred_element_type=F32)
        res = value * jax.nn.sigmoid(gate)
        for b in range(batch):
            glu[b, pl.ds(pad, length), pl.ds(pl.multiple_of(c * nc, nc), nc)] = (
                res[b * length:(b + 1) * length]
            )
        return 0

    for b in range(batch):
        glu[b, 0:pad, :] = jnp.zeros((pad, chan), F32)
        glu[b, pad + length:, :] = jnp.zeros((8, chan), F32)
    lax.fori_loop(0, chan // nc, glu_step, 0)
    relay((3,), (1,))

    lanes = chunk_of(chan, 128)
    span = chunk_of(length, 64)
    strips = chan // lanes

    def conv_step(i, _):
        q = lax.rem(i, strips)
        p = i // strips
        cols = pl.ds(pl.multiple_of(q * lanes, lanes), lanes)
        weights = cw_ref[:, cols]
        for b in range(batch):
            total = jnp.zeros((span, lanes), F32)
            for shift in range(8):
                acc = None
                for tap in range(taps):
                    if (lead + tap) % 8 != shift:
                        continue
                    base = lead + tap - shift
                    term = weights[tap:tap + 1, :] * glu[
                        b, pl.ds(pl.multiple_of(p * span + base, 8), span + 8), cols
                    ]
                    acc = term if acc is None else acc + term
                if acc is not None:
                    total = total + acc[shift:shift + span]
            conv[pl.ds(pl.multiple_of(b * length + p * span, span), span), cols] = total
        return 0

    lax.fori_loop(0, strips * (length // span), conv_step, 0)

    lane = lax.broadcasted_iota(jnp.int32, (count, 128), 1)

    def across_lanes(a, b):
        table = jnp.where(lane == 0, a, jnp.where(lane == 1, b, 0.0))
        return jnp.transpose(table)[0:8, :]

    def down_rows(top):
        full = jnp.concatenate([top, jnp.zeros((120, count), F32)], axis=0)
        return jnp.transpose(full)

    values = conv[...]
    local_sum = jnp.sum(values, axis=1, keepdims=True)
    dev = values - local_sum / chan
    st1[...] = across_lanes(local_sum, jnp.sum(dev * dev, axis=1, keepdims=True))
    sg1[me] = st1[...]
    for d in range(1, T):
        tp_send(1, st1, sg1.at[me], d).start()
    relay((4,), (1,))
    for d in range(1, T):
        peer = lax.rem(me + T - d, T)
        tp_send(1, st1, sg1.at[peer], d).wait_recv()
    sums = [sg1[t] for t in range(T)]
    mean = sum(s[0:1, :] for s in sums) / (chan * T)
    spread = sum(
        s[1:2, :] + chan * (s[0:1, :] / chan - mean) * (s[0:1, :] / chan - mean) for s in sums
    ) / (chan * T)
    inv = lax.rsqrt(spread + EPS)
    line = lax.broadcasted_iota(jnp.int32, (8, count), 0)
    table = down_rows(jnp.where(line == 0, mean, jnp.where(line == 1, inv, 0.0)))
    normed = (conv[...] - table[:, 0:1]) * table[:, 1:2] * cg_ref[...]
    act[...] = (normed * jax.nn.sigmoid(normed)).astype(BF16)

    settle((2,))

    def project(src, buf, part):
        dsh = buf.shape[2]
        for j in range(F):
            t, off = (j * dsh) // dt, (j * dsh) % dt
            prod = jnp.dot(src[...], buf[j], preferred_element_type=F32)
            part[t, :, off:off + dsh] = prod.astype(BF16)

    def scatter(k, part, got):
        for d in range(1, T):
            tp_send(k, part.at[lax.rem(me + d, T)], got.at[d - 1], d).start()

    def gathered(k, part, got):
        total = part[me].astype(F32)
        for d in range(1, T):
            tp_send(k, part.at[me], got.at[d - 1], d).wait_recv()
            total = total + got[d - 1].astype(F32)
        return total

    def piece(t):
        return remote(part2.at[t], got2.at[me], ts.at[4, t], tr.at[4, me], {"tp": t})

    def piece_in(t):
        return remote(part2.at[t], got2.at[t], ts.at[4, t], tr.at[4, t], {"tp": t})

    project(act, bo, part1)
    scatter(2, part1, got1)
    relay((5,), (1,))
    first = (x_ref[...].astype(F32) + gathered(2, part1, got1)).astype(BF16)
    firsts[me] = first
    for d in range(1, T):
        tp_send(3, firsts.at[me], firsts.at[me], d).start()
    relay((3,), (2,))
    for d in range(1, T):
        peer = lax.rem(me + T - d, T)
        tp_send(3, firsts.at[peer], firsts.at[peer], d).wait_recv()
    relay((4,), (2,))
    norm_rows(firsts, mg_ref)
    relay((5,), (2,))
    relay((3, 4), range(3, F))
    settle((3, 4))

    ff = bga.shape[2]
    nf = chunk_of(ff, 256)

    def ff_step(c, _):
        gate = jnp.dot(rows[...], columns(bga, c, nf), preferred_element_type=F32)
        up = jnp.dot(rows[...], columns(bup, c, nf), preferred_element_type=F32)
        hid[:, pl.ds(pl.multiple_of(c * nf, nf), nf)] = (
            gate * jax.nn.sigmoid(gate) * up
        ).astype(BF16)
        return 0

    lax.fori_loop(0, ff // nf, ff_step, 0)
    if F == T and bd.shape[2] == dt:
        def down(shard):
            prod = jnp.dot(hid[...], bd[shard], preferred_element_type=F32)
            part2[shard] = prod.astype(BF16)

            @pl.when(shard != me)
            def _():
                piece(shard).start()

        own[5].wait()
        down(f)
        for s in range(1, F):
            if s >= 3:
                relay((5,), (s,))
            for side in (0, 1):
                @pl.when(has(side, s))
                def _():
                    if split == 2:
                        across_in(5, side, s).wait_recv()
                    down(f - s if side == 0 else f + s)
    else:
        relay((5,), range(3, F))
        settle((5,))
        project(hid, bd, part2)
        for d in range(1, T):
            piece(lax.rem(me + d, T)).start()
    second = firsts[me].astype(F32) + part2[me].astype(F32)
    for d in range(1, T):
        peer = lax.rem(me + d, T)
        piece_in(peer).wait_recv()
        second = second + got2[peer].astype(F32)
    total = jnp.sum(second * second, axis=1, keepdims=True)
    conv[:, 0:dt] = second
    st2[...] = across_lanes(total, total)
    sg2[me] = st2[...]
    for d in range(1, T):
        tp_send(5, st2, sg2.at[me], d).start()
    for d in range(1, T):
        peer = lax.rem(me + T - d, T)
        tp_send(5, st2, sg2.at[peer], d).wait_recv()
    full = sum(sg2[t] for t in range(T))
    table = down_rows(full)
    scale = lax.rsqrt(table[:, 0:1] / width + EPS)
    out_ref[...] = (conv[:, 0:dt] * scale * fg_ref[...]).astype(BF16)

    for w in range(6):
        for side in (0, 1):
            for s in range(F):
                if s < F - 1:
                    @pl.when(sends(side, s))
                    def _():
                        hop(w, side, s).wait_send()
                if s >= 1 and split == 2:
                    @pl.when(has(side, s))
                    def _():
                        across(w, side, s).wait_send()
    for d in range(1, T):
        peer = lax.rem(me + d, T)
        tp_send(0, x_ref, xg.at[me], d).wait_send()
        tp_send(1, st1, sg1.at[me], d).wait_send()
        tp_send(2, part1.at[peer], got1.at[d - 1], d).wait_send()
        tp_send(3, firsts.at[me], firsts.at[me], d).wait_send()
        piece(peer).wait_send()
        tp_send(5, st2, sg2.at[me], d).wait_send()


PIECES = (2, 2, 2, 2, 2, 8)
FIRST = tuple(sum(PIECES[:w]) for w in range(6))
GROUP = (0, 0, 0, 1, 1, 2)


def fast_kernel(
    length,
    x_ref, ng_hbm, cw_hbm, cg_hbm, mg_hbm, fg_hbm,
    wv_ref, wg_ref, wo_ref, wga_ref, wup_ref, wd_ref,
    out_ref,
    ng_ref, cw_ref, cg_ref, mg_ref, fg_ref, bv, bg, bo, bga, bup, bd,
    xg, rows, accv, accg, glu, conv, act, part, got, q1, q1in, firsts, hid,
    accs, part2, got2, q2, q2in, sec, ssq, secb, secin, st1, sg1, st2, sg2, finin,
    small, own_sem, zs, zr, zr2, ms, mr, md, ys, yr, xos, xor_, ags, agr, sts, str_, rss, rsr, ds_, dr, qs, qr, os_, orr, fs_, fr,
):
    f = lax.axis_index("fs")
    me = lax.axis_index("tp")
    rep = lax.axis_index("rep")
    count, dt = x_ref.shape
    T = 4
    width = dt * T
    rows_all = 2 * count
    batch = count // length
    chan, ff = bv.shape[2], bga.shape[2]
    local = [wv_ref, wg_ref, wo_ref, wga_ref, wup_ref, wd_ref]
    bufs = [bv, bg, bo, bga, bup, bd]
    VAL, GATE, CVO, GA, UP, DOWN = range(6)
    outer = jnp.logical_or(f == 0, f == 3)
    near = 1 + f // 3
    po, pi, fo = 3 * (f - 1), 3 - f, 3 * (2 - f)
    sib = me + 1 - 2 * lax.rem(me, 2)
    mir = lax.rem(me + 2, T)
    dia = lax.rem(sib + 2, T)

    def view(ref, w, h, c):
        if w == DOWN:
            n, m = ref.shape[1] // 2, ref.shape[0] // 4
            k = n // 2
            return ref.at[pl.ds((c % 4) * m, m), pl.ds(pl.multiple_of(h * n + (c // 4) * k, k), k)]
        n = ref.shape[0] // 2
        k = n // PIECES[w]
        return ref.at[pl.ds(pl.multiple_of(h * n + c * k, k), k), :]

    barrier = pltpu.get_barrier_semaphore()

    def greet(**target):
        pl.semaphore_signal(barrier, inc=1, device_id=target, device_id_type=MESH)

    def zsend(w, hs, c):
        h = rep if hs == 0 else 1 - rep
        sem = zr2.at[(c + 1 if c > 5 else w + c // 4) if w == DOWN else w] if hs else zr.at[FIRST[w] + c]
        return remote(view(local[w], w, h, c), view(bufs[w].at[f], w, h, c), zs.at[GROUP[w]], sem, {"fs": near})

    def all_sent(sems, eighths):
        n = bd.shape[1] * eighths // 8
        for g, ref in enumerate((bufs[VAL].at[0:3], bufs[GA].at[0:2], bufs[DOWN].at[0, 0:n, :])):
            remote(ref, ref, sems.at[g], sems.at[g], {"fs": f}).wait_send()

    def xsend():
        return remote(x_ref, xg.at[me, 0], xos, xor_, {"fs": near})

    hn = dt // 2

    def ucols(j):
        if j == 0:
            return pl.ds(pl.multiple_of(rep * hn, hn), hn)
        if j > 3:
            return pl.ds(pl.multiple_of(rep * hn + (j - 4) * (hn // 2), hn // 2), hn // 2)
        return pl.ds(pl.multiple_of((1 - rep) * hn + min(j - 1, 1) * (hn // 2), hn // 2), hn // 2)

    def urows(j):
        return slice((j - 2) * count, (j - 1) * count) if j in (2, 3) else slice(0, rows_all)

    def result(cols, target):
        return remote(secb.at[:, cols], secin.at[:, cols], os_, orr, {"fs": target})

    smalls = [
        pltpu.make_async_copy(src, dst, small.at[k])
        for k, (src, dst) in enumerate(
            ((ng_hbm, ng_ref), (cw_hbm, cw_ref), (cg_hbm, cg_ref), (mg_hbm, mg_ref), (fg_hbm, fg_ref))
        )
    ]

    lane = lax.broadcasted_iota(jnp.int32, (count, 128), 1)
    line = lax.broadcasted_iota(jnp.int32, (8, count), 0)

    def across_lanes(a, b):
        table = jnp.where(lane == 0, a, jnp.where(lane == 1, b, 0.0))
        return jnp.transpose(table)[0:8, :]

    def down_rows(top):
        full = jnp.concatenate([top, jnp.zeros((120, count), F32)], axis=0)
        return jnp.transpose(full)

    @pl.when(outer)
    def _():
        greet(fs=near)
        smalls[4].start()
        pl.semaphore_wait(barrier, 1)
        order = [
            (VAL, 0), (GATE, 0), None, (CVO, 0), (VAL, 1), (GATE, 1), (CVO, 1),
            (GA, 0), (UP, 0), (GA, 1),
        ]
        for item in order:
            if item is None:
                xsend().start()
            else:
                for c in range(PIECES[item[0]]):
                    zsend(item[0], item[1], c).start()
        zsend(UP, 1, 0).start()
        zsend(DOWN, 0, 0).start()
        zsend(DOWN, 0, 1).start()
        zsend(UP, 1, 1).start()
        for c in range(2, PIECES[DOWN]):
            zsend(DOWN, 0, c).start()
        for c in (6, 7, 0, 1, 2, 3, 4, 5):
            zsend(DOWN, 1, c).start()
        xsend().wait_send()
        all_sent(zs, 8)
        smalls[4].wait()
        remote(secb, secin, os_, orr, {"fs": near}).wait_recv()
        remote(finin, finin, fs_, fr, {"fs": near}).wait_recv()
        full = sum(finin[t] for t in range(T))
        scale = lax.rsqrt(down_rows(full)[:, 0:1] / width + EPS)
        out_ref[...] = (secin[...].astype(F32) * scale * fg_ref[...]).astype(BF16)

    @pl.when(jnp.logical_not(outer))
    def _():
        greet(fs=po)
        greet(fs=pi)
        greet(rep=1 - rep)
        for t in (sib, mir):
            greet(tp=t)
        own = [pltpu.make_async_copy(local[w], bufs[w].at[f], own_sem.at[w]) for w in range(6)]
        load_x = pltpu.make_async_copy(x_ref, xg.at[me, 1], small.at[5])
        load_x.start()
        for copy in smalls:
            copy.start()
        for copy in own:
            copy.start()
        pl.semaphore_wait(barrier, 5)

        def arrived(ref, send, recv):
            remote(ref, ref, send, recv, {"fs": f}).wait_recv()

        def mid_own(w, c):
            return remote(
                view(local[w], w, rep, c), view(bufs[w].at[f], w, rep, c), ms.at[GROUP[w]], mr.at[0, FIRST[w] + c], {"fs": pi}
            )

        def mid_fwd(w, c):
            ref = view(bufs[w].at[po], w, rep, c)
            return remote(ref, ref, ms.at[GROUP[w]], mr.at[1, FIRST[w] + c], {"fs": pi})

        def mid_direct(c):
            ref = view(bufs[DOWN].at[po], DOWN, 1 - rep, c)
            return remote(ref, ref, md.at[0], md.at[1], {"fs": pi})

        def relay_direct(c):
            arrived(view(bufs[DOWN].at[po], DOWN, 1 - rep, c), zs.at[2], zr2.at[c + 1])
            mid_direct(c).start()

        def y_fwd(w, k, c):
            ref = view(bufs[w].at[fo if k else pi], w, rep, c)
            sem = yr.at[k, w + c // 4 if w == DOWN else w]
            return remote(ref, ref, ys.at[GROUP[w]], sem, {"rep": 1 - rep})

        def wait_z_down(j):
            n = bd.shape[1] // (1 if j == 1 else 2)
            arrived(bufs[DOWN].at[po, 0:n, ucols(j)], zs.at[2], zr2.at[DOWN + j - 1])

        def send_own(w):
            for c in range(PIECES[w]):
                mid_own(w, c).start()

        def relay_mid(w, c):
            arrived(view(bufs[w].at[po], w, rep, c), zs.at[GROUP[w]], zr.at[FIRST[w] + c])
            mid_fwd(w, c).start()

        def wait_mid(w, k, c):
            arrived(view(bufs[w].at[fo if k else pi], w, rep, c), ms.at[GROUP[w]], mr.at[k, FIRST[w] + c])

        def relay_y(w, k, c):
            wait_mid(w, k, c)
            y_fwd(w, k, c).start()

        def other(w, shard):
            n = bufs[w].shape[1] // 2
            return bufs[w].at[shard, pl.ds(pl.multiple_of((1 - rep) * n, n), n), :]

        def wait_z(w):
            arrived(other(w, po), zs.at[GROUP[w]], zr2.at[w])

        def wait_y(w, k):
            arrived(other(w, fo if k else pi), ys.at[GROUP[w]], yr.at[k, w])

        def wait_y_down(k, j):
            ref = bufs[DOWN].at[fo if k else pi, :, ucols(j)]
            arrived(ref, ys.at[2], yr.at[k, DOWN + j - 1])

        def wait_last():
            m = bd.shape[1] // 2
            arrived(bufs[DOWN].at[fo, 0:m, ucols(2)], ys.at[2], yr.at[1, 6])
            arrived(bufs[DOWN].at[fo, m:2 * m, ucols(2)], md.at[0], md.at[1])

        def ag(p, buf, slot, kind):
            ref = buf.at[mir if kind == 2 else me, slot]
            return remote(
                ref, ref, ags.at[p, slot], agr.at[p, slot, 1 if kind == 1 else 0], {"tp": mir if kind == 1 else sib}
            )

        def ag_start(p, buf, slot):
            ag(p, buf, slot, 1).start()
            ag(p, buf, slot, 0).start()

        def ag_forward(p, buf, slot):
            arrived(buf.at[mir, slot], ags.at[p, slot], agr.at[p, slot, 1])
            ag(p, buf, slot, 2).start()

        def ag_finish(p, buf, slot):
            arrived(buf.at[0:2, slot], ags.at[p, slot], agr.at[p, slot, 0])

        block = chunk_of(count, 32)

        def norm_rows(src, slot, gain):
            def step(i, _):
                r = pl.ds(pl.multiple_of(i * block, block), block)
                o = pl.ds(pl.multiple_of(slot * count + i * block, block), block)
                vals = [src[t, slot, r, :].astype(F32) for t in range(T)]
                ss = sum(jnp.sum(v * v, axis=1, keepdims=True) for v in vals)
                scale = lax.rsqrt(ss / width + EPS)
                for t in range(T):
                    rows[t, o, :] = (vals[t] * scale * gain[:, t * dt:(t + 1) * dt]).astype(BF16)
                return 0
            lax.fori_loop(0, count // block, step, 0)

        def stat(k, src, dst, d):
            return remote(src, dst, sts.at[k], str_.at[k], {"tp": lax.rem(me + d, T)})

        send_own(VAL)
        send_own(GATE)
        load_x.wait()
        ag_start(0, xg, 1)
        for c in range(2):
            relay_mid(VAL, c)
            relay_y(VAL, 0, c)
        relay_mid(GATE, 0)
        ag_forward(0, xg, 1)
        relay_y(GATE, 0, 0)
        relay_mid(GATE, 1)
        relay_y(GATE, 0, 1)
        send_own(CVO)
        ag_finish(0, xg, 1)
        for copy in smalls:
            copy.wait()
        norm_rows(xg, 1, ng_ref)
        relay_y(VAL, 1, 0)
        arrived(xg.at[me, 0], xos, xor_)
        ag_start(0, xg, 0)
        relay_y(VAL, 1, 1)
        relay_mid(CVO, 0)
        relay_y(GATE, 1, 0)
        relay_mid(CVO, 1)
        send_own(GA)
        send_own(UP)
        relay_y(GATE, 1, 1)
        ag_forward(0, xg, 0)
        ag_finish(0, xg, 0)
        norm_rows(xg, 0, ng_ref)
        relay_y(CVO, 0, 0)

        pad = glu.shape[1] - length - 8
        taps = cw_ref.shape[0]
        lead = pad - (taps - 1)
        nc = chunk_of(chan, 256)
        for b in range(2 * batch):
            glu[b, 0:pad, :] = jnp.zeros((pad, chan), F32)
            glu[b, pad + length:, :] = jnp.zeros((8, chan), F32)

        def s1(shard, first, last):
            def step(c, _):
                cols = pl.ds(pl.multiple_of(c * nc, nc), nc)
                value = jnp.dot(rows[shard], bv[shard, :, cols], preferred_element_type=F32)
                gate = jnp.dot(rows[shard], bg[shard, :, cols], preferred_element_type=F32)
                if not first:
                    value = value + accv[:, cols]
                    gate = gate + accg[:, cols]
                if last:
                    res = value * jax.nn.sigmoid(gate)
                    for b in range(2 * batch):
                        glu[b, pl.ds(pad, length), cols] = res[b * length:(b + 1) * length]
                else:
                    accv[:, cols] = value
                    accg[:, cols] = gate
                return 0
            lax.fori_loop(0, chan // nc, step, 0)

        own[VAL].wait()
        own[GATE].wait()
        s1(f, True, False)
        wait_y(VAL, 0)
        wait_y(GATE, 0)
        s1(pi, False, False)
        relay_y(CVO, 0, 1)
        wait_y(VAL, 1)
        wait_y(GATE, 1)
        s1(fo, False, False)
        relay_y(CVO, 1, 0)
        wait_z(VAL)
        wait_z(GATE)
        s1(po, False, True)
        relay_y(CVO, 1, 1)

        lanes = chunk_of(chan, 128)
        span = chunk_of(length, 64)
        strips = chan // lanes

        def convolve(slot):
            def step(i, _):
                s = lax.rem(i, strips)
                p = i // strips
                cols = pl.ds(pl.multiple_of(s * lanes, lanes), lanes)
                weights = cw_ref[:, cols]
                for b in range(batch):
                    total = jnp.zeros((span, lanes), F32)
                    for shift in range(8):
                        acc = None
                        for tap in range(taps):
                            if (lead + tap) % 8 != shift:
                                continue
                            base = lead + tap - shift
                            term = weights[tap:tap + 1, :] * glu[
                                slot * batch + b, pl.ds(pl.multiple_of(p * span + base, 8), span + 8), cols
                            ]
                            acc = term if acc is None else acc + term
                        if acc is not None:
                            total = total + acc[shift:shift + span]
                    at = pl.multiple_of(slot * count + b * length + p * span, span)
                    conv[pl.ds(at, span), cols] = total
                return 0
            lax.fori_loop(0, strips * (length // span), step, 0)

        def span_of(slot):
            return slice(slot * count, (slot + 1) * count)

        def conv_stats(slot):
            values = conv[span_of(slot), :]
            local_sum = jnp.sum(values, axis=1, keepdims=True)
            dev = values - local_sum / chan
            st1[slot] = across_lanes(local_sum, jnp.sum(dev * dev, axis=1, keepdims=True))
            sg1[slot, me] = st1[slot]
            for d in range(1, T):
                stat(slot, st1.at[slot], sg1.at[slot, me], d).start()

        def activate(slot):
            arrived(sg1.at[slot, 0:3], sts.at[slot], str_.at[slot])
            sums = [sg1[slot, t] for t in range(T)]
            mean = sum(s[0:1, :] for s in sums) / (chan * T)
            spread = sum(
                s[1:2, :] + chan * (s[0:1, :] / chan - mean) * (s[0:1, :] / chan - mean) for s in sums
            ) / (chan * T)
            inv = lax.rsqrt(spread + EPS)
            table = down_rows(jnp.where(line == 0, mean, jnp.where(line == 1, inv, 0.0)))
            normed = (conv[span_of(slot), :] - table[:, 0:1]) * table[:, 1:2] * cg_ref[...]
            act[span_of(slot), :] = (normed * jax.nn.sigmoid(normed)).astype(BF16)

        def rs(slot, kind):
            if kind == 2:
                return remote(q1.at[slot], q1in.at[slot], rss.at[slot], rsr.at[slot, 0], {"tp": mir})
            return remote(
                part.at[slot, dia if kind else sib], got.at[slot, kind], rss.at[slot], rsr.at[slot, kind], {"tp": sib}
            )

        def project(slot):
            def step(j, _):
                prod = jnp.dot(act[span_of(slot), :], bo[j], preferred_element_type=F32)
                part[slot, j] = prod.astype(BF16)
                return 0
            lax.fori_loop(0, T, step, 0)
            rs(slot, 1).start()
            rs(slot, 0).start()

        def pair_sum(slot):
            rs(slot, 1).wait_recv()
            q1[slot] = (part[slot, mir].astype(F32) + got[slot, 1].astype(F32)).astype(BF16)
            rs(slot, 2).start()

        def finish_first(slot):
            arrived(part.at[slot, 0:2], rss.at[slot], rsr.at[slot, 0])
            total = xg[me, slot].astype(F32) + (part[slot, me].astype(F32) + got[slot, 0].astype(F32))
            firsts[me, slot] = (total + q1in[slot].astype(F32)).astype(BF16)
            ag_start(1, firsts, slot)

        convolve(0)
        conv_stats(0)
        convolve(1)
        conv_stats(1)
        relay_y(GA, 0, 0)
        own[CVO].wait()
        wait_y(CVO, 0)
        wait_y(CVO, 1)
        wait_z(CVO)
        activate(0)
        project(0)
        activate(1)
        project(1)
        pair_sum(0)
        relay_y(GA, 0, 1)
        relay_mid(GA, 0)
        pair_sum(1)
        relay_y(UP, 0, 0)
        relay_mid(GA, 1)
        relay_y(UP, 0, 1)
        finish_first(0)
        relay_mid(UP, 0)
        relay_y(GA, 1, 0)
        finish_first(1)
        relay_mid(UP, 1)
        send_own(DOWN)
        relay_y(GA, 1, 1)
        relay_y(UP, 1, 0)
        ag_forward(1, firsts, 0)
        ag_finish(1, firsts, 0)
        norm_rows(firsts, 0, mg_ref)
        relay_y(UP, 1, 1)
        ag_forward(1, firsts, 1)
        ag_finish(1, firsts, 1)
        relay_y(DOWN, 0, 0)
        relay_y(DOWN, 0, 1)
        norm_rows(firsts, 1, mg_ref)
        relay_y(DOWN, 0, 2)
        relay_y(DOWN, 0, 3)

        nf = chunk_of(ff, 256)

        def s5(w, shards, keep):
            def step(c, _):
                cols = pl.ds(pl.multiple_of(c * nf, nf), nf)
                value = sum(jnp.dot(rows[t], bufs[w][t, :, cols], preferred_element_type=F32) for t in shards)
                if keep:
                    accs[w - GA, :, cols] = value
                else:
                    gate = accs[0, :, cols]
                    hid[:, cols] = (gate * jax.nn.sigmoid(gate) * (value + accs[1, :, cols])).astype(BF16)
                return 0
            lax.fori_loop(0, ff // nf, step, 0)

        own[GA].wait()
        own[UP].wait()
        wait_y(GA, 0)
        wait_y(GA, 1)
        wait_z(GA)
        relay_mid(DOWN, 0)
        s5(GA, (f, pi, po, fo), True)
        relay_mid(DOWN, 1)
        wait_y(UP, 0)
        s5(UP, (f, pi), True)
        relay_y(DOWN, 0, 4)
        for c in range(5, 8):
            relay_y(DOWN, 0, c)
        wait_z(UP)
        wait_y(UP, 1)
        s5(UP, (po, fo), False)

        def pair_send(b, j):
            at = (b, urows(j), ucols(j))
            return remote(part2.at[at], got2.at[at], ds_, dr.at[lax.rem(b // 2 + me // 2, 2), j], {"tp": sib})

        def cross(j):
            at = (urows(j), ucols(j))
            return remote(q2.at[at], q2in.at[at], qs, qr.at[j], {"tp": mir})

        def down(b, j):
            r, cols = urows(j), ucols(j)
            prod = jnp.dot(hid[r, :], bd[b, :, cols], preferred_element_type=F32)
            part2[b, r, cols] = prod.astype(BF16)

            @pl.when(jnp.logical_or(b == sib, b == dia))
            def _():
                pair_send(b, j).start()

        def combine(b, j):
            r, cols = urows(j), ucols(j)

            @pl.when(b == mir)
            def _():
                pair_send(b, j).wait_recv()
                q2[r, cols] = (part2[b, r, cols].astype(F32) + got2[b, r, cols].astype(F32)).astype(BF16)
                cross(j).start()

        def outer_stat(t):
            return remote(st2.at[0], finin.at[me], fs_, fr, {"fs": po, "tp": t})

        def finish(b, j):
            @pl.when(b == me)
            def _():
                pair_send(me, j).wait_recv()
                cross(j).wait_recv()
                cols = ucols(j)
                for slot in (j - 2,) if j in (2, 3) else (0, 1):
                    r = span_of(slot)
                    second = firsts[me, slot, :, cols].astype(F32) + part2[me, r, cols].astype(F32)
                    second = second + got2[me, r, cols].astype(F32) + q2in[r, cols].astype(F32)
                    total = jnp.sum(second * second, axis=1, keepdims=True)
                    if j not in (0, 4):
                        total = total + ssq[r, :]
                    if slot == 0:
                        secb[:, cols] = second.astype(BF16)
                    else:
                        sec[:, cols] = second
                    if j not in (2, 3):
                        ssq[r, :] = total
                    else:
                        st2[slot] = across_lanes(total, total)
                    if j == 2:
                        for t in (mir, dia, me, sib):
                            outer_stat(t).start()
                    if j == 3:
                        sg2[me] = st2[1]
                        for d in (2, 1, 3):
                            stat(2, st2.at[1], sg2.at[me], d).start()
                    if slot == 0:
                        result(cols, po).start()

        own[DOWN].wait()
        down(pi, 0)
        down(f, 0)
        relay_mid(DOWN, 2)
        relay_mid(DOWN, 3)
        combine(pi, 0)
        down(f, 1)
        combine(f, 0)
        wait_y_down(0, 1)
        down(pi, 1)
        relay_mid(DOWN, 4)
        relay_mid(DOWN, 5)
        relay_y(DOWN, 1, 0)
        relay_y(DOWN, 1, 1)
        combine(f, 1)
        combine(pi, 1)
        down(f, 2)
        down(f, 3)
        relay_mid(DOWN, 6)
        relay_mid(DOWN, 7)
        relay_y(DOWN, 1, 2)
        relay_y(DOWN, 1, 3)
        down(po, 0)
        down(fo, 4)
        relay_direct(6)
        relay_direct(7)
        relay_y(DOWN, 1, 4)
        relay_y(DOWN, 1, 5)
        combine(f, 2)
        combine(f, 3)
        combine(po, 0)
        combine(fo, 4)
        wait_y_down(0, 2)
        down(pi, 2)
        down(pi, 3)
        wait_mid(DOWN, 1, 6)
        wait_mid(DOWN, 1, 7)
        down(fo, 5)
        combine(pi, 2)
        combine(pi, 3)
        wait_y_down(1, 1)
        down(fo, 1)
        finish(f, 0)
        finish(pi, 0)
        combine(fo, 5)
        wait_z_down(1)
        down(po, 1)
        combine(fo, 1)
        wait_last()
        down(fo, 2)
        finish(f, 1)
        finish(pi, 1)
        combine(po, 1)
        down(fo, 3)
        wait_z_down(2)
        down(po, 2)
        combine(fo, 2)
        down(po, 3)
        finish(po, 0)
        combine(po, 2)
        combine(fo, 3)
        combine(po, 3)
        finish(fo, 4)
        finish(po, 1)
        finish(fo, 5)
        finish(fo, 1)
        for j in (2, 3):
            for b in (f, po, pi, fo):
                finish(b, j)
        arrived(sg2.at[0:3], sts.at[2], str_.at[2])
        table = down_rows(sum(sg2[t] for t in range(T)))
        scale = lax.rsqrt(table[:, 0:1] / width + EPS)
        out_ref[...] = (sec[...] * scale * fg_ref[...]).astype(BF16)

        def sent(ref, sem):
            remote(ref, ref, sem, sem, {"fs": f}).wait_send()

        all_sent(ms, 8)
        all_sent(ys, 7)
        sent(bufs[DOWN].at[f, 0:bd.shape[1] // 2, ucols(2)], md.at[0])
        for slot in range(2):
            sent(xg.at[0:3, slot], ags.at[0, slot])
            sent(firsts.at[0:3, slot], ags.at[1, slot])
            sent(part.at[slot, 0:3], rss.at[slot])
            sent(sg1.at[slot, 0:3], sts.at[slot])
        sent(sg2.at[0:3], sts.at[2])
        sent(part2.at[0:2], ds_)
        sent(q2, qs)
        sent(secb, os_)
        sent(finin, fs_)


def fast_body(
    activations, norm_gain, w_value, w_gate_conv, conv_weight, chan_gain,
    w_conv_out, mix_gain, w_gate, w_up, w_down, final_gain,
):
    batch, length, dt = activations.shape
    count = batch * length
    weights = (w_value, w_gate_conv, w_conv_out, w_gate, w_up, w_down)
    chan, ff = w_value.shape[1], w_gate.shape[1]
    T = 4
    pad = 8 * ((conv_weight.shape[0] - 1 + 7) // 8)
    rows_all = 2 * count
    vmem, hbm = pl.BlockSpec(memory_space=pltpu.VMEM), pl.BlockSpec(memory_space=pl.ANY)
    dma = pltpu.SemaphoreType.DMA
    V = pltpu.VMEM
    out = pl.pallas_call(
        functools.partial(fast_kernel, length),
        out_shape=pltpu.VMEM((count, dt), BF16),
        in_specs=[hbm] * 12,
        out_specs=vmem,
        scratch_shapes=[
            V((1, dt * T), F32),
            V(conv_weight.shape, F32),
            V((1, chan), F32),
            V((1, dt * T), F32),
            V((1, dt), F32),
        ] + [V((4,) + w.shape, BF16) for w in weights] + [
            V((T, 2, count, dt), BF16),
            V((T, rows_all, dt), BF16),
            V((rows_all, chan), F32),
            V((rows_all, chan), F32),
            V((2 * batch, pad + length + 8, chan), F32),
            V((rows_all, chan), F32),
            V((rows_all, chan), BF16),
            V((2, T, count, dt), BF16),
            V((2, 2, count, dt), BF16),
            V((2, count, dt), BF16),
            V((2, count, dt), BF16),
            V((T, 2, count, dt), BF16),
            V((rows_all, ff), BF16),
            V((2, rows_all, ff), F32),
            V((T, rows_all, dt), BF16),
            V((T, rows_all, dt), BF16),
            V((rows_all, dt), BF16),
            V((rows_all, dt), BF16),
            V((count, dt), F32),
            V((rows_all, 1), F32),
            V((count, dt), BF16),
            V((count, dt), BF16),
            V((2, 8, count), F32),
            V((2, T, 8, count), F32),
            V((2, 8, count), F32),
            V((T, 8, count), F32),
            V((T, 8, count), F32),
            dma((6,)),
            dma((6,)),
            dma((3,)),
            dma((sum(PIECES),)),
            dma((9,)),
            dma((3,)),
            dma((2, sum(PIECES))),
            dma((2,)),
            dma((3,)),
            dma((2, 7)),
            dma(()),
            dma(()),
            dma((2, 2)),
            dma((2, 2, 2)),
            dma((3,)),
            dma((3,)),
            dma((2,)),
            dma((2, 2)),
            dma(()),
            dma((2, 6)),
            dma(()),
            dma((6,)),
            dma(()),
            dma(()),
            dma(()),
            dma(()),
        ],
        compiler_params=pltpu.CompilerParams(
            collective_id=0, has_side_effects=True, vmem_limit_bytes=60 * 1024 * 1024
        ),
        name="block",
    )(
        activations.reshape(count, dt),
        norm_gain.reshape(1, dt * T),
        conv_weight,
        chan_gain.reshape(1, chan),
        mix_gain.reshape(1, dt * T),
        final_gain.reshape(1, dt),
        *weights,
    )
    return out.reshape(batch, length, dt)


def ring_body(
    activations, norm_gain, w_value, w_gate_conv, conv_weight, chan_gain,
    w_conv_out, mix_gain, w_gate, w_up, w_down, final_gain,
):
    batch, length, dt = activations.shape
    count = batch * length
    R, F, T = lax.axis_size("rep"), lax.axis_size("fs"), lax.axis_size("tp")
    weights = (w_value, w_gate_conv, w_conv_out, w_gate, w_up, w_down)
    split = 2 if R == 2 and all(w.shape[0] % 32 == 0 for w in weights) else 1
    width = dt * T
    chan, ff = w_value.shape[1], w_gate.shape[1]
    taps = conv_weight.shape[0]
    pad = 8 * ((taps - 1 + 7) // 8)
    vmem, hbm = pl.BlockSpec(memory_space=pltpu.VMEM), pl.BlockSpec(memory_space=pl.ANY)
    ysh = (2, 6, F) if split == 2 else (1,)
    dma = pltpu.SemaphoreType.DMA
    out = pl.pallas_call(
        functools.partial(ring_kernel, R, F, T, split, length),
        out_shape=jax.ShapeDtypeStruct((count, dt), BF16),
        in_specs=[vmem] * 6 + [hbm] * 6,
        out_specs=vmem,
        scratch_shapes=[pltpu.VMEM((F,) + w.shape, BF16) for w in weights] + [
            pltpu.VMEM((T, count, dt), BF16),
            pltpu.VMEM((count, width), BF16),
            pltpu.VMEM((batch, pad + length + 8, chan), F32),
            pltpu.VMEM((count, max(chan, dt)), F32),
            pltpu.VMEM((count, chan), BF16),
            pltpu.VMEM((T, count, dt), BF16),
            pltpu.VMEM((T, count, dt), BF16),
            pltpu.VMEM((T - 1, count, dt), BF16),
            pltpu.VMEM((T, count, dt), BF16),
            pltpu.VMEM((T, count, dt), BF16),
            pltpu.VMEM((count, ff), BF16),
            pltpu.VMEM((8, count), F32),
            pltpu.VMEM((8, count), F32),
            pltpu.VMEM((T, 8, count), F32),
            pltpu.VMEM((T, 8, count), F32),
            dma((6,)),
            dma((2, 6, F)),
            dma((2, 6, F)),
            dma(ysh),
            dma(ysh),
            dma((6, T)),
            dma((6, T)),
        ],
        compiler_params=pltpu.CompilerParams(
            collective_id=0, has_side_effects=True, vmem_limit_bytes=60 * 1024 * 1024
        ),
        name="block",
    )(
        activations.reshape(count, dt),
        norm_gain.reshape(T, dt),
        conv_weight,
        chan_gain.reshape(1, chan),
        mix_gain.reshape(T, dt),
        final_gain.reshape(1, dt),
        *weights,
    )
    return out.reshape(batch, length, dt)


def solution(mesh):
    in_specs = (
        P(("rep", "fs"), None, "tp"),
        P(),
        P("fs", "tp"),
        P("fs", "tp"),
        P(None, "tp"),
        P("tp"),
        P("tp", "fs"),
        P(),
        P("fs", "tp"),
        P("fs", "tp"),
        P("tp", "fs"),
        P("tp"),
    )
    out_specs = P(("rep", "fs"), None, "tp")
    fast = tuple(mesh.shape[a] for a in ("rep", "fs", "tp")) == (2, 4, 4)
    body = fast_body if fast else ring_body
    return jax.shard_map(body, mesh=mesh, in_specs=in_specs, out_specs=out_specs, check_vma=False)
```

```python
import functools

import jax
import jax.numpy as jnp
from jax import lax
from jax.experimental import pallas as pl
from jax.experimental.pallas import tpu as pltpu
from jax.sharding import PartitionSpec as P

EPS = 1e-06
MESH = pl.DeviceIdType.MESH
F32 = jnp.float32
BF16 = jnp.bfloat16


def remote(src, dst, send, recv, target):
    return pltpu.make_async_remote_copy(
        src_ref=src, dst_ref=dst, send_sem=send, recv_sem=recv, device_id=target, device_id_type=MESH
    )


def chunk_of(extent, want):
    return want if extent % want == 0 else extent


def ring_kernel(
    R, F, T, split, length,
    x_ref, ng_ref, cw_ref, cg_ref, mg_ref, fg_ref,
    wv_ref, wg_ref, wo_ref, wga_ref, wup_ref, wd_ref,
    out_ref,
    bv, bg, bo, bga, bup, bd,
    xg, rows, glu, conv, act, part1, part2, got1, got2, firsts, hid, st1, st2, sg1, sg2,
    own_sem, zs, zr, ys, yr, ts, tr,
):
    f = lax.axis_index("fs")
    me = lax.axis_index("tp")
    rep = lax.axis_index("rep")
    count, dt = x_ref.shape
    width = dt * T
    local = [wv_ref, wg_ref, wo_ref, wga_ref, wup_ref, wd_ref]
    bufs = [bv, bg, bo, bga, bup, bd]

    barrier = pltpu.get_barrier_semaphore()
    greeted = 0
    for target in (lax.rem(f + 1, F), lax.rem(f + F - 1, F)):
        pl.semaphore_signal(barrier, inc=1, device_id={"fs": target}, device_id_type=MESH)
        greeted += 1
    if split == 2:
        pl.semaphore_signal(barrier, inc=1, device_id={"rep": 1 - rep}, device_id_type=MESH)
        greeted += 1
    for d in range(1, T):
        pl.semaphore_signal(barrier, inc=1, device_id={"tp": lax.rem(me + d, T)}, device_id_type=MESH)
        greeted += 1
    own = [
        pltpu.make_async_copy(local[w], bufs[w].at[f], own_sem.at[w]) for w in range(6)
    ]
    for copy in own:
        copy.start()
    pl.semaphore_wait(barrier, greeted)

    def half(w):
        n = local[w].shape[0] // split
        return pl.ds(pl.multiple_of((rep if split == 2 else 0) * n, n), n)

    def other(w):
        n = local[w].shape[0] // split
        return pl.ds(pl.multiple_of((1 - rep) * n, n), n)

    def hop(w, side, s):
        shard = f - s if side == 0 else f + s
        target = f + 1 if side == 0 else f - 1
        src = local[w].at[half(w)] if s == 0 else bufs[w].at[shard, half(w)]
        return remote(src, bufs[w].at[shard, half(w)], zs.at[side, w, s], zr.at[side, w, s + 1], {"fs": target})

    def arrival(w, side, s):
        shard = f - s if side == 0 else f + s
        ref = bufs[w].at[shard, half(w)]
        return remote(ref, ref, zs.at[side, w, s], zr.at[side, w, s], {"fs": f})

    def across(w, side, s):
        shard = f - s if side == 0 else f + s
        ref = bufs[w].at[shard, half(w)]
        return remote(ref, ref, ys.at[side, w, s], yr.at[side, w, s], {"rep": 1 - rep})

    def across_in(w, side, s):
        shard = f - s if side == 0 else f + s
        ref = bufs[w].at[shard, other(w)]
        return remote(ref, ref, ys.at[side, w, s], yr.at[side, w, s], {"rep": 1 - rep})

    def has(side, s):
        return f >= s if side == 0 else f + s <= F - 1

    def sends(side, s):
        ahead = f < F - 1 if side == 0 else f > 0
        return jnp.logical_and(has(side, s), ahead)

    def launch(w):
        for side in (0, 1):
            @pl.when(sends(side, 0))
            def _():
                hop(w, side, 0).start()

    def relay(group, stages=range(1, F)):
        for s in stages:
            for w in group:
                for side in (0, 1):
                    @pl.when(has(side, s))
                    def _():
                        arrival(w, side, s).wait_recv()
                        if s < F - 1:
                            @pl.when(sends(side, s))
                            def _():
                                hop(w, side, s).start()
                        if split == 2:
                            across(w, side, s).start()

    def settle(group):
        for w in group:
            own[w].wait()
        if split == 2:
            for s in range(1, F):
                for w in group:
                    for side in (0, 1):
                        @pl.when(has(side, s))
                        def _():
                            across_in(w, side, s).wait_recv()

    def tp_send(k, src, dst_at, d):
        return remote(src, dst_at, ts.at[k, d], tr.at[k, d], {"tp": lax.rem(me + d, T)})

    for w in (0, 1):
        launch(w)
    for d in range(1, T):
        tp_send(0, x_ref, xg.at[me], d).start()
    launch(2)
    xg[me] = x_ref[...]
    for d in range(1, T):
        peer = lax.rem(me + T - d, T)
        tp_send(0, x_ref, xg.at[peer], d).wait_recv()

    block = chunk_of(count, 16)

    def norm_rows(src, gain):
        def step(i, _):
            r = pl.ds(pl.multiple_of(i * block, block), block)
            vals = [src[t, r, :].astype(F32) for t in range(T)]
            ss = sum(jnp.sum(v * v, axis=1, keepdims=True) for v in vals)
            scale = lax.rsqrt(ss / width + EPS)
            for t in range(T):
                rows[r, t * dt:(t + 1) * dt] = (
                    vals[t] * scale * gain[t:t + 1, :]
                ).astype(BF16)
            return 0
        lax.fori_loop(0, count // block, step, 0)

    norm_rows(xg, ng_ref)
    relay((0, 1, 2))
    for w in (3, 4, 5):
        launch(w)
    settle((0, 1))

    chan = bv.shape[2]
    batch = count // length
    taps = cw_ref.shape[0]
    pad = 8 * ((taps - 1 + 7) // 8)
    lead = pad - (taps - 1)

    def columns(buf, c, n):
        block_w = buf[:, :, pl.ds(pl.multiple_of(c * n, n), n)]
        return block_w.reshape(block_w.shape[0] * block_w.shape[1], n)

    nc = chunk_of(chan, 256)

    def glu_step(c, _):
        value = jnp.dot(rows[...], columns(bv, c, nc), preferred_element_type=F32)
        gate = jnp.dot(rows[...], columns(bg, c, nc), preferred_element_type=F32)
        res = value * jax.nn.sigmoid(gate)
        for b in range(batch):
            glu[b, pl.ds(pad, length), pl.ds(pl.multiple_of(c * nc, nc), nc)] = (
                res[b * length:(b + 1) * length]
            )
        return 0

    for b in range(batch):
        glu[b, 0:pad, :] = jnp.zeros((pad, chan), F32)
        glu[b, pad + length:, :] = jnp.zeros((8, chan), F32)
    lax.fori_loop(0, chan // nc, glu_step, 0)
    relay((3,), (1,))

    lanes = chunk_of(chan, 128)
    span = chunk_of(length, 64)
    strips = chan // lanes

    def conv_step(i, _):
        q = lax.rem(i, strips)
        p = i // strips
        cols = pl.ds(pl.multiple_of(q * lanes, lanes), lanes)
        weights = cw_ref[:, cols]
        for b in range(batch):
            total = jnp.zeros((span, lanes), F32)
            for shift in range(8):
                acc = None
                for tap in range(taps):
                    if (lead + tap) % 8 != shift:
                        continue
                    base = lead + tap - shift
                    term = weights[tap:tap + 1, :] * glu[
                        b, pl.ds(pl.multiple_of(p * span + base, 8), span + 8), cols
                    ]
                    acc = term if acc is None else acc + term
                if acc is not None:
                    total = total + acc[shift:shift + span]
            conv[pl.ds(pl.multiple_of(b * length + p * span, span), span), cols] = total
        return 0

    lax.fori_loop(0, strips * (length // span), conv_step, 0)

    lane = lax.broadcasted_iota(jnp.int32, (count, 128), 1)

    def across_lanes(a, b):
        table = jnp.where(lane == 0, a, jnp.where(lane == 1, b, 0.0))
        return jnp.transpose(table)[0:8, :]

    def down_rows(top):
        full = jnp.concatenate([top, jnp.zeros((120, count), F32)], axis=0)
        return jnp.transpose(full)

    values = conv[...]
    local_sum = jnp.sum(values, axis=1, keepdims=True)
    dev = values - local_sum / chan
    st1[...] = across_lanes(local_sum, jnp.sum(dev * dev, axis=1, keepdims=True))
    sg1[me] = st1[...]
    for d in range(1, T):
        tp_send(1, st1, sg1.at[me], d).start()
    relay((4,), (1,))
    for d in range(1, T):
        peer = lax.rem(me + T - d, T)
        tp_send(1, st1, sg1.at[peer], d).wait_recv()
    sums = [sg1[t] for t in range(T)]
    mean = sum(s[0:1, :] for s in sums) / (chan * T)
    spread = sum(
        s[1:2, :] + chan * (s[0:1, :] / chan - mean) * (s[0:1, :] / chan - mean) for s in sums
    ) / (chan * T)
    inv = lax.rsqrt(spread + EPS)
    line = lax.broadcasted_iota(jnp.int32, (8, count), 0)
    table = down_rows(jnp.where(line == 0, mean, jnp.where(line == 1, inv, 0.0)))
    normed = (conv[...] - table[:, 0:1]) * table[:, 1:2] * cg_ref[...]
    act[...] = (normed * jax.nn.sigmoid(normed)).astype(BF16)

    settle((2,))

    def project(src, buf, part):
        dsh = buf.shape[2]
        for j in range(F):
            t, off = (j * dsh) // dt, (j * dsh) % dt
            prod = jnp.dot(src[...], buf[j], preferred_element_type=F32)
            part[t, :, off:off + dsh] = prod.astype(BF16)

    def scatter(k, part, got):
        for d in range(1, T):
            tp_send(k, part.at[lax.rem(me + d, T)], got.at[d - 1], d).start()

    def gathered(k, part, got):
        total = part[me].astype(F32)
        for d in range(1, T):
            tp_send(k, part.at[me], got.at[d - 1], d).wait_recv()
            total = total + got[d - 1].astype(F32)
        return total

    def piece(t):
        return remote(part2.at[t], got2.at[me], ts.at[4, t], tr.at[4, me], {"tp": t})

    def piece_in(t):
        return remote(part2.at[t], got2.at[t], ts.at[4, t], tr.at[4, t], {"tp": t})

    project(act, bo, part1)
    scatter(2, part1, got1)
    relay((5,), (1,))
    first = (x_ref[...].astype(F32) + gathered(2, part1, got1)).astype(BF16)
    firsts[me] = first
    for d in range(1, T):
        tp_send(3, firsts.at[me], firsts.at[me], d).start()
    relay((3,), (2,))
    for d in range(1, T):
        peer = lax.rem(me + T - d, T)
        tp_send(3, firsts.at[peer], firsts.at[peer], d).wait_recv()
    relay((4,), (2,))
    norm_rows(firsts, mg_ref)
    relay((5,), (2,))
    relay((3, 4), range(3, F))
    settle((3, 4))

    ff = bga.shape[2]
    nf = chunk_of(ff, 256)

    def ff_step(c, _):
        gate = jnp.dot(rows[...], columns(bga, c, nf), preferred_element_type=F32)
        up = jnp.dot(rows[...], columns(bup, c, nf), preferred_element_type=F32)
        hid[:, pl.ds(pl.multiple_of(c * nf, nf), nf)] = (
            gate * jax.nn.sigmoid(gate) * up
        ).astype(BF16)
        return 0

    lax.fori_loop(0, ff // nf, ff_step, 0)
    if F == T and bd.shape[2] == dt:
        def down(shard):
            prod = jnp.dot(hid[...], bd[shard], preferred_element_type=F32)
            part2[shard] = prod.astype(BF16)

            @pl.when(shard != me)
            def _():
                piece(shard).start()

        own[5].wait()
        down(f)
        for s in range(1, F):
            if s >= 3:
                relay((5,), (s,))
            for side in (0, 1):
                @pl.when(has(side, s))
                def _():
                    if split == 2:
                        across_in(5, side, s).wait_recv()
                    down(f - s if side == 0 else f + s)
    else:
        relay((5,), range(3, F))
        settle((5,))
        project(hid, bd, part2)
        for d in range(1, T):
            piece(lax.rem(me + d, T)).start()
    second = firsts[me].astype(F32) + part2[me].astype(F32)
    for d in range(1, T):
        peer = lax.rem(me + d, T)
        piece_in(peer).wait_recv()
        second = second + got2[peer].astype(F32)
    total = jnp.sum(second * second, axis=1, keepdims=True)
    conv[:, 0:dt] = second
    st2[...] = across_lanes(total, total)
    sg2[me] = st2[...]
    for d in range(1, T):
        tp_send(5, st2, sg2.at[me], d).start()
    for d in range(1, T):
        peer = lax.rem(me + T - d, T)
        tp_send(5, st2, sg2.at[peer], d).wait_recv()
    full = sum(sg2[t] for t in range(T))
    table = down_rows(full)
    scale = lax.rsqrt(table[:, 0:1] / width + EPS)
    out_ref[...] = (conv[:, 0:dt] * scale * fg_ref[...]).astype(BF16)

    for w in range(6):
        for side in (0, 1):
            for s in range(F):
                if s < F - 1:
                    @pl.when(sends(side, s))
                    def _():
                        hop(w, side, s).wait_send()
                if s >= 1 and split == 2:
                    @pl.when(has(side, s))
                    def _():
                        across(w, side, s).wait_send()
    for d in range(1, T):
        peer = lax.rem(me + d, T)
        tp_send(0, x_ref, xg.at[me], d).wait_send()
        tp_send(1, st1, sg1.at[me], d).wait_send()
        tp_send(2, part1.at[peer], got1.at[d - 1], d).wait_send()
        tp_send(3, firsts.at[me], firsts.at[me], d).wait_send()
        piece(peer).wait_send()
        tp_send(5, st2, sg2.at[me], d).wait_send()


PIECES = (2, 2, 2, 2, 2, 8)
FIRST = tuple(sum(PIECES[:w]) for w in range(6))
GROUP = (0, 0, 0, 1, 1, 2)
SLOT = (0, 1, 2, 3, 0, 4)


def fast_kernel(
    length,
    x_ref, ng_hbm, cw_hbm, cg_hbm, mg_hbm, fg_hbm,
    wv_ref, wg_ref, wo_ref, wga_ref, wup_ref, wd_ref,
    out_ref,
    ng_ref, cw_ref, cg_ref, mg_ref, fg_ref, bv, bg, bo, bga, bup, bd,
    xg, rows, accv, accg, glu, conv, act, part, got, q1, q1in, firsts, hid,
    accs, part2, got2, q2, q2in, sec, ssq, secb, secin, st1, sg1, st2, sg2, finin,
    small, own_sem, zs, zr, zr2, ms, mr, md, ys, yr, xos, xor_, ags, agr, sts, str_, rss, rsr, ds_, dr, qs, qr, os_, orr, fs_, fr,
):
    f = lax.axis_index("fs")
    me = lax.axis_index("tp")
    rep = lax.axis_index("rep")
    count, dt = x_ref.shape
    T = 4
    width = dt * T
    rows_all = 2 * count
    batch = count // length
    chan, ff = bv.shape[2], bga.shape[2]
    local = [wv_ref, wg_ref, wo_ref, wga_ref, wup_ref, wd_ref]
    bufs = [bv, bg, bo, bga, bup, bd]
    VAL, GATE, CVO, GA, UP, DOWN = range(6)
    outer = jnp.logical_or(f == 0, f == 3)
    near = 1 + f // 3
    po, pi, fo = 3 * (f - 1), 3 - f, 3 * (2 - f)
    sib = me + 1 - 2 * lax.rem(me, 2)
    mir = lax.rem(me + 2, T)
    dia = lax.rem(sib + 2, T)

    def view(ref, w, h, c):
        if w == DOWN:
            n, m = ref.shape[1] // 2, ref.shape[0] // 4
            k = n // 2
            return ref.at[pl.ds((c % 4) * m, m), pl.ds(pl.multiple_of(h * n + (c // 4) * k, k), k)]
        n = ref.shape[0] // 2
        k = n // PIECES[w]
        return ref.at[pl.ds(pl.multiple_of(h * n + c * k, k), k), :]

    barrier = pltpu.get_barrier_semaphore()

    def greet(**target):
        pl.semaphore_signal(barrier, inc=1, device_id=target, device_id_type=MESH)

    def source(w):
        return bufs[w].at[f] if w == VAL else local[w]

    def zsend(w, hs, c):
        h = rep if hs == 0 else 1 - rep
        sem = zr2.at[w + c // 4 if w == DOWN else w] if hs else zr.at[FIRST[w] + c]
        return remote(view(source(w), w, h, c), view(bufs[w].at[f], w, h, c), zs.at[GROUP[w]], sem, {"fs": near})

    def all_sent(sems, eighths):
        n = bd.shape[1] * eighths // 8
        for g, ref in enumerate((bufs[VAL].at[0:3], bufs[GA].at[0:2], bufs[DOWN].at[0, 0:n, :])):
            remote(ref, ref, sems.at[g], sems.at[g], {"fs": f}).wait_send()

    def xsend():
        return remote(x_ref, xg.at[me, 0], xos, xor_, {"fs": near})

    hn = dt // 2

    def ucols(j):
        if j == 0:
            return pl.ds(pl.multiple_of(rep * hn, hn), hn)
        if j > 3:
            return pl.ds(pl.multiple_of(rep * hn + (j - 4) * (hn // 2), hn // 2), hn // 2)
        return pl.ds(pl.multiple_of((1 - rep) * hn + min(j - 1, 1) * (hn // 2), hn // 2), hn // 2)

    def urows(j):
        return slice((j - 2) * count, (j - 1) * count) if j in (2, 3) else slice(0, rows_all)

    def result(cols, target):
        return remote(secb.at[:, cols], secin.at[:, cols], os_, orr, {"fs": target})

    smalls = [
        pltpu.make_async_copy(src, dst, small.at[k])
        for k, (src, dst) in enumerate(
            ((ng_hbm, ng_ref), (cw_hbm, cw_ref), (cg_hbm, cg_ref), (mg_hbm, mg_ref), (fg_hbm, fg_ref))
        )
    ]

    lane = lax.broadcasted_iota(jnp.int32, (count, 128), 1)
    line = lax.broadcasted_iota(jnp.int32, (8, count), 0)

    def across_lanes(a, b):
        table = jnp.where(lane == 0, a, jnp.where(lane == 1, b, 0.0))
        return jnp.transpose(table)[0:8, :]

    def down_rows(top):
        full = jnp.concatenate([top, jnp.zeros((120, count), F32)], axis=0)
        return jnp.transpose(full)

    @pl.when(outer)
    def _():
        greet(fs=near)
        first = pltpu.make_async_copy(local[VAL], bufs[VAL].at[f], own_sem.at[VAL])
        first.start()
        smalls[4].start()
        pl.semaphore_wait(barrier, 1)
        first.wait()
        order = [
            (VAL, 0), (GATE, 0), None, (CVO, 0), (VAL, 1), (GATE, 1), (CVO, 1),
            (GA, 0), (UP, 0), (GA, 1),
        ]
        for item in order:
            if item is None:
                xsend().start()
            else:
                for c in range(PIECES[item[0]]):
                    zsend(item[0], item[1], c).start()
        zsend(UP, 1, 0).start()
        zsend(DOWN, 0, 0).start()
        zsend(DOWN, 0, 1).start()
        zsend(UP, 1, 1).start()
        for c in range(2, PIECES[DOWN]):
            zsend(DOWN, 0, c).start()
        for c in range(PIECES[DOWN]):
            zsend(DOWN, 1, c).start()
        xsend().wait_send()
        all_sent(zs, 8)
        smalls[4].wait()
        remote(secb, secin, os_, orr, {"fs": near}).wait_recv()
        remote(finin, finin, fs_, fr, {"fs": near}).wait_recv()
        full = sum(finin[t] for t in range(T))
        scale = lax.rsqrt(down_rows(full)[:, 0:1] / width + EPS)
        out_ref[...] = (secin[...].astype(F32) * scale * fg_ref[...]).astype(BF16)

    @pl.when(jnp.logical_not(outer))
    def _():
        greet(fs=po)
        greet(fs=pi)
        greet(rep=1 - rep)
        for t in (sib, mir):
            greet(tp=t)
        own = [pltpu.make_async_copy(local[w], bufs[w].at[f], own_sem.at[w]) for w in range(6)]
        load_x = pltpu.make_async_copy(x_ref, xg.at[me, 1], small.at[5])
        load_x.start()
        for copy in smalls:
            copy.start()
        for copy in own:
            copy.start()
        pl.semaphore_wait(barrier, 5)

        def arrived(ref, send, recv):
            remote(ref, ref, send, recv, {"fs": f}).wait_recv()

        def mid_own(w, c):
            return remote(
                view(source(w), w, rep, c), view(bufs[w].at[f], w, rep, c), ms.at[GROUP[w]], mr.at[0, FIRST[w] + c], {"fs": pi}
            )

        def mid_fwd(w, c):
            ref = view(bufs[w].at[po], w, rep, c)
            return remote(ref, ref, ms.at[GROUP[w]], mr.at[1, FIRST[w] + c], {"fs": pi})

        def mid_direct(c):
            return remote(
                view(local[DOWN], DOWN, 1 - rep, c), view(bufs[DOWN].at[f], DOWN, 1 - rep, c), md.at[0], md.at[1], {"fs": pi}
            )

        def y_fwd(w, k, c):
            ref = view(bufs[w].at[fo if k else pi], w, rep, c)
            sem = yr.at[k, w + c // 4 if w == DOWN else w]
            return remote(ref, ref, ys.at[GROUP[w]], sem, {"rep": 1 - rep})

        def wait_z_down(j):
            arrived(bufs[DOWN].at[po, :, ucols(j)], zs.at[2], zr2.at[DOWN + j - 1])

        def send_own(w):
            for c in range(PIECES[w]):
                mid_own(w, c).start()

        def relay_mid(w, c):
            arrived(view(bufs[w].at[po], w, rep, c), zs.at[GROUP[w]], zr.at[FIRST[w] + c])
            mid_fwd(w, c).start()

        def wait_mid(w, k, c):
            arrived(view(bufs[w].at[fo if k else pi], w, rep, c), ms.at[GROUP[w]], mr.at[k, FIRST[w] + c])

        def relay_y(w, k, c):
            wait_mid(w, k, c)
            y_fwd(w, k, c).start()

        def other(w, shard):
            n = bufs[w].shape[1] // 2
            return bufs[w].at[shard, pl.ds(pl.multiple_of((1 - rep) * n, n), n), :]

        def wait_z(w):
            arrived(other(w, po), zs.at[GROUP[w]], zr2.at[w])

        def wait_y(w, k):
            arrived(other(w, fo if k else pi), ys.at[GROUP[w]], yr.at[k, w])

        def wait_y_down(k, j):
            ref = bufs[DOWN].at[fo if k else pi, :, ucols(j)]
            arrived(ref, ys.at[2], yr.at[k, DOWN + j - 1])

        def wait_last():
            m = bd.shape[1] // 2
            arrived(bufs[DOWN].at[pi, 0:m, ucols(2)], ys.at[2], yr.at[0, 6])
            arrived(bufs[DOWN].at[pi, m:2 * m, ucols(2)], md.at[0], md.at[1])

        def ag(p, buf, slot, kind):
            ref = buf.at[mir if kind == 2 else me, slot]
            return remote(
                ref, ref, ags.at[p, slot], agr.at[p, slot, 1 if kind == 1 else 0], {"tp": mir if kind == 1 else sib}
            )

        def ag_start(p, buf, slot):
            ag(p, buf, slot, 1).start()
            ag(p, buf, slot, 0).start()

        def ag_forward(p, buf, slot):
            arrived(buf.at[mir, slot], ags.at[p, slot], agr.at[p, slot, 1])
            ag(p, buf, slot, 2).start()

        def ag_finish(p, buf, slot):
            arrived(buf.at[0:2, slot], ags.at[p, slot], agr.at[p, slot, 0])

        block = chunk_of(count, 32)

        def norm_rows(src, slot, gain):
            def step(i, _):
                r = pl.ds(pl.multiple_of(i * block, block), block)
                o = pl.ds(pl.multiple_of(slot * count + i * block, block), block)
                vals = [src[t, slot, r, :].astype(F32) for t in range(T)]
                ss = sum(jnp.sum(v * v, axis=1, keepdims=True) for v in vals)
                scale = lax.rsqrt(ss / width + EPS)
                for t in range(T):
                    rows[t, o, :] = (vals[t] * scale * gain[:, t * dt:(t + 1) * dt]).astype(BF16)
                return 0
            lax.fori_loop(0, count // block, step, 0)

        def stat(k, src, dst, d):
            return remote(src, dst, sts.at[k], str_.at[k], {"tp": lax.rem(me + d, T)})

        own[VAL].wait()
        send_own(VAL)
        send_own(GATE)
        load_x.wait()
        ag_start(0, xg, 1)
        for c in range(2):
            relay_mid(VAL, c)
            relay_y(VAL, 0, c)
        relay_mid(GATE, 0)
        ag_forward(0, xg, 1)
        relay_y(GATE, 0, 0)
        relay_mid(GATE, 1)
        relay_y(GATE, 0, 1)
        send_own(CVO)
        ag_finish(0, xg, 1)
        for copy in smalls:
            copy.wait()
        norm_rows(xg, 1, ng_ref)
        relay_y(VAL, 1, 0)
        arrived(xg.at[me, 0], xos, xor_)
        ag_start(0, xg, 0)
        relay_y(VAL, 1, 1)
        relay_mid(CVO, 0)
        relay_y(GATE, 1, 0)
        relay_mid(CVO, 1)
        send_own(GA)
        send_own(UP)
        relay_y(GATE, 1, 1)
        ag_forward(0, xg, 0)
        ag_finish(0, xg, 0)
        norm_rows(xg, 0, ng_ref)
        relay_y(CVO, 0, 0)

        pad = glu.shape[1] - length - 8
        taps = cw_ref.shape[0]
        lead = pad - (taps - 1)
        nc = chunk_of(chan, 256)
        for b in range(2 * batch):
            glu[b, 0:pad, :] = jnp.zeros((pad, chan), F32)
            glu[b, pad + length:, :] = jnp.zeros((8, chan), F32)

        def s1(shard, first, last):
            def step(c, _):
                cols = pl.ds(pl.multiple_of(c * nc, nc), nc)
                value = jnp.dot(rows[shard], bv[shard, :, cols], preferred_element_type=F32)
                gate = jnp.dot(rows[shard], bg[shard, :, cols], preferred_element_type=F32)
                if not first:
                    value = value + accv[:, cols]
                    gate = gate + accg[:, cols]
                if last:
                    res = value * jax.nn.sigmoid(gate)
                    for b in range(2 * batch):
                        glu[b, pl.ds(pad, length), cols] = res[b * length:(b + 1) * length]
                else:
                    accv[:, cols] = value
                    accg[:, cols] = gate
                return 0
            lax.fori_loop(0, chan // nc, step, 0)

        own[GATE].wait()
        s1(f, True, False)
        wait_y(VAL, 0)
        wait_y(GATE, 0)
        s1(pi, False, False)
        relay_y(CVO, 0, 1)
        wait_y(VAL, 1)
        wait_y(GATE, 1)
        s1(fo, False, False)
        relay_y(CVO, 1, 0)
        wait_z(VAL)
        wait_z(GATE)
        s1(po, False, True)
        relay_y(CVO, 1, 1)

        lanes = chunk_of(chan, 128)
        span = chunk_of(length, 64)
        strips = chan // lanes

        def convolve(slot):
            def step(i, _):
                s = lax.rem(i, strips)
                p = i // strips
                cols = pl.ds(pl.multiple_of(s * lanes, lanes), lanes)
                weights = cw_ref[:, cols]
                for b in range(batch):
                    total = jnp.zeros((span, lanes), F32)
                    for shift in range(8):
                        acc = None
                        for tap in range(taps):
                            if (lead + tap) % 8 != shift:
                                continue
                            base = lead + tap - shift
                            term = weights[tap:tap + 1, :] * glu[
                                slot * batch + b, pl.ds(pl.multiple_of(p * span + base, 8), span + 8), cols
                            ]
                            acc = term if acc is None else acc + term
                        if acc is not None:
                            total = total + acc[shift:shift + span]
                    at = pl.multiple_of(slot * count + b * length + p * span, span)
                    conv[pl.ds(at, span), cols] = total
                return 0
            lax.fori_loop(0, strips * (length // span), step, 0)

        def span_of(slot):
            return slice(slot * count, (slot + 1) * count)

        def conv_stats(slot):
            values = conv[span_of(slot), :]
            local_sum = jnp.sum(values, axis=1, keepdims=True)
            dev = values - local_sum / chan
            st1[slot] = across_lanes(local_sum, jnp.sum(dev * dev, axis=1, keepdims=True))
            sg1[slot, me] = st1[slot]
            for d in range(1, T):
                stat(slot, st1.at[slot], sg1.at[slot, me], d).start()

        def activate(slot):
            arrived(sg1.at[slot, 0:3], sts.at[slot], str_.at[slot])
            sums = [sg1[slot, t] for t in range(T)]
            mean = sum(s[0:1, :] for s in sums) / (chan * T)
            spread = sum(
                s[1:2, :] + chan * (s[0:1, :] / chan - mean) * (s[0:1, :] / chan - mean) for s in sums
            ) / (chan * T)
            inv = lax.rsqrt(spread + EPS)
            table = down_rows(jnp.where(line == 0, mean, jnp.where(line == 1, inv, 0.0)))
            normed = (conv[span_of(slot), :] - table[:, 0:1]) * table[:, 1:2] * cg_ref[...]
            act[span_of(slot), :] = (normed * jax.nn.sigmoid(normed)).astype(BF16)

        def rs(slot, kind):
            if kind == 2:
                return remote(q1.at[slot], q1in.at[slot], rss.at[slot], rsr.at[slot, 0], {"tp": mir})
            return remote(
                part.at[slot, dia if kind else sib], got.at[slot, kind], rss.at[slot], rsr.at[slot, kind], {"tp": sib}
            )

        def project(slot):
            def step(j, _):
                prod = jnp.dot(act[span_of(slot), :], bo[j], preferred_element_type=F32)
                part[slot, j] = prod.astype(BF16)
                return 0
            lax.fori_loop(0, T, step, 0)
            rs(slot, 1).start()
            rs(slot, 0).start()

        def pair_sum(slot):
            rs(slot, 1).wait_recv()
            q1[slot] = (part[slot, mir].astype(F32) + got[slot, 1].astype(F32)).astype(BF16)
            rs(slot, 2).start()

        def finish_first(slot):
            arrived(part.at[slot, 0:2], rss.at[slot], rsr.at[slot, 0])
            total = xg[me, slot].astype(F32) + (part[slot, me].astype(F32) + got[slot, 0].astype(F32))
            firsts[me, slot] = (total + q1in[slot].astype(F32)).astype(BF16)
            ag_start(1, firsts, slot)

        convolve(0)
        conv_stats(0)
        convolve(1)
        conv_stats(1)
        relay_y(GA, 0, 0)
        own[CVO].wait()
        wait_y(CVO, 0)
        wait_y(CVO, 1)
        wait_z(CVO)
        activate(0)
        project(0)
        activate(1)
        project(1)
        pair_sum(0)
        relay_y(GA, 0, 1)
        relay_mid(GA, 0)
        pair_sum(1)
        relay_y(UP, 0, 0)
        relay_mid(GA, 1)
        relay_y(UP, 0, 1)
        finish_first(0)
        relay_mid(UP, 0)
        relay_y(GA, 1, 0)
        finish_first(1)
        relay_mid(UP, 1)
        send_own(DOWN)
        relay_y(GA, 1, 1)
        relay_y(UP, 1, 0)
        ag_forward(1, firsts, 0)
        ag_finish(1, firsts, 0)
        norm_rows(firsts, 0, mg_ref)
        relay_y(UP, 1, 1)
        ag_forward(1, firsts, 1)
        ag_finish(1, firsts, 1)
        relay_y(DOWN, 0, 0)
        relay_y(DOWN, 0, 1)
        norm_rows(firsts, 1, mg_ref)
        relay_y(DOWN, 0, 2)
        relay_y(DOWN, 0, 3)

        nf = chunk_of(ff, 256)

        def s5(w, shards, keep):
            def step(c, _):
                cols = pl.ds(pl.multiple_of(c * nf, nf), nf)
                value = sum(jnp.dot(rows[t], bufs[w][t, :, cols], preferred_element_type=F32) for t in shards)
                if keep:
                    accs[w - GA, :, cols] = value
                else:
                    gate = accs[0, :, cols]
                    hid[:, cols] = (gate * jax.nn.sigmoid(gate) * (value + accs[1, :, cols])).astype(BF16)
                return 0
            lax.fori_loop(0, ff // nf, step, 0)

        own[GA].wait()
        own[UP].wait()
        wait_y(GA, 0)
        wait_y(GA, 1)
        wait_z(GA)
        relay_mid(DOWN, 0)
        s5(GA, (f, pi, po, fo), True)
        relay_mid(DOWN, 1)
        wait_y(UP, 0)
        s5(UP, (f, pi), True)
        relay_y(DOWN, 0, 4)
        relay_y(DOWN, 0, 5)
        wait_z(UP)
        wait_y(UP, 1)
        s5(UP, (po, fo), False)

        def pair_send(b, j):
            at = (b, urows(j), ucols(j))
            return remote(part2.at[at], got2.at[at], ds_, dr.at[lax.rem(b // 2 + me // 2, 2), SLOT[j]], {"tp": sib})

        def cross(j):
            at = (urows(j), ucols(j))
            return remote(q2.at[at], q2in.at[at], qs, qr.at[SLOT[j]], {"tp": mir})

        def down(b, j):
            r, cols = urows(j), ucols(j)
            prod = jnp.dot(hid[r, :], bd[b, :, cols], preferred_element_type=F32)
            part2[b, r, cols] = prod.astype(BF16)

            @pl.when(jnp.logical_or(b == sib, b == dia))
            def _():
                pair_send(b, j).start()

        def combine(b, j):
            r, cols = urows(j), ucols(j)

            @pl.when(b == mir)
            def _():
                pair_send(b, j).wait_recv()
                q2[r, cols] = (part2[b, r, cols].astype(F32) + got2[b, r, cols].astype(F32)).astype(BF16)
                cross(j).start()

        def outer_stat(t):
            return remote(st2.at[0], finin.at[me], fs_, fr, {"fs": po, "tp": t})

        def finish(b, j):
            @pl.when(b == me)
            def _():
                pair_send(me, j).wait_recv()
                cross(j).wait_recv()
                cols = ucols(j)
                for slot in (j - 2,) if j in (2, 3) else (0, 1):
                    r = span_of(slot)
                    second = firsts[me, slot, :, cols].astype(F32) + part2[me, r, cols].astype(F32)
                    second = second + got2[me, r, cols].astype(F32) + q2in[r, cols].astype(F32)
                    total = jnp.sum(second * second, axis=1, keepdims=True)
                    if j not in (0, 4):
                        total = total + ssq[r, :]
                    if slot == 0:
                        secb[:, cols] = second.astype(BF16)
                    else:
                        sec[:, cols] = second
                    if j not in (2, 3):
                        ssq[r, :] = total
                    else:
                        st2[slot] = across_lanes(total, total)
                    if j == 2:
                        for t in (mir, dia, me, sib):
                            outer_stat(t).start()
                    if j == 3:
                        sg2[me] = st2[1]
                        for d in (2, 1, 3):
                            stat(2, st2.at[1], sg2.at[me], d).start()
                    if slot == 0:
                        result(cols, po).start()

        own[DOWN].wait()
        for c in range(6, 8):
            wait_mid(DOWN, 0, c)
        down(pi, 0)
        down(f, 0)
        relay_mid(DOWN, 2)
        relay_mid(DOWN, 3)
        combine(pi, 0)
        down(f, 1)
        combine(f, 0)
        wait_y_down(0, 1)
        down(pi, 1)
        relay_mid(DOWN, 4)
        relay_mid(DOWN, 5)
        relay_y(DOWN, 1, 0)
        relay_y(DOWN, 1, 1)
        combine(f, 1)
        combine(pi, 1)
        down(f, 2)
        down(f, 3)
        relay_mid(DOWN, 6)
        relay_mid(DOWN, 7)
        mid_direct(6).start()
        mid_direct(7).start()
        relay_y(DOWN, 1, 2)
        relay_y(DOWN, 1, 3)
        down(po, 0)
        down(fo, 4)
        relay_y(DOWN, 1, 4)
        relay_y(DOWN, 1, 5)
        combine(f, 2)
        combine(f, 3)
        combine(po, 0)
        combine(fo, 4)
        relay_y(DOWN, 1, 6)
        relay_y(DOWN, 1, 7)
        down(fo, 5)
        wait_y_down(1, 1)
        down(fo, 1)
        finish(f, 0)
        finish(pi, 0)
        combine(fo, 5)
        wait_z_down(1)
        down(po, 1)
        combine(fo, 1)
        wait_last()
        down(pi, 2)
        down(pi, 3)
        finish(f, 1)
        finish(pi, 1)
        combine(po, 1)
        wait_z_down(2)
        down(po, 2)
        down(po, 3)
        combine(pi, 2)
        combine(pi, 3)
        finish(po, 0)
        wait_y_down(1, 2)
        down(fo, 2)
        combine(po, 2)
        down(fo, 3)
        combine(fo, 2)
        combine(po, 3)
        combine(fo, 3)
        finish(fo, 4)
        finish(po, 1)
        finish(fo, 5)
        finish(fo, 1)
        for j in (2, 3):
            for b in (f, po, pi, fo):
                finish(b, j)
        arrived(sg2.at[0:3], sts.at[2], str_.at[2])
        table = down_rows(sum(sg2[t] for t in range(T)))
        scale = lax.rsqrt(table[:, 0:1] / width + EPS)
        out_ref[...] = (sec[...] * scale * fg_ref[...]).astype(BF16)

        def sent(ref, sem):
            remote(ref, ref, sem, sem, {"fs": f}).wait_send()

        all_sent(ms, 8)
        all_sent(ys, 7)
        sent(bufs[DOWN].at[f, 0:bd.shape[1] // 2, ucols(2)], md.at[0])
        for slot in range(2):
            sent(xg.at[0:3, slot], ags.at[0, slot])
            sent(firsts.at[0:3, slot], ags.at[1, slot])
            sent(part.at[slot, 0:3], rss.at[slot])
            sent(sg1.at[slot, 0:3], sts.at[slot])
        sent(sg2.at[0:3], sts.at[2])
        sent(part2.at[0:2], ds_)
        sent(q2, qs)
        sent(secb, os_)
        sent(finin, fs_)


def fast_body(
    activations, norm_gain, w_value, w_gate_conv, conv_weight, chan_gain,
    w_conv_out, mix_gain, w_gate, w_up, w_down, final_gain,
):
    batch, length, dt = activations.shape
    count = batch * length
    weights = (w_value, w_gate_conv, w_conv_out, w_gate, w_up, w_down)
    chan, ff = w_value.shape[1], w_gate.shape[1]
    T = 4
    pad = 8 * ((conv_weight.shape[0] - 1 + 7) // 8)
    rows_all = 2 * count
    vmem, hbm = pl.BlockSpec(memory_space=pltpu.VMEM), pl.BlockSpec(memory_space=pl.ANY)
    dma = pltpu.SemaphoreType.DMA
    V = pltpu.VMEM
    out = pl.pallas_call(
        functools.partial(fast_kernel, length),
        out_shape=pltpu.VMEM((count, dt), BF16),
        in_specs=[hbm] * 12,
        out_specs=vmem,
        scratch_shapes=[
            V((1, dt * T), F32),
            V(conv_weight.shape, F32),
            V((1, chan), F32),
            V((1, dt * T), F32),
            V((1, dt), F32),
        ] + [V((4,) + w.shape, BF16) for w in weights] + [
            V((T, 2, count, dt), BF16),
            V((T, rows_all, dt), BF16),
            V((rows_all, chan), F32),
            V((rows_all, chan), F32),
            V((2 * batch, pad + length + 8, chan), F32),
            V((rows_all, chan), F32),
            V((rows_all, chan), BF16),
            V((2, T, count, dt), BF16),
            V((2, 2, count, dt), BF16),
            V((2, count, dt), BF16),
            V((2, count, dt), BF16),
            V((T, 2, count, dt), BF16),
            V((rows_all, ff), BF16),
            V((2, rows_all, ff), F32),
            V((T, rows_all, dt), BF16),
            V((T, rows_all, dt), BF16),
            V((rows_all, dt), BF16),
            V((rows_all, dt), BF16),
            V((count, dt), F32),
            V((rows_all, 1), F32),
            V((count, dt), BF16),
            V((count, dt), BF16),
            V((2, 8, count), F32),
            V((2, T, 8, count), F32),
            V((2, 8, count), F32),
            V((T, 8, count), F32),
            V((T, 8, count), F32),
            dma((6,)),
            dma((6,)),
            dma((3,)),
            dma((sum(PIECES),)),
            dma((7,)),
            dma((3,)),
            dma((2, sum(PIECES))),
            dma((2,)),
            dma((3,)),
            dma((2, 7)),
            dma(()),
            dma(()),
            dma((2, 2)),
            dma((2, 2, 2)),
            dma((3,)),
            dma((3,)),
            dma((2,)),
            dma((2, 2)),
            dma(()),
            dma((2, 5)),
            dma(()),
            dma((5,)),
            dma(()),
            dma(()),
            dma(()),
            dma(()),
        ],
        compiler_params=pltpu.CompilerParams(
            collective_id=0, has_side_effects=True, vmem_limit_bytes=60 * 1024 * 1024
        ),
        name="block",
    )(
        activations.reshape(count, dt),
        norm_gain.reshape(1, dt * T),
        conv_weight,
        chan_gain.reshape(1, chan),
        mix_gain.reshape(1, dt * T),
        final_gain.reshape(1, dt),
        *weights,
    )
    return out.reshape(batch, length, dt)


def ring_body(
    activations, norm_gain, w_value, w_gate_conv, conv_weight, chan_gain,
    w_conv_out, mix_gain, w_gate, w_up, w_down, final_gain,
):
    batch, length, dt = activations.shape
    count = batch * length
    R, F, T = lax.axis_size("rep"), lax.axis_size("fs"), lax.axis_size("tp")
    weights = (w_value, w_gate_conv, w_conv_out, w_gate, w_up, w_down)
    split = 2 if R == 2 and all(w.shape[0] % 32 == 0 for w in weights) else 1
    width = dt * T
    chan, ff = w_value.shape[1], w_gate.shape[1]
    taps = conv_weight.shape[0]
    pad = 8 * ((taps - 1 + 7) // 8)
    vmem, hbm = pl.BlockSpec(memory_space=pltpu.VMEM), pl.BlockSpec(memory_space=pl.ANY)
    ysh = (2, 6, F) if split == 2 else (1,)
    dma = pltpu.SemaphoreType.DMA
    out = pl.pallas_call(
        functools.partial(ring_kernel, R, F, T, split, length),
        out_shape=jax.ShapeDtypeStruct((count, dt), BF16),
        in_specs=[vmem] * 6 + [hbm] * 6,
        out_specs=vmem,
        scratch_shapes=[pltpu.VMEM((F,) + w.shape, BF16) for w in weights] + [
            pltpu.VMEM((T, count, dt), BF16),
            pltpu.VMEM((count, width), BF16),
            pltpu.VMEM((batch, pad + length + 8, chan), F32),
            pltpu.VMEM((count, max(chan, dt)), F32),
            pltpu.VMEM((count, chan), BF16),
            pltpu.VMEM((T, count, dt), BF16),
            pltpu.VMEM((T, count, dt), BF16),
            pltpu.VMEM((T - 1, count, dt), BF16),
            pltpu.VMEM((T, count, dt), BF16),
            pltpu.VMEM((T, count, dt), BF16),
            pltpu.VMEM((count, ff), BF16),
            pltpu.VMEM((8, count), F32),
            pltpu.VMEM((8, count), F32),
            pltpu.VMEM((T, 8, count), F32),
            pltpu.VMEM((T, 8, count), F32),
            dma((6,)),
            dma((2, 6, F)),
            dma((2, 6, F)),
            dma(ysh),
            dma(ysh),
            dma((6, T)),
            dma((6, T)),
        ],
        compiler_params=pltpu.CompilerParams(
            collective_id=0, has_side_effects=True, vmem_limit_bytes=60 * 1024 * 1024
        ),
        name="block",
    )(
        activations.reshape(count, dt),
        norm_gain.reshape(T, dt),
        conv_weight,
        chan_gain.reshape(1, chan),
        mix_gain.reshape(T, dt),
        final_gain.reshape(1, dt),
        *weights,
    )
    return out.reshape(batch, length, dt)


def solution(mesh):
    in_specs = (
        P(("rep", "fs"), None, "tp"),
        P(),
        P("fs", "tp"),
        P("fs", "tp"),
        P(None, "tp"),
        P("tp"),
        P("tp", "fs"),
        P(),
        P("fs", "tp"),
        P("fs", "tp"),
        P("tp", "fs"),
        P("tp"),
    )
    out_specs = P(("rep", "fs"), None, "tp")
    fast = tuple(mesh.shape[a] for a in ("rep", "fs", "tp")) == (2, 4, 4)
    body = fast_body if fast else ring_body
    return jax.shard_map(body, mesh=mesh, in_specs=in_specs, out_specs=out_specs, check_vma=False)
```
